256 devices in a mesh: sp: 32 (over z, x), tp: 8 (over y, core).
Axes of the slice: x: 4, y: 4, z: 8, core: 2. Of those that a mesh axis runs over, the one named last changes fastest.
Arguments:
- tokens: bfloat16 [16384, 2048], P(('sp', 'tp')), may hold values from -6 to 6
- input_gain: bfloat16 [2048], replicated, may hold values from 0.099609375 to 1.8984375
- weight_query: bfloat16 [2048, 1024], P(None, 'tp'), may hold values from -0.125 to 0.125
- weight_key: bfloat16 [2048, 1024], P(None, 'tp'), may hold values from -0.125 to 0.125
- weight_value: bfloat16 [2048, 2048], P(None, 'tp'), may hold values from -8 to 8
- weight_outgate: bfloat16 [2048, 2048], P(None, 'tp'), may hold values from -0.125 to 0.125
- weight_ingate: bfloat16 [2048, 8], replicated, may hold values from -0.125 to 0.125
- weight_forget: bfloat16 [2048, 8], replicated, may hold values from -0.125 to 0.125
- forget_shift: float32 [16384, 8], P('sp', 'tp'), may hold values from 0 to 20
- mem_gain: bfloat16 [2048], replicated, may hold values from 0.099609375 to 1.8984375
- query_down_weight: bfloat16 [2048, 768], P(None, 'tp'), may hold values from -0.125 to 0.125
- latent_down_weight: bfloat16 [2048, 512], P(None, 'tp'), may hold values from -0.125 to 0.125
- down_rotary: bfloat16 [2048, 64], replicated, may hold values from -0.125 to 0.125
- query_gain: float32 [768], replicated, may hold values from 0.15 to 12
- latent_gain: float32 [512], replicated, may hold values from 0.15 to 12
- query_up_weight: bfloat16 [768, 1536], P(None, 'tp'), may hold values from -0.4375 to 0.4375
- key_up_weight: bfloat16 [512, 1024], P(None, 'tp'), may hold values from -0.25 to 0.25
- value_up_weight: bfloat16 [512, 1024], P(None, 'tp'), may hold values from -0.25 to 0.25
- out_memory: bfloat16 [2048, 2048], P('tp'), may hold values from -0.5 to 0.5
- out_attend: bfloat16 [1024, 2048], P('tp'), may hold values from -0.75 to 0.75
Outputs:
- mixed: bfloat16 [16384, 2048], P(('sp', 'tp'))
The draws below stay inside these ranges and needn't reach their ends.
All inputs are finite; a program needn't handle non-finite values.
Results may differ from the reference program's by a relative error of at most 0.04.
The reference program's roundings to bfloat16 on the way count: a program that leaves them out, or rounds other values in their place, can miss the bound.
Values may be sent and summed in bfloat16 or wider, within the bound.
A program may use at most 128 MiB of HBM per device.

```python
import jax
import jax.numpy as jnp
from jax import lax

MODEL_WIDTH = 2048
MEMORY_HEADS = 8
M_QK = 128
M_V = 256
ATTEND_HEADS = 8
PLAIN_CHANNELS = 128
ROTARY_CHANNELS = 64
VALUE_CHANNELS = 128
QUERY_LATENT = 768
LATENT_WIDTH = 512
BLOCK = 64
TOK_DEV = 512
SEQUENCE_LENGTH = 16384
N_TP = 8


def draw_forget_shift(key, part):
    random_keys = jax.random.split(key, 5)
    shuffled = jax.random.permutation(random_keys[0], MEMORY_HEADS)
    quick_heads = shuffled[:MEMORY_HEADS // 2]
    fast_head = jnp.any(jnp.arange(MEMORY_HEADS)[None, :] == quick_heads[:, None], axis=0)
    block_total = SEQUENCE_LENGTH // TOK_DEV
    factor = jnp.exp(jax.random.uniform(random_keys[1], (block_total, MEMORY_HEADS), jnp.float32, -0.7, 0.7))
    factor = jnp.repeat(factor, TOK_DEV, axis=0)
    jitter = jnp.exp(jax.random.uniform(random_keys[2], (SEQUENCE_LENGTH, MEMORY_HEADS), jnp.float32, -0.35, 0.35))
    decay_rate = jnp.where(fast_head[None, :], 1.0 / 40.0, 0.4 / SEQUENCE_LENGTH) * factor * jitter
    score_retained = -jnp.log(jnp.expm1(decay_rate))
    spike_position = jax.random.randint(random_keys[3], (4, MEMORY_HEADS), 0, SEQUENCE_LENGTH)
    spike_retained = jax.random.uniform(random_keys[4], (4, MEMORY_HEADS), jnp.float32, 0.5, 0.8)
    spike_score = jnp.log(spike_retained / (1.0 - spike_retained))
    spike_matches = jnp.arange(SEQUENCE_LENGTH)[:, None, None] == spike_position[None, :, :]
    spike_amount = jnp.min(jnp.where(spike_matches, spike_score[None], 1000000000.0), axis=1)
    score_retained = jnp.minimum(score_retained, spike_amount)
    ratio = jnp.clip(score_retained, 0.0, 13.5) / 15.0
    return 7.5 * jnp.log((1.0 + ratio) / (1.0 - ratio))


def gain_entries(key, length):
    return 1.0 + 0.18 * jnp.clip(jax.random.normal(key, (length,), jnp.float32), -4.5, 4.5)


def draw_query_gain(key, part):
    return gain_entries(jax.random.fold_in(key, 11), QUERY_LATENT)


def draw_latent_gain(key, part):
    return gain_entries(jax.random.fold_in(key, 23), LATENT_WIDTH)


def draw_weight_value(key, part):
    position = jnp.arange(MEMORY_HEADS, dtype=jnp.float32) / max(MEMORY_HEADS - 1, 1)
    top_scale = 3.0
    head_scale = jnp.repeat(jnp.power(top_scale, position), M_V)
    base = jnp.clip(jax.random.normal(jax.random.fold_in(key, 37), (MODEL_WIDTH, MEMORY_HEADS * M_V), jnp.float32), -6.0, 6.0)
    return (base * head_scale[None, :] * MODEL_WIDTH ** (-0.5)).astype(jnp.bfloat16)


def levels(key, shape, pieces, low, largest):
    level = 1.0
    for dim, parts in pieces:
        draws = jax.random.uniform(jax.random.fold_in(jax.random.fold_in(key, 6), dim), (parts,), jnp.float32, low / len(pieces), largest / len(pieces))
        level = level * jnp.repeat(jnp.exp(draws), shape[dim] // parts).reshape((-1,) + (1,) * (len(shape) - 1 - dim))
    return level


def bell_draw(key, dims, spread, most, shards=(), kind=jnp.bfloat16):
    level = levels(key, dims, shards, -0.22, 0.18) if shards else 1.0
    values = jax.random.normal(key, dims, jnp.float32) * spread * level
    return jnp.minimum(jnp.maximum(values, -most), most).astype(kind)


def setup_inputs(seed: int = 0) -> dict:
    key_list = jax.random.split(jax.random.key(seed), 21)
    tokens = bell_draw(key_list[0], (SEQUENCE_LENGTH, MODEL_WIDTH), 1.0, 6.0, ((0, 256),))
    input_gain = jnp.clip(1.0 + 0.18 * jax.random.normal(key_list[1], (MODEL_WIDTH,), jnp.float32), 0.099609375, 1.8984375).astype(jnp.bfloat16)
    weight_query = bell_draw(key_list[2], (MODEL_WIDTH, MEMORY_HEADS * M_QK), MODEL_WIDTH ** -0.5, 0.125, ((1, 8),))
    weight_key = bell_draw(key_list[3], (MODEL_WIDTH, MEMORY_HEADS * M_QK), MODEL_WIDTH ** -0.5, 0.125, ((1, 8),))
    weight_value = draw_weight_value(jax.random.fold_in(key_list[20], 71), 0)
    weight_outgate = bell_draw(key_list[5], (MODEL_WIDTH, MEMORY_HEADS * M_V), MODEL_WIDTH ** -0.5, 0.125, ((1, 8),))
    weight_ingate = bell_draw(key_list[6], (MODEL_WIDTH, MEMORY_HEADS), MODEL_WIDTH ** -0.5, 0.125)
    weight_forget = bell_draw(key_list[7], (MODEL_WIDTH, MEMORY_HEADS), MODEL_WIDTH ** -0.5, 0.125)
    forget_shift = draw_forget_shift(jax.random.fold_in(key_list[20], 71), 0)
    mem_gain = jnp.clip(1.0 + 0.18 * jax.random.normal(key_list[9], (MEMORY_HEADS * M_V,), jnp.float32), 0.099609375, 1.8984375).astype(jnp.bfloat16)
    query_down_weight = bell_draw(key_list[10], (MODEL_WIDTH, QUERY_LATENT), MODEL_WIDTH ** -0.5, 0.125, ((1, 8),))
    latent_down_weight = bell_draw(key_list[11], (MODEL_WIDTH, LATENT_WIDTH), MODEL_WIDTH ** -0.5, 0.125, ((1, 8),))
    down_rotary = bell_draw(key_list[12], (MODEL_WIDTH, ROTARY_CHANNELS), MODEL_WIDTH ** -0.5, 0.125)
    query_gain = draw_query_gain(jax.random.fold_in(key_list[20], 71), 0)
    latent_gain = draw_latent_gain(jax.random.fold_in(key_list[20], 71), 0)
    query_up_weight = bell_draw(key_list[15], (QUERY_LATENT, ATTEND_HEADS * (PLAIN_CHANNELS + ROTARY_CHANNELS)), (QUERY_LATENT // 4) ** -0.5, 0.4375, ((1, 8),))
    key_up_weight = bell_draw(key_list[16], (LATENT_WIDTH, ATTEND_HEADS * PLAIN_CHANNELS), LATENT_WIDTH ** -0.5, 0.25, ((1, 8),))
    value_up_weight = bell_draw(key_list[17], (LATENT_WIDTH, ATTEND_HEADS * VALUE_CHANNELS), LATENT_WIDTH ** -0.5, 0.25, ((1, 8),))
    out_memory = bell_draw(key_list[18], (MEMORY_HEADS * M_V, MODEL_WIDTH), (MEMORY_HEADS * M_V // 16) ** -0.5, 0.5, ((0, 8),))
    out_attend = bell_draw(key_list[19], (ATTEND_HEADS * VALUE_CHANNELS, MODEL_WIDTH), (ATTEND_HEADS * VALUE_CHANNELS // 16) ** -0.5, 0.75, ((0, 8),))
    return dict(tokens=tokens, input_gain=input_gain, weight_query=weight_query, weight_key=weight_key, weight_value=weight_value, weight_outgate=weight_outgate, weight_ingate=weight_ingate, weight_forget=weight_forget, forget_shift=forget_shift, mem_gain=mem_gain, query_down_weight=query_down_weight, latent_down_weight=latent_down_weight, down_rotary=down_rotary, query_gain=query_gain, latent_gain=latent_gain, query_up_weight=query_up_weight, key_up_weight=key_up_weight, value_up_weight=value_up_weight, out_memory=out_memory, out_attend=out_attend)


SMALL_CONSTANT = 1e-06
SOFTCAP = 15.0
ROTARY_BASE = 10000.0
PRECISE = lax.Precision.HIGHEST

def rms_scale(values, gain):
    widened = values.astype(jnp.float32)
    return widened * lax.rsqrt(lax.optimization_barrier(jnp.mean(widened * widened, axis=-1, keepdims=True)) + SMALL_CONSTANT) * gain.astype(jnp.float32)

def rotate(values, positions):
    halfway = values.shape[-1] // 2
    inverse = jnp.power(ROTARY_BASE, -jnp.arange(halfway, dtype=jnp.float32) / halfway)
    angles = positions.astype(jnp.float32)[:, None] * inverse
    cosine = jnp.cos(angles)
    sine_part = jnp.sin(angles)
    if values.ndim == 3:
        cosine = cosine[:, None, :]
        sine_part = sine_part[:, None, :]
    widened = values.astype(jnp.float32)
    first = widened[..., :halfway]
    second = widened[..., halfway:]
    turned = jnp.concatenate([first * cosine - second * sine_part, second * cosine + first * sine_part], axis=-1)
    return turned.astype(jnp.bfloat16)

def update_state(carried, key_rows, value_rows, input_gate, cumulative):
    matrix, normal, stabilizer = carried
    last_total = cumulative[:, -1]
    weight_log = last_total[:, None] - cumulative + input_gate
    new_max = jnp.maximum(last_total + stabilizer, lax.optimization_barrier(jnp.max(weight_log, axis=-1)))
    weights = jnp.exp(weight_log - new_max[:, None])
    decay = jnp.exp(last_total + stabilizer - new_max)
    matrix = decay[:, None, None] * matrix + jnp.einsum('hsv,hsd->hvd', weights[:, :, None] * value_rows, key_rows, precision=PRECISE)
    normal = decay[:, None] * normal + jnp.einsum('hs,hsd->hd', weights, key_rows, precision=PRECISE)
    return (matrix, normal, new_max)

def block_step(carried, inputs):
    query_rows, key_rows, value_rows, input_gate, log_forget = inputs
    matrix, normal, stabilizer = carried
    cumulative = jnp.cumsum(log_forget, axis=-1)
    block_len = log_forget.shape[-1]
    causal = jnp.tril(jnp.ones((block_len, block_len), dtype=bool))
    pair_log = cumulative[:, :, None] - cumulative[:, None, :] + input_gate[:, None, :]
    pair_log = jnp.where(causal, pair_log, -jnp.inf)
    carried_log = cumulative + stabilizer[:, None]
    row_max = jnp.maximum(carried_log, lax.optimization_barrier(jnp.max(pair_log, axis=-1)))
    within = jnp.exp(pair_log - row_max[:, :, None])
    across = jnp.exp(carried_log - row_max)
    affinity = jnp.einsum('hjd,hsd->hjs', query_rows, key_rows, precision=PRECISE) * within
    numerator = jnp.einsum('hjs,hsv->hjv', affinity, value_rows, precision=PRECISE)
    numerator = numerator + across[:, :, None] * jnp.einsum('hjd,hvd->hjv', query_rows, matrix, precision=PRECISE)
    denominator = lax.optimization_barrier(jnp.sum(affinity, axis=-1)) + across * jnp.einsum('hjd,hd->hj', query_rows, normal, precision=PRECISE)
    output = numerator / jnp.maximum(jnp.abs(denominator), jnp.exp(-row_max))[:, :, None]
    return (update_state(carried, key_rows, value_rows, input_gate, cumulative), output)

def memory_cell(queries, keys_in, values, input_gate, log_forget):
    length, head_count, query_width = queries.shape
    value_width = values.shape[-1]
    block_count = length // BLOCK

    def to_blocks(array, width):
        return array.astype(jnp.float32).reshape(block_count, BLOCK, head_count, width).transpose(0, 2, 1, 3)

    def gate_blocks(array):
        return array.reshape(block_count, BLOCK, head_count).transpose(0, 2, 1)
    initial = (jnp.zeros((head_count, value_width, query_width), jnp.float32), jnp.zeros((head_count, query_width), jnp.float32), jnp.zeros((head_count,), jnp.float32))
    inputs = (to_blocks(queries, query_width), to_blocks(keys_in, query_width) * query_width ** (-0.5), to_blocks(values, value_width), gate_blocks(input_gate), gate_blocks(log_forget))
    _, outputs = lax.scan(block_step, initial, inputs)
    return outputs.transpose(0, 2, 1, 3).reshape(length, head_count, value_width)

def latent_attention(queries, key_nope, key_rot, values):
    length = queries.shape[0]
    size = min(512, length)
    factor = (PLAIN_CHANNELS + ROTARY_CHANNELS) ** (-0.5)
    results = []
    for block_number in range(length // size):
        lower = block_number * size
        upper = lower + size
        query_nope = queries[lower:upper, :, :PLAIN_CHANNELS].astype(jnp.float32)
        query_rot = queries[lower:upper, :, PLAIN_CHANNELS:].astype(jnp.float32)
        scores = jnp.einsum('qhd,khd->hqk', query_nope, key_nope[:upper].astype(jnp.float32))
        scores = (scores + jnp.einsum('qhd,kd->hqk', query_rot, key_rot[:upper].astype(jnp.float32))) * factor
        allowed = jnp.arange(upper)[None, :] <= (lower + jnp.arange(size))[:, None]
        scores = jnp.where(allowed[None], scores, -jnp.inf)
        row_max = lax.optimization_barrier(jnp.max(scores, axis=-1, keepdims=True))
        probs = jnp.exp(scores - row_max)
        summed = lax.optimization_barrier(jnp.sum(probs, axis=-1))
        rounded = lax.optimization_barrier(probs.astype(jnp.bfloat16)).astype(jnp.float32)
        numerator = jnp.einsum('hqk,khd->qhd', rounded, values[:upper].astype(jnp.float32))
        results.append((numerator / summed.T[:, :, None]).astype(jnp.bfloat16))
    return jnp.concatenate(results, axis=0)

def reference(tokens, input_gain, weight_query, weight_key, weight_value, weight_outgate, weight_ingate, weight_forget, forget_shift, mem_gain, query_down_weight, latent_down_weight, down_rotary, query_gain, latent_gain, query_up_weight, key_up_weight, value_up_weight, out_memory, out_attend):
    length = tokens.shape[0]
    normed = rms_scale(tokens, input_gain).astype(jnp.bfloat16)

    def project(weight):
        return jnp.dot(normed, weight, preferred_element_type=jnp.float32)
    stored = (project(weight_query).astype(jnp.bfloat16), project(weight_key).astype(jnp.bfloat16), project(weight_value).astype(jnp.bfloat16), project(weight_outgate).astype(jnp.bfloat16))
    mem_query, mem_key, mem_value, mem_outgate = lax.optimization_barrier(stored)
    in_pre = project(weight_ingate)
    forget_pre = project(weight_forget) + forget_shift
    in_gate = SOFTCAP * jnp.tanh(in_pre / SOFTCAP)
    log_forget = jax.nn.log_sigmoid(SOFTCAP * jnp.tanh(forget_pre / SOFTCAP))
    query_latent = project(query_down_weight).astype(jnp.bfloat16)
    keyval_latent = project(latent_down_weight).astype(jnp.bfloat16)
    key_raw = project(down_rotary).astype(jnp.bfloat16)
    positions = jnp.arange(length, dtype=jnp.int32)
    cell = memory_cell(mem_query.reshape(length, MEMORY_HEADS, M_QK), mem_key.reshape(length, MEMORY_HEADS, M_QK), mem_value.reshape(length, MEMORY_HEADS, M_V), in_gate, log_forget)
    cell = cell.reshape(length, MEMORY_HEADS * M_V)
    gated = rms_scale(cell, mem_gain)
    gated = gated * jax.nn.sigmoid(mem_outgate.astype(jnp.float32))
    gated = gated.astype(jnp.bfloat16)
    normed_query = rms_scale(query_latent, query_gain).astype(jnp.bfloat16)
    normed_latent = rms_scale(keyval_latent, latent_gain).astype(jnp.bfloat16)
    query_all = jnp.dot(normed_query, query_up_weight, preferred_element_type=jnp.float32).astype(jnp.bfloat16)
    query_all = query_all.reshape(length, ATTEND_HEADS, PLAIN_CHANNELS + ROTARY_CHANNELS)
    queries = jnp.concatenate([query_all[..., :PLAIN_CHANNELS], rotate(query_all[..., PLAIN_CHANNELS:], positions)], axis=-1)
    key_nope = jnp.dot(normed_latent, key_up_weight, preferred_element_type=jnp.float32).astype(jnp.bfloat16)
    values = jnp.dot(normed_latent, value_up_weight, preferred_element_type=jnp.float32).astype(jnp.bfloat16)
    key_rot = rotate(key_raw, positions)
    attended = latent_attention(queries, key_nope.reshape(length, ATTEND_HEADS, PLAIN_CHANNELS), key_rot, values.reshape(length, ATTEND_HEADS, VALUE_CHANNELS)).reshape(length, ATTEND_HEADS * VALUE_CHANNELS)
    mem_share = MEMORY_HEADS // N_TP * M_V
    att_share = ATTEND_HEADS // N_TP * VALUE_CHANNELS
    summed = jnp.zeros((length, tokens.shape[1]), jnp.float32)
    for share in range(N_TP):
        partial_value = jnp.dot(gated[:, share * mem_share:(share + 1) * mem_share], out_memory[share * mem_share:(share + 1) * mem_share], preferred_element_type=jnp.float32)
        partial_value = partial_value + jnp.dot(attended[:, share * att_share:(share + 1) * att_share], out_attend[share * att_share:(share + 1) * att_share], preferred_element_type=jnp.float32)
        summed = summed + lax.optimization_barrier(partial_value.astype(jnp.bfloat16)).astype(jnp.float32)
    return summed.astype(jnp.bfloat16)
```

```python
import jax
import jax.numpy as jnp
from jax import lax
from jax.experimental import pallas as pl
from jax.experimental.pallas import tpu as pltpu
from jax.sharding import Mesh
from jax.sharding import PartitionSpec as P

MEMORY_HEADS = 8
M_QK = 128
M_V = 256
PLAIN_CHANNELS = 128
ROTARY_CHANNELS = 64
VALUE_CHANNELS = 128
BLOCK = 64
SP = ("z", "x")
TP = ("y", "c")
SP_TP = ("z", "x", "y", "c")


SMALL_CONSTANT = 1e-06
SOFTCAP = 15.0
ROTARY_BASE = 10000.0
PRECISE = lax.Precision.HIGHEST
FAR_BELOW = -1e30


def copy_for_each(shard, axis):
    copies = jnp.broadcast_to(shard, (lax.axis_size(axis), *shard.shape))
    return lax.all_to_all(copies, axis, split_axis=0, concat_axis=0, tiled=True)


def laid_out(tiles, dim):
    shape = list(tiles.shape[1:])
    shape[dim] *= tiles.shape[0]
    return jnp.moveaxis(tiles, 0, dim).reshape(shape)


def gather_directly(shard, axis, dim):
    tiles = copy_for_each(shard, axis)
    return laid_out(tiles, dim)


def nothing_yet(shard, identity):
    return jax.tree.map(
        lambda a, e: jnp.broadcast_to(jnp.asarray(e, a.dtype), a.shape), shard, identity
    )


def gathered_once(shard, axis):
    leaves = jax.tree.leaves(shard)
    order = sorted(range(len(leaves)), key=lambda k: -leaves[k].size)
    width = (1, *leaves[order[0]].shape)[-1]
    lines = [
        jnp.pad(leaves[k].reshape(-1), (0, -leaves[k].size % width)).reshape(-1, width)
        for k in order
    ]
    both, at, found = (lax.all_gather(jnp.concatenate(lines), axis), 0, {})
    for k, line in zip(order, lines):
        slab = both[:, at : at + len(line)].reshape(len(both), -1)
        found[k] = slab[:, : leaves[k].size].reshape(-1, *leaves[k].shape)
        at += len(line)
    numbers = iter(range(len(leaves)))
    return jax.tree.map(lambda _: found[next(numbers)], shard)


def entering(shard, axes, combine, identity):
    before = start = nothing_yet(shard, identity)
    running = shard
    for axis in reversed(axes):
        peers, index = (lax.axis_size(axis), lax.axis_index(axis))
        pieces = gathered_once(running, axis)
        inside, running = (start, start)
        for k in range(peers):
            passed = k < index
            running = combine(running, jax.tree.map(lambda part: part[k], pieces))
            inside = jax.tree.map(lambda new, old: jnp.where(passed, new, old), running, inside)
        before = combine(inside, before)
    return before


def in_blocks(shard, dim, peers):
    shape = shard.shape
    tiles = shard.reshape(*shape[:dim], peers, shape[dim] // peers, *shape[dim + 1 :])
    return jnp.moveaxis(tiles, dim, 0)


def sum_at_owner(shard, axis, dim):
    tiles = in_blocks(shard, dim, lax.axis_size(axis))
    arrived = lax.all_to_all(tiles, axis, split_axis=0, concat_axis=0, tiled=True)
    return arrived.astype(jnp.float32).sum(axis=0)


def rms_scale(values, gain):
    widened = values.astype(jnp.float32)
    return (
        widened
        * lax.rsqrt(jnp.mean(widened * widened, axis=-1, keepdims=True) + SMALL_CONSTANT)
        * gain.astype(jnp.float32)
    )


def rotate(values, positions):
    halfway = values.shape[-1] // 2
    inverse = jnp.power(ROTARY_BASE, -jnp.arange(halfway, dtype=jnp.float32) / halfway)
    angles = positions.astype(jnp.float32)[:, None] * inverse
    cosine = jnp.cos(angles)
    sine_part = jnp.sin(angles)
    if values.ndim == 3:
        cosine = cosine[:, None, :]
        sine_part = sine_part[:, None, :]
    widened = values.astype(jnp.float32)
    first = widened[..., :halfway]
    second = widened[..., halfway:]
    turned = jnp.concatenate(
        [first * cosine - second * sine_part, second * cosine + first * sine_part], axis=-1
    )
    return turned.astype(jnp.bfloat16)


def merge_states(earlier, later):
    decayed = later[3] + earlier[2]
    joined = jnp.maximum(decayed, later[2])
    early_part = jnp.exp(decayed - joined)
    late_part = jnp.exp(later[2] - joined)
    return (
        early_part[:, None, None] * earlier[0] + late_part[:, None, None] * later[0],
        early_part[:, None] * earlier[1] + late_part[:, None] * later[1],
        joined,
        earlier[3] + later[3],
    )


LOG2E = 1.4426950408889634
N_Z = 8
N_X = 4
ROWS = 512
MESH_ID = pl.DeviceIdType.MESH
CONTRACT_LAST = (((1,), (1,)), ((), ()))


def attend_kernel(
    q_ref,
    kv_ref,
    o_ref,
    q_all,
    kv_all,
    k_cat,
    top,
    total,
    accum,
    part_out,
    stat_out,
    part_in,
    stat_in,
    q_send,
    q_recv,
    up_send,
    up_recv,
    down_send,
    down_recv,
    part_send,
    part_recv,
    stat_send,
    stat_recv,
):
    z = lax.axis_index("z")
    x = lax.axis_index("x")
    above, below = lax.rem(z + 1, N_Z), lax.rem(z + N_Z - 1, N_Z)
    peers = [lax.rem(x + d, N_X) for d in range(1, N_X)]

    barrier = pltpu.get_barrier_semaphore()
    for other in (above, below):
        pl.semaphore_signal(barrier, inc=1, device_id={"z": other}, device_id_type=MESH_ID)
    for other in peers:
        pl.semaphore_signal(barrier, inc=1, device_id={"x": other}, device_id_type=MESH_ID)
    pl.semaphore_wait(barrier, N_X + 1)

    half = kv_ref.shape[0] // 2
    width = PLAIN_CHANNELS

    def kv_copy(up, step, h):
        shift = (N_Z - step + 1) if up else (step - 1)
        owner = lax.rem(z + shift, N_Z)
        rows = pl.ds(h * half, half)
        source = kv_ref.at[rows] if step == 1 else kv_all.at[owner, rows]
        send, recv = (up_send, up_recv) if up else (down_send, down_recv)
        return pltpu.make_async_remote_copy(
            src_ref=source,
            dst_ref=kv_all.at[owner, rows],
            send_sem=send.at[step - 1, h],
            recv_sem=recv.at[step - 1, h],
            device_id={"z": above if up else below},
            device_id_type=MESH_ID,
        )

    def q_copy(d):
        return pltpu.make_async_remote_copy(
            src_ref=q_ref,
            dst_ref=q_all.at[x],
            send_sem=q_send.at[d],
            recv_sem=q_recv.at[d],
            device_id={"x": peers[d]},
            device_id_type=MESH_ID,
        )

    def part_copy(d):
        return pltpu.make_async_remote_copy(
            src_ref=part_out.at[d],
            dst_ref=part_in.at[d],
            send_sem=part_send.at[d],
            recv_sem=part_recv.at[d],
            device_id={"x": peers[d]},
            device_id_type=MESH_ID,
        )

    def stat_copy(d):
        return pltpu.make_async_remote_copy(
            src_ref=stat_out.at[d],
            dst_ref=stat_in.at[d],
            send_sem=stat_send.at[d],
            recv_sem=stat_recv.at[d],
            device_id={"x": peers[d]},
            device_id_type=MESH_ID,
        )

    started = []
    for h in range(2):
        for up in (True, False):
            copy = kv_copy(up, 1, h)
            copy.start()
            started.append(copy)
    for d in range(N_X - 1):
        copy = q_copy(d)
        copy.start()
        started.append(copy)

    q_all[x] = q_ref[...]
    top[...] = jnp.full(top.shape, FAR_BELOW, jnp.float32)
    total[...] = jnp.zeros(total.shape, jnp.float32)
    accum[...] = jnp.zeros(accum.shape, jnp.float32)

    lane = lax.broadcasted_iota(jnp.int32, (ROWS // 2, width), 1)
    low = (lane < ROTARY_CHANNELS).astype(jnp.bfloat16)
    high = (lane >= ROTARY_CHANNELS).astype(jnp.bfloat16)
    scale = LOG2E * (PLAIN_CHANNELS + ROTARY_CHANNELS) ** (-0.5)
    tall = 256

    def keys_from(ref):
        k_cat[:, :width] = ref[:ROWS]
        packed = ref[2 * ROWS :]
        k_cat[: ROWS // 2, width:] = packed * low
        k_cat[ROWS // 2 :, width:] = packed * high

    def attend(first, last, values, masked):
        def one(t, carry):
            shard = t // (ROWS // tall)
            rows = pl.ds(pl.multiple_of(t * tall, tall), tall)
            inner = pl.ds(pl.multiple_of((t % (ROWS // tall)) * tall, tall), tall)
            queries = q_all[shard, inner]
            scores = lax.dot_general(
                queries, k_cat[...], CONTRACT_LAST, preferred_element_type=jnp.float32
            )
            scores = scores * scale
            if masked:
                row = lax.broadcasted_iota(jnp.int32, scores.shape, 0) + t * tall
                col = lax.broadcasted_iota(jnp.int32, scores.shape, 1) + x * ROWS
                scores = jnp.where(col <= row, scores, -jnp.inf)
            old = top[rows]
            new = jnp.maximum(old, jnp.max(scores, axis=1, keepdims=True))
            probs = jnp.exp2(scores - new[:, :1])
            shrink = jnp.exp2(old - new)
            total[rows] = total[rows] * shrink + jnp.sum(probs, axis=1, keepdims=True)
            accum[rows] = accum[rows] * shrink + jnp.dot(
                probs.astype(jnp.bfloat16), values(), preferred_element_type=jnp.float32
            )
            top[rows] = new
            return carry

        lax.fori_loop(first, last, one, 0)

    steps = ROWS // tall
    keys_from(kv_ref)
    own_values = lambda: kv_ref[ROWS : 2 * ROWS]
    attend(x * steps, (x + 1) * steps, own_values, True)
    for d in range(N_X - 1):
        q_copy(d).wait_recv()
    attend((x + 1) * steps, N_X * steps, own_values, False)

    def arrived(owner, useful):
        @pl.when(useful)
        def _():
            keys_from(kv_all.at[owner])
            attend(0, N_X * steps, lambda: kv_all[owner, ROWS : 2 * ROWS], False)

    last = N_Z // 2
    for step in range(1, last + 1):
        for h in range(2):
            for up in (True, False):
                if step == last and up != (h == 0):
                    continue
                kv_copy(up, step, h).wait_recv()
                if step < last - 1 or (step == last - 1 and up == (h == 0)):
                    copy = kv_copy(up, step + 1, h)
                    copy.start()
                    started.append(copy)
        if step < last:
            arrived(lax.rem(z + N_Z - step, N_Z), z >= step)
            arrived(lax.rem(z + step, N_Z), z + step >= N_Z)
        else:
            arrived(lax.rem(z + step, N_Z), z >= step)

    def finish(shard):
        rows = pl.ds(pl.multiple_of(shard * ROWS, ROWS), ROWS)
        summed = jnp.maximum(total[rows], 1.0)
        seen = total[rows] > 0.0
        log_total = jnp.where(seen, top[rows] + jnp.log2(summed), FAR_BELOW)
        return accum[rows] / summed, log_total

    for d in range(N_X - 1):
        part, log_total = finish(peers[d])
        part_out[d] = part.astype(jnp.bfloat16)
        stat_out[d] = log_total.T[:8]
        for copy in (part_copy(d), stat_copy(d)):
            copy.start()
            started.append(copy)
    own, own_log = finish(x)
    parts, logs = [], []
    for d in range(N_X - 1):
        part_copy(d).wait_recv()
        stat_copy(d).wait_recv()
        logs.append(jnp.broadcast_to(stat_in[d, 0:1, :], (width, ROWS)).T)
    highest = own_log
    for one in logs:
        highest = jnp.maximum(highest, one)
    weight = jnp.exp2(own_log - highest)
    numerator = own * weight
    denominator = weight
    for d in range(N_X - 1):
        weight = jnp.exp2(logs[d] - highest)
        numerator = numerator + part_in[d].astype(jnp.float32) * weight
        denominator = denominator + weight
    o_ref[...] = (numerator / denominator).astype(jnp.bfloat16)
    for copy in started:
        copy.wait_send()


def attend(queries, keys_values):
    f32, bf16 = jnp.float32, jnp.bfloat16
    last = N_Z // 2
    dma = pltpu.SemaphoreType.DMA
    return pl.pallas_call(
        attend_kernel,
        out_shape=jax.ShapeDtypeStruct((ROWS, VALUE_CHANNELS), bf16),
        in_specs=[pl.BlockSpec(memory_space=pltpu.VMEM)] * 2,
        out_specs=pl.BlockSpec(memory_space=pltpu.VMEM),
        scratch_shapes=[
            pltpu.VMEM((N_X, ROWS, 256), bf16),
            pltpu.VMEM((N_Z, *keys_values.shape), bf16),
            pltpu.VMEM((ROWS, 256), bf16),
            pltpu.VMEM((N_X * ROWS, 128), f32),
            pltpu.VMEM((N_X * ROWS, 128), f32),
            pltpu.VMEM((N_X * ROWS, VALUE_CHANNELS), f32),
            pltpu.VMEM((N_X - 1, ROWS, VALUE_CHANNELS), bf16),
            pltpu.VMEM((N_X - 1, 8, ROWS), f32),
            pltpu.VMEM((N_X - 1, ROWS, VALUE_CHANNELS), bf16),
            pltpu.VMEM((N_X - 1, 8, ROWS), f32),
            dma((N_X - 1,)),
            dma((N_X - 1,)),
            dma((last, 2)),
            dma((last, 2)),
            dma((last, 2)),
            dma((last, 2)),
            dma((N_X - 1,)),
            dma((N_X - 1,)),
            dma((N_X - 1,)),
            dma((N_X - 1,)),
        ],
        compiler_params=pltpu.CompilerParams(
            collective_id=1, has_side_effects=True, vmem_limit_bytes=48 * 1024 * 1024
        ),
        cost_estimate=pl.CostEstimate(
            flops=4 * 10**9, bytes_accessed=10**7, transcendentals=4 * 10**6
        ),
        name="attend",
    )(queries, keys_values)


def per_device(
    tokens,
    input_gain,
    weight_query,
    weight_key,
    weight_value,
    weight_outgate,
    weight_ingate,
    weight_forget,
    forget_shift,
    mem_gain,
    query_down_weight,
    latent_down_weight,
    down_rotary,
    query_gain,
    latent_gain,
    query_up_weight,
    key_up_weight,
    value_up_weight,
    out_memory,
    out_attend,
):
    normed = rms_scale(tokens, input_gain).astype(jnp.bfloat16)
    tp_index = lax.axis_index(TP)
    mem_heads = weight_query.shape[1] // M_QK
    att_heads = key_up_weight.shape[1] // PLAIN_CHANNELS
    ingate_cols = lax.dynamic_slice_in_dim(weight_ingate, tp_index * mem_heads, mem_heads, 1)
    forget_cols = lax.dynamic_slice_in_dim(weight_forget, tp_index * mem_heads, mem_heads, 1)
    weight_list = (
        weight_query,
        weight_key,
        weight_value,
        weight_outgate,
        query_down_weight,
        latent_down_weight,
        down_rotary,
        ingate_cols,
        forget_cols,
    )

    def project(portion):
        return jnp.concatenate(
            [
                jnp.dot(portion, weight, preferred_element_type=jnp.float32)
                for weight in weight_list
            ],
            axis=1,
        )

    projected = project(gather_directly(normed, TP, 0))
    sections = []
    offset = 0
    for weight in weight_list:
        sections.append(projected[:, offset : offset + weight.shape[1]])
        offset = offset + weight.shape[1]
    stored = tuple((section.astype(jnp.bfloat16) for section in sections[:7]))
    mem_query, mem_key, mem_value, mem_outgate, query_latent, keyval_latent, key_raw = (
        lax.optimization_barrier(stored)
    )
    in_gate = SOFTCAP * jnp.tanh(sections[7] / SOFTCAP)
    log_forget = jax.nn.log_sigmoid(SOFTCAP * jnp.tanh((sections[8] + forget_shift) / SOFTCAP))
    length = projected.shape[0]
    positions = lax.axis_index(SP) * length + jnp.arange(length, dtype=jnp.int32)
    query_whole, latent_whole = (
        lax.all_gather(query_latent, TP, axis=1, tiled=True),
        lax.all_gather(keyval_latent, TP, axis=1, tiled=True),
    )
    normed_query = rms_scale(query_whole, query_gain).astype(jnp.bfloat16)
    normed_latent = rms_scale(latent_whole, latent_gain).astype(jnp.bfloat16)
    cumulative = jnp.cumsum(log_forget[:, 0])
    relative = in_gate[:, 0] - cumulative
    running = lax.cummax(relative)
    ends_at = running[-1]
    key_scale = M_QK ** (-0.5)
    wide_value = mem_value.astype(jnp.float32)
    weights = jnp.exp(relative - ends_at) * key_scale
    local_matrix = lax.dot_general(
        weights[:, None] * wide_value,
        mem_key.astype(jnp.float32),
        (((0,), (0,)), ((), ())),
        precision=PRECISE,
    )
    local_normal = jnp.sum(weights[:, None] * mem_key.astype(jnp.float32), axis=0)
    local_state = (
        local_matrix[None],
        local_normal[None],
        (cumulative[-1] + ends_at)[None],
        cumulative[-1:],
    )
    identity = (
        jnp.zeros((mem_heads, M_V, M_QK), jnp.float32),
        jnp.zeros((mem_heads, M_QK), jnp.float32),
        jnp.full((mem_heads,), FAR_BELOW, jnp.float32),
        jnp.zeros((mem_heads,), jnp.float32),
    )
    prefix = entering(local_state, SP, merge_states, identity)
    start_max = jnp.maximum(prefix[3], prefix[2])
    rescale = jnp.exp(prefix[2] - start_max)
    start_matrix = (prefix[0] * rescale[:, None, None])[0]
    start_normal = (prefix[1] * rescale[:, None])[0]
    highest = jnp.maximum(start_max[0], running)
    causal = jnp.tril(jnp.ones((length, length), dtype=bool))
    within = jnp.where(causal, relative[None, :] - highest[:, None], -jnp.inf)
    affinity = lax.dot_general(
        mem_query, mem_key, (((1,), (1,)), ((), ())), preferred_element_type=jnp.float32
    )
    affinity = affinity * (jnp.exp(within) * key_scale)
    across = jnp.exp(start_max[0] - highest)
    wide_query = mem_query.astype(jnp.float32)
    numerator = jnp.dot(affinity, wide_value, precision=PRECISE) + across[:, None] * lax.dot_general(
        wide_query, start_matrix, (((1,), (1,)), ((), ())), precision=PRECISE
    )
    denominator = jnp.sum(affinity, axis=1) + across * jnp.sum(
        wide_query * start_normal[None, :], axis=1
    )
    floor = jnp.exp(-(cumulative + highest))
    cell = numerator / jnp.maximum(jnp.abs(denominator), floor)[:, None]
    cell_total = lax.psum(jnp.sum(cell * cell, axis=1), TP)
    gain_part = lax.dynamic_slice_in_dim(mem_gain, tp_index * mem_heads * M_V, mem_heads * M_V, 0)
    gated = (
        cell
        * lax.rsqrt(cell_total / (MEMORY_HEADS * M_V) + SMALL_CONSTANT)[:, None]
        * gain_part.astype(jnp.float32)
    )
    gated = gated * jax.nn.sigmoid(mem_outgate.astype(jnp.float32))
    gated = gated.astype(jnp.bfloat16)
    query_all = jnp.dot(normed_query, query_up_weight, preferred_element_type=jnp.float32).astype(
        jnp.bfloat16
    )
    query_all = query_all.reshape(length, att_heads, PLAIN_CHANNELS + ROTARY_CHANNELS)
    query_nope = query_all[..., :PLAIN_CHANNELS]
    query_rot = rotate(query_all[..., PLAIN_CHANNELS:], positions)
    key_rot = rotate(key_raw, positions)
    own_nope = jnp.dot(normed_latent, key_up_weight, preferred_element_type=jnp.float32).astype(
        jnp.bfloat16
    )
    own_values = jnp.dot(normed_latent, value_up_weight, preferred_element_type=jnp.float32).astype(
        jnp.bfloat16
    )
    turned = query_rot.reshape(length, ROTARY_CHANNELS)
    queries = jnp.concatenate([query_nope.reshape(length, PLAIN_CHANNELS), turned, turned], axis=1)
    packed = jnp.concatenate([key_rot[: length // 2], key_rot[length // 2 :]], axis=1)
    attended = attend(queries, jnp.concatenate([own_nope, own_values, packed], axis=0))
    mixed = sum_at_owner(
        (
            jnp.dot(gated, out_memory, preferred_element_type=jnp.float32)
            + jnp.dot(attended, out_attend, preferred_element_type=jnp.float32)
        ).astype(jnp.bfloat16),
        TP,
        0,
    )
    return mixed.astype(jnp.bfloat16)


def solution(mesh):
    torus = Mesh(mesh.devices.reshape(N_Z, N_X, 4, 2), SP_TP)
    in_specs = (
        P(SP_TP, None),
        P(),
        P(None, TP),
        P(None, TP),
        P(None, TP),
        P(None, TP),
        P(),
        P(),
        P(SP, TP),
        P(),
        P(None, TP),
        P(None, TP),
        P(),
        P(),
        P(),
        P(None, TP),
        P(None, TP),
        P(None, TP),
        P(TP, None),
        P(TP, None),
    )
    out_specs = P(SP_TP, None)
    return jax.shard_map(
        per_device, mesh=torus, in_specs=in_specs, out_specs=out_specs, check_vma=False
    )
```

```python
import jax
import jax.numpy as jnp
from jax import lax
from jax.experimental import pallas as pl
from jax.experimental.pallas import tpu as pltpu
from jax.sharding import Mesh
from jax.sharding import PartitionSpec as P

MEMORY_HEADS = 8
M_QK = 128
M_V = 256
PLAIN_CHANNELS = 128
ROTARY_CHANNELS = 64
VALUE_CHANNELS = 128
BLOCK = 64
SP = ("z", "x")
TP = ("y", "c")
SP_TP = ("z", "x", "y", "c")


SMALL_CONSTANT = 1e-06
SOFTCAP = 15.0
ROTARY_BASE = 10000.0
PRECISE = lax.Precision.HIGHEST
FAR_BELOW = -1e30


def nothing_yet(shard, identity):
    return jax.tree.map(
        lambda a, e: jnp.broadcast_to(jnp.asarray(e, a.dtype), a.shape), shard, identity
    )


def gathered_once(shard, axis):
    leaves = jax.tree.leaves(shard)
    order = sorted(range(len(leaves)), key=lambda k: -leaves[k].size)
    width = (1, *leaves[order[0]].shape)[-1]
    lines = [
        jnp.pad(leaves[k].reshape(-1), (0, -leaves[k].size % width)).reshape(-1, width)
        for k in order
    ]
    both, at, found = (lax.all_gather(jnp.concatenate(lines), axis), 0, {})
    for k, line in zip(order, lines):
        slab = both[:, at : at + len(line)].reshape(len(both), -1)
        found[k] = slab[:, : leaves[k].size].reshape(-1, *leaves[k].shape)
        at += len(line)
    numbers = iter(range(len(leaves)))
    return jax.tree.map(lambda _: found[next(numbers)], shard)


def entering(shard, axes, combine, identity):
    before = start = nothing_yet(shard, identity)
    running = shard
    for axis in reversed(axes):
        peers, index = (lax.axis_size(axis), lax.axis_index(axis))
        pieces = gathered_once(running, axis)
        inside, running = (start, start)
        for k in range(peers):
            passed = k < index
            running = combine(running, jax.tree.map(lambda part: part[k], pieces))
            inside = jax.tree.map(lambda new, old: jnp.where(passed, new, old), running, inside)
        before = combine(inside, before)
    return before


def merge_states(earlier, later):
    decayed = later[3] + earlier[2]
    joined = jnp.maximum(decayed, later[2])
    early_part = jnp.exp(decayed - joined)
    late_part = jnp.exp(later[2] - joined)
    return (
        early_part[:, None, None] * earlier[0] + late_part[:, None, None] * later[0],
        early_part[:, None] * earlier[1] + late_part[:, None] * later[1],
        joined,
        earlier[3] + later[3],
    )


LOG2E = 1.4426950408889634
N_Z = 8
N_X = 4
ROWS = 512
MESH_ID = pl.DeviceIdType.MESH
CONTRACT_LAST = (((1,), (1,)), ((), ()))


def attend_kernel(
    q_ref,
    kv_ref,
    o_ref,
    q_all,
    kv_all,
    k_cat,
    top,
    total,
    accum,
    part_out,
    stat_out,
    part_in,
    stat_in,
    q_send,
    q_recv,
    up_send,
    up_recv,
    down_send,
    down_recv,
    part_send,
    part_recv,
    stat_send,
    stat_recv,
):
    z = lax.axis_index("z")
    x = lax.axis_index("x")
    above, below = lax.rem(z + 1, N_Z), lax.rem(z + N_Z - 1, N_Z)
    peers = [lax.rem(x + d, N_X) for d in range(1, N_X)]

    barrier = pltpu.get_barrier_semaphore()
    for other in (above, below):
        pl.semaphore_signal(barrier, inc=1, device_id={"z": other}, device_id_type=MESH_ID)
    for other in peers:
        pl.semaphore_signal(barrier, inc=1, device_id={"x": other}, device_id_type=MESH_ID)
    pl.semaphore_wait(barrier, N_X + 1)

    half = kv_ref.shape[0] // 2
    width = PLAIN_CHANNELS

    def kv_copy(up, step, h):
        shift = (N_Z - step + 1) if up else (step - 1)
        owner = lax.rem(z + shift, N_Z)
        rows = pl.ds(h * half, half)
        source = kv_ref.at[rows] if step == 1 else kv_all.at[owner, rows]
        send, recv = (up_send, up_recv) if up else (down_send, down_recv)
        return pltpu.make_async_remote_copy(
            src_ref=source,
            dst_ref=kv_all.at[owner, rows],
            send_sem=send.at[step - 1, h],
            recv_sem=recv.at[step - 1, h],
            device_id={"z": above if up else below},
            device_id_type=MESH_ID,
        )

    def q_copy(d):
        return pltpu.make_async_remote_copy(
            src_ref=q_ref,
            dst_ref=q_all.at[x],
            send_sem=q_send.at[d],
            recv_sem=q_recv.at[d],
            device_id={"x": peers[d]},
            device_id_type=MESH_ID,
        )

    def part_copy(d):
        return pltpu.make_async_remote_copy(
            src_ref=part_out.at[d],
            dst_ref=part_in.at[d],
            send_sem=part_send.at[d],
            recv_sem=part_recv.at[d],
            device_id={"x": peers[d]},
            device_id_type=MESH_ID,
        )

    def stat_copy(d):
        return pltpu.make_async_remote_copy(
            src_ref=stat_out.at[d],
            dst_ref=stat_in.at[d],
            send_sem=stat_send.at[d],
            recv_sem=stat_recv.at[d],
            device_id={"x": peers[d]},
            device_id_type=MESH_ID,
        )

    started = []
    for h in range(2):
        for up in (True, False):
            copy = kv_copy(up, 1, h)
            copy.start()
            started.append(copy)
    for d in range(N_X - 1):
        copy = q_copy(d)
        copy.start()
        started.append(copy)

    q_all[x] = q_ref[...]
    top[...] = jnp.full(top.shape, FAR_BELOW, jnp.float32)
    total[...] = jnp.zeros(total.shape, jnp.float32)
    accum[...] = jnp.zeros(accum.shape, jnp.float32)

    lane = lax.broadcasted_iota(jnp.int32, (ROWS // 2, width), 1)
    low = (lane < ROTARY_CHANNELS).astype(jnp.bfloat16)
    high = (lane >= ROTARY_CHANNELS).astype(jnp.bfloat16)
    scale = LOG2E * (PLAIN_CHANNELS + ROTARY_CHANNELS) ** (-0.5)
    tall = 256

    def keys_from(ref):
        k_cat[:, :width] = ref[:ROWS]
        packed = ref[2 * ROWS :]
        k_cat[: ROWS // 2, width:] = packed * low
        k_cat[ROWS // 2 :, width:] = packed * high

    def attend(first, last, values, masked):
        def one(t, carry):
            shard = t // (ROWS // tall)
            rows = pl.ds(pl.multiple_of(t * tall, tall), tall)
            inner = pl.ds(pl.multiple_of((t % (ROWS // tall)) * tall, tall), tall)
            queries = q_all[shard, inner]
            scores = lax.dot_general(
                queries, k_cat[...], CONTRACT_LAST, preferred_element_type=jnp.float32
            )
            scores = scores * scale
            if masked:
                row = lax.broadcasted_iota(jnp.int32, scores.shape, 0) + t * tall
                col = lax.broadcasted_iota(jnp.int32, scores.shape, 1) + x * ROWS
                scores = jnp.where(col <= row, scores, -jnp.inf)
            old = top[rows]
            new = jnp.maximum(old, jnp.max(scores, axis=1, keepdims=True))
            probs = jnp.exp2(scores - new[:, :1])
            shrink = jnp.exp2(old - new)
            total[rows] = total[rows] * shrink + jnp.sum(probs, axis=1, keepdims=True)
            accum[rows] = accum[rows] * shrink + jnp.dot(
                probs.astype(jnp.bfloat16), values(), preferred_element_type=jnp.float32
            )
            top[rows] = new
            return carry

        lax.fori_loop(first, last, one, 0)

    steps = ROWS // tall
    keys_from(kv_ref)
    own_values = lambda: kv_ref[ROWS : 2 * ROWS]
    attend(x * steps, (x + 1) * steps, own_values, True)
    for d in range(N_X - 1):
        q_copy(d).wait_recv()
    attend((x + 1) * steps, N_X * steps, own_values, False)

    def arrived(owner, useful):
        @pl.when(useful)
        def _():
            keys_from(kv_all.at[owner])
            attend(0, N_X * steps, lambda: kv_all[owner, ROWS : 2 * ROWS], False)

    last = N_Z // 2
    for step in range(1, last + 1):
        for h in range(2):
            for up in (True, False):
                if step == last and up != (h == 0):
                    continue
                kv_copy(up, step, h).wait_recv()
                if step < last - 1 or (step == last - 1 and up == (h == 0)):
                    copy = kv_copy(up, step + 1, h)
                    copy.start()
                    started.append(copy)
        if step < last:
            arrived(lax.rem(z + N_Z - step, N_Z), z >= step)
            arrived(lax.rem(z + step, N_Z), z + step >= N_Z)
        else:
            arrived(lax.rem(z + step, N_Z), z >= step)

    def finish(shard):
        rows = pl.ds(pl.multiple_of(shard * ROWS, ROWS), ROWS)
        summed = jnp.maximum(total[rows], 1.0)
        seen = total[rows] > 0.0
        log_total = jnp.where(seen, top[rows] + jnp.log2(summed), FAR_BELOW)
        return accum[rows] / summed, log_total

    for d in range(N_X - 1):
        part, log_total = finish(peers[d])
        part_out[d] = part.astype(jnp.bfloat16)
        stat_out[d] = log_total.T[:8]
        for copy in (part_copy(d), stat_copy(d)):
            copy.start()
            started.append(copy)
    own, own_log = finish(x)
    parts, logs = [], []
    for d in range(N_X - 1):
        part_copy(d).wait_recv()
        stat_copy(d).wait_recv()
        logs.append(jnp.broadcast_to(stat_in[d, 0:1, :], (width, ROWS)).T)
    highest = own_log
    for one in logs:
        highest = jnp.maximum(highest, one)
    weight = jnp.exp2(own_log - highest)
    numerator = own * weight
    denominator = weight
    for d in range(N_X - 1):
        weight = jnp.exp2(logs[d] - highest)
        numerator = numerator + part_in[d].astype(jnp.float32) * weight
        denominator = denominator + weight
    o_ref[...] = (numerator / denominator).astype(jnp.bfloat16)
    for copy in started:
        copy.wait_send()


def attend(queries, keys_values):
    f32, bf16 = jnp.float32, jnp.bfloat16
    last = N_Z // 2
    dma = pltpu.SemaphoreType.DMA
    return pl.pallas_call(
        attend_kernel,
        out_shape=jax.ShapeDtypeStruct((ROWS, VALUE_CHANNELS), bf16),
        in_specs=[pl.BlockSpec(memory_space=pltpu.VMEM)] * 2,
        out_specs=pl.BlockSpec(memory_space=pltpu.VMEM),
        scratch_shapes=[
            pltpu.VMEM((N_X, ROWS, 256), bf16),
            pltpu.VMEM((N_Z, *keys_values.shape), bf16),
            pltpu.VMEM((ROWS, 256), bf16),
            pltpu.VMEM((N_X * ROWS, 128), f32),
            pltpu.VMEM((N_X * ROWS, 128), f32),
            pltpu.VMEM((N_X * ROWS, VALUE_CHANNELS), f32),
            pltpu.VMEM((N_X - 1, ROWS, VALUE_CHANNELS), bf16),
            pltpu.VMEM((N_X - 1, 8, ROWS), f32),
            pltpu.VMEM((N_X - 1, ROWS, VALUE_CHANNELS), bf16),
            pltpu.VMEM((N_X - 1, 8, ROWS), f32),
            dma((N_X - 1,)),
            dma((N_X - 1,)),
            dma((last, 2)),
            dma((last, 2)),
            dma((last, 2)),
            dma((last, 2)),
            dma((N_X - 1,)),
            dma((N_X - 1,)),
            dma((N_X - 1,)),
            dma((N_X - 1,)),
        ],
        compiler_params=pltpu.CompilerParams(
            collective_id=1, has_side_effects=True, vmem_limit_bytes=48 * 1024 * 1024
        ),
        cost_estimate=pl.CostEstimate(
            flops=4 * 10**9, bytes_accessed=10**7, transcendentals=4 * 10**6
        ),
        name="attend",
    )(queries, keys_values)


N_Y = 4
N_C = 2
SHARE = 64
QUERY_LATENT = 768
LATENT_WIDTH = 512
QUERY_PART = QUERY_LATENT // (N_Y * N_C)
LATENT_PART = LATENT_WIDTH // (N_Y * N_C)
PARAMS = pltpu.CompilerParams


class TpGather:
    def __init__(self, full, sends, recvs):
        self.full, self.sends, self.recvs = full, sends, recvs
        self.y, self.c = lax.axis_index("y"), lax.axis_index("c")
        self.half = full.shape[1] // 2
        self.started = []

    def _copy(self, number, shift, part, target):
        slot = lax.rem(self.y + shift, N_Y) * N_C + self.c
        if part is None:
            ref = self.full.at[slot]
        else:
            ref = self.full.at[slot, pl.ds(part * self.half, self.half)]
        if target == "core":
            device = {"c": 1 - self.c}
        else:
            device = {"y": lax.rem(self.y + (1 if target == "up" else N_Y - 1), N_Y)}
        return pltpu.make_async_remote_copy(
            src_ref=ref,
            dst_ref=ref,
            send_sem=self.sends.at[number],
            recv_sem=self.recvs.at[number],
            device_id=device,
            device_id_type=MESH_ID,
        )

    def _start(self, *what):
        copy = self._copy(*what)
        copy.start()
        self.started.append(copy)

    def start(self):
        self._start(0, 0, 0, "up")
        self._start(3, 0, 1, "down")
        self._start(1, 0, 1, "up")
        self._start(2, 0, 0, "down")
        self._start(6, 0, None, "core")

    def relay(self):
        self._copy(0, 0, 0, "up").wait_recv()
        self._start(4, N_Y - 1, 0, "up")
        self._copy(3, 0, 1, "down").wait_recv()
        self._start(5, 1, 1, "down")
        self._copy(1, 0, 1, "up").wait_recv()
        self._start(7, N_Y - 1, None, "core")
        self._copy(2, 0, 0, "down").wait_recv()
        self._start(8, 1, None, "core")

    def near(self):
        for number, shift in ((6, 0), (7, N_Y - 1), (8, 1)):
            self._copy(number, shift, None, "core").wait_recv()

    def far(self):
        self._copy(4, 0, 0, "up").wait_recv()
        self._start(9, 2, 0, "core")
        self._copy(5, 0, 1, "down").wait_recv()
        self._start(10, 2, 1, "core")
        for part in range(2):
            self._copy(9 + part, 2, part, "core").wait_recv()

    def finish(self):
        for copy in self.started:
            copy.wait_send()


def greet_tp(barrier):
    y, c = lax.axis_index("y"), lax.axis_index("c")
    for device in (
        {"c": 1 - c},
        {"y": lax.rem(y + 1, N_Y)},
        {"y": lax.rem(y + N_Y - 1, N_Y)},
    ):
        pl.semaphore_signal(barrier, inc=1, device_id=device, device_id_type=MESH_ID)


def project_kernel(
    tokens,
    gain,
    small_hbm,
    query_hbm,
    key_hbm,
    value_hbm,
    outgate_hbm,
    query_up,
    key_up,
    value_up,
    gains,
    cosine,
    sine_part,
    mem_ref,
    gate_ref,
    q_ref,
    kv_ref,
    rows_all,
    latents,
    small,
    big,
    up_query,
    up_latent,
    wide_query,
    wide_latent,
    load_sem,
    row_send,
    row_recv,
    lat_send,
    lat_recv,
):
    f32, bf16 = jnp.float32, jnp.bfloat16
    y, c = lax.axis_index("y"), lax.axis_index("c")
    mine = y * N_C + c
    width = 128
    loads = [pltpu.make_async_copy(small_hbm, small, load_sem.at[0])]
    at = 0
    for k, ref in enumerate((query_hbm, key_hbm, value_hbm, outgate_hbm)):
        columns = ref.shape[1]
        loads.append(
            pltpu.make_async_copy(ref, big.at[:, pl.ds(at, columns)], load_sem.at[1 + k])
        )
        at += columns
    for load in loads:
        load.start()

    wide = tokens[...].astype(f32)
    inverse = lax.rsqrt(jnp.mean(wide * wide, axis=1, keepdims=True) + SMALL_CONSTANT)
    rows_all[mine] = (wide * inverse * gain[...].astype(f32)).astype(bf16)

    barrier = pltpu.get_barrier_semaphore()
    greet_tp(barrier)
    pl.semaphore_wait(barrier, 3)
    gather = TpGather(rows_all, row_send, row_recv)
    gather.start()

    up_query[...] = jnp.zeros(up_query.shape, bf16)
    for s in range(N_Y * N_C):
        up_query[s * width : s * width + QUERY_PART] = query_up[
            s * QUERY_PART : (s + 1) * QUERY_PART
        ]
        part = slice(s * LATENT_PART, (s + 1) * LATENT_PART)
        for h in range(2):
            at = s * width + h * LATENT_PART
            up_latent[at : at + LATENT_PART, :width] = key_up[part]
            up_latent[at : at + LATENT_PART, width:] = value_up[part]
    for load in loads:
        load.wait()

    lane = lax.broadcasted_iota(jnp.int32, (1, width), 1)
    row_id = lax.broadcasted_iota(jnp.int32, (width, width), 0)
    col_id = lax.broadcasted_iota(jnp.int32, (width, width), 1)
    channels = lax.rem(col_id, ROTARY_CHANNELS)
    halfway = ROTARY_CHANNELS // 2
    twin = (row_id == channels).astype(bf16)
    partner = lax.rem(channels + halfway, ROTARY_CHANNELS)
    sign = jnp.where(channels < halfway, -1.0, 1.0)

    def duplicated(values, offset):
        return jnp.dot(
            values, (row_id == channels + offset).astype(bf16), preferred_element_type=f32
        )

    def rotated(values, offset):
        swap = jnp.where(row_id == partner + offset, sign, 0.0).astype(bf16)
        turned = jnp.dot(values, swap, preferred_element_type=f32)
        return duplicated(values, offset) * cosine[...] + turned * sine_part[...]

    def chip_rows(chip):
        slots = [rows_all[chip * N_C + k] for k in range(N_C)]
        return jnp.concatenate(slots, axis=0)

    span = N_C * SHARE
    tile = 256

    def project_small(chip):
        rows = pl.ds(pl.multiple_of(chip * span, span), span)
        made = jnp.dot(chip_rows(chip), small[...], preferred_element_type=f32)
        gate_ref[rows] = made[:, :width]
        rounded = made.astype(bf16)
        latents[mine, rows] = rounded[:, :width]
        wide_latent[rows, :width] = rounded[:, width:]

    def project_big(chip):
        rows = pl.ds(pl.multiple_of(chip * span, span), span)

        def one(t, carry):
            columns = pl.ds(pl.multiple_of(t * tile, tile), tile)
            made = jnp.dot(chip_rows(chip), big[:, columns], preferred_element_type=f32)
            mem_ref[rows, columns] = made.astype(bf16)
            return carry

        lax.fori_loop(0, big.shape[1] // tile, one, 0)

    gather.relay()
    gather.near()
    near = [y, lax.rem(y + N_Y - 1, N_Y), lax.rem(y + 1, N_Y)]
    for chip in near:
        project_small(chip)
    opposite = lax.rem(y + 2, N_Y)
    gather.far()
    project_small(opposite)

    second = wide_latent[:, :width]
    both = duplicated(second, 0)
    half = ROWS // 2
    packed = jnp.where(lane < LATENT_PART, both[:half], both[half:])
    latents[mine, ROWS:] = packed.astype(bf16)
    exchange = TpGather(latents, lat_send, lat_recv)
    exchange.start()
    for chip in near[:2]:
        project_big(chip)
    exchange.relay()
    for chip in (near[2], opposite):
        project_big(chip)
    key_turned = rotated(second, LATENT_PART)
    kv_ref[2 * ROWS :] = jnp.where(
        lane < ROTARY_CHANNELS, key_turned[:half], key_turned[half:]
    ).astype(bf16)
    exchange.near()
    exchange.far()

    query_mask = (lane < QUERY_PART).astype(f32)
    squares = jnp.zeros((ROWS, width), f32)
    low_squares = jnp.zeros((half, width), f32)
    for s in range(N_Y * N_C):
        part = latents[s, :ROWS].astype(f32) * query_mask
        squares = squares + part * part
        part = latents[s, ROWS:].astype(f32)
        low_squares = low_squares + part * part
    query_scale = lax.rsqrt(
        jnp.sum(squares, axis=1, keepdims=True) / QUERY_LATENT + SMALL_CONSTANT
    )
    low = lane < LATENT_PART
    low_scale = lax.rsqrt(
        jnp.sum(jnp.where(low, low_squares, 0.0), axis=1, keepdims=True) / LATENT_WIDTH
        + SMALL_CONSTANT
    )
    high_scale = lax.rsqrt(
        jnp.sum(jnp.where(low, 0.0, low_squares), axis=1, keepdims=True) / LATENT_WIDTH
        + SMALL_CONSTANT
    )
    latent_scale = jnp.where(low, low_scale, high_scale)
    for s in range(N_Y * N_C):
        columns = slice(s * width, (s + 1) * width)
        part = latents[s, :ROWS].astype(f32) * query_mask
        wide_query[:, columns] = (part * query_scale * gains[s : s + 1]).astype(bf16)
        part = latents[s, ROWS:].astype(f32)
        made = (part * latent_scale * gains[8 + s : 9 + s]).astype(bf16)
        wide_latent[:half, columns] = jnp.where(low, made, jnp.zeros_like(made))
        wide_latent[half:, columns] = jnp.where(low, jnp.zeros_like(made), made)
    made = jnp.dot(wide_query[...], up_query[...], preferred_element_type=f32).astype(bf16)
    q_ref[:, :width] = made[:, :width]
    turning = jnp.concatenate([made[:, width:], jnp.zeros((ROWS, ROTARY_CHANNELS), bf16)], axis=1)
    q_ref[:, width:] = rotated(turning, 0).astype(bf16)
    made = jnp.dot(wide_latent[...], up_latent[...], preferred_element_type=f32).astype(bf16)
    kv_ref[:ROWS] = made[:, :width]
    kv_ref[ROWS : 2 * ROWS] = made[:, width:]
    gather.finish()
    exchange.finish()


def project(tokens, gain, small, query, key, value, outgate, ups, gains, cosine, sine_part):
    f32, bf16 = jnp.float32, jnp.bfloat16
    depth = tokens.shape[1]
    dma = pltpu.SemaphoreType.DMA
    vmem = pl.BlockSpec(memory_space=pltpu.VMEM)
    hbm = pl.BlockSpec(memory_space=pl.ANY)
    mem_width = query.shape[1] + key.shape[1] + value.shape[1] + outgate.shape[1]
    return pl.pallas_call(
        project_kernel,
        out_shape=(
            jax.ShapeDtypeStruct((ROWS, mem_width), bf16),
            jax.ShapeDtypeStruct((ROWS, 128), f32),
            jax.ShapeDtypeStruct((ROWS, 256), bf16),
            jax.ShapeDtypeStruct((ROWS * 5 // 2, 128), bf16),
        ),
        in_specs=[vmem] * 2 + [hbm] * 5 + [vmem] * 6,
        out_specs=[vmem] * 4,
        scratch_shapes=[
            pltpu.VMEM((N_Y * N_C, SHARE, depth), bf16),
            pltpu.VMEM((N_Y * N_C, ROWS * 3 // 2, 128), bf16),
            pltpu.VMEM((depth, 256), bf16),
            pltpu.VMEM((depth, mem_width), bf16),
            pltpu.VMEM((1024, PLAIN_CHANNELS + ROTARY_CHANNELS), bf16),
            pltpu.VMEM((1024, 256), bf16),
            pltpu.VMEM((ROWS, 1024), bf16),
            pltpu.VMEM((ROWS, 1024), bf16),
            dma((5,)),
            dma((11,)),
            dma((11,)),
            dma((11,)),
            dma((11,)),
        ],
        compiler_params=PARAMS(
            collective_id=2, has_side_effects=True, vmem_limit_bytes=48 * 1024 * 1024
        ),
        cost_estimate=pl.CostEstimate(
            flops=3 * 10**9, bytes_accessed=10**7, transcendentals=10**4
        ),
        name="project",
    )(tokens, gain, small, query, key, value, outgate, *ups, gains, cosine, sine_part)


def output_kernel(
    gated,
    attended,
    out_memory,
    out_attend,
    o_ref,
    to_core,
    from_core,
    sums,
    passing,
    from_below,
    from_above,
    relay_in,
    core_send,
    core_recv,
    relay_send,
    relay_recv,
    up_send,
    up_recv,
    down_send,
    down_recv,
):
    f32, bf16 = jnp.float32, jnp.bfloat16
    y, c = lax.axis_index("y"), lax.axis_index("c")
    above, below = lax.rem(y + 1, N_Y), lax.rem(y + N_Y - 1, N_Y)
    opposite = lax.rem(y + 2, N_Y)
    half = out_memory.shape[1] // 2
    tile = 512

    barrier = pltpu.get_barrier_semaphore()
    greet_tp(barrier)

    def remote(source, target, send, recv, device):
        return pltpu.make_async_remote_copy(
            src_ref=source,
            dst_ref=target,
            send_sem=send,
            recv_sem=recv,
            device_id=device,
            device_id_type=MESH_ID,
        )

    def rows_of(ref, core):
        picked = [ref[pl.ds(pl.multiple_of((k * N_C + core) * SHARE, SHARE), SHARE)] for k in range(N_Y)]
        return jnp.concatenate(picked, axis=0)

    def partial(core, h, store):
        memory_rows, attend_rows = rows_of(gated, core), rows_of(attended, core)
        for t in range(half // tile):
            columns = slice(h * half + t * tile, h * half + (t + 1) * tile)
            made = jnp.dot(memory_rows, out_memory[:, columns], preferred_element_type=f32)
            made = made + jnp.dot(attend_rows, out_attend[:, columns], preferred_element_type=f32)
            store(t * tile, made.astype(bf16).reshape(N_Y, SHARE, tile))

    def core_copy(h):
        return remote(
            to_core.at[h], from_core.at[h], core_send.at[h], core_recv.at[h], {"c": 1 - c}
        )

    def relay_copy(h):
        return remote(
            passing.at[h],
            relay_in.at[h],
            relay_send.at[h],
            relay_recv.at[h],
            {"y": above if h == 0 else below},
        )

    def up_copy(h):
        return remote(
            passing.at[2 + h], from_below.at[h], up_send.at[h], up_recv.at[h], {"y": above}
        )

    def down_copy(h):
        return remote(
            passing.at[4 + h], from_above.at[h], down_send.at[h], down_recv.at[h], {"y": below}
        )

    started = []

    def start(copy):
        copy.start()
        started.append(copy)

    for h in range(2):

        def keep(at, block, h=h):
            to_core[h, :, :, at : at + tile] = block

        partial(1 - c, h, keep)
        if h == 0:
            pl.semaphore_wait(barrier, 3)
        start(core_copy(h))
    for h in range(2):

        def keep(at, block, h=h):
            sums[h, :, :, at : at + tile] = block.astype(f32)

        partial(c, h, keep)
    for h in range(2):
        core_copy(h).wait_recv()
        sums[h] = sums[h] + from_core[h].astype(f32)
        passing[h] = sums[h, opposite].astype(bf16)
        start(relay_copy(h))
        if h == 0:
            passing[4] = sums[0, below].astype(bf16)
            start(down_copy(0))
        else:
            passing[3] = sums[1, above].astype(bf16)
            start(up_copy(1))
    relay_copy(0).wait_recv()
    passing[2] = (sums[0, above] + relay_in[0].astype(f32)).astype(bf16)
    start(up_copy(0))
    relay_copy(1).wait_recv()
    passing[5] = (sums[1, below] + relay_in[1].astype(f32)).astype(bf16)
    start(down_copy(1))
    for h in (1, 0):
        up_copy(h).wait_recv()
        down_copy(h).wait_recv()
        made = sums[h, y] + from_below[h].astype(f32) + from_above[h].astype(f32)
        o_ref[:, h * half : (h + 1) * half] = made.astype(bf16)
    for copy in started:
        copy.wait_send()


def project_out(gated, attended, out_memory, out_attend):
    f32, bf16 = jnp.float32, jnp.bfloat16
    dma = pltpu.SemaphoreType.DMA
    vmem = pl.BlockSpec(memory_space=pltpu.VMEM)
    half = out_memory.shape[1] // 2
    block = (2, SHARE, half)
    return pl.pallas_call(
        output_kernel,
        out_shape=jax.ShapeDtypeStruct((SHARE, 2 * half), bf16),
        in_specs=[vmem] * 4,
        out_specs=vmem,
        scratch_shapes=[
            pltpu.VMEM((2, N_Y, SHARE, half), bf16),
            pltpu.VMEM((2, N_Y, SHARE, half), bf16),
            pltpu.VMEM((2, N_Y, SHARE, half), f32),
            pltpu.VMEM((6, SHARE, half), bf16),
            pltpu.VMEM(block, bf16),
            pltpu.VMEM(block, bf16),
            pltpu.VMEM(block, bf16),
        ]
        + [dma((2,))] * 8,
        compiler_params=PARAMS(
            collective_id=3, has_side_effects=True, vmem_limit_bytes=48 * 1024 * 1024
        ),
        cost_estimate=pl.CostEstimate(flops=10**9, bytes_accessed=10**7, transcendentals=0),
        name="project_out",
    )(gated, attended, out_memory, out_attend)


def per_device(
    tokens,
    input_gain,
    weight_query,
    weight_key,
    weight_value,
    weight_outgate,
    weight_ingate,
    weight_forget,
    forget_shift,
    mem_gain,
    query_down_weight,
    latent_down_weight,
    down_rotary,
    query_gain,
    latent_gain,
    query_up_weight,
    key_up_weight,
    value_up_weight,
    out_memory,
    out_attend,
):
    tp_index = lax.axis_index(TP)
    mem_heads = weight_query.shape[1] // M_QK
    length = forget_shift.shape[0]
    small = jnp.concatenate(
        [
            query_down_weight,
            weight_ingate,
            weight_forget,
            jnp.zeros((tokens.shape[1], 16), jnp.bfloat16),
            latent_down_weight,
            down_rotary,
        ],
        axis=1,
    )
    latent_rows = latent_gain.reshape(8, LATENT_PART)
    gains = jnp.concatenate(
        [
            jnp.pad(query_gain.reshape(8, QUERY_PART), ((0, 0), (0, 128 - QUERY_PART))),
            jnp.concatenate([latent_rows, latent_rows], axis=1),
        ],
        axis=0,
    )
    positions = lax.axis_index(SP) * length + jnp.arange(length, dtype=jnp.int32)
    halfway = ROTARY_CHANNELS // 2
    inverse = jnp.power(ROTARY_BASE, -jnp.arange(halfway, dtype=jnp.float32) / halfway)
    angles = positions.astype(jnp.float32)[:, None] * inverse
    cosine, sine_part = (jnp.tile(made, (1, 4)) for made in (jnp.cos(angles), jnp.sin(angles)))
    memory_inputs, pre_gates, queries, keys_values = project(
        tokens,
        input_gain[None, :],
        small,
        weight_query,
        weight_key,
        weight_value,
        weight_outgate,
        (query_up_weight, key_up_weight, value_up_weight),
        gains,
        cosine,
        sine_part,
    )
    mem_query = memory_inputs[:, :M_QK]
    mem_key = memory_inputs[:, M_QK : 2 * M_QK]
    mem_value = memory_inputs[:, 2 * M_QK : 2 * M_QK + M_V]
    mem_outgate = memory_inputs[:, 2 * M_QK + M_V :]
    in_pre = lax.dynamic_slice_in_dim(pre_gates, QUERY_PART + tp_index, 1, 1)
    forget_pre = lax.dynamic_slice_in_dim(pre_gates, QUERY_PART + 8 + tp_index, 1, 1)
    in_gate = SOFTCAP * jnp.tanh(in_pre / SOFTCAP)
    log_forget = jax.nn.log_sigmoid(SOFTCAP * jnp.tanh((forget_pre + forget_shift) / SOFTCAP))
    cumulative = jnp.cumsum(log_forget[:, 0])
    relative = in_gate[:, 0] - cumulative
    running = lax.cummax(relative)
    ends_at = running[-1]
    key_scale = M_QK ** (-0.5)
    wide_value = mem_value.astype(jnp.float32)
    weights = jnp.exp(relative - ends_at) * key_scale
    local_matrix = lax.dot_general(
        weights[:, None] * wide_value,
        mem_key.astype(jnp.float32),
        (((0,), (0,)), ((), ())),
        precision=PRECISE,
    )
    local_normal = jnp.sum(weights[:, None] * mem_key.astype(jnp.float32), axis=0)
    local_state = (
        local_matrix[None],
        local_normal[None],
        (cumulative[-1] + ends_at)[None],
        cumulative[-1:],
    )
    identity = (
        jnp.zeros((mem_heads, M_V, M_QK), jnp.float32),
        jnp.zeros((mem_heads, M_QK), jnp.float32),
        jnp.full((mem_heads,), FAR_BELOW, jnp.float32),
        jnp.zeros((mem_heads,), jnp.float32),
    )
    prefix = entering(local_state, SP, merge_states, identity)
    start_max = jnp.maximum(prefix[3], prefix[2])
    rescale = jnp.exp(prefix[2] - start_max)
    start_matrix = (prefix[0] * rescale[:, None, None])[0]
    start_normal = (prefix[1] * rescale[:, None])[0]
    highest = jnp.maximum(start_max[0], running)
    causal = jnp.tril(jnp.ones((length, length), dtype=bool))
    within = jnp.where(causal, relative[None, :] - highest[:, None], -jnp.inf)
    affinity = lax.dot_general(
        mem_query, mem_key, (((1,), (1,)), ((), ())), preferred_element_type=jnp.float32
    )
    affinity = affinity * (jnp.exp(within) * key_scale)
    across = jnp.exp(start_max[0] - highest)
    wide_query = mem_query.astype(jnp.float32)
    numerator = jnp.dot(affinity, wide_value, precision=PRECISE) + across[:, None] * lax.dot_general(
        wide_query, start_matrix, (((1,), (1,)), ((), ())), precision=PRECISE
    )
    denominator = jnp.sum(affinity, axis=1) + across * jnp.sum(
        wide_query * start_normal[None, :], axis=1
    )
    floor = jnp.exp(-(cumulative + highest))
    cell = numerator / jnp.maximum(jnp.abs(denominator), floor)[:, None]
    cell_total = lax.psum(jnp.sum(cell * cell, axis=1), TP)
    gain_part = lax.dynamic_slice_in_dim(mem_gain, tp_index * mem_heads * M_V, mem_heads * M_V, 0)
    gated = (
        cell
        * lax.rsqrt(cell_total / (MEMORY_HEADS * M_V) + SMALL_CONSTANT)[:, None]
        * gain_part.astype(jnp.float32)
    )
    gated = gated * jax.nn.sigmoid(mem_outgate.astype(jnp.float32))
    gated = gated.astype(jnp.bfloat16)
    attended = attend(queries, keys_values)
    return project_out(gated, attended, out_memory, out_attend)


def solution(mesh):
    torus = Mesh(mesh.devices.reshape(N_Z, N_X, 4, 2), SP_TP)
    in_specs = (
        P(SP_TP, None),
        P(),
        P(None, TP),
        P(None, TP),
        P(None, TP),
        P(None, TP),
        P(),
        P(),
        P(SP, TP),
        P(),
        P(None, TP),
        P(None, TP),
        P(),
        P(),
        P(),
        P(None, TP),
        P(None, TP),
        P(None, TP),
        P(TP, None),
        P(TP, None),
    )
    out_specs = P(SP_TP, None)
    return jax.shard_map(
        per_device, mesh=torus, in_specs=in_specs, out_specs=out_specs, check_vma=False
    )
```

```python
import jax
import jax.numpy as jnp
from jax import lax
from jax.experimental import pallas as pl
from jax.experimental.pallas import tpu as pltpu
from jax.sharding import Mesh
from jax.sharding import PartitionSpec as P

MEMORY_HEADS = 8
M_QK = 128
M_V = 256
PLAIN_CHANNELS = 128
ROTARY_CHANNELS = 64
VALUE_CHANNELS = 128
SP = ("z", "x")
TP = ("y", "c")
SP_TP = ("z", "x", "y", "c")


SMALL_CONSTANT = 1e-06
SOFTCAP = 15.0
ROTARY_BASE = 10000.0
PRECISE = lax.Precision.HIGHEST
FAR_BELOW = -1e30

N_Y = 4
N_C = 2
SHARE = 64
QUERY_LATENT = 768
LATENT_WIDTH = 512
QUERY_PART = QUERY_LATENT // (N_Y * N_C)
LATENT_PART = LATENT_WIDTH // (N_Y * N_C)
PARAMS = pltpu.CompilerParams


LOG2E = 1.4426950408889634
N_Z = 8
N_X = 4
ROWS = 512
MESH_ID = pl.DeviceIdType.MESH
CONTRACT_LAST = (((1,), (1,)), ((), ()))
CHUNK = M_QK // N_X
STATE_ROWS = CHUNK + 8
NORMAL_ROW, TOP_ROW, DECAY_ROW = CHUNK, CHUNK + 1, CHUNK + 2


def merge_states(early, late):
    moved = early[TOP_ROW : TOP_ROW + 1] + late[DECAY_ROW : DECAY_ROW + 1]
    late_top = late[TOP_ROW : TOP_ROW + 1]
    joined = jnp.maximum(moved, late_top)
    both = early * jnp.exp(moved - joined) + late * jnp.exp(late_top - joined)
    row = lax.broadcasted_iota(jnp.int32, both.shape, 0)
    decay = early[DECAY_ROW : DECAY_ROW + 1] + late[DECAY_ROW : DECAY_ROW + 1]
    return jnp.where(row == TOP_ROW, joined, jnp.where(row == DECAY_ROW, decay, both))


def in_two(values):
    high = values.astype(jnp.bfloat16)
    return high, (values - high.astype(jnp.float32)).astype(jnp.bfloat16)


def as_columns(row, width):
    return jnp.broadcast_to(row, (width, row.shape[1])).T


def attend_kernel(
    q_ref,
    kv_ref,
    mem_ref,
    gate_ref,
    gain_ref,
    o_ref,
    gated_ref,
    q_all,
    kv_all,
    k_cat,
    top,
    total,
    accum,
    part_out,
    stat_out,
    part_in,
    stat_in,
    cell,
    cell_sum,
    cell_top,
    first_out,
    first_in,
    column_out,
    column_in,
    start_out,
    start_in,
    square_out,
    square_in,
    q_send,
    q_recv,
    up_send,
    up_recv,
    down_send,
    down_recv,
    part_send,
    part_recv,
    stat_send,
    stat_recv,
    first_send,
    first_recv,
    column_send,
    column_recv,
    start_send,
    start_recv,
    square_send,
    square_recv,
):
    f32, bf16 = jnp.float32, jnp.bfloat16
    z, x = lax.axis_index("z"), lax.axis_index("x")
    y, c = lax.axis_index("y"), lax.axis_index("c")
    above, below = lax.rem(z + 1, N_Z), lax.rem(z + N_Z - 1, N_Z)
    peers = [lax.rem(x + d, N_X) for d in range(1, N_X)]
    right, left = peers[0], peers[-1]
    rows_y = [lax.rem(y + d, N_Y) for d in range(1, N_Y)]
    half = kv_ref.shape[0] // 2
    width = PLAIN_CHANNELS

    barrier = pltpu.get_barrier_semaphore()
    devices = [{"z": lax.rem(z + d, N_Z)} for d in range(1, N_Z)]
    devices += [{"x": other} for other in peers] + [{"y": other} for other in rows_y]
    devices.append({"c": 1 - c})
    for device in devices:
        pl.semaphore_signal(barrier, inc=1, device_id=device, device_id_type=MESH_ID)
    pl.semaphore_wait(barrier, len(devices))

    def remote(source, target, send, recv, device):
        return pltpu.make_async_remote_copy(
            src_ref=source,
            dst_ref=target,
            send_sem=send,
            recv_sem=recv,
            device_id=device,
            device_id_type=MESH_ID,
        )

    def kv_copy(up, step, h):
        shift = (N_Z - step + 1) if up else (step - 1)
        owner = lax.rem(z + shift, N_Z)
        rows = pl.ds(h * half, half)
        source = kv_ref.at[rows] if step == 1 else kv_all.at[owner, rows]
        send, recv = (up_send, up_recv) if up else (down_send, down_recv)
        return remote(
            source,
            kv_all.at[owner, rows],
            send.at[step - 1, h],
            recv.at[step - 1, h],
            {"z": above if up else below},
        )

    q_half = ROWS // 2

    def q_copy(number):
        shift, part, to_right = (
            (0, 0, True),
            (0, 1, True),
            (0, 0, False),
            (0, 1, False),
            (N_X - 1, 0, True),
            (1, 1, False),
        )[number]
        owner = lax.rem(x + shift, N_X)
        rows = pl.ds(part * q_half, q_half)
        source = q_ref.at[rows] if shift == 0 else q_all.at[owner, rows]
        return remote(
            source,
            q_all.at[owner, rows],
            q_send.at[number],
            q_recv.at[number],
            {"x": right if to_right else left},
        )

    def part_copy(d):
        return remote(
            part_out.at[d], part_in.at[d], part_send.at[d], part_recv.at[d], {"x": peers[d]}
        )

    def stat_copy(d):
        return remote(
            stat_out.at[d], stat_in.at[d], stat_send.at[d], stat_recv.at[d], {"x": peers[d]}
        )

    def first_copy(d):
        return remote(
            first_out.at[peers[d]],
            first_in.at[x],
            first_send.at[d],
            first_recv.at[d],
            {"x": peers[d]},
        )

    def column_copy(target):
        return remote(
            column_out,
            column_in.at[z],
            column_send.at[target],
            column_recv.at[z],
            {"z": target},
        )

    def column_arrival(source):
        return remote(
            column_out,
            column_in.at[source],
            column_send.at[source],
            column_recv.at[source],
            {"z": source},
        )

    def start_copy(d):
        return remote(
            start_out.at[peers[d]],
            start_in.at[x],
            start_send.at[d],
            start_recv.at[d],
            {"x": peers[d]},
        )

    def square_copy(number):
        device = {"c": 1 - c} if number == 0 else {"y": rows_y[number - 1]}
        return remote(
            square_out.at[min(number, 1)],
            square_in.at[number],
            square_send.at[number],
            square_recv.at[number],
            device,
        )

    started = []

    def start(copy):
        copy.start()
        started.append(copy)

    for h in range(2):
        for up in (True, False):
            start(kv_copy(up, 1, h))
    for number in (0, 3, 1, 2):
        start(q_copy(number))

    q_all[x] = q_ref[...]
    top[...] = jnp.full(top.shape, FAR_BELOW, f32)
    total[...] = jnp.zeros(total.shape, f32)
    accum[...] = jnp.zeros(accum.shape, f32)

    relative, cumulative = gate_ref[0:1], gate_ref[1:2]
    key_scale = M_QK ** (-0.5)
    tall = 256
    for t in range(ROWS // tall):
        rows, seen = slice(t * tall, (t + 1) * tall), (t + 1) * tall
        row = lax.broadcasted_iota(jnp.int32, (tall, seen), 0) + t * tall
        col = lax.broadcasted_iota(jnp.int32, (tall, seen), 1)
        logs = jnp.where(col <= row, relative[:, :seen], -jnp.inf)
        highest = jnp.max(logs, axis=1, keepdims=True)
        affinity = lax.dot_general(
            mem_ref[rows, :M_QK],
            mem_ref[:seen, M_QK : 2 * M_QK],
            CONTRACT_LAST,
            preferred_element_type=f32,
        )
        affinity = affinity * (jnp.exp(logs - highest) * key_scale)
        values = mem_ref[:seen, 2 * M_QK : 2 * M_QK + M_V]
        cell[rows] = sum(
            jnp.dot(piece, values, preferred_element_type=f32) for piece in in_two(affinity)
        )
        cell_sum[rows] = jnp.broadcast_to(
            jnp.sum(affinity, axis=1, keepdims=True), (tall, width)
        )
        cell_top[rows] = jnp.broadcast_to(highest, (tall, width))
    ends_at = jnp.max(relative, axis=1, keepdims=True)
    weights = jnp.exp(relative - ends_at) * key_scale
    wide_key = mem_ref[:, M_QK : 2 * M_QK].astype(f32)
    normal = jnp.sum(as_columns(weights, width) * wide_key, axis=0, keepdims=True)
    values = mem_ref[:, 2 * M_QK : 2 * M_QK + M_V]
    matrix = sum(
        jnp.dot(piece, values, preferred_element_type=f32)
        for piece in in_two(wide_key.T * weights)
    )
    decay = cumulative[:, ROWS - 1 : ROWS]
    row = lax.broadcasted_iota(jnp.int32, (8, M_V), 0)
    lines = jnp.concatenate([normal, jnp.zeros_like(normal)], axis=1)
    notes = jnp.where(
        row == 0, lines, jnp.where(row == 1, ends_at + decay, jnp.where(row == 2, decay, 0.0))
    )
    for k in range(N_X):
        first_out[k, :CHUNK] = matrix[k * CHUNK : (k + 1) * CHUNK]
        first_out[k, CHUNK:] = notes
    for d in range(N_X - 1):
        start(first_copy(d))
    first_in[x] = first_out[x]

    lane = lax.broadcasted_iota(jnp.int32, (ROWS // 2, width), 1)
    low = (lane < ROTARY_CHANNELS).astype(bf16)
    high = (lane >= ROTARY_CHANNELS).astype(bf16)
    scale = LOG2E * (PLAIN_CHANNELS + ROTARY_CHANNELS) ** (-0.5)

    def keys_from(ref):
        k_cat[:, :width] = ref[:ROWS]
        packed = ref[2 * ROWS :]
        k_cat[: ROWS // 2, width:] = packed * low
        k_cat[ROWS // 2 :, width:] = packed * high

    def attend_rows(first, last, values, masked):
        def one(t, carry):
            shard = t // (ROWS // tall)
            rows = pl.ds(pl.multiple_of(t * tall, tall), tall)
            inner = pl.ds(pl.multiple_of((t % (ROWS // tall)) * tall, tall), tall)
            queries = q_all[shard, inner]
            scores = lax.dot_general(
                queries, k_cat[...], CONTRACT_LAST, preferred_element_type=f32
            )
            scores = scores * scale
            if masked:
                row = lax.broadcasted_iota(jnp.int32, scores.shape, 0) + t * tall
                col = lax.broadcasted_iota(jnp.int32, scores.shape, 1) + x * ROWS
                scores = jnp.where(col <= row, scores, -jnp.inf)
            old = top[rows]
            new = jnp.maximum(old, jnp.max(scores, axis=1, keepdims=True))
            probs = jnp.exp2(scores - new[:, :1])
            shrink = jnp.exp2(old - new)
            total[rows] = total[rows] * shrink + jnp.sum(probs, axis=1, keepdims=True)
            accum[rows] = accum[rows] * shrink + jnp.dot(
                probs.astype(bf16), values(), preferred_element_type=f32
            )
            top[rows] = new
            return carry

        lax.fori_loop(first, last, one, 0)

    def arrived(owner, useful):
        @pl.when(useful)
        def _():
            keys_from(kv_all.at[owner])
            attend_rows(0, N_X * steps, lambda: kv_all[owner, ROWS : 2 * ROWS], False)

    last = N_Z // 2

    def take(step):
        for h in range(2):
            for up in (True, False):
                if step == last and up != (h == 0):
                    continue
                kv_copy(up, step, h).wait_recv()
                if step < last - 1 or (step == last - 1 and up == (h == 0)):
                    start(kv_copy(up, step + 1, h))

    def use(step):
        arrived(lax.rem(z + N_Z - step, N_Z), z >= step)
        if step < last:
            arrived(lax.rem(z + step, N_Z), z + step >= N_Z)

    steps = ROWS // tall
    keys_from(kv_ref)
    own_values = lambda: kv_ref[ROWS : 2 * ROWS]
    attend_rows(x * steps, (x + 1) * steps, own_values, True)

    for d in range(N_X - 1):
        first_copy(d).wait_recv()
    column = first_in[0]
    for k in range(1, N_X):
        column = merge_states(column, first_in[k])
    column_out[...] = column
    for target in range(1, N_Z):

        @pl.when(target > z)
        def _(target=target):
            column_copy(target).start()

    q_copy(0).wait_recv()
    start(q_copy(4))
    q_copy(3).wait_recv()
    start(q_copy(5))
    take(1)
    for number in (1, 2, 4, 5):
        q_copy(number).wait_recv()
    attend_rows((x + 1) * steps, N_X * steps, own_values, False)

    def gather_column(k, state):
        column_arrival(k).wait_recv()
        return merge_states(state, column_in[k])

    state = lax.fori_loop(0, z, gather_column, jnp.zeros((STATE_ROWS, M_V), f32))
    for k in range(N_X):
        start_out[k] = state
        if k < N_X - 1:
            state = merge_states(state, first_in[k])
    for d in range(N_X - 1):
        start(start_copy(d))
    start_in[x] = start_out[x]
    use(1)
    take(2)

    for d in range(N_X - 1):
        start_copy(d).wait_recv()
    carried = jnp.concatenate([start_in[k, :CHUNK] for k in range(N_X)], axis=0)
    carried_normal = start_in[0, NORMAL_ROW : NORMAL_ROW + 1, :M_QK]
    carried_top = start_in[0, TOP_ROW : TOP_ROW + 1, :width]
    queries = mem_ref[:, :M_QK]
    from_start = sum(
        jnp.dot(queries, piece, preferred_element_type=f32) for piece in in_two(carried)
    )
    highest = jnp.maximum(carried_top, cell_top[...])
    across, within = jnp.exp(carried_top - highest), jnp.exp(cell_top[...] - highest)
    twice = lambda one: jnp.concatenate([one, one], axis=1)
    numerator = cell[...] * twice(within) + from_start * twice(across)
    denominator = cell_sum[...] * within + across * jnp.sum(
        queries.astype(f32) * carried_normal, axis=1, keepdims=True
    )
    floor = jnp.exp(-(as_columns(cumulative, width) + highest))
    made = numerator / twice(jnp.maximum(jnp.abs(denominator), floor))
    cell[...] = made
    squares = jnp.sum(made * made, axis=1, keepdims=True)
    square_out[0] = jnp.broadcast_to(squares, (ROWS, width)).T[:8]
    start(square_copy(0))

    use(2)
    take(3)
    square_copy(0).wait_recv()
    square_out[1] = square_out[0] + square_in[0]
    for number in range(1, N_Y):
        start(square_copy(number))
    use(3)
    take(4)
    use(4)

    def finish(shard):
        rows = pl.ds(pl.multiple_of(shard * ROWS, ROWS), ROWS)
        summed = jnp.maximum(total[rows], 1.0)
        seen = total[rows] > 0.0
        log_total = jnp.where(seen, top[rows] + jnp.log2(summed), FAR_BELOW)
        return accum[rows] / summed, log_total

    for d in (1, 0, 2):
        part, log_total = finish(peers[d])
        part_out[d] = part.astype(bf16)
        stat_out[d] = log_total.T[:8]
        start(part_copy(d))
        start(stat_copy(d))

    squares = square_out[1]
    for number in range(1, N_Y):
        square_copy(number).wait_recv()
        squares = squares + square_in[number]
    inverse = lax.rsqrt(squares[:1] / (MEMORY_HEADS * M_V) + SMALL_CONSTANT)
    gated = cell[...] * twice(as_columns(inverse, width)) * gain_ref[...].astype(f32)
    gated = gated * jax.nn.sigmoid(mem_ref[:, 2 * M_QK + M_V :].astype(f32))
    gated_ref[...] = gated.astype(bf16)

    own, own_log = finish(x)
    logs = []
    for d in range(N_X - 1):
        stat_copy(d).wait_recv()
        logs.append(as_columns(stat_in[d, 0:1, :], width))
    highest = own_log
    for one in logs:
        highest = jnp.maximum(highest, one)
    weight = jnp.exp2(own_log - highest)
    numerator = own * weight
    denominator = weight
    for d in range(N_X - 1):
        part_copy(d).wait_recv()
        weight = jnp.exp2(logs[d] - highest)
        numerator = numerator + part_in[d].astype(f32) * weight
        denominator = denominator + weight
    o_ref[...] = (numerator / denominator).astype(bf16)
    for copy in started:
        copy.wait_send()
    for target in range(1, N_Z):

        @pl.when(target > z)
        def _(target=target):
            column_copy(target).wait_send()


def attend(queries, keys_values, memory_inputs, gates, gain):
    f32, bf16 = jnp.float32, jnp.bfloat16
    last = N_Z // 2
    dma = pltpu.SemaphoreType.DMA
    vmem = pl.BlockSpec(memory_space=pltpu.VMEM)
    state = (STATE_ROWS, M_V)
    peers = (N_X - 1,)
    return pl.pallas_call(
        attend_kernel,
        out_shape=(
            jax.ShapeDtypeStruct((ROWS, VALUE_CHANNELS), bf16),
            jax.ShapeDtypeStruct((ROWS, M_V), bf16),
        ),
        in_specs=[vmem] * 5,
        out_specs=[vmem] * 2,
        scratch_shapes=[
            pltpu.VMEM((N_X, ROWS, 256), bf16),
            pltpu.VMEM((N_Z, *keys_values.shape), bf16),
            pltpu.VMEM((ROWS, 256), bf16),
            pltpu.VMEM((N_X * ROWS, 128), f32),
            pltpu.VMEM((N_X * ROWS, 128), f32),
            pltpu.VMEM((N_X * ROWS, VALUE_CHANNELS), f32),
            pltpu.VMEM((N_X - 1, ROWS, VALUE_CHANNELS), bf16),
            pltpu.VMEM((N_X - 1, 8, ROWS), f32),
            pltpu.VMEM((N_X - 1, ROWS, VALUE_CHANNELS), bf16),
            pltpu.VMEM((N_X - 1, 8, ROWS), f32),
            pltpu.VMEM((ROWS, M_V), f32),
            pltpu.VMEM((ROWS, 128), f32),
            pltpu.VMEM((ROWS, 128), f32),
            pltpu.VMEM((N_X, *state), f32),
            pltpu.VMEM((N_X, *state), f32),
            pltpu.VMEM(state, f32),
            pltpu.VMEM((N_Z, *state), f32),
            pltpu.VMEM((N_X, *state), f32),
            pltpu.VMEM((N_X, *state), f32),
            pltpu.VMEM((2, 8, ROWS), f32),
            pltpu.VMEM((N_Y, 8, ROWS), f32),
            dma((6,)),
            dma((6,)),
            dma((last, 2)),
            dma((last, 2)),
            dma((last, 2)),
            dma((last, 2)),
            dma(peers),
            dma(peers),
            dma(peers),
            dma(peers),
            dma(peers),
            dma(peers),
            dma((N_Z,)),
            dma((N_Z,)),
            dma(peers),
            dma(peers),
            dma((N_Y,)),
            dma((N_Y,)),
        ],
        compiler_params=pltpu.CompilerParams(
            collective_id=1, has_side_effects=True, vmem_limit_bytes=48 * 1024 * 1024
        ),
        cost_estimate=pl.CostEstimate(
            flops=4 * 10**9, bytes_accessed=10**7, transcendentals=4 * 10**6
        ),
        name="attend",
    )(queries, keys_values, memory_inputs, gates, gain)


class TpGather:
    def __init__(self, full, sends, recvs):
        self.full, self.sends, self.recvs = full, sends, recvs
        self.y, self.c = lax.axis_index("y"), lax.axis_index("c")
        self.half = full.shape[1] // 2
        self.started = []

    def _copy(self, number, shift, part, target):
        slot = lax.rem(self.y + shift, N_Y) * N_C + self.c
        if part is None:
            ref = self.full.at[slot]
        else:
            ref = self.full.at[slot, pl.ds(part * self.half, self.half)]
        if target == "core":
            device = {"c": 1 - self.c}
        else:
            device = {"y": lax.rem(self.y + (1 if target == "up" else N_Y - 1), N_Y)}
        return pltpu.make_async_remote_copy(
            src_ref=ref,
            dst_ref=ref,
            send_sem=self.sends.at[number],
            recv_sem=self.recvs.at[number],
            device_id=device,
            device_id_type=MESH_ID,
        )

    def _start(self, *what):
        copy = self._copy(*what)
        copy.start()
        self.started.append(copy)

    def start(self):
        self._start(0, 0, 0, "up")
        self._start(3, 0, 1, "down")
        self._start(1, 0, 1, "up")
        self._start(2, 0, 0, "down")
        self._start(6, 0, None, "core")

    def relay(self):
        self._copy(0, 0, 0, "up").wait_recv()
        self._start(4, N_Y - 1, 0, "up")
        self._copy(3, 0, 1, "down").wait_recv()
        self._start(5, 1, 1, "down")
        self._copy(1, 0, 1, "up").wait_recv()
        self._start(7, N_Y - 1, None, "core")
        self._copy(2, 0, 0, "down").wait_recv()
        self._start(8, 1, None, "core")

    def near(self):
        for number, shift in ((6, 0), (7, N_Y - 1), (8, 1)):
            self._copy(number, shift, None, "core").wait_recv()

    def far(self):
        self._copy(4, 0, 0, "up").wait_recv()
        self._start(9, 2, 0, "core")
        self._copy(5, 0, 1, "down").wait_recv()
        self._start(10, 2, 1, "core")
        for part in range(2):
            self._copy(9 + part, 2, part, "core").wait_recv()

    def finish(self):
        for copy in self.started:
            copy.wait_send()


def greet_tp(barrier):
    y, c = lax.axis_index("y"), lax.axis_index("c")
    for device in (
        {"c": 1 - c},
        {"y": lax.rem(y + 1, N_Y)},
        {"y": lax.rem(y + N_Y - 1, N_Y)},
    ):
        pl.semaphore_signal(barrier, inc=1, device_id=device, device_id_type=MESH_ID)


def project_kernel(
    tokens,
    gain,
    gains,
    cosine,
    sine_part,
    shift_row,
    narrow_query,
    narrow_latent,
    narrow_rotary,
    narrow_ingate,
    narrow_forget,
    query_hbm,
    key_hbm,
    value_hbm,
    outgate_hbm,
    query_up_hbm,
    key_up_hbm,
    value_up_hbm,
    mem_ref,
    gate_ref,
    q_ref,
    kv_ref,
    rows_all,
    latents,
    small,
    ingate,
    forget,
    big,
    query_up,
    key_up,
    value_up,
    pre_gates,
    up_query,
    up_latent,
    wide_query,
    wide_latent,
    load_sem,
    row_send,
    row_recv,
    lat_send,
    lat_recv,
):
    f32, bf16 = jnp.float32, jnp.bfloat16
    y, c = lax.axis_index("y"), lax.axis_index("c")
    mine = y * N_C + c
    width = 128
    sources = (
        (narrow_query, small.at[pl.ds(0, QUERY_PART)]),
        (narrow_latent, small.at[pl.ds(width, LATENT_PART)]),
        (narrow_rotary, small.at[pl.ds(width + LATENT_PART, ROTARY_CHANNELS)]),
        (narrow_ingate, ingate),
        (narrow_forget, forget),
        (query_up_hbm, query_up),
        (key_up_hbm, key_up),
        (value_up_hbm, value_up),
    )
    loads = [
        pltpu.make_async_copy(source, target, load_sem.at[k])
        for k, (source, target) in enumerate(sources)
    ]
    at = 0
    for k, ref in enumerate((query_hbm, key_hbm, value_hbm, outgate_hbm)):
        columns = ref.shape[1]
        loads.append(
            pltpu.make_async_copy(ref, big.at[:, pl.ds(at, columns)], load_sem.at[8 + k])
        )
        at += columns
    for load in loads:
        load.start()

    wide = tokens[...].astype(f32)
    inverse = lax.rsqrt(jnp.mean(wide * wide, axis=1, keepdims=True) + SMALL_CONSTANT)
    rows_all[mine] = (wide * inverse * gain[...].astype(f32)).astype(bf16)
    small[QUERY_PART:width] = jnp.zeros((width - QUERY_PART, small.shape[1]), bf16)

    barrier = pltpu.get_barrier_semaphore()
    greet_tp(barrier)
    pl.semaphore_wait(barrier, 3)
    gather = TpGather(rows_all, row_send, row_recv)
    gather.start()

    for load in loads:
        load.wait()
    up_query[...] = jnp.zeros(up_query.shape, bf16)
    for s in range(N_Y * N_C):
        up_query[s * width : s * width + QUERY_PART] = query_up[
            s * QUERY_PART : (s + 1) * QUERY_PART
        ]
        part = slice(s * LATENT_PART, (s + 1) * LATENT_PART)
        for h in range(2):
            at = s * width + h * LATENT_PART
            up_latent[at : at + LATENT_PART, :width] = key_up[part]
            up_latent[at : at + LATENT_PART, width:] = value_up[part]

    lane = lax.broadcasted_iota(jnp.int32, (1, width), 1)
    row_id = lax.broadcasted_iota(jnp.int32, (width, width), 0)
    col_id = lax.broadcasted_iota(jnp.int32, (width, width), 1)
    channels = lax.rem(col_id, ROTARY_CHANNELS)
    halfway = ROTARY_CHANNELS // 2
    twin = (row_id == channels).astype(bf16)
    partner = lax.rem(channels + halfway, ROTARY_CHANNELS)
    sign = jnp.where(channels < halfway, -1.0, 1.0)

    def duplicated(values, offset):
        return jnp.dot(
            values, (row_id == channels + offset).astype(bf16), preferred_element_type=f32
        )

    def rotated(values, offset):
        swap = jnp.where(row_id == partner + offset, sign, 0.0).astype(bf16)
        turned = jnp.dot(values, swap, preferred_element_type=f32)
        return duplicated(values, offset) * cosine[...] + turned * sine_part[...]

    def chip_rows(chip):
        slots = [rows_all[chip * N_C + k] for k in range(N_C)]
        return jnp.concatenate(slots, axis=0)

    span = N_C * SHARE
    tile = 256

    def project_small(chip):
        rows = pl.ds(pl.multiple_of(chip * span, span), span)
        here = chip_rows(chip)
        made = lax.dot_general(here, small[...], CONTRACT_LAST, preferred_element_type=f32)
        for k, ref in enumerate((ingate, forget)):
            pre_gates[k, :, rows] = lax.dot_general(
                ref[...], here, CONTRACT_LAST, preferred_element_type=f32
            )
        rounded = made.astype(bf16)
        latents[mine, rows] = rounded[:, :width]
        wide_latent[rows, :width] = rounded[:, width:]

    def project_big(chip):
        rows = pl.ds(pl.multiple_of(chip * span, span), span)

        def one(t, carry):
            columns = pl.ds(pl.multiple_of(t * tile, tile), tile)
            made = jnp.dot(chip_rows(chip), big[:, columns], preferred_element_type=f32)
            mem_ref[rows, columns] = made.astype(bf16)
            return carry

        lax.fori_loop(0, big.shape[1] // tile, one, 0)

    gather.relay()
    gather.near()
    near = [y, lax.rem(y + N_Y - 1, N_Y), lax.rem(y + 1, N_Y)]
    for chip in near:
        project_small(chip)
    opposite = lax.rem(y + 2, N_Y)
    gather.far()
    project_small(opposite)

    second = wide_latent[:, :width]
    both = duplicated(second, 0)
    half = ROWS // 2
    packed = jnp.where(lane < LATENT_PART, both[:half], both[half:])
    latents[mine, ROWS:] = packed.astype(bf16)
    exchange = TpGather(latents, lat_send, lat_recv)
    exchange.start()
    for chip in near[:2]:
        project_big(chip)
    exchange.relay()
    for chip in (near[2], opposite):
        project_big(chip)
    heads = lax.broadcasted_iota(jnp.int32, (8, ROWS), 0) == mine
    in_pre, forget_pre = (
        jnp.sum(jnp.where(heads, pre_gates[k], 0.0), axis=0, keepdims=True) for k in range(2)
    )
    in_gate = SOFTCAP * jnp.tanh(in_pre / SOFTCAP)
    capped = SOFTCAP * jnp.tanh((forget_pre + shift_row[...]) / SOFTCAP)
    small_part = jnp.exp(-jnp.abs(capped))
    above_one = 1.0 + small_part
    grown = jnp.where(
        above_one == 1.0, small_part, jnp.log(above_one) * small_part / (above_one - 1.0)
    )
    log_forget = jnp.minimum(capped, 0.0) - grown
    earlier = lax.broadcasted_iota(jnp.int32, (ROWS, ROWS), 0) <= lax.broadcasted_iota(
        jnp.int32, (ROWS, ROWS), 1
    )
    cumulative = jnp.dot(
        jnp.broadcast_to(log_forget, (8, ROWS)),
        earlier.astype(f32),
        precision=PRECISE,
        preferred_element_type=f32,
    )
    top_rows = lax.broadcasted_iota(jnp.int32, (8, ROWS), 0) == 0
    gate_ref[...] = jnp.where(top_rows, in_gate - cumulative, cumulative)
    key_turned = rotated(second, LATENT_PART)
    kv_ref[2 * ROWS :] = jnp.where(
        lane < ROTARY_CHANNELS, key_turned[:half], key_turned[half:]
    ).astype(bf16)
    exchange.near()
    exchange.far()

    query_mask = (lane < QUERY_PART).astype(f32)
    squares = jnp.zeros((ROWS, width), f32)
    low_squares = jnp.zeros((half, width), f32)
    for s in range(N_Y * N_C):
        part = latents[s, :ROWS].astype(f32) * query_mask
        squares = squares + part * part
        part = latents[s, ROWS:].astype(f32)
        low_squares = low_squares + part * part
    query_scale = lax.rsqrt(
        jnp.sum(squares, axis=1, keepdims=True) / QUERY_LATENT + SMALL_CONSTANT
    )
    low = lane < LATENT_PART
    low_scale = lax.rsqrt(
        jnp.sum(jnp.where(low, low_squares, 0.0), axis=1, keepdims=True) / LATENT_WIDTH
        + SMALL_CONSTANT
    )
    high_scale = lax.rsqrt(
        jnp.sum(jnp.where(low, 0.0, low_squares), axis=1, keepdims=True) / LATENT_WIDTH
        + SMALL_CONSTANT
    )
    latent_scale = jnp.where(low, low_scale, high_scale)
    for s in range(N_Y * N_C):
        columns = slice(s * width, (s + 1) * width)
        part = latents[s, :ROWS].astype(f32) * query_mask
        wide_query[:, columns] = (part * query_scale * gains[s : s + 1]).astype(bf16)
        part = latents[s, ROWS:].astype(f32)
        made = (part * latent_scale * gains[8 + s : 9 + s]).astype(bf16)
        wide_latent[:half, columns] = jnp.where(low, made, jnp.zeros_like(made))
        wide_latent[half:, columns] = jnp.where(low, jnp.zeros_like(made), made)
    made = jnp.dot(wide_query[...], up_query[...], preferred_element_type=f32).astype(bf16)
    q_ref[:, :width] = made[:, :width]
    turning = jnp.concatenate([made[:, width:], jnp.zeros((ROWS, ROTARY_CHANNELS), bf16)], axis=1)
    q_ref[:, width:] = rotated(turning, 0).astype(bf16)
    made = jnp.dot(wide_latent[...], up_latent[...], preferred_element_type=f32).astype(bf16)
    kv_ref[:ROWS] = made[:, :width]
    kv_ref[ROWS : 2 * ROWS] = made[:, width:]
    gather.finish()
    exchange.finish()


def project(dense, narrow, weights):
    f32, bf16 = jnp.float32, jnp.bfloat16
    depth = weights[0].shape[0]
    dma = pltpu.SemaphoreType.DMA
    vmem = pl.BlockSpec(memory_space=pltpu.VMEM)
    hbm = pl.BlockSpec(memory_space=pl.ANY)
    mem_width = sum(one.shape[1] for one in weights[:4])
    return pl.pallas_call(
        project_kernel,
        out_shape=(
            jax.ShapeDtypeStruct((ROWS, mem_width), bf16),
            jax.ShapeDtypeStruct((8, ROWS), f32),
            jax.ShapeDtypeStruct((ROWS, 256), bf16),
            jax.ShapeDtypeStruct((ROWS * 5 // 2, 128), bf16),
        ),
        in_specs=[vmem] * len(dense) + [hbm] * (len(narrow) + len(weights)),
        out_specs=[vmem] * 4,
        scratch_shapes=[
            pltpu.VMEM((N_Y * N_C, SHARE, depth), bf16),
            pltpu.VMEM((N_Y * N_C, ROWS * 3 // 2, 128), bf16),
            pltpu.VMEM((256, depth), bf16),
            pltpu.VMEM((8, depth), bf16),
            pltpu.VMEM((8, depth), bf16),
            pltpu.VMEM((depth, mem_width), bf16),
            *(pltpu.VMEM(one.shape, bf16) for one in weights[4:]),
            pltpu.VMEM((2, 8, ROWS), f32),
            pltpu.VMEM((1024, PLAIN_CHANNELS + ROTARY_CHANNELS), bf16),
            pltpu.VMEM((1024, 256), bf16),
            pltpu.VMEM((ROWS, 1024), bf16),
            pltpu.VMEM((ROWS, 1024), bf16),
            dma((12,)),
            dma((11,)),
            dma((11,)),
            dma((11,)),
            dma((11,)),
        ],
        compiler_params=PARAMS(
            collective_id=2, has_side_effects=True, vmem_limit_bytes=48 * 1024 * 1024
        ),
        cost_estimate=pl.CostEstimate(
            flops=3 * 10**9, bytes_accessed=10**7, transcendentals=10**4
        ),
        name="project",
    )(*dense, *narrow, *weights)


def output_kernel(
    gated,
    attended,
    out_memory,
    out_attend,
    o_ref,
    to_core,
    from_core,
    sums,
    passing,
    from_below,
    from_above,
    relay_in,
    core_send,
    core_recv,
    relay_send,
    relay_recv,
    up_send,
    up_recv,
    down_send,
    down_recv,
):
    f32, bf16 = jnp.float32, jnp.bfloat16
    y, c = lax.axis_index("y"), lax.axis_index("c")
    above, below = lax.rem(y + 1, N_Y), lax.rem(y + N_Y - 1, N_Y)
    opposite = lax.rem(y + 2, N_Y)
    half = out_memory.shape[1] // 2
    tile = 512

    barrier = pltpu.get_barrier_semaphore()
    greet_tp(barrier)

    def remote(source, target, send, recv, device):
        return pltpu.make_async_remote_copy(
            src_ref=source,
            dst_ref=target,
            send_sem=send,
            recv_sem=recv,
            device_id=device,
            device_id_type=MESH_ID,
        )

    def rows_of(ref, core):
        picked = [ref[pl.ds(pl.multiple_of((k * N_C + core) * SHARE, SHARE), SHARE)] for k in range(N_Y)]
        return jnp.concatenate(picked, axis=0)

    def partial(core, h, store):
        memory_rows, attend_rows = rows_of(gated, core), rows_of(attended, core)
        for t in range(half // tile):
            columns = slice(h * half + t * tile, h * half + (t + 1) * tile)
            made = jnp.dot(memory_rows, out_memory[:, columns], preferred_element_type=f32)
            made = made + jnp.dot(attend_rows, out_attend[:, columns], preferred_element_type=f32)
            store(t * tile, made.astype(bf16).reshape(N_Y, SHARE, tile))

    def core_copy(h):
        return remote(
            to_core.at[h], from_core.at[h], core_send.at[h], core_recv.at[h], {"c": 1 - c}
        )

    def relay_copy(h):
        return remote(
            passing.at[h],
            relay_in.at[h],
            relay_send.at[h],
            relay_recv.at[h],
            {"y": above if h == 0 else below},
        )

    def up_copy(h):
        return remote(
            passing.at[2 + h], from_below.at[h], up_send.at[h], up_recv.at[h], {"y": above}
        )

    def down_copy(h):
        return remote(
            passing.at[4 + h], from_above.at[h], down_send.at[h], down_recv.at[h], {"y": below}
        )

    started = []

    def start(copy):
        copy.start()
        started.append(copy)

    for h in range(2):

        def keep(at, block, h=h):
            to_core[h, :, :, at : at + tile] = block

        partial(1 - c, h, keep)
        if h == 0:
            pl.semaphore_wait(barrier, 3)
        start(core_copy(h))
    for h in range(2):

        def keep(at, block, h=h):
            sums[h, :, :, at : at + tile] = block.astype(f32)

        partial(c, h, keep)
    for h in range(2):
        core_copy(h).wait_recv()
        sums[h] = sums[h] + from_core[h].astype(f32)
        passing[h] = sums[h, opposite].astype(bf16)
        start(relay_copy(h))
        if h == 0:
            passing[4] = sums[0, below].astype(bf16)
            start(down_copy(0))
        else:
            passing[3] = sums[1, above].astype(bf16)
            start(up_copy(1))
    relay_copy(0).wait_recv()
    passing[2] = (sums[0, above] + relay_in[0].astype(f32)).astype(bf16)
    start(up_copy(0))
    relay_copy(1).wait_recv()
    passing[5] = (sums[1, below] + relay_in[1].astype(f32)).astype(bf16)
    start(down_copy(1))
    for h in (1, 0):
        up_copy(h).wait_recv()
        down_copy(h).wait_recv()
        made = sums[h, y] + from_below[h].astype(f32) + from_above[h].astype(f32)
        o_ref[:, h * half : (h + 1) * half] = made.astype(bf16)
    for copy in started:
        copy.wait_send()


def project_out(gated, attended, out_memory, out_attend):
    f32, bf16 = jnp.float32, jnp.bfloat16
    dma = pltpu.SemaphoreType.DMA
    vmem = pl.BlockSpec(memory_space=pltpu.VMEM)
    half = out_memory.shape[1] // 2
    block = (2, SHARE, half)
    return pl.pallas_call(
        output_kernel,
        out_shape=jax.ShapeDtypeStruct((SHARE, 2 * half), bf16),
        in_specs=[vmem] * 4,
        out_specs=vmem,
        scratch_shapes=[
            pltpu.VMEM((2, N_Y, SHARE, half), bf16),
            pltpu.VMEM((2, N_Y, SHARE, half), bf16),
            pltpu.VMEM((2, N_Y, SHARE, half), f32),
            pltpu.VMEM((6, SHARE, half), bf16),
            pltpu.VMEM(block, bf16),
            pltpu.VMEM(block, bf16),
            pltpu.VMEM(block, bf16),
        ]
        + [dma((2,))] * 8,
        compiler_params=PARAMS(
            collective_id=3, has_side_effects=True, vmem_limit_bytes=48 * 1024 * 1024
        ),
        cost_estimate=pl.CostEstimate(flops=10**9, bytes_accessed=10**7, transcendentals=0),
        name="project_out",
    )(gated, attended, out_memory, out_attend)


def per_device(
    tokens,
    input_gain,
    weight_query,
    weight_key,
    weight_value,
    weight_outgate,
    weight_ingate,
    weight_forget,
    forget_shift,
    mem_gain,
    query_down_weight,
    latent_down_weight,
    down_rotary,
    query_gain,
    latent_gain,
    query_up_weight,
    key_up_weight,
    value_up_weight,
    out_memory,
    out_attend,
):
    length = forget_shift.shape[0]
    latent_rows = latent_gain.reshape(8, LATENT_PART)
    gains = jnp.concatenate(
        [
            jnp.pad(query_gain.reshape(8, QUERY_PART), ((0, 0), (0, 128 - QUERY_PART))),
            jnp.concatenate([latent_rows, latent_rows], axis=1),
        ],
        axis=0,
    )
    positions = lax.axis_index(SP) * length + jnp.arange(length, dtype=jnp.int32)
    halfway = ROTARY_CHANNELS // 2
    inverse = jnp.power(ROTARY_BASE, -jnp.arange(halfway, dtype=jnp.float32) / halfway)
    angles = positions.astype(jnp.float32)[:, None] * inverse
    cosine, sine_part = (jnp.tile(made, (1, 4)) for made in (jnp.cos(angles), jnp.sin(angles)))
    memory_inputs, gates, queries, keys_values = project(
        (tokens, input_gain[None, :], gains, cosine, sine_part, forget_shift.T),
        (
            query_down_weight.T,
            latent_down_weight.T,
            down_rotary.T,
            weight_ingate.T,
            weight_forget.T,
        ),
        (
            weight_query,
            weight_key,
            weight_value,
            weight_outgate,
            query_up_weight,
            key_up_weight,
            value_up_weight,
        ),
    )
    gain_part = lax.dynamic_slice_in_dim(mem_gain, lax.axis_index(TP) * M_V, M_V, 0)
    attended, gated = attend(queries, keys_values, memory_inputs, gates, gain_part[None, :])
    return project_out(gated, attended, out_memory, out_attend)


def solution(mesh):
    torus = Mesh(mesh.devices.reshape(N_Z, N_X, 4, 2), SP_TP)
    in_specs = (
        P(SP_TP, None),
        P(),
        P(None, TP),
        P(None, TP),
        P(None, TP),
        P(None, TP),
        P(),
        P(),
        P(SP, TP),
        P(),
        P(None, TP),
        P(None, TP),
        P(),
        P(),
        P(),
        P(None, TP),
        P(None, TP),
        P(None, TP),
        P(TP, None),
        P(TP, None),
    )
    out_specs = P(SP_TP, None)
    return jax.shard_map(
        per_device, mesh=torus, in_specs=in_specs, out_specs=out_specs, check_vma=False
    )
```

```python
import functools

import jax
import jax.numpy as jnp
from jax import lax
from jax.experimental import pallas as pl
from jax.experimental.pallas import tpu as pltpu
from jax.sharding import Mesh
from jax.sharding import PartitionSpec as P

MEMORY_HEADS = 8
M_QK = 128
M_V = 256
PLAIN_CHANNELS = 128
ROTARY_CHANNELS = 64
VALUE_CHANNELS = 128
SP = ("z", "x")
TP = ("y", "c")
SP_TP = ("z", "x", "y", "c")


SMALL_CONSTANT = 1e-06
SOFTCAP = 15.0
ROTARY_BASE = 10000.0
PRECISE = lax.Precision.HIGHEST
FAR_BELOW = -1e30

N_Y = 4
N_C = 2
SHARE = 64
QUERY_LATENT = 768
LATENT_WIDTH = 512
QUERY_PART = QUERY_LATENT // (N_Y * N_C)
LATENT_PART = LATENT_WIDTH // (N_Y * N_C)
LOG2E = 1.4426950408889634
N_Z = 8
N_X = 4
ROWS = 512
MESH_ID = pl.DeviceIdType.MESH
CONTRACT_LAST = (((1,), (1,)), ((), ()))
CHUNK = M_QK // N_X
TALL = 512
GROUP = 1
STATE_ROWS = CHUNK + 8
NORMAL_ROW, TOP_ROW, DECAY_ROW = CHUNK, CHUNK + 1, CHUNK + 2


def merge_states(early, late):
    moved = early[TOP_ROW : TOP_ROW + 1] + late[DECAY_ROW : DECAY_ROW + 1]
    late_top = late[TOP_ROW : TOP_ROW + 1]
    joined = jnp.maximum(moved, late_top)
    both = early * jnp.exp(moved - joined) + late * jnp.exp(late_top - joined)
    row = lax.broadcasted_iota(jnp.int32, both.shape, 0)
    decay = early[DECAY_ROW : DECAY_ROW + 1] + late[DECAY_ROW : DECAY_ROW + 1]
    return jnp.where(row == TOP_ROW, joined, jnp.where(row == DECAY_ROW, decay, both))


def in_two(values):
    high = values.astype(jnp.bfloat16)
    return high, (values - high.astype(jnp.float32)).astype(jnp.bfloat16)


def as_columns(row, width):
    return jnp.broadcast_to(row, (width, row.shape[1])).T


def attend_phase(
    q_ref,
    kv_ref,
    mem_ref,
    gate_ref,
    gain_ref,
    attended_ref,
    gated_ref,
    q_all,
    kv_all,
    k_cat,
    top,
    total,
    accum,
    part_out,
    stat_out,
    part_in,
    stat_in,
    cell,
    cell_sum,
    cell_top,
    first_out,
    first_in,
    column_out,
    column_in,
    start_out,
    start_in,
    square_out,
    square_in,
    passed,
    q_send,
    q_recv,
    up_send,
    up_recv,
    down_send,
    down_recv,
    part_send,
    part_recv,
    stat_send,
    stat_recv,
    first_send,
    first_recv,
    column_send,
    column_recv,
    start_send,
    start_recv,
    square_send,
    square_recv,
    passed_send,
    passed_recv,
):
    f32, bf16 = jnp.float32, jnp.bfloat16
    z, x = lax.axis_index("z"), lax.axis_index("x")
    y, c = lax.axis_index("y"), lax.axis_index("c")
    above, below = lax.rem(z + 1, N_Z), lax.rem(z + N_Z - 1, N_Z)
    peers = [lax.rem(x + d, N_X) for d in range(1, N_X)]
    right, left = peers[0], peers[-1]
    rows_y = [lax.rem(y + d, N_Y) for d in range(1, N_Y)]
    me_tp = y * N_C + c
    half = kv_ref.shape[0] // 2
    width = PLAIN_CHANNELS

    def remote(source, target, send, recv, device):
        return pltpu.make_async_remote_copy(
            src_ref=source,
            dst_ref=target,
            send_sem=send,
            recv_sem=recv,
            device_id=device,
            device_id_type=MESH_ID,
        )

    def kv_copy(up, step, h):
        shift = (N_Z - step + 1) if up else (step - 1)
        owner = lax.rem(z + shift, N_Z)
        rows = pl.ds(h * half, half)
        source = kv_ref.at[rows] if step == 1 else kv_all.at[owner, rows]
        send, recv = (up_send, up_recv) if up else (down_send, down_recv)
        return remote(
            source,
            kv_all.at[owner, rows],
            send.at[step - 1, h],
            recv.at[step - 1, h],
            {"z": above if up else below},
        )

    q_half = ROWS // 2

    def q_copy(number):
        shift, part, to_right = (
            (0, 0, True),
            (0, 1, True),
            (0, 0, False),
            (0, 1, False),
            (N_X - 1, 0, True),
            (1, 1, False),
        )[number]
        owner = lax.rem(x + shift, N_X)
        rows = pl.ds(part * q_half, q_half)
        source = q_ref.at[rows] if shift == 0 else q_all.at[owner, rows]
        return remote(
            source,
            q_all.at[owner, rows],
            q_send.at[number],
            q_recv.at[number],
            {"x": right if to_right else left},
        )

    def part_copy(d):
        return remote(
            part_out.at[d], part_in.at[d], part_send.at[d], part_recv.at[d], {"x": peers[d]}
        )

    def far_copy(h, hop):
        rows = pl.ds(h * q_half, q_half)
        return remote(
            part_out.at[1, rows] if hop == 0 else passed.at[h],
            passed.at[h] if hop == 0 else part_in.at[1, rows],
            passed_send.at[hop, h],
            passed_recv.at[hop, h],
            {"x": right if h == 0 else left},
        )

    def stat_copy(d):
        return remote(
            stat_out.at[d], stat_in.at[d], stat_send.at[d], stat_recv.at[d], {"x": peers[d]}
        )

    def first_copy(d):
        return remote(
            first_out.at[peers[d]],
            first_in.at[x],
            first_send.at[d],
            first_recv.at[d],
            {"x": peers[d]},
        )

    def column_copy(target):
        return remote(
            column_out,
            column_in.at[z],
            column_send.at[target],
            column_recv.at[z],
            {"z": target},
        )

    def column_arrival(source):
        return remote(
            column_out,
            column_in.at[source],
            column_send.at[source],
            column_recv.at[source],
            {"z": source},
        )

    def start_copy(d):
        return remote(
            start_out.at[peers[d]],
            start_in.at[x],
            start_send.at[d],
            start_recv.at[d],
            {"x": peers[d]},
        )

    def square_copy(number):
        device = {"c": 1 - c} if number == 0 else {"y": rows_y[number - 1]}
        return remote(
            square_out.at[min(number, 1)],
            square_in.at[number],
            square_send.at[number],
            square_recv.at[number],
            device,
        )

    started = []

    def start(copy):
        copy.start()
        started.append(copy)

    for h in range(2):
        for up in (True, False):
            start(kv_copy(up, 1, h))
    top[...] = jnp.full(top.shape, FAR_BELOW, f32)
    total[...] = jnp.zeros(total.shape, f32)
    for number in (0, 3, 1, 2):
        start(q_copy(number))
    accum[...] = jnp.zeros(accum.shape, f32)
    q_all[x] = q_ref[...]

    relative, cumulative = gate_ref[0:1], gate_ref[1:2]
    key_scale = M_QK ** (-0.5)
    tall = 256
    for t in range(ROWS // tall):
        rows, seen = slice(t * tall, (t + 1) * tall), (t + 1) * tall
        row = lax.broadcasted_iota(jnp.int32, (tall, seen), 0) + t * tall
        col = lax.broadcasted_iota(jnp.int32, (tall, seen), 1)
        logs = jnp.where(col <= row, relative[:, :seen], -jnp.inf)
        highest = jnp.max(logs, axis=1, keepdims=True)
        affinity = lax.dot_general(
            mem_ref[rows, :M_QK],
            mem_ref[:seen, M_QK : 2 * M_QK],
            CONTRACT_LAST,
            preferred_element_type=f32,
        )
        affinity = affinity * (jnp.exp(logs - highest) * key_scale)
        values = mem_ref[:seen, 2 * M_QK : 2 * M_QK + M_V]
        cell[rows] = sum(
            jnp.dot(piece, values, preferred_element_type=f32) for piece in in_two(affinity)
        )
        cell_sum[rows] = jnp.broadcast_to(
            jnp.sum(affinity, axis=1, keepdims=True), (tall, width)
        )
        cell_top[rows] = jnp.broadcast_to(highest, (tall, width))
    ends_at = jnp.max(relative, axis=1, keepdims=True)
    weights = jnp.exp(relative - ends_at) * key_scale
    wide_key = mem_ref[:, M_QK : 2 * M_QK].astype(f32)
    normal = jnp.sum(as_columns(weights, width) * wide_key, axis=0, keepdims=True)
    values = mem_ref[:, 2 * M_QK : 2 * M_QK + M_V]
    matrix = sum(
        jnp.dot(piece, values, preferred_element_type=f32)
        for piece in in_two(wide_key.T * weights)
    )
    decay = cumulative[:, ROWS - 1 : ROWS]
    row = lax.broadcasted_iota(jnp.int32, (8, M_V), 0)
    lines = jnp.concatenate([normal, jnp.zeros_like(normal)], axis=1)
    notes = jnp.where(
        row == 0, lines, jnp.where(row == 1, ends_at + decay, jnp.where(row == 2, decay, 0.0))
    )
    for k in range(N_X):
        first_out[k, :CHUNK] = matrix[k * CHUNK : (k + 1) * CHUNK]
        first_out[k, CHUNK:] = notes
    for d in range(N_X - 1):
        start(first_copy(d))
    first_in[x] = first_out[x]

    lane = lax.broadcasted_iota(jnp.int32, (ROWS // 2, width), 1)
    low = (lane < ROTARY_CHANNELS).astype(bf16)
    high = (lane >= ROTARY_CHANNELS).astype(bf16)
    scale = LOG2E * (PLAIN_CHANNELS + ROTARY_CHANNELS) ** (-0.5)

    def keys_from(ref):
        k_cat[:, :width] = ref[:ROWS]
        packed = ref[2 * ROWS :]
        k_cat[: ROWS // 2, width:] = packed * low
        k_cat[ROWS // 2 :, width:] = packed * high

    def attend_tile(t, keys, values, masked):
        shard = t // (ROWS // TALL)
        rows = pl.ds(pl.multiple_of(t * TALL, TALL), TALL)
        inner = pl.ds(pl.multiple_of((t % (ROWS // TALL)) * TALL, TALL), TALL)
        scores = lax.dot_general(
            q_all[shard, inner], keys, CONTRACT_LAST, preferred_element_type=f32
        )
        scores = scores * scale
        if masked:
            row = lax.broadcasted_iota(jnp.int32, scores.shape, 0) + t * TALL
            col = lax.broadcasted_iota(jnp.int32, scores.shape, 1) + x * ROWS
            scores = jnp.where(col <= row, scores, -jnp.inf)
        old = top[rows]
        new = jnp.maximum(old, jnp.max(scores, axis=1, keepdims=True))
        probs = jnp.exp2(scores - jnp.concatenate([new] * (ROWS // width), axis=1))
        shrink = jnp.exp2(old - new)
        added = sum(probs[:, k : k + width] for k in range(0, ROWS, width))
        total[rows] = total[rows] * shrink + added
        accum[rows] = accum[rows] * shrink + jnp.dot(
            probs.astype(bf16), values, preferred_element_type=f32
        )
        top[rows] = new

    def attend_rows(first, last, values, masked):
        def one(g, carry):
            for u in range(GROUP):
                attend_tile(g * GROUP + u, k_cat[...], values(), masked)
            return carry

        lax.fori_loop(first, last, one, 0)

    last = N_Z // 2
    steps = ROWS // (TALL * GROUP)

    def arrived(owner, useful):
        @pl.when(useful)
        def _():
            keys_from(kv_all.at[owner])
            attend_rows(0, N_X * steps, lambda: kv_all[owner, ROWS : 2 * ROWS], False)

    def take(step, h):
        for up in (True, False):
            if step == last and up != (h == 0):
                continue
            kv_copy(up, step, h).wait_recv()
            if step < last - 1 or (step == last - 1 and up == (h == 0)):
                start(kv_copy(up, step + 1, h))

    def use_up(step):
        arrived(lax.rem(z + N_Z - step, N_Z), z >= step)

    def use_down(step):
        arrived(lax.rem(z + step, N_Z), z + step >= N_Z)

    keys_from(kv_ref)
    own_values = lambda: kv_ref[ROWS : 2 * ROWS]
    attend_rows(x * steps, (x + 1) * steps, own_values, True)

    q_copy(0).wait_recv()
    start(q_copy(4))
    q_copy(3).wait_recv()
    start(q_copy(5))
    for d in range(N_X - 1):
        first_copy(d).wait_recv()
    column = first_in[0]
    for k in range(1, N_X):
        column = merge_states(column, first_in[k])
    column_out[...] = column
    for target in range(1, N_Z):

        @pl.when(target > z)
        def _(target=target):
            column_copy(target).start()

    take(1, 0)
    for number in (1, 2, 4, 5):
        q_copy(number).wait_recv()
    attend_rows((x + 1) * steps, N_X * steps, own_values, False)
    take(1, 1)
    take(2, 0)
    use_up(1)
    take(2, 1)
    use_down(1)

    def gather_column(k, state):
        column_arrival(k).wait_recv()
        return merge_states(state, column_in[k])

    state = lax.fori_loop(0, z, gather_column, jnp.zeros((STATE_ROWS, M_V), f32))
    for k in range(N_X):
        start_out[k] = state
        if k < N_X - 1:
            state = merge_states(state, first_in[k])
    for d in range(N_X - 1):
        start(start_copy(d))
    start_in[x] = start_out[x]
    take(3, 0)
    use_up(2)
    take(3, 1)
    use_down(2)

    for d in range(N_X - 1):
        start_copy(d).wait_recv()
    carried = jnp.concatenate([start_in[k, :CHUNK] for k in range(N_X)], axis=0)
    carried_normal = start_in[0, NORMAL_ROW : NORMAL_ROW + 1, :M_QK]
    carried_top = start_in[0, TOP_ROW : TOP_ROW + 1, :width]
    queries = mem_ref[:, :M_QK]
    from_start = sum(
        jnp.dot(queries, piece, preferred_element_type=f32) for piece in in_two(carried)
    )
    highest = jnp.maximum(carried_top, cell_top[...])
    across, within = jnp.exp(carried_top - highest), jnp.exp(cell_top[...] - highest)
    twice = lambda one: jnp.concatenate([one, one], axis=1)
    numerator = cell[...] * twice(within) + from_start * twice(across)
    denominator = cell_sum[...] * within + across * jnp.sum(
        queries.astype(f32) * carried_normal, axis=1, keepdims=True
    )
    floor = jnp.exp(-(as_columns(cumulative, width) + highest))
    made = numerator / twice(jnp.maximum(jnp.abs(denominator), floor))
    cell[...] = made
    squares = jnp.sum(made * made, axis=1, keepdims=True)
    square_out[0] = jnp.broadcast_to(squares, (ROWS, width)).T[:8]
    start(square_copy(0))

    use_up(3)
    square_copy(0).wait_recv()
    square_out[1] = square_out[0] + square_in[0]
    for number in range(1, N_Y):
        start(square_copy(number))
    use_down(3)
    take(4, 0)
    take(4, 1)

    opposite = lax.rem(z + last, N_Z)

    @pl.when(z >= last)
    def _():
        keys_from(kv_all.at[opposite])

    def finish(shard):
        @pl.when(z >= last)
        def _():
            attend_rows(
                shard * steps,
                (shard + 1) * steps,
                lambda: kv_all[opposite, ROWS : 2 * ROWS],
                False,
            )

        rows = pl.ds(pl.multiple_of(shard * ROWS, ROWS), ROWS)
        summed = jnp.sum(total[rows], axis=1, keepdims=True)
        seen = summed > 0.0
        summed = jnp.maximum(summed, 1.0)
        log_total = jnp.where(seen, top[rows] + jnp.log2(summed), FAR_BELOW)
        return accum[rows] / summed, log_total

    for d in (1, 0, 2):
        part, log_total = finish(peers[d])
        part_out[d] = part.astype(bf16)
        stat_out[d] = log_total.T[:8]
        if d == 1:
            start(far_copy(0, 0))
            start(far_copy(1, 0))
        else:
            start(part_copy(d))
        start(stat_copy(d))
    own, own_log = finish(x)

    squares = square_out[1]
    for number in range(1, N_Y):
        square_copy(number).wait_recv()
        squares = squares + square_in[number]
    inverse = lax.rsqrt(squares[:1] / (MEMORY_HEADS * M_V) + SMALL_CONSTANT)
    gated = cell[...] * twice(as_columns(inverse, width)) * gain_ref[pl.ds(pl.multiple_of(me_tp * M_V, M_V), M_V)].astype(f32).reshape(1, M_V)
    gated = gated * jax.nn.sigmoid(mem_ref[:, 2 * M_QK + M_V :].astype(f32))
    gated_ref[...] = gated.astype(bf16)
    for h in range(2):
        far_copy(h, 0).wait_recv()
        start(far_copy(h, 1))

    logs = []
    for d in range(N_X - 1):
        stat_copy(d).wait_recv()
        logs.append(as_columns(stat_in[d, 0:1, :], width))
    highest = own_log
    for one in logs:
        highest = jnp.maximum(highest, one)
    weight = jnp.exp2(own_log - highest)
    numerator = own * weight
    denominator = weight
    for d in (0, 2, 1):
        if d == 1:
            far_copy(0, 1).wait_recv()
            far_copy(1, 1).wait_recv()
        else:
            part_copy(d).wait_recv()
        weight = jnp.exp2(logs[d] - highest)
        numerator = numerator + part_in[d].astype(f32) * weight
        denominator = denominator + weight
    attended_ref[...] = (numerator / denominator).astype(bf16)
    def finish_columns():
        for target in range(1, N_Z):

            @pl.when(target > z)
            def _(target=target):
                column_copy(target).wait_send()

    return started, finish_columns


class TpGather:
    def __init__(self, full, sends, recvs):
        self.full, self.sends, self.recvs = full, sends, recvs
        self.y, self.c = lax.axis_index("y"), lax.axis_index("c")
        self.half = full.shape[1] // 2
        self.started = []

    def _copy(self, number, shift, part, target):
        slot = lax.rem(self.y + shift, N_Y) * N_C + self.c
        if part is None:
            ref = self.full.at[slot]
        else:
            ref = self.full.at[slot, pl.ds(part * self.half, self.half)]
        if target == "core":
            device = {"c": 1 - self.c}
        else:
            device = {"y": lax.rem(self.y + (1 if target == "up" else N_Y - 1), N_Y)}
        return pltpu.make_async_remote_copy(
            src_ref=ref,
            dst_ref=ref,
            send_sem=self.sends.at[number],
            recv_sem=self.recvs.at[number],
            device_id=device,
            device_id_type=MESH_ID,
        )

    def _start(self, *what):
        copy = self._copy(*what)
        copy.start()
        self.started.append(copy)

    def start(self):
        self._start(0, 0, 0, "up")
        self._start(3, 0, 1, "down")
        self._start(1, 0, 1, "up")
        self._start(2, 0, 0, "down")
        self._start(6, 0, None, "core")

    def relay(self):
        self._copy(0, 0, 0, "up").wait_recv()
        self._start(4, N_Y - 1, 0, "up")
        self._copy(3, 0, 1, "down").wait_recv()
        self._start(5, 1, 1, "down")
        self._copy(1, 0, 1, "up").wait_recv()
        self._start(7, N_Y - 1, None, "core")
        self._copy(2, 0, 0, "down").wait_recv()
        self._start(8, 1, None, "core")

    def near(self):
        for number, shift in ((6, 0), (7, N_Y - 1), (8, 1)):
            self._copy(number, shift, None, "core").wait_recv()

    def far(self):
        self._copy(4, 0, 0, "up").wait_recv()
        self._start(9, 2, 0, "core")
        self._copy(5, 0, 1, "down").wait_recv()
        self._start(10, 2, 1, "core")
        for part in range(2):
            self._copy(9 + part, 2, part, "core").wait_recv()

    def finish(self):
        for copy in self.started:
            copy.wait_send()


def project_phase(
    greeted,
    tokens_hbm,
    gain,
    query_gain,
    latent_gain,
    cosine,
    sine_part,
    shift_hbm,
    narrow_query,
    narrow_latent,
    narrow_rotary,
    narrow_ingate,
    narrow_forget,
    query_hbm,
    key_hbm,
    value_hbm,
    outgate_hbm,
    query_up_hbm,
    key_up_hbm,
    value_up_hbm,
    mem_ref,
    gate_ref,
    q_ref,
    kv_ref,
    rows_all,
    latents,
    small,
    ingate,
    forget,
    big,
    query_up,
    key_up,
    value_up,
    tokens,
    shift_row,
    pre_gates,
    up_query,
    up_latent,
    wide_query,
    wide_latent,
    load_sem,
    row_send,
    row_recv,
    lat_send,
    lat_recv,
):
    f32, bf16 = jnp.float32, jnp.bfloat16
    y, c = lax.axis_index("y"), lax.axis_index("c")
    mine = y * N_C + c
    width = 128
    sources = (
        (narrow_query, small.at[pl.ds(0, QUERY_PART)]),
        (narrow_latent, small.at[pl.ds(width, LATENT_PART)]),
        (narrow_rotary, small.at[pl.ds(width + LATENT_PART, ROTARY_CHANNELS)]),
        (narrow_ingate, ingate),
        (narrow_forget, forget),
        (query_up_hbm, query_up),
        (key_up_hbm, key_up),
        (value_up_hbm, value_up),
        (shift_hbm, shift_row),
    )
    loads = [
        pltpu.make_async_copy(source, target, load_sem.at[k])
        for k, (source, target) in enumerate(sources)
    ]
    at = 0
    for k, ref in enumerate((query_hbm, key_hbm, value_hbm, outgate_hbm)):
        columns = ref.shape[1]
        loads.append(
            pltpu.make_async_copy(ref, big.at[:, pl.ds(at, columns)], load_sem.at[9 + k])
        )
        at += columns
    arrival = pltpu.make_async_copy(tokens_hbm, tokens, load_sem.at[13])
    arrival.start()
    for load in loads:
        load.start()
    arrival.wait()
    wide = tokens[...].astype(f32)
    inverse = lax.rsqrt(jnp.mean(wide * wide, axis=1, keepdims=True) + SMALL_CONSTANT)
    rows_all[mine] = (wide * inverse * gain[...].astype(f32).reshape(1, -1)).astype(bf16)
    small[QUERY_PART:width] = jnp.zeros((width - QUERY_PART, small.shape[1]), bf16)

    greeted()
    gather = TpGather(rows_all, row_send, row_recv)
    gather.start()

    for load in loads:
        load.wait()
    up_query[...] = jnp.zeros(up_query.shape, bf16)
    query_rows = query_up[...].astype(f32).T.astype(bf16)
    for s in range(N_Y * N_C):
        up_query[s * width : s * width + QUERY_PART] = query_rows[
            s * QUERY_PART : (s + 1) * QUERY_PART
        ]
        part = slice(s * LATENT_PART, (s + 1) * LATENT_PART)
        for h in range(2):
            at = s * width + h * LATENT_PART
            up_latent[at : at + LATENT_PART, :width] = key_up[part]
            up_latent[at : at + LATENT_PART, width:] = value_up[part]

    lane = lax.broadcasted_iota(jnp.int32, (1, width), 1)
    row_id = lax.broadcasted_iota(jnp.int32, (width, width), 0)
    col_id = lax.broadcasted_iota(jnp.int32, (width, width), 1)
    channels = lax.rem(col_id, ROTARY_CHANNELS)
    halfway = ROTARY_CHANNELS // 2
    twin = (row_id == channels).astype(bf16)
    partner = lax.rem(channels + halfway, ROTARY_CHANNELS)
    sign = jnp.where(channels < halfway, -1.0, 1.0)

    def duplicated(values, offset):
        return jnp.dot(
            values, (row_id == channels + offset).astype(bf16), preferred_element_type=f32
        )

    def rotated(values, offset):
        swap = jnp.where(row_id == partner + offset, sign, 0.0).astype(bf16)
        turned = jnp.dot(values, swap, preferred_element_type=f32)
        return duplicated(values, offset) * cosine[...] + turned * sine_part[...]

    def chip_rows(chip):
        slots = [rows_all[chip * N_C + k] for k in range(N_C)]
        return jnp.concatenate(slots, axis=0)

    span = N_C * SHARE
    tile = 256

    def project_small(chip):
        rows = pl.ds(pl.multiple_of(chip * span, span), span)
        here = chip_rows(chip)
        made = lax.dot_general(here, small[...], CONTRACT_LAST, preferred_element_type=f32)
        for k, ref in enumerate((ingate, forget)):
            pre_gates[k, :, rows] = lax.dot_general(
                ref[...], here, CONTRACT_LAST, preferred_element_type=f32
            )
        rounded = made.astype(bf16)
        latents[mine, rows] = rounded[:, :width]
        wide_latent[rows, :width] = rounded[:, width:]

    def project_big(chip):
        rows = pl.ds(pl.multiple_of(chip * span, span), span)

        def one(t, carry):
            columns = pl.ds(pl.multiple_of(t * tile, tile), tile)
            made = jnp.dot(chip_rows(chip), big[:, columns], preferred_element_type=f32)
            mem_ref[rows, columns] = made.astype(bf16)
            return carry

        lax.fori_loop(0, big.shape[1] // tile, one, 0)

    gather.relay()
    gather.near()
    near = [y, lax.rem(y + N_Y - 1, N_Y), lax.rem(y + 1, N_Y)]
    for chip in near:
        project_small(chip)
    opposite = lax.rem(y + 2, N_Y)
    gather.far()
    project_small(opposite)

    second = wide_latent[:, :width]
    both = duplicated(second, 0)
    half = ROWS // 2
    packed = jnp.where(lane < LATENT_PART, both[:half], both[half:])
    latents[mine, ROWS:] = packed.astype(bf16)
    exchange = TpGather(latents, lat_send, lat_recv)
    exchange.start()
    for chip in near[:2]:
        project_big(chip)
    exchange.relay()
    for chip in (near[2], opposite):
        project_big(chip)
    heads = lax.broadcasted_iota(jnp.int32, (8, ROWS), 0) == mine
    in_pre, forget_pre = (
        jnp.sum(jnp.where(heads, pre_gates[k], 0.0), axis=0, keepdims=True) for k in range(2)
    )
    in_gate = SOFTCAP * jnp.tanh(in_pre / SOFTCAP)
    capped = SOFTCAP * jnp.tanh((forget_pre + shift_row[...]) / SOFTCAP)
    small_part = jnp.exp(-jnp.abs(capped))
    above_one = 1.0 + small_part
    grown = jnp.where(
        above_one == 1.0, small_part, jnp.log(above_one) * small_part / (above_one - 1.0)
    )
    log_forget = jnp.minimum(capped, 0.0) - grown
    earlier = lax.broadcasted_iota(jnp.int32, (ROWS, ROWS), 0) <= lax.broadcasted_iota(
        jnp.int32, (ROWS, ROWS), 1
    )
    cumulative = jnp.dot(
        jnp.broadcast_to(log_forget, (8, ROWS)),
        earlier.astype(f32),
        precision=PRECISE,
        preferred_element_type=f32,
    )
    top_rows = lax.broadcasted_iota(jnp.int32, (8, ROWS), 0) == 0
    gate_ref[...] = jnp.where(top_rows, in_gate - cumulative, cumulative)
    key_turned = rotated(second, LATENT_PART)
    kv_ref[2 * ROWS :] = jnp.where(
        lane < ROTARY_CHANNELS, key_turned[:half], key_turned[half:]
    ).astype(bf16)
    exchange.near()
    exchange.far()

    query_mask = (lane < QUERY_PART).astype(f32)
    squares = jnp.zeros((ROWS, width), f32)
    low_squares = jnp.zeros((half, width), f32)
    for s in range(N_Y * N_C):
        part = latents[s, :ROWS].astype(f32) * query_mask
        squares = squares + part * part
        part = latents[s, ROWS:].astype(f32)
        low_squares = low_squares + part * part
    query_scale = lax.rsqrt(
        jnp.sum(squares, axis=1, keepdims=True) / QUERY_LATENT + SMALL_CONSTANT
    )
    low = lane < LATENT_PART
    low_scale = lax.rsqrt(
        jnp.sum(jnp.where(low, low_squares, 0.0), axis=1, keepdims=True) / LATENT_WIDTH
        + SMALL_CONSTANT
    )
    high_scale = lax.rsqrt(
        jnp.sum(jnp.where(low, 0.0, low_squares), axis=1, keepdims=True) / LATENT_WIDTH
        + SMALL_CONSTANT
    )
    latent_scale = jnp.where(low, low_scale, high_scale)
    query_gains = jnp.broadcast_to(query_gain[...].reshape(1, -1), (8, QUERY_LATENT))
    latent_gains = jnp.broadcast_to(latent_gain[...].reshape(1, -1), (8, LATENT_WIDTH))

    def latent_gain_of(s):
        pair = latent_gains[:1, (s // 2) * width : (s // 2 + 1) * width]
        turned = pltpu.roll(latent_gains, LATENT_PART, 1)
        other = turned[:1, (s // 2) * width : (s // 2 + 1) * width]
        if s % 2:
            other = pltpu.roll(latent_gains, LATENT_WIDTH - LATENT_PART, 1)
            other = other[:1, (s // 2) * width : (s // 2 + 1) * width]
            return jnp.where(low, other, pair)
        return jnp.where(low, pair, other)

    def query_gain_of(s):
        turned = query_gains
        if s:
            turned = pltpu.roll(query_gains, QUERY_LATENT - s * QUERY_PART, 1)
        return turned[:1, :width]

    for s in range(N_Y * N_C):
        columns = slice(s * width, (s + 1) * width)
        part = latents[s, :ROWS].astype(f32) * query_mask
        wide_query[:, columns] = (part * query_scale * query_gain_of(s)).astype(bf16)
        part = latents[s, ROWS:].astype(f32)
        made = (part * latent_scale * latent_gain_of(s)).astype(bf16)
        wide_latent[:half, columns] = jnp.where(low, made, jnp.zeros_like(made))
        wide_latent[half:, columns] = jnp.where(low, jnp.zeros_like(made), made)
    made = jnp.dot(wide_latent[...], up_latent[...], preferred_element_type=f32).astype(bf16)
    kv_ref[:ROWS] = made[:, :width]
    kv_ref[ROWS : 2 * ROWS] = made[:, width:]
    made = jnp.dot(wide_query[...], up_query[...], preferred_element_type=f32).astype(bf16)
    q_ref[:, :width] = made[:, :width]
    turning = jnp.concatenate([made[:, width:], jnp.zeros((ROWS, ROTARY_CHANNELS), bf16)], axis=1)
    q_ref[:, width:] = rotated(turning, 0).astype(bf16)
    return gather.started + exchange.started


def output_phase(
    gated,
    attended,
    out_memory,
    out_attend,
    o_ref,
    to_core,
    from_core,
    sums,
    passing,
    from_below,
    from_above,
    relay_in,
    core_send,
    core_recv,
    relay_send,
    relay_recv,
    up_send,
    up_recv,
    down_send,
    down_recv,
):
    f32, bf16 = jnp.float32, jnp.bfloat16
    y, c = lax.axis_index("y"), lax.axis_index("c")
    above, below = lax.rem(y + 1, N_Y), lax.rem(y + N_Y - 1, N_Y)
    opposite = lax.rem(y + 2, N_Y)
    half = out_memory.shape[1] // 2
    tile = 512

    def remote(source, target, send, recv, device):
        return pltpu.make_async_remote_copy(
            src_ref=source,
            dst_ref=target,
            send_sem=send,
            recv_sem=recv,
            device_id=device,
            device_id_type=MESH_ID,
        )

    def rows_of(ref, core):
        picked = [ref[pl.ds(pl.multiple_of((k * N_C + core) * SHARE, SHARE), SHARE)] for k in range(N_Y)]
        return jnp.concatenate(picked, axis=0)

    def partial(core, h, store):
        memory_rows, attend_rows = rows_of(gated, core), rows_of(attended, core)
        for t in range(half // tile):
            columns = slice(h * half + t * tile, h * half + (t + 1) * tile)
            made = jnp.dot(memory_rows, out_memory[:, columns], preferred_element_type=f32)
            made = made + jnp.dot(attend_rows, out_attend[:, columns], preferred_element_type=f32)
            store(t * tile, made.astype(bf16).reshape(N_Y, SHARE, tile))

    def core_copy(h):
        return remote(
            to_core.at[h], from_core.at[h], core_send.at[h], core_recv.at[h], {"c": 1 - c}
        )

    def relay_copy(h):
        return remote(
            passing.at[h],
            relay_in.at[h],
            relay_send.at[h],
            relay_recv.at[h],
            {"y": above if h == 0 else below},
        )

    def up_copy(h):
        return remote(
            passing.at[2 + h], from_below.at[h], up_send.at[h], up_recv.at[h], {"y": above}
        )

    def down_copy(h):
        return remote(
            passing.at[4 + h], from_above.at[h], down_send.at[h], down_recv.at[h], {"y": below}
        )

    started = []

    def start(copy):
        copy.start()
        started.append(copy)

    for h in range(2):

        def keep(at, block, h=h):
            to_core[h, :, :, at : at + tile] = block

        partial(1 - c, h, keep)
        start(core_copy(h))
    for h in range(2):

        def keep(at, block, h=h):
            sums[h, :, :, at : at + tile] = block.astype(f32)

        partial(c, h, keep)
    for h in range(2):
        core_copy(h).wait_recv()
        sums[h] = sums[h] + from_core[h].astype(f32)
        passing[h] = sums[h, opposite].astype(bf16)
        start(relay_copy(h))
        if h == 0:
            passing[4] = sums[0, below].astype(bf16)
            start(down_copy(0))
        else:
            passing[3] = sums[1, above].astype(bf16)
            start(up_copy(1))
    relay_copy(0).wait_recv()
    passing[2] = (sums[0, above] + relay_in[0].astype(f32)).astype(bf16)
    start(up_copy(0))
    relay_copy(1).wait_recv()
    passing[5] = (sums[1, below] + relay_in[1].astype(f32)).astype(bf16)
    start(down_copy(1))
    for h in (1, 0):
        up_copy(h).wait_recv()
        down_copy(h).wait_recv()
        made = sums[h, y] + from_below[h].astype(f32) + from_above[h].astype(f32)
        o_ref[:, h * half : (h + 1) * half] = made.astype(bf16)
    return started


INPUTS = (
    "tokens_hbm",
    "shift_hbm",
    "narrow_query",
    "narrow_latent",
    "narrow_rotary",
    "narrow_ingate",
    "narrow_forget",
    "query_hbm",
    "key_hbm",
    "value_hbm",
    "outgate_hbm",
    "query_up_hbm",
    "key_up_hbm",
    "value_up_hbm",
    "out_memory_hbm",
    "out_attend_hbm",
    "input_gain",
    "query_gain",
    "latent_gain",
    "mem_gain",
    "cosine",
    "sine_part",
)

HBM_INPUTS = 16


def scratch(depth, mem_width):
    f32, bf16 = jnp.float32, jnp.bfloat16
    dma = pltpu.SemaphoreType.DMA
    return dict(
        rows_all=pltpu.VMEM((N_Y * N_C, SHARE, depth), bf16),
        latents=pltpu.VMEM((N_Y * N_C, ROWS * 3 // 2, 128), bf16),
        small=pltpu.VMEM((256, depth), bf16),
        ingate=pltpu.VMEM((8, depth), bf16),
        forget=pltpu.VMEM((8, depth), bf16),
        big=pltpu.VMEM((depth, mem_width), bf16),
        query_up=pltpu.VMEM((PLAIN_CHANNELS + ROTARY_CHANNELS, QUERY_LATENT), bf16),
        key_up=pltpu.VMEM((LATENT_WIDTH, PLAIN_CHANNELS), bf16),
        value_up=pltpu.VMEM((LATENT_WIDTH, VALUE_CHANNELS), bf16),
        tokens=pltpu.VMEM((SHARE, depth), bf16),
        shift_row=pltpu.VMEM((1, ROWS), f32),
        pre_gates=pltpu.VMEM((2, 8, ROWS), f32),
        up_query=pltpu.VMEM((1024, PLAIN_CHANNELS + ROTARY_CHANNELS), bf16),
        up_latent=pltpu.VMEM((1024, 256), bf16),
        wide_query=pltpu.VMEM((ROWS, 1024), bf16),
        wide_latent=pltpu.VMEM((ROWS, 1024), bf16),
        load_sem=dma((16,)),
        row_send=dma((11,)),
        row_recv=dma((11,)),
        lat_send=dma((11,)),
        lat_recv=dma((11,)),
        mem_ref=pltpu.VMEM((ROWS, mem_width), bf16),
        gate_ref=pltpu.VMEM((8, ROWS), f32),
        q_ref=pltpu.VMEM((ROWS, 256), bf16),
        kv_ref=pltpu.VMEM((ROWS * 5 // 2, 128), bf16),
        attended_ref=pltpu.VMEM((ROWS, VALUE_CHANNELS), bf16),
        gated_ref=pltpu.VMEM((ROWS, M_V), bf16),
        q_all=pltpu.VMEM((N_X, ROWS, 256), bf16),
        kv_all=pltpu.VMEM((N_Z, ROWS * 5 // 2, 128), bf16),
        k_cat=pltpu.VMEM((ROWS, 256), bf16),
        top=pltpu.VMEM((N_X * ROWS, 128), f32),
        total=pltpu.VMEM((N_X * ROWS, 128), f32),
        accum=pltpu.VMEM((N_X * ROWS, VALUE_CHANNELS), f32),
        part_out=pltpu.VMEM((N_X - 1, ROWS, VALUE_CHANNELS), bf16),
        stat_out=pltpu.VMEM((N_X - 1, 8, ROWS), f32),
        part_in=pltpu.VMEM((N_X - 1, ROWS, VALUE_CHANNELS), bf16),
        stat_in=pltpu.VMEM((N_X - 1, 8, ROWS), f32),
        cell=pltpu.VMEM((ROWS, M_V), f32),
        cell_sum=pltpu.VMEM((ROWS, 128), f32),
        cell_top=pltpu.VMEM((ROWS, 128), f32),
        first_out=pltpu.VMEM((N_X, STATE_ROWS, M_V), f32),
        first_in=pltpu.VMEM((N_X, STATE_ROWS, M_V), f32),
        column_out=pltpu.VMEM((STATE_ROWS, M_V), f32),
        column_in=pltpu.VMEM((N_Z, STATE_ROWS, M_V), f32),
        start_out=pltpu.VMEM((N_X, STATE_ROWS, M_V), f32),
        start_in=pltpu.VMEM((N_X, STATE_ROWS, M_V), f32),
        square_out=pltpu.VMEM((2, 8, ROWS), f32),
        square_in=pltpu.VMEM((N_Y, 8, ROWS), f32),
        passed=pltpu.VMEM((2, ROWS // 2, VALUE_CHANNELS), bf16),
        q_send=dma((6,)),
        q_recv=dma((6,)),
        up_send=dma((N_Z // 2, 2)),
        up_recv=dma((N_Z // 2, 2)),
        down_send=dma((N_Z // 2, 2)),
        down_recv=dma((N_Z // 2, 2)),
        part_send=dma((N_X - 1,)),
        part_recv=dma((N_X - 1,)),
        stat_send=dma((N_X - 1,)),
        stat_recv=dma((N_X - 1,)),
        first_send=dma((N_X - 1,)),
        first_recv=dma((N_X - 1,)),
        column_send=dma((N_Z,)),
        column_recv=dma((N_Z,)),
        start_send=dma((N_X - 1,)),
        start_recv=dma((N_X - 1,)),
        square_send=dma((N_Y,)),
        square_recv=dma((N_Y,)),
        passed_send=dma((2, 2)),
        passed_recv=dma((2, 2)),
        out_memory=pltpu.VMEM((M_V, depth), bf16),
        out_attend=pltpu.VMEM((VALUE_CHANNELS, depth), bf16),
        to_core=pltpu.VMEM((2, N_Y, SHARE, depth // 2), bf16),
        from_core=pltpu.VMEM((2, N_Y, SHARE, depth // 2), bf16),
        sums=pltpu.VMEM((2, N_Y, SHARE, depth // 2), f32),
        passing=pltpu.VMEM((6, SHARE, depth // 2), bf16),
        from_below=pltpu.VMEM((2, SHARE, depth // 2), bf16),
        from_above=pltpu.VMEM((2, SHARE, depth // 2), bf16),
        relay_in=pltpu.VMEM((2, SHARE, depth // 2), bf16),
        core_send=dma((2,)),
        core_recv=dma((2,)),
        relay_send=dma((2,)),
        relay_recv=dma((2,)),
        out_up_send=dma((2,)),
        out_up_recv=dma((2,)),
        out_down_send=dma((2,)),
        out_down_recv=dma((2,)),
    )


def layer_kernel(names, *refs):
    at = dict(zip(names, refs))
    y, c = lax.axis_index("y"), lax.axis_index("c")
    z, x = lax.axis_index("z"), lax.axis_index("x")
    barrier = pltpu.get_barrier_semaphore()
    devices = [{"c": 1 - c}]
    devices += [{"y": lax.rem(y + d, N_Y)} for d in range(1, N_Y)]
    devices += [{"x": lax.rem(x + d, N_X)} for d in range(1, N_X)]
    devices += [{"z": lax.rem(z + d, N_Z)} for d in range(1, N_Z)]
    for device in devices:
        pl.semaphore_signal(barrier, inc=1, device_id=device, device_id_type=MESH_ID)
    loads = [
        pltpu.make_async_copy(at[name + "_hbm"], at[name], at["load_sem"].at[14 + k])
        for k, name in enumerate(("out_memory", "out_attend"))
    ]
    started = project_phase(
        lambda: pl.semaphore_wait(barrier, len(devices)),
        *(at[name] for name in PROJECT_REFS),
    )
    for load in loads:
        load.start()
    more, finish_columns = attend_phase(*(at[name] for name in ATTEND_REFS))
    started += more
    for load in loads:
        load.wait()
    started += output_phase(*(at[name] for name in OUTPUT_REFS))
    for copy in started:
        copy.wait_send()
    finish_columns()


PROJECT_REFS = (
    "tokens_hbm",
    "input_gain",
    "query_gain",
    "latent_gain",
    "cosine",
    "sine_part",
    "shift_hbm",
    "narrow_query",
    "narrow_latent",
    "narrow_rotary",
    "narrow_ingate",
    "narrow_forget",
    "query_hbm",
    "key_hbm",
    "value_hbm",
    "outgate_hbm",
    "query_up_hbm",
    "key_up_hbm",
    "value_up_hbm",
    "mem_ref",
    "gate_ref",
    "q_ref",
    "kv_ref",
    "rows_all",
    "latents",
    "small",
    "ingate",
    "forget",
    "big",
    "query_up",
    "key_up",
    "value_up",
    "tokens",
    "shift_row",
    "pre_gates",
    "up_query",
    "up_latent",
    "wide_query",
    "wide_latent",
    "load_sem",
    "row_send",
    "row_recv",
    "lat_send",
    "lat_recv",
)
ATTEND_REFS = (
    "q_ref",
    "kv_ref",
    "mem_ref",
    "gate_ref",
    "mem_gain",
    "attended_ref",
    "gated_ref",
    "q_all",
    "kv_all",
    "k_cat",
    "top",
    "total",
    "accum",
    "part_out",
    "stat_out",
    "part_in",
    "stat_in",
    "cell",
    "cell_sum",
    "cell_top",
    "first_out",
    "first_in",
    "column_out",
    "column_in",
    "start_out",
    "start_in",
    "square_out",
    "square_in",
    "passed",
    "q_send",
    "q_recv",
    "up_send",
    "up_recv",
    "down_send",
    "down_recv",
    "part_send",
    "part_recv",
    "stat_send",
    "stat_recv",
    "first_send",
    "first_recv",
    "column_send",
    "column_recv",
    "start_send",
    "start_recv",
    "square_send",
    "square_recv",
    "passed_send",
    "passed_recv",
)
OUTPUT_REFS = (
    "gated_ref",
    "attended_ref",
    "out_memory",
    "out_attend",
    "o_ref",
    "to_core",
    "from_core",
    "sums",
    "passing",
    "from_below",
    "from_above",
    "relay_in",
    "core_send",
    "core_recv",
    "relay_send",
    "relay_recv",
    "out_up_send",
    "out_up_recv",
    "out_down_send",
    "out_down_recv",
)


def layer(*inputs):
    depth = inputs[0].shape[1]
    mem_width = sum(one.shape[1] for one in inputs[7:11])
    made = scratch(depth, mem_width)
    names = (*INPUTS, "o_ref", *made)
    vmem = pl.BlockSpec(memory_space=pltpu.VMEM)
    hbm = pl.BlockSpec(memory_space=pltpu.HBM)
    return pl.pallas_call(
        functools.partial(layer_kernel, names),
        out_shape=jax.ShapeDtypeStruct((SHARE, depth), jnp.bfloat16),
        in_specs=[hbm] * HBM_INPUTS + [vmem] * (len(inputs) - HBM_INPUTS),
        out_specs=vmem,
        scratch_shapes=list(made.values()),
        compiler_params=pltpu.CompilerParams(
            collective_id=1, has_side_effects=True, vmem_limit_bytes=67_000_000
        ),
        cost_estimate=pl.CostEstimate(
            flops=8 * 10**9, bytes_accessed=2 * 10**7, transcendentals=4 * 10**6
        ),
        name="layer",
    )(*inputs)


def per_device(
    tokens,
    input_gain,
    weight_query,
    weight_key,
    weight_value,
    weight_outgate,
    weight_ingate,
    weight_forget,
    forget_shift,
    mem_gain,
    query_down_weight,
    latent_down_weight,
    down_rotary,
    query_gain,
    latent_gain,
    query_up_weight,
    key_up_weight,
    value_up_weight,
    out_memory,
    out_attend,
):
    length = forget_shift.shape[0]
    positions = lax.axis_index(SP) * length + jnp.arange(length, dtype=jnp.int32)
    halfway = ROTARY_CHANNELS // 2
    inverse = jnp.power(ROTARY_BASE, -jnp.arange(halfway, dtype=jnp.float32) / halfway)
    angles = positions.astype(jnp.float32)[:, None] * inverse
    cosine, sine_part = (jnp.tile(made, (1, 4)) for made in (jnp.cos(angles), jnp.sin(angles)))
    return layer(
        tokens,
        forget_shift.T,
        query_down_weight.T,
        latent_down_weight.T,
        down_rotary.T,
        weight_ingate.T,
        weight_forget.T,
        weight_query,
        weight_key,
        weight_value,
        weight_outgate,
        query_up_weight.T,
        key_up_weight,
        value_up_weight,
        out_memory,
        out_attend,
        input_gain,
        query_gain,
        latent_gain,
        mem_gain,
        cosine,
        sine_part,
    )


def solution(mesh):
    torus = Mesh(mesh.devices.reshape(N_Z, N_X, 4, 2), SP_TP)
    in_specs = (
        P(SP_TP, None),
        P(),
        P(None, TP),
        P(None, TP),
        P(None, TP),
        P(None, TP),
        P(),
        P(),
        P(SP, TP),
        P(),
        P(None, TP),
        P(None, TP),
        P(),
        P(),
        P(),
        P(None, TP),
        P(None, TP),
        P(None, TP),
        P(TP, None),
        P(TP, None),
    )
    out_specs = P(SP_TP, None)
    return jax.shard_map(
        per_device, mesh=torus, in_specs=in_specs, out_specs=out_specs, check_vma=False
    )
```

```python
import functools

import jax
import jax.numpy as jnp
from jax import lax
from jax.experimental import pallas as pl
from jax.experimental.pallas import tpu as pltpu
from jax.sharding import Mesh
from jax.sharding import PartitionSpec as P

MEMORY_HEADS = 8
M_QK = 128
M_V = 256
PLAIN_CHANNELS = 128
ROTARY_CHANNELS = 64
VALUE_CHANNELS = 128
SP = ("z", "x")
TP = ("y", "c")
SP_TP = ("z", "x", "y", "c")


SMALL_CONSTANT = 1e-06
SOFTCAP = 15.0
ROTARY_BASE = 10000.0
PRECISE = lax.Precision.HIGHEST
FAR_BELOW = -1e30

N_Y = 4
N_C = 2
SHARE = 64
QUERY_LATENT = 768
LATENT_WIDTH = 512
QUERY_PART = QUERY_LATENT // (N_Y * N_C)
LATENT_PART = LATENT_WIDTH // (N_Y * N_C)
LOG2E = 1.4426950408889634
N_Z = 8
N_X = 4
ROWS = 512
MESH_ID = pl.DeviceIdType.MESH
CONTRACT_LAST = (((1,), (1,)), ((), ()))
CHUNK = M_QK // N_X
TALL = 512
GROUP = 1
STATE_ROWS = CHUNK + 8
NORMAL_ROW, TOP_ROW, DECAY_ROW = CHUNK, CHUNK + 1, CHUNK + 2


def merge_states(early, late):
    moved = early[TOP_ROW : TOP_ROW + 1] + late[DECAY_ROW : DECAY_ROW + 1]
    late_top = late[TOP_ROW : TOP_ROW + 1]
    joined = jnp.maximum(moved, late_top)
    both = early * jnp.exp(moved - joined) + late * jnp.exp(late_top - joined)
    row = lax.broadcasted_iota(jnp.int32, both.shape, 0)
    decay = early[DECAY_ROW : DECAY_ROW + 1] + late[DECAY_ROW : DECAY_ROW + 1]
    return jnp.where(row == TOP_ROW, joined, jnp.where(row == DECAY_ROW, decay, both))


def in_two(values):
    high = values.astype(jnp.bfloat16)
    return high, (values - high.astype(jnp.float32)).astype(jnp.bfloat16)


def as_columns(row, width):
    return jnp.broadcast_to(row, (width, row.shape[1])).T


def attend_phase(
    q_ref,
    kv_ref,
    mem_ref,
    gate_ref,
    gain_ref,
    attended_ref,
    gated_ref,
    q_all,
    kv_all,
    k_cat,
    top,
    total,
    accum,
    part_out,
    stat_out,
    part_in,
    stat_in,
    cell,
    cell_sum,
    cell_top,
    first_out,
    first_in,
    column_out,
    column_in,
    start_out,
    start_in,
    square_out,
    square_in,
    passed,
    q_send,
    q_recv,
    up_send,
    up_recv,
    down_send,
    down_recv,
    part_send,
    part_recv,
    stat_send,
    stat_recv,
    first_send,
    first_recv,
    column_send,
    column_recv,
    start_send,
    start_recv,
    square_send,
    square_recv,
    passed_send,
    passed_recv,
):
    f32, bf16 = jnp.float32, jnp.bfloat16
    z, x = lax.axis_index("z"), lax.axis_index("x")
    y, c = lax.axis_index("y"), lax.axis_index("c")
    above, below = lax.rem(z + 1, N_Z), lax.rem(z + N_Z - 1, N_Z)
    peers = [lax.rem(x + d, N_X) for d in range(1, N_X)]
    right, left = peers[0], peers[-1]
    rows_y = [lax.rem(y + d, N_Y) for d in range(1, N_Y)]
    me_tp = y * N_C + c
    half = kv_ref.shape[0] // 2
    width = PLAIN_CHANNELS

    def remote(source, target, send, recv, device):
        return pltpu.make_async_remote_copy(
            src_ref=source,
            dst_ref=target,
            send_sem=send,
            recv_sem=recv,
            device_id=device,
            device_id_type=MESH_ID,
        )

    def kv_copy(up, step, h):
        shift = (N_Z - step + 1) if up else (step - 1)
        owner = lax.rem(z + shift, N_Z)
        rows = pl.ds(h * half, half)
        source = kv_ref.at[rows] if step == 1 else kv_all.at[owner, rows]
        send, recv = (up_send, up_recv) if up else (down_send, down_recv)
        return remote(
            source,
            kv_all.at[owner, rows],
            send.at[step - 1, h],
            recv.at[step - 1, h],
            {"z": above if up else below},
        )

    q_half = ROWS // 2

    def q_copy(number):
        shift, part, to_right = (
            (0, 0, True),
            (0, 1, True),
            (0, 0, False),
            (0, 1, False),
            (N_X - 1, 0, True),
            (1, 1, False),
        )[number]
        owner = lax.rem(x + shift, N_X)
        rows = pl.ds(part * q_half, q_half)
        source = q_ref.at[rows] if shift == 0 else q_all.at[owner, rows]
        return remote(
            source,
            q_all.at[owner, rows],
            q_send.at[number],
            q_recv.at[number],
            {"x": right if to_right else left},
        )

    def part_copy(d):
        return remote(
            part_out.at[d], part_in.at[d], part_send.at[d], part_recv.at[d], {"x": peers[d]}
        )

    def far_copy(h, hop):
        rows = pl.ds(h * q_half, q_half)
        return remote(
            part_out.at[1, rows] if hop == 0 else passed.at[h],
            passed.at[h] if hop == 0 else part_in.at[1, rows],
            passed_send.at[hop, h],
            passed_recv.at[hop, h],
            {"x": right if h == 0 else left},
        )

    def stat_copy(d):
        return remote(
            stat_out.at[d], stat_in.at[d], stat_send.at[d], stat_recv.at[d], {"x": peers[d]}
        )

    def first_copy(d):
        return remote(
            first_out.at[peers[d]],
            first_in.at[x],
            first_send.at[d],
            first_recv.at[d],
            {"x": peers[d]},
        )

    def column_copy(target):
        return remote(
            column_out,
            column_in.at[z],
            column_send.at[target],
            column_recv.at[z],
            {"z": target},
        )

    def column_arrival(source):
        return remote(
            column_out,
            column_in.at[source],
            column_send.at[source],
            column_recv.at[source],
            {"z": source},
        )

    def start_copy(d):
        return remote(
            start_out.at[peers[d]],
            start_in.at[x],
            start_send.at[d],
            start_recv.at[d],
            {"x": peers[d]},
        )

    def square_copy(number):
        device = {"c": 1 - c} if number == 0 else {"y": rows_y[number - 1]}
        return remote(
            square_out.at[min(number, 1)],
            square_in.at[number],
            square_send.at[number],
            square_recv.at[number],
            device,
        )

    started = []

    def start(copy):
        copy.start()
        started.append(copy)

    relative, cumulative = gate_ref[0:1], gate_ref[1:2]
    key_scale = M_QK ** (-0.5)
    tall = 256
    for t in range(ROWS // tall):
        rows, seen = slice(t * tall, (t + 1) * tall), (t + 1) * tall
        row = lax.broadcasted_iota(jnp.int32, (tall, seen), 0) + t * tall
        col = lax.broadcasted_iota(jnp.int32, (tall, seen), 1)
        logs = jnp.where(col <= row, relative[:, :seen], -jnp.inf)
        highest = jnp.max(logs, axis=1, keepdims=True)
        affinity = lax.dot_general(
            mem_ref[rows, :M_QK],
            mem_ref[:seen, M_QK : 2 * M_QK],
            CONTRACT_LAST,
            preferred_element_type=f32,
        )
        affinity = affinity * (jnp.exp(logs - highest) * key_scale)
        values = mem_ref[:seen, 2 * M_QK : 2 * M_QK + M_V]
        cell[rows] = sum(
            jnp.dot(piece, values, preferred_element_type=f32) for piece in in_two(affinity)
        )
        cell_sum[rows] = jnp.broadcast_to(
            jnp.sum(affinity, axis=1, keepdims=True), (tall, width)
        )
        cell_top[rows] = jnp.broadcast_to(highest, (tall, width))
    ends_at = jnp.max(relative, axis=1, keepdims=True)
    weights = jnp.exp(relative - ends_at) * key_scale
    wide_key = mem_ref[:, M_QK : 2 * M_QK].astype(f32)
    normal = jnp.sum(as_columns(weights, width) * wide_key, axis=0, keepdims=True)
    values = mem_ref[:, 2 * M_QK : 2 * M_QK + M_V]
    matrix = sum(
        jnp.dot(piece, values, preferred_element_type=f32)
        for piece in in_two(wide_key.T * weights)
    )
    decay = cumulative[:, ROWS - 1 : ROWS]
    row = lax.broadcasted_iota(jnp.int32, (8, M_V), 0)
    lines = jnp.concatenate([normal, jnp.zeros_like(normal)], axis=1)
    notes = jnp.where(
        row == 0, lines, jnp.where(row == 1, ends_at + decay, jnp.where(row == 2, decay, 0.0))
    )
    for k in range(N_X):
        first_out[k, :CHUNK] = matrix[k * CHUNK : (k + 1) * CHUNK]
        first_out[k, CHUNK:] = notes
    for d in range(N_X - 1):
        start(first_copy(d))
    first_in[x] = first_out[x]

    yield

    for d in range(N_X - 1):
        first_copy(d).wait_recv()
    column = first_in[0]
    for k in range(1, N_X):
        column = merge_states(column, first_in[k])
    column_out[...] = column
    for target in range(1, N_Z):

        @pl.when(target > z)
        def _(target=target):
            column_copy(target).start()

    yield

    for h in range(2):
        for up in (True, False):
            start(kv_copy(up, 1, h))
    top[...] = jnp.full(top.shape, FAR_BELOW, f32)
    total[...] = jnp.zeros(total.shape, f32)
    for number in (0, 3, 1, 2):
        start(q_copy(number))
    accum[...] = jnp.zeros(accum.shape, f32)
    q_all[x] = q_ref[...]

    lane = lax.broadcasted_iota(jnp.int32, (ROWS // 2, width), 1)
    low = (lane < ROTARY_CHANNELS).astype(bf16)
    high = (lane >= ROTARY_CHANNELS).astype(bf16)
    scale = LOG2E * (PLAIN_CHANNELS + ROTARY_CHANNELS) ** (-0.5)

    def keys_from(ref):
        k_cat[:, :width] = ref[:ROWS]
        packed = ref[2 * ROWS :]
        k_cat[: ROWS // 2, width:] = packed * low
        k_cat[ROWS // 2 :, width:] = packed * high

    def attend_tile(t, keys, values, masked):
        shard = t // (ROWS // TALL)
        rows = pl.ds(pl.multiple_of(t * TALL, TALL), TALL)
        inner = pl.ds(pl.multiple_of((t % (ROWS // TALL)) * TALL, TALL), TALL)
        scores = lax.dot_general(
            q_all[shard, inner], keys, CONTRACT_LAST, preferred_element_type=f32
        )
        scores = scores * scale
        if masked:
            row = lax.broadcasted_iota(jnp.int32, scores.shape, 0) + t * TALL
            col = lax.broadcasted_iota(jnp.int32, scores.shape, 1) + x * ROWS
            scores = jnp.where(col <= row, scores, -jnp.inf)
        old = top[rows]
        new = jnp.maximum(old, jnp.max(scores, axis=1, keepdims=True))
        probs = jnp.exp2(scores - jnp.concatenate([new] * (ROWS // width), axis=1))
        shrink = jnp.exp2(old - new)
        added = sum(probs[:, k : k + width] for k in range(0, ROWS, width))
        total[rows] = total[rows] * shrink + added
        accum[rows] = accum[rows] * shrink + jnp.dot(
            probs.astype(bf16), values, preferred_element_type=f32
        )
        top[rows] = new

    def attend_rows(first, last, values, masked):
        def one(g, carry):
            for u in range(GROUP):
                attend_tile(g * GROUP + u, k_cat[...], values(), masked)
            return carry

        lax.fori_loop(first, last, one, 0)

    last = N_Z // 2
    steps = ROWS // (TALL * GROUP)

    def arrived(owner, useful):
        @pl.when(useful)
        def _():
            keys_from(kv_all.at[owner])
            attend_rows(0, N_X * steps, lambda: kv_all[owner, ROWS : 2 * ROWS], False)

    def take(step, h):
        for up in (True, False):
            if step == last and up != (h == 0):
                continue
            kv_copy(up, step, h).wait_recv()
            if step < last - 1 or (step == last - 1 and up == (h == 0)):
                start(kv_copy(up, step + 1, h))

    def use_up(step):
        arrived(lax.rem(z + N_Z - step, N_Z), z >= step)

    def use_down(step):
        arrived(lax.rem(z + step, N_Z), z + step >= N_Z)

    keys_from(kv_ref)
    own_values = lambda: kv_ref[ROWS : 2 * ROWS]
    attend_rows(x * steps, (x + 1) * steps, own_values, True)

    q_copy(0).wait_recv()
    start(q_copy(4))
    q_copy(3).wait_recv()
    start(q_copy(5))

    def gather_column(k, state):
        column_arrival(k).wait_recv()
        return merge_states(state, column_in[k])

    state = lax.fori_loop(0, z, gather_column, jnp.zeros((STATE_ROWS, M_V), f32))
    for k in range(N_X):
        start_out[k] = state
        if k < N_X - 1:
            state = merge_states(state, first_in[k])
    for d in range(N_X - 1):
        start(start_copy(d))
    start_in[x] = start_out[x]
    take(1, 0)
    for number in (1, 2, 4, 5):
        q_copy(number).wait_recv()
    attend_rows((x + 1) * steps, N_X * steps, own_values, False)
    take(1, 1)
    take(2, 0)
    use_up(1)
    take(2, 1)
    use_down(1)

    for d in range(N_X - 1):
        start_copy(d).wait_recv()
    carried = jnp.concatenate([start_in[k, :CHUNK] for k in range(N_X)], axis=0)
    carried_normal = start_in[0, NORMAL_ROW : NORMAL_ROW + 1, :M_QK]
    carried_top = start_in[0, TOP_ROW : TOP_ROW + 1, :width]
    queries = mem_ref[:, :M_QK]
    from_start = sum(
        jnp.dot(queries, piece, preferred_element_type=f32) for piece in in_two(carried)
    )
    highest = jnp.maximum(carried_top, cell_top[...])
    across, within = jnp.exp(carried_top - highest), jnp.exp(cell_top[...] - highest)
    twice = lambda one: jnp.concatenate([one, one], axis=1)
    numerator = cell[...] * twice(within) + from_start * twice(across)
    denominator = cell_sum[...] * within + across * jnp.sum(
        queries.astype(f32) * carried_normal, axis=1, keepdims=True
    )
    floor = jnp.exp(-(as_columns(cumulative, width) + highest))
    made = numerator / twice(jnp.maximum(jnp.abs(denominator), floor))
    cell[...] = made
    squares = jnp.sum(made * made, axis=1, keepdims=True)
    square_out[0] = jnp.broadcast_to(squares, (ROWS, width)).T[:8]
    start(square_copy(0))

    take(3, 0)
    use_up(2)
    square_copy(0).wait_recv()
    square_out[1] = square_out[0] + square_in[0]
    for number in range(1, N_Y):
        start(square_copy(number))
    take(3, 1)
    use_down(2)
    use_up(3)
    use_down(3)

    squares = square_out[1]
    for number in range(1, N_Y):
        square_copy(number).wait_recv()
        squares = squares + square_in[number]
    inverse = lax.rsqrt(squares[:1] / (MEMORY_HEADS * M_V) + SMALL_CONSTANT)
    gated = cell[...] * twice(as_columns(inverse, width)) * gain_ref[pl.ds(pl.multiple_of(me_tp * M_V, M_V), M_V)].astype(f32).reshape(1, M_V)
    gated = gated * jax.nn.sigmoid(mem_ref[:, 2 * M_QK + M_V :].astype(f32))
    gated_ref[...] = gated.astype(bf16)
    take(4, 0)
    take(4, 1)

    opposite = lax.rem(z + last, N_Z)

    @pl.when(z >= last)
    def _():
        keys_from(kv_all.at[opposite])

    def finish(shard):
        @pl.when(z >= last)
        def _():
            attend_rows(
                shard * steps,
                (shard + 1) * steps,
                lambda: kv_all[opposite, ROWS : 2 * ROWS],
                False,
            )

        rows = pl.ds(pl.multiple_of(shard * ROWS, ROWS), ROWS)
        summed = jnp.sum(total[rows], axis=1, keepdims=True)
        seen = summed > 0.0
        summed = jnp.maximum(summed, 1.0)
        log_total = jnp.where(seen, top[rows] + jnp.log2(summed), FAR_BELOW)
        return accum[rows] / summed, log_total

    for d in (1, 0, 2):
        part, log_total = finish(peers[d])
        part_out[d] = part.astype(bf16)
        stat_out[d] = log_total.T[:8]
        if d == 1:
            start(far_copy(0, 0))
            start(far_copy(1, 0))
        else:
            start(part_copy(d))
        start(stat_copy(d))
    own, own_log = finish(x)

    for h in range(2):
        far_copy(h, 0).wait_recv()
        start(far_copy(h, 1))

    logs = []
    for d in range(N_X - 1):
        stat_copy(d).wait_recv()
        logs.append(as_columns(stat_in[d, 0:1, :], width))
    highest = own_log
    for one in logs:
        highest = jnp.maximum(highest, one)
    weight = jnp.exp2(own_log - highest)
    numerator = own * weight
    denominator = weight
    for d in (0, 2, 1):
        if d == 1:
            far_copy(0, 1).wait_recv()
            far_copy(1, 1).wait_recv()
        else:
            part_copy(d).wait_recv()
        weight = jnp.exp2(logs[d] - highest)
        numerator = numerator + part_in[d].astype(f32) * weight
        denominator = denominator + weight
    attended_ref[...] = (numerator / denominator).astype(bf16)
    def finish_columns():
        for target in range(1, N_Z):

            @pl.when(target > z)
            def _(target=target):
                column_copy(target).wait_send()

    yield started, finish_columns


class TpGather:
    def __init__(self, full, sends, recvs):
        self.full, self.sends, self.recvs = full, sends, recvs
        self.y, self.c = lax.axis_index("y"), lax.axis_index("c")
        self.half = full.shape[1] // 2
        self.started = []

    def _copy(self, number, shift, part, target):
        slot = lax.rem(self.y + shift, N_Y) * N_C + self.c
        if part is None:
            ref = self.full.at[slot]
        else:
            ref = self.full.at[slot, pl.ds(part * self.half, self.half)]
        if target == "core":
            device = {"c": 1 - self.c}
        else:
            device = {"y": lax.rem(self.y + (1 if target == "up" else N_Y - 1), N_Y)}
        return pltpu.make_async_remote_copy(
            src_ref=ref,
            dst_ref=ref,
            send_sem=self.sends.at[number],
            recv_sem=self.recvs.at[number],
            device_id=device,
            device_id_type=MESH_ID,
        )

    def _start(self, *what):
        copy = self._copy(*what)
        copy.start()
        self.started.append(copy)

    def start(self):
        self._start(0, 0, 0, "up")
        self._start(3, 0, 1, "down")
        self._start(1, 0, 1, "up")
        self._start(2, 0, 0, "down")
        self._start(6, 0, None, "core")

    def relay(self):
        self._copy(0, 0, 0, "up").wait_recv()
        self._start(4, N_Y - 1, 0, "up")
        self._copy(3, 0, 1, "down").wait_recv()
        self._start(5, 1, 1, "down")
        self._copy(1, 0, 1, "up").wait_recv()
        self._start(7, N_Y - 1, None, "core")
        self._copy(2, 0, 0, "down").wait_recv()
        self._start(8, 1, None, "core")

    def near(self):
        for number, shift in ((6, 0), (7, N_Y - 1), (8, 1)):
            self._copy(number, shift, None, "core").wait_recv()

    def far(self):
        self._copy(4, 0, 0, "up").wait_recv()
        self._start(9, 2, 0, "core")
        self._copy(5, 0, 1, "down").wait_recv()
        self._start(10, 2, 1, "core")
        for part in range(2):
            self._copy(9 + part, 2, part, "core").wait_recv()

    def finish(self):
        for copy in self.started:
            copy.wait_send()


def project_phase(
    greeted,
    after_gates,
    after_exchange,
    tokens_hbm,
    gain,
    query_gain,
    latent_gain,
    cosine_row,
    sine_row,
    shift_hbm,
    narrow_query,
    narrow_latent,
    narrow_rotary,
    narrow_ingate,
    narrow_forget,
    query_hbm,
    key_hbm,
    value_hbm,
    outgate_hbm,
    query_up_hbm,
    key_up_hbm,
    value_up_hbm,
    mem_ref,
    gate_ref,
    q_ref,
    kv_ref,
    rows_all,
    latents,
    small,
    ingate,
    forget,
    big,
    query_up,
    key_up,
    value_up,
    tokens,
    shift_row,
    pre_gates,
    up_query,
    up_latent,
    wide_query,
    wide_latent,
    load_sem,
    row_send,
    row_recv,
    lat_send,
    lat_recv,
):
    f32, bf16 = jnp.float32, jnp.bfloat16
    y, c = lax.axis_index("y"), lax.axis_index("c")
    mine = y * N_C + c
    width = 128
    sources = (
        (narrow_query, small.at[pl.ds(0, QUERY_PART)]),
        (narrow_latent, small.at[pl.ds(width, LATENT_PART)]),
        (narrow_rotary, small.at[pl.ds(width + LATENT_PART, ROTARY_CHANNELS)]),
        (narrow_ingate, ingate),
        (narrow_forget, forget),
        (query_up_hbm, query_up),
        (key_up_hbm, key_up),
        (value_up_hbm, value_up),
        (shift_hbm, shift_row),
    )
    loads = [
        pltpu.make_async_copy(source, target, load_sem.at[k])
        for k, (source, target) in enumerate(sources)
    ]
    at = 0
    for k, ref in enumerate((query_hbm, key_hbm, value_hbm, outgate_hbm)):
        columns = ref.shape[1]
        loads.append(
            pltpu.make_async_copy(ref, big.at[:, pl.ds(at, columns)], load_sem.at[9 + k])
        )
        at += columns
    arrival = pltpu.make_async_copy(tokens_hbm, tokens, load_sem.at[13])
    arrival.start()
    for load in loads:
        load.start()
    arrival.wait()
    wide = tokens[...].astype(f32)
    inverse = lax.rsqrt(jnp.mean(wide * wide, axis=1, keepdims=True) + SMALL_CONSTANT)
    rows_all[mine] = (wide * inverse * gain[...].astype(f32).reshape(1, -1)).astype(bf16)
    small[QUERY_PART:width] = jnp.zeros((width - QUERY_PART, small.shape[1]), bf16)

    greeted()
    gather = TpGather(rows_all, row_send, row_recv)
    gather.start()

    for load in loads:
        load.wait()
    small[QUERY_PART : QUERY_PART + 8] = ingate[...]
    small[QUERY_PART + 16 : QUERY_PART + 24] = forget[...]
    up_query[...] = jnp.zeros(up_query.shape, bf16)
    query_rows = query_up[...].astype(f32).T.astype(bf16)
    for s in range(N_Y * N_C):
        up_query[s * width : s * width + QUERY_PART] = query_rows[
            s * QUERY_PART : (s + 1) * QUERY_PART
        ]
        part = slice(s * LATENT_PART, (s + 1) * LATENT_PART)
        for h in range(2):
            at = s * width + h * LATENT_PART
            up_latent[at : at + LATENT_PART, :width] = key_up[part]
            up_latent[at : at + LATENT_PART, width:] = value_up[part]

    lane = lax.broadcasted_iota(jnp.int32, (1, width), 1)
    cosine, sine_part = (
        jnp.concatenate([ref[...]] * 4, axis=0).T for ref in (cosine_row, sine_row)
    )
    row_id = lax.broadcasted_iota(jnp.int32, (width, width), 0)
    col_id = lax.broadcasted_iota(jnp.int32, (width, width), 1)
    channels = lax.rem(col_id, ROTARY_CHANNELS)
    halfway = ROTARY_CHANNELS // 2
    twin = (row_id == channels).astype(bf16)
    partner = lax.rem(channels + halfway, ROTARY_CHANNELS)
    sign = jnp.where(channels < halfway, -1.0, 1.0)

    def duplicated(values, offset):
        return jnp.dot(
            values, (row_id == channels + offset).astype(bf16), preferred_element_type=f32
        )

    def rotated(values, offset):
        swap = jnp.where(row_id == partner + offset, sign, 0.0).astype(bf16)
        turned = jnp.dot(values, swap, preferred_element_type=f32)
        return duplicated(values, offset) * cosine + turned * sine_part

    def chip_rows(chip):
        slots = [rows_all[chip * N_C + k] for k in range(N_C)]
        return jnp.concatenate(slots, axis=0)

    span = N_C * SHARE
    tile = 256

    def project_small(chip):
        rows = pl.ds(pl.multiple_of(chip * span, span), span)
        here = chip_rows(chip)
        made = lax.dot_general(here, small[...], CONTRACT_LAST, preferred_element_type=f32)
        turned = made[:, :width].T
        for k in range(2):
            at = QUERY_PART + 16 * k
            pre_gates[k, :, rows] = turned[at : at + 8]
        rounded = made.astype(bf16)
        latents[mine, rows] = rounded[:, :width]
        wide_latent[rows, :width] = rounded[:, width:]

    def project_big():
        def one(t, carry):
            columns = pl.ds(pl.multiple_of(t * tile, tile), tile)
            rows = rows_all[...].reshape(ROWS, rows_all.shape[2])
            made = jnp.dot(rows, big[:, columns], preferred_element_type=f32)
            mem_ref[:, columns] = made.astype(bf16)
            return carry

        lax.fori_loop(0, big.shape[1] // tile, one, 0)

    gather.relay()
    gather.near()
    near = [y, lax.rem(y + N_Y - 1, N_Y), lax.rem(y + 1, N_Y)]
    for chip in near:
        project_small(chip)
    opposite = lax.rem(y + 2, N_Y)
    gather.far()
    project_small(opposite)

    second = wide_latent[:, :width]
    both = duplicated(second, 0)
    half = ROWS // 2
    packed = jnp.where(lane < LATENT_PART, both[:half], both[half:])
    latents[mine, ROWS:] = packed.astype(bf16)
    exchange = TpGather(latents, lat_send, lat_recv)
    exchange.start()
    project_big()
    heads = lax.broadcasted_iota(jnp.int32, (8, ROWS), 0) == mine
    in_pre, forget_pre = (
        jnp.sum(jnp.where(heads, pre_gates[k], 0.0), axis=0, keepdims=True) for k in range(2)
    )
    in_gate = SOFTCAP * jnp.tanh(in_pre / SOFTCAP)
    capped = SOFTCAP * jnp.tanh((forget_pre + shift_row[...]) / SOFTCAP)
    small_part = jnp.exp(-jnp.abs(capped))
    above_one = 1.0 + small_part
    grown = jnp.where(
        above_one == 1.0, small_part, jnp.log(above_one) * small_part / (above_one - 1.0)
    )
    log_forget = jnp.minimum(capped, 0.0) - grown
    earlier = lax.broadcasted_iota(jnp.int32, (ROWS, ROWS), 0) <= lax.broadcasted_iota(
        jnp.int32, (ROWS, ROWS), 1
    )
    cumulative = jnp.dot(
        jnp.broadcast_to(log_forget, (8, ROWS)),
        earlier.astype(f32),
        precision=PRECISE,
        preferred_element_type=f32,
    )
    top_rows = lax.broadcasted_iota(jnp.int32, (8, ROWS), 0) == 0
    gate_ref[...] = jnp.where(top_rows, in_gate - cumulative, cumulative)
    exchange.relay()
    after_gates()
    key_turned = rotated(second, LATENT_PART)
    kv_ref[2 * ROWS :] = jnp.where(
        lane < ROTARY_CHANNELS, key_turned[:half], key_turned[half:]
    ).astype(bf16)
    exchange.near()
    after_exchange()
    exchange.far()

    query_mask = (lane < QUERY_PART).astype(f32)
    squares = jnp.zeros((ROWS, width), f32)
    low_squares = jnp.zeros((half, width), f32)
    for s in range(N_Y * N_C):
        part = latents[s, :ROWS].astype(f32) * query_mask
        squares = squares + part * part
        part = latents[s, ROWS:].astype(f32)
        low_squares = low_squares + part * part
    query_scale = lax.rsqrt(
        jnp.sum(squares, axis=1, keepdims=True) / QUERY_LATENT + SMALL_CONSTANT
    )
    low = lane < LATENT_PART
    low_scale = lax.rsqrt(
        jnp.sum(jnp.where(low, low_squares, 0.0), axis=1, keepdims=True) / LATENT_WIDTH
        + SMALL_CONSTANT
    )
    high_scale = lax.rsqrt(
        jnp.sum(jnp.where(low, 0.0, low_squares), axis=1, keepdims=True) / LATENT_WIDTH
        + SMALL_CONSTANT
    )
    latent_scale = jnp.where(low, low_scale, high_scale)
    query_gains = jnp.broadcast_to(query_gain[...].reshape(1, -1), (8, QUERY_LATENT))
    latent_gains = jnp.broadcast_to(latent_gain[...].reshape(1, -1), (8, LATENT_WIDTH))

    def latent_gain_of(s):
        pair = latent_gains[:1, (s // 2) * width : (s // 2 + 1) * width]
        turned = pltpu.roll(latent_gains, LATENT_PART, 1)
        other = turned[:1, (s // 2) * width : (s // 2 + 1) * width]
        if s % 2:
            other = pltpu.roll(latent_gains, LATENT_WIDTH - LATENT_PART, 1)
            other = other[:1, (s // 2) * width : (s // 2 + 1) * width]
            return jnp.where(low, other, pair)
        return jnp.where(low, pair, other)

    def query_gain_of(s):
        turned = query_gains
        if s:
            turned = pltpu.roll(query_gains, QUERY_LATENT - s * QUERY_PART, 1)
        return turned[:1, :width]

    for s in range(N_Y * N_C):
        columns = slice(s * width, (s + 1) * width)
        part = latents[s, :ROWS].astype(f32) * query_mask
        wide_query[:, columns] = (part * query_scale * query_gain_of(s)).astype(bf16)
        part = latents[s, ROWS:].astype(f32)
        made = (part * latent_scale * latent_gain_of(s)).astype(bf16)
        wide_latent[:half, columns] = jnp.where(low, made, jnp.zeros_like(made))
        wide_latent[half:, columns] = jnp.where(low, jnp.zeros_like(made), made)
    made = jnp.dot(wide_latent[...], up_latent[...], preferred_element_type=f32).astype(bf16)
    kv_ref[:ROWS] = made[:, :width]
    kv_ref[ROWS : 2 * ROWS] = made[:, width:]
    made = jnp.dot(wide_query[...], up_query[...], preferred_element_type=f32).astype(bf16)
    q_ref[:, :width] = made[:, :width]
    turning = jnp.concatenate([made[:, width:], jnp.zeros((ROWS, ROTARY_CHANNELS), bf16)], axis=1)
    q_ref[:, width:] = rotated(turning, 0).astype(bf16)
    return gather.started + exchange.started


def output_phase(
    gated,
    attended,
    out_memory,
    out_attend,
    o_ref,
    to_core,
    from_core,
    sums,
    passing,
    from_below,
    from_above,
    relay_in,
    core_send,
    core_recv,
    relay_send,
    relay_recv,
    up_send,
    up_recv,
    down_send,
    down_recv,
):
    f32, bf16 = jnp.float32, jnp.bfloat16
    y, c = lax.axis_index("y"), lax.axis_index("c")
    above, below = lax.rem(y + 1, N_Y), lax.rem(y + N_Y - 1, N_Y)
    opposite = lax.rem(y + 2, N_Y)
    half = out_memory.shape[1] // 2
    tile = 512

    def remote(source, target, send, recv, device):
        return pltpu.make_async_remote_copy(
            src_ref=source,
            dst_ref=target,
            send_sem=send,
            recv_sem=recv,
            device_id=device,
            device_id_type=MESH_ID,
        )

    def rows_of(ref, core):
        picked = [ref[pl.ds(pl.multiple_of((k * N_C + core) * SHARE, SHARE), SHARE)] for k in range(N_Y)]
        return jnp.concatenate(picked, axis=0)

    def partial(core, h, store):
        memory_rows, attend_rows = rows_of(gated, core), rows_of(attended, core)
        for t in range(half // tile):
            columns = slice(h * half + t * tile, h * half + (t + 1) * tile)
            made = jnp.dot(memory_rows, out_memory[:, columns], preferred_element_type=f32)
            made = made + jnp.dot(attend_rows, out_attend[:, columns], preferred_element_type=f32)
            store(t * tile, made.astype(bf16).reshape(N_Y, SHARE, tile))

    def core_copy(h):
        return remote(
            to_core.at[h], from_core.at[h], core_send.at[h], core_recv.at[h], {"c": 1 - c}
        )

    def relay_copy(h):
        return remote(
            passing.at[h],
            relay_in.at[h],
            relay_send.at[h],
            relay_recv.at[h],
            {"y": above if h == 0 else below},
        )

    def up_copy(h):
        return remote(
            passing.at[2 + h], from_below.at[h], up_send.at[h], up_recv.at[h], {"y": above}
        )

    def down_copy(h):
        return remote(
            passing.at[4 + h], from_above.at[h], down_send.at[h], down_recv.at[h], {"y": below}
        )

    started = []

    def start(copy):
        copy.start()
        started.append(copy)

    for h in range(2):

        def keep(at, block, h=h):
            to_core[h, :, :, at : at + tile] = block

        partial(1 - c, h, keep)
        start(core_copy(h))
    for h in range(2):

        def keep(at, block, h=h):
            sums[h, :, :, at : at + tile] = block.astype(f32)

        partial(c, h, keep)
    for h in range(2):
        core_copy(h).wait_recv()
        sums[h] = sums[h] + from_core[h].astype(f32)
        passing[h] = sums[h, opposite].astype(bf16)
        start(relay_copy(h))
        if h == 0:
            passing[4] = sums[0, below].astype(bf16)
            start(down_copy(0))
        else:
            passing[3] = sums[1, above].astype(bf16)
            start(up_copy(1))
    relay_copy(0).wait_recv()
    passing[2] = (sums[0, above] + relay_in[0].astype(f32)).astype(bf16)
    start(up_copy(0))
    relay_copy(1).wait_recv()
    passing[5] = (sums[1, below] + relay_in[1].astype(f32)).astype(bf16)
    start(down_copy(1))
    for h in (1, 0):
        up_copy(h).wait_recv()
        down_copy(h).wait_recv()
        made = sums[h, y] + from_below[h].astype(f32) + from_above[h].astype(f32)
        o_ref[:, h * half : (h + 1) * half] = made.astype(bf16)
    return started


def scratch(depth, mem_width):
    f32, bf16 = jnp.float32, jnp.bfloat16
    dma = pltpu.SemaphoreType.DMA
    between = (
        pltpu.VMEM((ROWS, VALUE_CHANNELS), bf16),
        pltpu.VMEM((ROWS, M_V), bf16),
        pltpu.VMEM((ROWS, mem_width), bf16),
        pltpu.VMEM((8, ROWS), f32),
        pltpu.VMEM((ROWS, 256), bf16),
        pltpu.VMEM((ROWS * 5 // 2, 128), bf16),
        pltpu.VMEM((M_V, depth), bf16),
        pltpu.VMEM((VALUE_CHANNELS, depth), bf16),
        dma((2,)),
    )
    for_project = (
        pltpu.VMEM((N_Y * N_C, SHARE, depth), bf16),
        pltpu.VMEM((N_Y * N_C, ROWS * 3 // 2, 128), bf16),
        pltpu.VMEM((256, depth), bf16),
        pltpu.VMEM((8, depth), bf16),
        pltpu.VMEM((8, depth), bf16),
        pltpu.VMEM((depth, mem_width), bf16),
        pltpu.VMEM((PLAIN_CHANNELS + ROTARY_CHANNELS, QUERY_LATENT), bf16),
        pltpu.VMEM((LATENT_WIDTH, PLAIN_CHANNELS), bf16),
        pltpu.VMEM((LATENT_WIDTH, VALUE_CHANNELS), bf16),
        pltpu.VMEM((SHARE, depth), bf16),
        pltpu.VMEM((1, ROWS), f32),
        pltpu.VMEM((2, 8, ROWS), f32),
        pltpu.VMEM((1024, PLAIN_CHANNELS + ROTARY_CHANNELS), bf16),
        pltpu.VMEM((1024, 256), bf16),
        pltpu.VMEM((ROWS, 1024), bf16),
        pltpu.VMEM((ROWS, 1024), bf16),
        dma((16,)),
        dma((11,)),
        dma((11,)),
        dma((11,)),
        dma((11,)),
    )
    for_attend = (
        pltpu.VMEM((N_X, ROWS, 256), bf16),
        pltpu.VMEM((N_Z, ROWS * 5 // 2, 128), bf16),
        pltpu.VMEM((ROWS, 256), bf16),
        pltpu.VMEM((N_X * ROWS, 128), f32),
        pltpu.VMEM((N_X * ROWS, 128), f32),
        pltpu.VMEM((N_X * ROWS, VALUE_CHANNELS), f32),
        pltpu.VMEM((N_X - 1, ROWS, VALUE_CHANNELS), bf16),
        pltpu.VMEM((N_X - 1, 8, ROWS), f32),
        pltpu.VMEM((N_X - 1, ROWS, VALUE_CHANNELS), bf16),
        pltpu.VMEM((N_X - 1, 8, ROWS), f32),
        pltpu.VMEM((ROWS, M_V), f32),
        pltpu.VMEM((ROWS, 128), f32),
        pltpu.VMEM((ROWS, 128), f32),
        pltpu.VMEM((N_X, STATE_ROWS, M_V), f32),
        pltpu.VMEM((N_X, STATE_ROWS, M_V), f32),
        pltpu.VMEM((STATE_ROWS, M_V), f32),
        pltpu.VMEM((N_Z, STATE_ROWS, M_V), f32),
        pltpu.VMEM((N_X, STATE_ROWS, M_V), f32),
        pltpu.VMEM((N_X, STATE_ROWS, M_V), f32),
        pltpu.VMEM((2, 8, ROWS), f32),
        pltpu.VMEM((N_Y, 8, ROWS), f32),
        pltpu.VMEM((2, ROWS // 2, VALUE_CHANNELS), bf16),
        dma((6,)),
        dma((6,)),
        dma((N_Z // 2, 2)),
        dma((N_Z // 2, 2)),
        dma((N_Z // 2, 2)),
        dma((N_Z // 2, 2)),
        dma((N_X - 1,)),
        dma((N_X - 1,)),
        dma((N_X - 1,)),
        dma((N_X - 1,)),
        dma((N_X - 1,)),
        dma((N_X - 1,)),
        dma((N_Z,)),
        dma((N_Z,)),
        dma((N_X - 1,)),
        dma((N_X - 1,)),
        dma((N_Y,)),
        dma((N_Y,)),
        dma((2, 2)),
        dma((2, 2)),
    )
    for_output = (
        pltpu.VMEM((2, N_Y, SHARE, depth // 2), bf16),
        pltpu.VMEM((2, N_Y, SHARE, depth // 2), bf16),
        pltpu.VMEM((2, N_Y, SHARE, depth // 2), f32),
        pltpu.VMEM((6, SHARE, depth // 2), bf16),
        pltpu.VMEM((2, SHARE, depth // 2), bf16),
        pltpu.VMEM((2, SHARE, depth // 2), bf16),
        pltpu.VMEM((2, SHARE, depth // 2), bf16),
        dma((2,)),
        dma((2,)),
        dma((2,)),
        dma((2,)),
        dma((2,)),
        dma((2,)),
        dma((2,)),
        dma((2,)),
    )
    return between, for_project, for_attend, for_output


N_INPUTS = 22
N_PROJECT_INPUTS = 19
IN_VMEM = (1, 2, 3, 4, 5, 19)


def layer_kernel(counts, *refs):
    y, c = lax.axis_index("y"), lax.axis_index("c")
    z, x = lax.axis_index("z"), lax.axis_index("x")
    project_inputs = refs[:N_PROJECT_INPUTS]
    mem_gain, out_memory_hbm, out_attend_hbm, out_ref = refs[N_PROJECT_INPUTS : N_INPUTS + 1]
    groups, at = [], N_INPUTS + 1
    for count in counts:
        groups.append(refs[at : at + count])
        at += count
    between, for_project, for_attend, for_output = groups
    attended, gated, mem, gates, queries, keys_values, out_memory, out_attend, out_sem = between

    barrier = pltpu.get_barrier_semaphore()
    devices = [{"c": 1 - c}]
    devices += [{"y": lax.rem(y + d, N_Y)} for d in range(1, N_Y)]
    devices += [{"x": lax.rem(x + d, N_X)} for d in range(1, N_X)]
    devices += [{"z": lax.rem(z + d, N_Z)} for d in range(1, N_Z)]
    for device in devices:
        pl.semaphore_signal(barrier, inc=1, device_id=device, device_id_type=MESH_ID)
    loads = [
        pltpu.make_async_copy(out_memory_hbm, out_memory, out_sem.at[0]),
        pltpu.make_async_copy(out_attend_hbm, out_attend, out_sem.at[1]),
    ]
    attending = attend_phase(
        queries, keys_values, mem, gates, mem_gain, attended, gated, *for_attend
    )
    started = project_phase(
        lambda: pl.semaphore_wait(barrier, len(devices)),
        lambda: next(attending),
        lambda: next(attending),
        *project_inputs,
        mem,
        gates,
        queries,
        keys_values,
        *for_project,
    )
    for load in loads:
        load.start()
    more, finish_columns = next(attending)
    started += more
    for load in loads:
        load.wait()
    started += output_phase(gated, attended, out_memory, out_attend, out_ref, *for_output)
    for copy in started:
        copy.wait_send()
    finish_columns()


def layer(*inputs):
    depth = inputs[0].shape[1]
    mem_width = 2 * M_QK + 2 * M_V
    groups = scratch(depth, mem_width)
    vmem = pl.BlockSpec(memory_space=pltpu.VMEM)
    hbm = pl.BlockSpec(memory_space=pltpu.HBM)
    return pl.pallas_call(
        functools.partial(layer_kernel, tuple(len(group) for group in groups)),
        out_shape=jax.ShapeDtypeStruct((SHARE, depth), jnp.bfloat16),
        in_specs=[vmem if k in IN_VMEM else hbm for k in range(N_INPUTS)],
        out_specs=vmem,
        scratch_shapes=[one for group in groups for one in group],
        compiler_params=pltpu.CompilerParams(
            collective_id=1, has_side_effects=True, vmem_limit_bytes=67_000_000
        ),
        cost_estimate=pl.CostEstimate(
            flops=8 * 10**9, bytes_accessed=2 * 10**7, transcendentals=4 * 10**6
        ),
        name="layer",
    )(*inputs)


def per_device(
    tokens,
    input_gain,
    weight_query,
    weight_key,
    weight_value,
    weight_outgate,
    weight_ingate,
    weight_forget,
    forget_shift,
    mem_gain,
    query_down_weight,
    latent_down_weight,
    down_rotary,
    query_gain,
    latent_gain,
    query_up_weight,
    key_up_weight,
    value_up_weight,
    out_memory,
    out_attend,
):
    length = forget_shift.shape[0]
    positions = lax.axis_index(SP) * length + jnp.arange(length, dtype=jnp.int32)
    halfway = ROTARY_CHANNELS // 2
    inverse = jnp.power(ROTARY_BASE, -jnp.arange(halfway, dtype=jnp.float32) / halfway)
    angles = positions.astype(jnp.float32)[None, :] * inverse[:, None]
    return layer(
        tokens,
        input_gain,
        query_gain,
        latent_gain,
        jnp.cos(angles),
        jnp.sin(angles),
        forget_shift.T,
        query_down_weight.T,
        latent_down_weight.T,
        down_rotary.T,
        weight_ingate.T,
        weight_forget.T,
        weight_query,
        weight_key,
        weight_value,
        weight_outgate,
        query_up_weight.T,
        key_up_weight,
        value_up_weight,
        mem_gain,
        out_memory,
        out_attend,
    )


def solution(mesh):
    torus = Mesh(mesh.devices.reshape(N_Z, N_X, 4, 2), SP_TP)
    in_specs = (
        P(SP_TP, None),
        P(),
        P(None, TP),
        P(None, TP),
        P(None, TP),
        P(None, TP),
        P(),
        P(),
        P(SP, TP),
        P(),
        P(None, TP),
        P(None, TP),
        P(),
        P(),
        P(),
        P(None, TP),
        P(None, TP),
        P(None, TP),
        P(TP, None),
        P(TP, None),
    )
    out_specs = P(SP_TP, None)
    return jax.shard_map(
        per_device, mesh=torus, in_specs=in_specs, out_specs=out_specs, check_vma=False
    )
```

```python
import functools

import jax
import jax.numpy as jnp
from jax import lax
from jax.experimental import pallas as pl
from jax.experimental.pallas import tpu as pltpu
from jax.sharding import Mesh
from jax.sharding import PartitionSpec as P

MEMORY_HEADS = 8
M_QK = 128
M_V = 256
PLAIN_CHANNELS = 128
ROTARY_CHANNELS = 64
VALUE_CHANNELS = 128
SP = ("z", "x")
TP = ("y", "c")
SP_TP = ("z", "x", "y", "c")


SMALL_CONSTANT = 1e-06
SOFTCAP = 15.0
ROTARY_BASE = 10000.0
PRECISE = lax.Precision.HIGHEST
FAR_BELOW = -1e30

N_Y = 4
N_C = 2
SHARE = 64
QUERY_LATENT = 768
LATENT_WIDTH = 512
QUERY_PART = QUERY_LATENT // (N_Y * N_C)
LATENT_PART = LATENT_WIDTH // (N_Y * N_C)
LOG2E = 1.4426950408889634
N_Z = 8
N_X = 4
ROWS = 512
MESH_ID = pl.DeviceIdType.MESH
CONTRACT_LAST = (((1,), (1,)), ((), ()))
CHUNK = M_QK // N_X
TALL = 512
GROUP = 1
STATE_ROWS = CHUNK + 8
NORMAL_ROW, TOP_ROW, DECAY_ROW = CHUNK, CHUNK + 1, CHUNK + 2


def merge_states(early, late):
    moved = early[TOP_ROW : TOP_ROW + 1] + late[DECAY_ROW : DECAY_ROW + 1]
    late_top = late[TOP_ROW : TOP_ROW + 1]
    joined = jnp.maximum(moved, late_top)
    both = early * jnp.exp(moved - joined) + late * jnp.exp(late_top - joined)
    row = lax.broadcasted_iota(jnp.int32, both.shape, 0)
    decay = early[DECAY_ROW : DECAY_ROW + 1] + late[DECAY_ROW : DECAY_ROW + 1]
    return jnp.where(row == TOP_ROW, joined, jnp.where(row == DECAY_ROW, decay, both))


def in_two(values):
    high = values.astype(jnp.bfloat16)
    return high, (values - high.astype(jnp.float32)).astype(jnp.bfloat16)


def as_columns(row, width):
    return jnp.broadcast_to(row, (width, row.shape[1])).T


def attend_phase(
    q_ref,
    kv_ref,
    mem_ref,
    gate_ref,
    gain_ref,
    attended_ref,
    gated_ref,
    q_all,
    kv_all,
    k_cat,
    top,
    total,
    accum,
    part_out,
    stat_out,
    part_in,
    stat_in,
    cell,
    cell_sum,
    cell_top,
    first_out,
    first_in,
    column_out,
    column_in,
    start_out,
    start_in,
    square_out,
    square_in,
    passed,
    q_send,
    q_recv,
    up_send,
    up_recv,
    down_send,
    down_recv,
    part_send,
    part_recv,
    stat_send,
    stat_recv,
    first_send,
    first_recv,
    column_send,
    column_recv,
    start_send,
    start_recv,
    square_send,
    square_recv,
    passed_send,
    passed_recv,
):
    f32, bf16 = jnp.float32, jnp.bfloat16
    z, x = lax.axis_index("z"), lax.axis_index("x")
    y, c = lax.axis_index("y"), lax.axis_index("c")
    above, below = lax.rem(z + 1, N_Z), lax.rem(z + N_Z - 1, N_Z)
    peers = [lax.rem(x + d, N_X) for d in range(1, N_X)]
    right, left = peers[0], peers[-1]
    rows_y = [lax.rem(y + d, N_Y) for d in range(1, N_Y)]
    me_tp = y * N_C + c
    half = kv_ref.shape[0] // 2
    width = PLAIN_CHANNELS

    def remote(source, target, send, recv, device):
        return pltpu.make_async_remote_copy(
            src_ref=source,
            dst_ref=target,
            send_sem=send,
            recv_sem=recv,
            device_id=device,
            device_id_type=MESH_ID,
        )

    def kv_copy(up, step, h):
        shift = (N_Z - step + 1) if up else (step - 1)
        owner = lax.rem(z + shift, N_Z)
        rows = pl.ds(h * half, half)
        source = kv_ref.at[rows] if step == 1 else kv_all.at[owner, rows]
        send, recv = (up_send, up_recv) if up else (down_send, down_recv)
        return remote(
            source,
            kv_all.at[owner, rows],
            send.at[step - 1, h],
            recv.at[step - 1, h],
            {"z": above if up else below},
        )

    q_half = ROWS // 2

    def q_copy(number):
        shift, part, to_right = (
            (0, 0, True),
            (0, 1, True),
            (0, 0, False),
            (0, 1, False),
            (N_X - 1, 0, True),
            (1, 1, False),
        )[number]
        owner = lax.rem(x + shift, N_X)
        rows = pl.ds(part * q_half, q_half)
        source = q_ref.at[rows] if shift == 0 else q_all.at[owner, rows]
        return remote(
            source,
            q_all.at[owner, rows],
            q_send.at[number],
            q_recv.at[number],
            {"x": right if to_right else left},
        )

    def part_copy(d):
        return remote(
            part_out.at[d], part_in.at[d], part_send.at[d], part_recv.at[d], {"x": peers[d]}
        )

    def far_copy(h, hop):
        rows = pl.ds(h * q_half, q_half)
        return remote(
            part_out.at[1, rows] if hop == 0 else passed.at[h],
            passed.at[h] if hop == 0 else part_in.at[1, rows],
            passed_send.at[hop, h],
            passed_recv.at[hop, h],
            {"x": right if h == 0 else left},
        )

    def stat_copy(d):
        return remote(
            stat_out.at[d], stat_in.at[d], stat_send.at[d], stat_recv.at[d], {"x": peers[d]}
        )

    def first_copy(d):
        return remote(
            first_out.at[peers[d]],
            first_in.at[x],
            first_send.at[d],
            first_recv.at[d],
            {"x": peers[d]},
        )

    def column_copy(target):
        return remote(
            column_out,
            column_in.at[z],
            column_send.at[target],
            column_recv.at[z],
            {"z": target},
        )

    def column_arrival(source):
        return remote(
            column_out,
            column_in.at[source],
            column_send.at[source],
            column_recv.at[source],
            {"z": source},
        )

    def start_copy(d):
        return remote(
            start_out.at[peers[d]],
            start_in.at[x],
            start_send.at[d],
            start_recv.at[d],
            {"x": peers[d]},
        )

    def square_copy(number):
        device = {"c": 1 - c} if number == 0 else {"y": rows_y[number - 1]}
        return remote(
            square_out.at[min(number, 1)],
            square_in.at[number],
            square_send.at[number],
            square_recv.at[number],
            device,
        )

    started = []

    def start(copy):
        copy.start()
        started.append(copy)

    relative, cumulative = gate_ref[0:1], gate_ref[1:2]
    key_scale = M_QK ** (-0.5)
    tall = 256
    for t in range(ROWS // tall):
        rows, seen = slice(t * tall, (t + 1) * tall), (t + 1) * tall
        row = lax.broadcasted_iota(jnp.int32, (tall, seen), 0) + t * tall
        col = lax.broadcasted_iota(jnp.int32, (tall, seen), 1)
        logs = jnp.where(col <= row, relative[:, :seen], -jnp.inf)
        highest = jnp.max(logs, axis=1, keepdims=True)
        affinity = lax.dot_general(
            mem_ref[rows, :M_QK],
            mem_ref[:seen, M_QK : 2 * M_QK],
            CONTRACT_LAST,
            preferred_element_type=f32,
        )
        affinity = affinity * (jnp.exp(logs - highest) * key_scale)
        values = mem_ref[:seen, 2 * M_QK : 2 * M_QK + M_V]
        cell[rows] = sum(
            jnp.dot(piece, values, preferred_element_type=f32) for piece in in_two(affinity)
        )
        cell_sum[rows] = jnp.broadcast_to(
            jnp.sum(affinity, axis=1, keepdims=True), (tall, width)
        )
        cell_top[rows] = jnp.broadcast_to(highest, (tall, width))
    ends_at = jnp.max(relative, axis=1, keepdims=True)
    weights = jnp.exp(relative - ends_at) * key_scale
    wide_key = mem_ref[:, M_QK : 2 * M_QK].astype(f32)
    normal = jnp.sum(as_columns(weights, width) * wide_key, axis=0, keepdims=True)
    values = mem_ref[:, 2 * M_QK : 2 * M_QK + M_V]
    matrix = sum(
        jnp.dot(piece, values, preferred_element_type=f32)
        for piece in in_two(wide_key.T * weights)
    )
    decay = cumulative[:, ROWS - 1 : ROWS]
    row = lax.broadcasted_iota(jnp.int32, (8, M_V), 0)
    lines = jnp.concatenate([normal, jnp.zeros_like(normal)], axis=1)
    notes = jnp.where(
        row == 0, lines, jnp.where(row == 1, ends_at + decay, jnp.where(row == 2, decay, 0.0))
    )
    for k in range(N_X):
        first_out[k, :CHUNK] = matrix[k * CHUNK : (k + 1) * CHUNK]
        first_out[k, CHUNK:] = notes
    for d in range(N_X - 1):
        start(first_copy(d))
    first_in[x] = first_out[x]

    yield

    for d in range(N_X - 1):
        first_copy(d).wait_recv()
    column = first_in[0]
    for k in range(1, N_X):
        column = merge_states(column, first_in[k])
    column_out[...] = column
    for target in range(1, N_Z):

        @pl.when(target > z)
        def _(target=target):
            column_copy(target).start()

    yield

    for h in range(2):
        for up in (True, False):
            start(kv_copy(up, 1, h))
    yield

    top[...] = jnp.full(top.shape, FAR_BELOW, f32)
    total[...] = jnp.zeros(total.shape, f32)
    for number in (0, 3, 1, 2):
        start(q_copy(number))
    accum[...] = jnp.zeros(accum.shape, f32)
    q_all[x] = q_ref[...]

    lane = lax.broadcasted_iota(jnp.int32, (ROWS // 2, width), 1)
    low = (lane < ROTARY_CHANNELS).astype(bf16)
    high = (lane >= ROTARY_CHANNELS).astype(bf16)
    scale = LOG2E * (PLAIN_CHANNELS + ROTARY_CHANNELS) ** (-0.5)

    def keys_from(ref):
        k_cat[:, :width] = ref[:ROWS]
        packed = ref[2 * ROWS :]
        k_cat[: ROWS // 2, width:] = packed * low
        k_cat[ROWS // 2 :, width:] = packed * high

    def attend_tile(t, keys, values, masked):
        shard = t // (ROWS // TALL)
        rows = pl.ds(pl.multiple_of(t * TALL, TALL), TALL)
        inner = pl.ds(pl.multiple_of((t % (ROWS // TALL)) * TALL, TALL), TALL)
        scores = lax.dot_general(
            q_all[shard, inner], keys, CONTRACT_LAST, preferred_element_type=f32
        )
        scores = scores * scale
        if masked:
            row = lax.broadcasted_iota(jnp.int32, scores.shape, 0) + t * TALL
            col = lax.broadcasted_iota(jnp.int32, scores.shape, 1) + x * ROWS
            scores = jnp.where(col <= row, scores, -jnp.inf)
        old = top[rows]
        new = jnp.maximum(old, jnp.max(scores, axis=1, keepdims=True))
        probs = jnp.exp2(scores - jnp.concatenate([new] * (ROWS // width), axis=1))
        shrink = jnp.exp2(old - new)
        added = sum(probs[:, k : k + width] for k in range(0, ROWS, width))
        total[rows] = total[rows] * shrink + added
        accum[rows] = accum[rows] * shrink + jnp.dot(
            probs.astype(bf16), values, preferred_element_type=f32
        )
        top[rows] = new

    def attend_rows(first, last, values, masked):
        def one(g, carry):
            for u in range(GROUP):
                attend_tile(g * GROUP + u, k_cat[...], values(), masked)
            return carry

        lax.fori_loop(first, last, one, 0)

    last = N_Z // 2
    steps = ROWS // (TALL * GROUP)

    def arrived(owner, useful):
        @pl.when(useful)
        def _():
            keys_from(kv_all.at[owner])
            attend_rows(0, N_X * steps, lambda: kv_all[owner, ROWS : 2 * ROWS], False)

    def take(step, h):
        for up in (True, False):
            if step == last and up != (h == 0):
                continue
            kv_copy(up, step, h).wait_recv()
            if step < last - 1 or (step == last - 1 and up == (h == 0)):
                start(kv_copy(up, step + 1, h))

    def use_up(step):
        arrived(lax.rem(z + N_Z - step, N_Z), z >= step)

    def use_down(step):
        arrived(lax.rem(z + step, N_Z), z + step >= N_Z)

    keys_from(kv_ref)
    own_values = lambda: kv_ref[ROWS : 2 * ROWS]
    attend_rows(x * steps, (x + 1) * steps, own_values, True)

    q_copy(0).wait_recv()
    start(q_copy(4))
    q_copy(3).wait_recv()
    start(q_copy(5))

    def gather_column(k, state):
        column_arrival(k).wait_recv()
        return merge_states(state, column_in[k])

    state = lax.fori_loop(0, z, gather_column, jnp.zeros((STATE_ROWS, M_V), f32))
    for k in range(N_X):
        start_out[k] = state
        if k < N_X - 1:
            state = merge_states(state, first_in[k])
    for d in range(N_X - 1):
        start(start_copy(d))
    start_in[x] = start_out[x]
    take(1, 0)
    for number in (1, 2, 4, 5):
        q_copy(number).wait_recv()
    attend_rows((x + 1) * steps, N_X * steps, own_values, False)
    take(1, 1)
    take(2, 0)
    use_up(1)
    take(2, 1)
    use_down(1)

    for d in range(N_X - 1):
        start_copy(d).wait_recv()
    carried = jnp.concatenate([start_in[k, :CHUNK] for k in range(N_X)], axis=0)
    carried_normal = start_in[0, NORMAL_ROW : NORMAL_ROW + 1, :M_QK]
    carried_top = start_in[0, TOP_ROW : TOP_ROW + 1, :width]
    queries = mem_ref[:, :M_QK]
    from_start = sum(
        jnp.dot(queries, piece, preferred_element_type=f32) for piece in in_two(carried)
    )
    highest = jnp.maximum(carried_top, cell_top[...])
    across, within = jnp.exp(carried_top - highest), jnp.exp(cell_top[...] - highest)
    twice = lambda one: jnp.concatenate([one, one], axis=1)
    numerator = cell[...] * twice(within) + from_start * twice(across)
    denominator = cell_sum[...] * within + across * jnp.sum(
        queries.astype(f32) * carried_normal, axis=1, keepdims=True
    )
    floor = jnp.exp(-(as_columns(cumulative, width) + highest))
    made = numerator / twice(jnp.maximum(jnp.abs(denominator), floor))
    cell[...] = made
    squares = jnp.sum(made * made, axis=1, keepdims=True)
    square_out[0] = jnp.broadcast_to(squares, (ROWS, width)).T[:8]
    start(square_copy(0))

    take(3, 0)
    use_up(2)
    square_copy(0).wait_recv()
    square_out[1] = square_out[0] + square_in[0]
    for number in range(1, N_Y):
        start(square_copy(number))
    take(3, 1)
    use_down(2)
    use_up(3)
    use_down(3)

    squares = square_out[1]
    for number in range(1, N_Y):
        square_copy(number).wait_recv()
        squares = squares + square_in[number]
    inverse = lax.rsqrt(squares[:1] / (MEMORY_HEADS * M_V) + SMALL_CONSTANT)
    gated = cell[...] * twice(as_columns(inverse, width)) * gain_ref[pl.ds(pl.multiple_of(me_tp * M_V, M_V), M_V)].astype(f32).reshape(1, M_V)
    gated = gated * jax.nn.sigmoid(mem_ref[:, 2 * M_QK + M_V :].astype(f32))
    gated_ref[...] = gated.astype(bf16)
    take(4, 0)
    take(4, 1)

    opposite = lax.rem(z + last, N_Z)

    @pl.when(z >= last)
    def _():
        keys_from(kv_all.at[opposite])

    def finish(shard):
        @pl.when(z >= last)
        def _():
            attend_rows(
                shard * steps,
                (shard + 1) * steps,
                lambda: kv_all[opposite, ROWS : 2 * ROWS],
                False,
            )

        rows = pl.ds(pl.multiple_of(shard * ROWS, ROWS), ROWS)
        summed = jnp.sum(total[rows], axis=1, keepdims=True)
        seen = summed > 0.0
        summed = jnp.maximum(summed, 1.0)
        log_total = jnp.where(seen, top[rows] + jnp.log2(summed), FAR_BELOW)
        return accum[rows] / summed, log_total

    for d in (1, 0, 2):
        part, log_total = finish(peers[d])
        part_out[d] = part.astype(bf16)
        stat_out[d] = log_total.T[:8]
        if d == 1:
            start(far_copy(0, 0))
            start(far_copy(1, 0))
        else:
            start(part_copy(d))
        start(stat_copy(d))
    own, own_log = finish(x)

    for h in range(2):
        far_copy(h, 0).wait_recv()
        start(far_copy(h, 1))

    logs = []
    for d in range(N_X - 1):
        stat_copy(d).wait_recv()
        logs.append(as_columns(stat_in[d, 0:1, :], width))
    highest = own_log
    for one in logs:
        highest = jnp.maximum(highest, one)
    weight = jnp.exp2(own_log - highest)
    numerator = own * weight
    denominator = weight
    for d in (0, 2, 1):
        if d == 1:
            far_copy(0, 1).wait_recv()
            far_copy(1, 1).wait_recv()
        else:
            part_copy(d).wait_recv()
        weight = jnp.exp2(logs[d] - highest)
        numerator = numerator + part_in[d].astype(f32) * weight
        denominator = denominator + weight
    attended_ref[...] = (numerator / denominator).astype(bf16)
    def finish_columns():
        for target in range(1, N_Z):

            @pl.when(target > z)
            def _(target=target):
                column_copy(target).wait_send()

    yield started, finish_columns


class TpGather:
    def __init__(self, full, sends, recvs):
        self.full, self.sends, self.recvs = full, sends, recvs
        self.y, self.c = lax.axis_index("y"), lax.axis_index("c")
        self.half = full.shape[1] // 2
        self.started = []

    def _copy(self, number, shift, part, target):
        slot = lax.rem(self.y + shift, N_Y) * N_C + self.c
        if part is None:
            ref = self.full.at[slot]
        else:
            ref = self.full.at[slot, pl.ds(part * self.half, self.half)]
        if target == "core":
            device = {"c": 1 - self.c}
        else:
            device = {"y": lax.rem(self.y + (1 if target == "up" else N_Y - 1), N_Y)}
        return pltpu.make_async_remote_copy(
            src_ref=ref,
            dst_ref=ref,
            send_sem=self.sends.at[number],
            recv_sem=self.recvs.at[number],
            device_id=device,
            device_id_type=MESH_ID,
        )

    def _start(self, *what):
        copy = self._copy(*what)
        copy.start()
        self.started.append(copy)

    def start(self):
        self._start(0, 0, 0, "up")
        self._start(3, 0, 1, "down")
        self._start(1, 0, 1, "up")
        self._start(2, 0, 0, "down")
        self._start(6, 0, None, "core")

    def relay(self):
        self._copy(0, 0, 0, "up").wait_recv()
        self._start(4, N_Y - 1, 0, "up")
        self._copy(3, 0, 1, "down").wait_recv()
        self._start(5, 1, 1, "down")
        self._copy(1, 0, 1, "up").wait_recv()
        self._start(7, N_Y - 1, None, "core")
        self._copy(2, 0, 0, "down").wait_recv()
        self._start(8, 1, None, "core")

    def near(self):
        for number, shift in ((6, 0), (7, N_Y - 1), (8, 1)):
            self._copy(number, shift, None, "core").wait_recv()

    def far(self):
        self._copy(4, 0, 0, "up").wait_recv()
        self._start(9, 2, 0, "core")
        self._copy(5, 0, 1, "down").wait_recv()
        self._start(10, 2, 1, "core")
        for part in range(2):
            self._copy(9 + part, 2, part, "core").wait_recv()

    def finish(self):
        for copy in self.started:
            copy.wait_send()


def project_phase(
    greeted,
    after_gates,
    after_exchange,
    after_keys,
    tokens_hbm,
    gain,
    query_gain,
    latent_gain,
    cosine_row,
    sine_row,
    shift_hbm,
    narrow_query,
    narrow_latent,
    narrow_rotary,
    narrow_ingate,
    narrow_forget,
    query_hbm,
    key_hbm,
    value_hbm,
    outgate_hbm,
    query_up_hbm,
    key_up_hbm,
    value_up_hbm,
    mem_ref,
    gate_ref,
    q_ref,
    kv_ref,
    rows_all,
    query_latents,
    latents,
    small,
    ingate,
    forget,
    big,
    query_up,
    key_up,
    value_up,
    tokens,
    shift_row,
    pre_gates,
    up_query,
    up_latent,
    wide_query,
    wide_latent,
    load_sem,
    row_send,
    row_recv,
    lat_send,
    lat_recv,
    query_send,
    query_recv,
):
    f32, bf16 = jnp.float32, jnp.bfloat16
    y, c = lax.axis_index("y"), lax.axis_index("c")
    mine = y * N_C + c
    width = 128
    sources = (
        (narrow_query, small.at[pl.ds(0, QUERY_PART)]),
        (narrow_latent, small.at[pl.ds(width, LATENT_PART)]),
        (narrow_rotary, small.at[pl.ds(width + LATENT_PART, ROTARY_CHANNELS)]),
        (narrow_ingate, ingate),
        (narrow_forget, forget),
        (query_up_hbm, query_up),
        (key_up_hbm, key_up),
        (value_up_hbm, value_up),
        (shift_hbm, shift_row),
    )
    loads = [
        pltpu.make_async_copy(source, target, load_sem.at[k])
        for k, (source, target) in enumerate(sources)
    ]
    at = 0
    for k, ref in enumerate((query_hbm, key_hbm, value_hbm, outgate_hbm)):
        columns = ref.shape[1]
        loads.append(
            pltpu.make_async_copy(ref, big.at[:, pl.ds(at, columns)], load_sem.at[9 + k])
        )
        at += columns
    arrival = pltpu.make_async_copy(tokens_hbm, tokens, load_sem.at[13])
    arrival.start()
    for load in loads:
        load.start()
    arrival.wait()
    wide = tokens[...].astype(f32)
    inverse = lax.rsqrt(jnp.mean(wide * wide, axis=1, keepdims=True) + SMALL_CONSTANT)
    rows_all[mine] = (wide * inverse * gain[...].astype(f32).reshape(1, -1)).astype(bf16)
    small[QUERY_PART:width] = jnp.zeros((width - QUERY_PART, small.shape[1]), bf16)

    greeted()
    gather = TpGather(rows_all, row_send, row_recv)
    gather.start()

    for load in loads:
        load.wait()
    small[QUERY_PART : QUERY_PART + 8] = ingate[...]
    small[QUERY_PART + 16 : QUERY_PART + 24] = forget[...]
    up_query[...] = jnp.zeros(up_query.shape, bf16)
    query_rows = query_up[...].astype(f32).T.astype(bf16)
    for s in range(N_Y * N_C):
        up_query[s * width : s * width + QUERY_PART] = query_rows[
            s * QUERY_PART : (s + 1) * QUERY_PART
        ]
        part = slice(s * LATENT_PART, (s + 1) * LATENT_PART)
        for h in range(2):
            at = s * width + h * LATENT_PART
            up_latent[at : at + LATENT_PART, :width] = key_up[part]
            up_latent[at : at + LATENT_PART, width:] = value_up[part]

    lane = lax.broadcasted_iota(jnp.int32, (1, width), 1)
    cosine, sine_part = (
        jnp.concatenate([ref[...]] * 4, axis=0).T for ref in (cosine_row, sine_row)
    )
    row_id = lax.broadcasted_iota(jnp.int32, (width, width), 0)
    col_id = lax.broadcasted_iota(jnp.int32, (width, width), 1)
    channels = lax.rem(col_id, ROTARY_CHANNELS)
    halfway = ROTARY_CHANNELS // 2
    twin = (row_id == channels).astype(bf16)
    partner = lax.rem(channels + halfway, ROTARY_CHANNELS)
    sign = jnp.where(channels < halfway, -1.0, 1.0)

    def duplicated(values, offset):
        return jnp.dot(
            values, (row_id == channels + offset).astype(bf16), preferred_element_type=f32
        )

    def rotated(values, offset):
        swap = jnp.where(row_id == partner + offset, sign, 0.0).astype(bf16)
        turned = jnp.dot(values, swap, preferred_element_type=f32)
        return duplicated(values, offset) * cosine + turned * sine_part

    def chip_rows(chip):
        slots = [rows_all[chip * N_C + k] for k in range(N_C)]
        return jnp.concatenate(slots, axis=0)

    span = N_C * SHARE
    tile = 256

    def project_small(chip):
        rows = pl.ds(pl.multiple_of(chip * span, span), span)
        here = chip_rows(chip)
        made = lax.dot_general(here, small[...], CONTRACT_LAST, preferred_element_type=f32)
        turned = made[:, :width].T
        for k in range(2):
            at = QUERY_PART + 16 * k
            pre_gates[k, :, rows] = turned[at : at + 8]
        rounded = made.astype(bf16)
        query_latents[mine, rows] = rounded[:, :width]
        wide_latent[rows, :width] = rounded[:, width:]

    def project_big():
        def one(t, carry):
            columns = pl.ds(pl.multiple_of(t * tile, tile), tile)
            rows = rows_all[...].reshape(ROWS, rows_all.shape[2])
            made = jnp.dot(rows, big[:, columns], preferred_element_type=f32)
            mem_ref[:, columns] = made.astype(bf16)
            return carry

        lax.fori_loop(0, big.shape[1] // tile, one, 0)

    gather.relay()
    gather.near()
    near = [y, lax.rem(y + N_Y - 1, N_Y), lax.rem(y + 1, N_Y)]
    for chip in near:
        project_small(chip)
    opposite = lax.rem(y + 2, N_Y)
    gather.far()
    project_small(opposite)

    second = wide_latent[:, :width]
    both = duplicated(second, 0)
    half = ROWS // 2
    packed = jnp.where(lane < LATENT_PART, both[:half], both[half:])
    latents[mine] = packed.astype(bf16)
    exchange = TpGather(latents, lat_send, lat_recv)
    query_exchange = TpGather(query_latents, query_send, query_recv)
    exchange.start()
    query_exchange.start()
    project_big()
    heads = lax.broadcasted_iota(jnp.int32, (8, ROWS), 0) == mine
    in_pre, forget_pre = (
        jnp.sum(jnp.where(heads, pre_gates[k], 0.0), axis=0, keepdims=True) for k in range(2)
    )
    in_gate = SOFTCAP * jnp.tanh(in_pre / SOFTCAP)
    capped = SOFTCAP * jnp.tanh((forget_pre + shift_row[...]) / SOFTCAP)
    small_part = jnp.exp(-jnp.abs(capped))
    above_one = 1.0 + small_part
    grown = jnp.where(
        above_one == 1.0, small_part, jnp.log(above_one) * small_part / (above_one - 1.0)
    )
    log_forget = jnp.minimum(capped, 0.0) - grown
    earlier = lax.broadcasted_iota(jnp.int32, (ROWS, ROWS), 0) <= lax.broadcasted_iota(
        jnp.int32, (ROWS, ROWS), 1
    )
    cumulative = jnp.dot(
        jnp.broadcast_to(log_forget, (8, ROWS)),
        earlier.astype(f32),
        precision=PRECISE,
        preferred_element_type=f32,
    )
    top_rows = lax.broadcasted_iota(jnp.int32, (8, ROWS), 0) == 0
    gate_ref[...] = jnp.where(top_rows, in_gate - cumulative, cumulative)
    after_gates()
    exchange.relay()
    query_exchange.relay()
    key_turned = rotated(second, LATENT_PART)
    kv_ref[2 * ROWS :] = jnp.where(
        lane < ROTARY_CHANNELS, key_turned[:half], key_turned[half:]
    ).astype(bf16)
    exchange.near()
    after_exchange()
    exchange.far()

    squares = jnp.zeros((half, width), f32)
    for s in range(N_Y * N_C):
        part = latents[s].astype(f32)
        squares = squares + part * part
    low = lane < LATENT_PART
    low_scale, high_scale = (
        lax.rsqrt(
            jnp.sum(jnp.where(low == first, squares, 0.0), axis=1, keepdims=True) / LATENT_WIDTH
            + SMALL_CONSTANT
        )
        for first in (True, False)
    )
    latent_scale = jnp.where(low, low_scale, high_scale)
    query_gains = jnp.broadcast_to(query_gain[...].reshape(1, -1), (8, QUERY_LATENT))
    latent_gains = jnp.broadcast_to(latent_gain[...].reshape(1, -1), (8, LATENT_WIDTH))

    def latent_gain_of(s):
        pair = slice((s // 2) * width, (s // 2 + 1) * width)
        shift = LATENT_WIDTH - LATENT_PART if s % 2 else LATENT_PART
        here = latent_gains[:1, pair]
        other = pltpu.roll(latent_gains, shift, 1)[:1, pair]
        return jnp.where(low, other, here) if s % 2 else jnp.where(low, here, other)

    def query_gain_of(s):
        turned = query_gains
        if s:
            turned = pltpu.roll(query_gains, QUERY_LATENT - s * QUERY_PART, 1)
        return turned[:1, :width]

    for s in range(N_Y * N_C):
        columns = slice(s * width, (s + 1) * width)
        part = latents[s].astype(f32)
        made = (part * latent_scale * latent_gain_of(s)).astype(bf16)
        wide_latent[:half, columns] = jnp.where(low, made, jnp.zeros_like(made))
        wide_latent[half:, columns] = jnp.where(low, jnp.zeros_like(made), made)
    made = jnp.dot(wide_latent[...], up_latent[...], preferred_element_type=f32).astype(bf16)
    kv_ref[:ROWS] = made[:, :width]
    kv_ref[ROWS : 2 * ROWS] = made[:, width:]
    after_keys()

    query_exchange.near()
    query_exchange.far()
    query_mask = (lane < QUERY_PART).astype(f32)
    squares = jnp.zeros((ROWS, width), f32)
    for s in range(N_Y * N_C):
        part = query_latents[s].astype(f32) * query_mask
        squares = squares + part * part
    query_scale = lax.rsqrt(
        jnp.sum(squares, axis=1, keepdims=True) / QUERY_LATENT + SMALL_CONSTANT
    )
    for s in range(N_Y * N_C):
        columns = slice(s * width, (s + 1) * width)
        part = query_latents[s].astype(f32) * query_mask
        wide_query[:, columns] = (part * query_scale * query_gain_of(s)).astype(bf16)
    made = jnp.dot(wide_query[...], up_query[...], preferred_element_type=f32).astype(bf16)
    q_ref[:, :width] = made[:, :width]
    turning = jnp.concatenate([made[:, width:], jnp.zeros((ROWS, ROTARY_CHANNELS), bf16)], axis=1)
    q_ref[:, width:] = rotated(turning, 0).astype(bf16)
    return gather.started + exchange.started + query_exchange.started


def output_phase(
    gated,
    attended,
    out_memory,
    out_attend,
    o_ref,
    to_core,
    from_core,
    sums,
    passing,
    from_below,
    from_above,
    relay_in,
    core_send,
    core_recv,
    relay_send,
    relay_recv,
    up_send,
    up_recv,
    down_send,
    down_recv,
):
    f32, bf16 = jnp.float32, jnp.bfloat16
    y, c = lax.axis_index("y"), lax.axis_index("c")
    above, below = lax.rem(y + 1, N_Y), lax.rem(y + N_Y - 1, N_Y)
    opposite = lax.rem(y + 2, N_Y)
    half = out_memory.shape[1] // 2
    tile = 512

    def remote(source, target, send, recv, device):
        return pltpu.make_async_remote_copy(
            src_ref=source,
            dst_ref=target,
            send_sem=send,
            recv_sem=recv,
            device_id=device,
            device_id_type=MESH_ID,
        )

    def rows_of(ref, core):
        picked = [ref[pl.ds(pl.multiple_of((k * N_C + core) * SHARE, SHARE), SHARE)] for k in range(N_Y)]
        return jnp.concatenate(picked, axis=0)

    def partial(core, h, store):
        memory_rows, attend_rows = rows_of(gated, core), rows_of(attended, core)
        for t in range(half // tile):
            columns = slice(h * half + t * tile, h * half + (t + 1) * tile)
            made = jnp.dot(memory_rows, out_memory[:, columns], preferred_element_type=f32)
            made = made + jnp.dot(attend_rows, out_attend[:, columns], preferred_element_type=f32)
            store(t * tile, made.astype(bf16).reshape(N_Y, SHARE, tile))

    def core_copy(h):
        return remote(
            to_core.at[h], from_core.at[h], core_send.at[h], core_recv.at[h], {"c": 1 - c}
        )

    def relay_copy(h):
        return remote(
            passing.at[h],
            relay_in.at[h],
            relay_send.at[h],
            relay_recv.at[h],
            {"y": above if h == 0 else below},
        )

    def up_copy(h):
        return remote(
            passing.at[2 + h], from_below.at[h], up_send.at[h], up_recv.at[h], {"y": above}
        )

    def down_copy(h):
        return remote(
            passing.at[4 + h], from_above.at[h], down_send.at[h], down_recv.at[h], {"y": below}
        )

    started = []

    def start(copy):
        copy.start()
        started.append(copy)

    for h in range(2):

        def keep(at, block, h=h):
            to_core[h, :, :, at : at + tile] = block

        partial(1 - c, h, keep)
        start(core_copy(h))
    for h in range(2):

        def keep(at, block, h=h):
            sums[h, :, :, at : at + tile] = block.astype(f32)

        partial(c, h, keep)
    for h in range(2):
        core_copy(h).wait_recv()
        sums[h] = sums[h] + from_core[h].astype(f32)
        passing[h] = sums[h, opposite].astype(bf16)
        start(relay_copy(h))
        if h == 0:
            passing[4] = sums[0, below].astype(bf16)
            start(down_copy(0))
        else:
            passing[3] = sums[1, above].astype(bf16)
            start(up_copy(1))
    relay_copy(0).wait_recv()
    passing[2] = (sums[0, above] + relay_in[0].astype(f32)).astype(bf16)
    start(up_copy(0))
    relay_copy(1).wait_recv()
    passing[5] = (sums[1, below] + relay_in[1].astype(f32)).astype(bf16)
    start(down_copy(1))
    for h in (1, 0):
        up_copy(h).wait_recv()
        down_copy(h).wait_recv()
        made = sums[h, y] + from_below[h].astype(f32) + from_above[h].astype(f32)
        o_ref[:, h * half : (h + 1) * half] = made.astype(bf16)
    return started


def scratch(depth, mem_width):
    f32, bf16 = jnp.float32, jnp.bfloat16
    dma = pltpu.SemaphoreType.DMA
    between = (
        pltpu.VMEM((ROWS, VALUE_CHANNELS), bf16),
        pltpu.VMEM((ROWS, M_V), bf16),
        pltpu.VMEM((ROWS, mem_width), bf16),
        pltpu.VMEM((8, ROWS), f32),
        pltpu.VMEM((ROWS, 256), bf16),
        pltpu.VMEM((ROWS * 5 // 2, 128), bf16),
        pltpu.VMEM((M_V, depth), bf16),
        pltpu.VMEM((VALUE_CHANNELS, depth), bf16),
        dma((2,)),
    )
    for_project = (
        pltpu.VMEM((N_Y * N_C, SHARE, depth), bf16),
        pltpu.VMEM((N_Y * N_C, ROWS, 128), bf16),
        pltpu.VMEM((N_Y * N_C, ROWS // 2, 128), bf16),
        pltpu.VMEM((256, depth), bf16),
        pltpu.VMEM((8, depth), bf16),
        pltpu.VMEM((8, depth), bf16),
        pltpu.VMEM((depth, mem_width), bf16),
        pltpu.VMEM((PLAIN_CHANNELS + ROTARY_CHANNELS, QUERY_LATENT), bf16),
        pltpu.VMEM((LATENT_WIDTH, PLAIN_CHANNELS), bf16),
        pltpu.VMEM((LATENT_WIDTH, VALUE_CHANNELS), bf16),
        pltpu.VMEM((SHARE, depth), bf16),
        pltpu.VMEM((1, ROWS), f32),
        pltpu.VMEM((2, 8, ROWS), f32),
        pltpu.VMEM((1024, PLAIN_CHANNELS + ROTARY_CHANNELS), bf16),
        pltpu.VMEM((1024, 256), bf16),
        pltpu.VMEM((ROWS, 1024), bf16),
        pltpu.VMEM((ROWS, 1024), bf16),
        dma((16,)),
        dma((11,)),
        dma((11,)),
        dma((11,)),
        dma((11,)),
        dma((11,)),
        dma((11,)),
    )
    for_attend = (
        pltpu.VMEM((N_X, ROWS, 256), bf16),
        pltpu.VMEM((N_Z, ROWS * 5 // 2, 128), bf16),
        pltpu.VMEM((ROWS, 256), bf16),
        pltpu.VMEM((N_X * ROWS, 128), f32),
        pltpu.VMEM((N_X * ROWS, 128), f32),
        pltpu.VMEM((N_X * ROWS, VALUE_CHANNELS), f32),
        pltpu.VMEM((N_X - 1, ROWS, VALUE_CHANNELS), bf16),
        pltpu.VMEM((N_X - 1, 8, ROWS), f32),
        pltpu.VMEM((N_X - 1, ROWS, VALUE_CHANNELS), bf16),
        pltpu.VMEM((N_X - 1, 8, ROWS), f32),
        pltpu.VMEM((ROWS, M_V), f32),
        pltpu.VMEM((ROWS, 128), f32),
        pltpu.VMEM((ROWS, 128), f32),
        pltpu.VMEM((N_X, STATE_ROWS, M_V), f32),
        pltpu.VMEM((N_X, STATE_ROWS, M_V), f32),
        pltpu.VMEM((STATE_ROWS, M_V), f32),
        pltpu.VMEM((N_Z, STATE_ROWS, M_V), f32),
        pltpu.VMEM((N_X, STATE_ROWS, M_V), f32),
        pltpu.VMEM((N_X, STATE_ROWS, M_V), f32),
        pltpu.VMEM((2, 8, ROWS), f32),
        pltpu.VMEM((N_Y, 8, ROWS), f32),
        pltpu.VMEM((2, ROWS // 2, VALUE_CHANNELS), bf16),
        dma((6,)),
        dma((6,)),
        dma((N_Z // 2, 2)),
        dma((N_Z // 2, 2)),
        dma((N_Z // 2, 2)),
        dma((N_Z // 2, 2)),
        dma((N_X - 1,)),
        dma((N_X - 1,)),
        dma((N_X - 1,)),
        dma((N_X - 1,)),
        dma((N_X - 1,)),
        dma((N_X - 1,)),
        dma((N_Z,)),
        dma((N_Z,)),
        dma((N_X - 1,)),
        dma((N_X - 1,)),
        dma((N_Y,)),
        dma((N_Y,)),
        dma((2, 2)),
        dma((2, 2)),
    )
    for_output = (
        pltpu.VMEM((2, N_Y, SHARE, depth // 2), bf16),
        pltpu.VMEM((2, N_Y, SHARE, depth // 2), bf16),
        pltpu.VMEM((2, N_Y, SHARE, depth // 2), f32),
        pltpu.VMEM((6, SHARE, depth // 2), bf16),
        pltpu.VMEM((2, SHARE, depth // 2), bf16),
        pltpu.VMEM((2, SHARE, depth // 2), bf16),
        pltpu.VMEM((2, SHARE, depth // 2), bf16),
        dma((2,)),
        dma((2,)),
        dma((2,)),
        dma((2,)),
        dma((2,)),
        dma((2,)),
        dma((2,)),
        dma((2,)),
    )
    return between, for_project, for_attend, for_output


N_INPUTS = 22
N_PROJECT_INPUTS = 19
IN_VMEM = (1, 2, 3, 4, 5, 19)


def layer_kernel(counts, *refs):
    y, c = lax.axis_index("y"), lax.axis_index("c")
    z, x = lax.axis_index("z"), lax.axis_index("x")
    project_inputs = refs[:N_PROJECT_INPUTS]
    mem_gain, out_memory_hbm, out_attend_hbm, out_ref = refs[N_PROJECT_INPUTS : N_INPUTS + 1]
    groups, at = [], N_INPUTS + 1
    for count in counts:
        groups.append(refs[at : at + count])
        at += count
    between, for_project, for_attend, for_output = groups
    attended, gated, mem, gates, queries, keys_values, out_memory, out_attend, out_sem = between

    barrier = pltpu.get_barrier_semaphore()
    devices = [{"c": 1 - c}]
    devices += [{"y": lax.rem(y + d, N_Y)} for d in range(1, N_Y)]
    devices += [{"x": lax.rem(x + d, N_X)} for d in range(1, N_X)]
    devices += [{"z": lax.rem(z + d, N_Z)} for d in range(1, N_Z)]
    for device in devices:
        pl.semaphore_signal(barrier, inc=1, device_id=device, device_id_type=MESH_ID)
    loads = [
        pltpu.make_async_copy(out_memory_hbm, out_memory, out_sem.at[0]),
        pltpu.make_async_copy(out_attend_hbm, out_attend, out_sem.at[1]),
    ]
    attending = attend_phase(
        queries, keys_values, mem, gates, mem_gain, attended, gated, *for_attend
    )
    started = project_phase(
        lambda: pl.semaphore_wait(barrier, len(devices)),
        *[lambda: next(attending)] * 3,
        *project_inputs,
        mem,
        gates,
        queries,
        keys_values,
        *for_project,
    )
    for load in loads:
        load.start()
    more, finish_columns = next(attending)
    started += more
    for load in loads:
        load.wait()
    started += output_phase(gated, attended, out_memory, out_attend, out_ref, *for_output)
    for copy in started:
        copy.wait_send()
    finish_columns()


def layer(*inputs):
    depth = inputs[0].shape[1]
    mem_width = 2 * M_QK + 2 * M_V
    groups = scratch(depth, mem_width)
    vmem = pl.BlockSpec(memory_space=pltpu.VMEM)
    hbm = pl.BlockSpec(memory_space=pltpu.HBM)
    return pl.pallas_call(
        functools.partial(layer_kernel, tuple(len(group) for group in groups)),
        out_shape=jax.ShapeDtypeStruct((SHARE, depth), jnp.bfloat16),
        in_specs=[vmem if k in IN_VMEM else hbm for k in range(N_INPUTS)],
        out_specs=vmem,
        scratch_shapes=[one for group in groups for one in group],
        compiler_params=pltpu.CompilerParams(
            collective_id=1, has_side_effects=True, vmem_limit_bytes=67_000_000
        ),
        cost_estimate=pl.CostEstimate(
            flops=8 * 10**9, bytes_accessed=2 * 10**7, transcendentals=4 * 10**6
        ),
        name="layer",
    )(*inputs)


def per_device(
    tokens,
    input_gain,
    weight_query,
    weight_key,
    weight_value,
    weight_outgate,
    weight_ingate,
    weight_forget,
    forget_shift,
    mem_gain,
    query_down_weight,
    latent_down_weight,
    down_rotary,
    query_gain,
    latent_gain,
    query_up_weight,
    key_up_weight,
    value_up_weight,
    out_memory,
    out_attend,
):
    length = forget_shift.shape[0]
    positions = lax.axis_index(SP) * length + jnp.arange(length, dtype=jnp.int32)
    halfway = ROTARY_CHANNELS // 2
    inverse = jnp.power(ROTARY_BASE, -jnp.arange(halfway, dtype=jnp.float32) / halfway)
    angles = positions.astype(jnp.float32)[None, :] * inverse[:, None]
    return layer(
        tokens,
        input_gain,
        query_gain,
        latent_gain,
        jnp.cos(angles),
        jnp.sin(angles),
        forget_shift.T,
        query_down_weight.T,
        latent_down_weight.T,
        down_rotary.T,
        weight_ingate.T,
        weight_forget.T,
        weight_query,
        weight_key,
        weight_value,
        weight_outgate,
        query_up_weight.T,
        key_up_weight,
        value_up_weight,
        mem_gain,
        out_memory,
        out_attend,
    )


def solution(mesh):
    torus = Mesh(mesh.devices.reshape(N_Z, N_X, 4, 2), SP_TP)
    in_specs = (
        P(SP_TP, None),
        P(),
        P(None, TP),
        P(None, TP),
        P(None, TP),
        P(None, TP),
        P(),
        P(),
        P(SP, TP),
        P(),
        P(None, TP),
        P(None, TP),
        P(),
        P(),
        P(),
        P(None, TP),
        P(None, TP),
        P(None, TP),
        P(TP, None),
        P(TP, None),
    )
    out_specs = P(SP_TP, None)
    return jax.shard_map(
        per_device, mesh=torus, in_specs=in_specs, out_specs=out_specs, check_vma=False
    )
```

```python
import functools

import jax
import jax.numpy as jnp
from jax import lax
from jax.experimental import pallas as pl
from jax.experimental.pallas import tpu as pltpu
from jax.sharding import Mesh
from jax.sharding import PartitionSpec as P

MEMORY_HEADS = 8
M_QK = 128
M_V = 256
PLAIN_CHANNELS = 128
ROTARY_CHANNELS = 64
VALUE_CHANNELS = 128
SP = ("z", "x")
TP = ("y", "c")
SP_TP = ("z", "x", "y", "c")


SMALL_CONSTANT = 1e-06
SOFTCAP = 15.0
ROTARY_BASE = 10000.0
PRECISE = lax.Precision.HIGHEST
FAR_BELOW = -1e30

N_Y = 4
N_C = 2
SHARE = 64
QUERY_LATENT = 768
LATENT_WIDTH = 512
QUERY_PART = QUERY_LATENT // (N_Y * N_C)
LATENT_PART = LATENT_WIDTH // (N_Y * N_C)
LOG2E = 1.4426950408889634
N_Z = 8
N_X = 4
ROWS = 512
MESH_ID = pl.DeviceIdType.MESH
CONTRACT_LAST = (((1,), (1,)), ((), ()))
CHUNK = M_QK // N_X
TALL = 512
GROUP = 1
STATE_ROWS = CHUNK + 8
NORMAL_ROW, TOP_ROW, DECAY_ROW = CHUNK, CHUNK + 1, CHUNK + 2


def merge_states(early, late):
    moved = early[TOP_ROW : TOP_ROW + 1] + late[DECAY_ROW : DECAY_ROW + 1]
    late_top = late[TOP_ROW : TOP_ROW + 1]
    joined = jnp.maximum(moved, late_top)
    both = early * jnp.exp(moved - joined) + late * jnp.exp(late_top - joined)
    row = lax.broadcasted_iota(jnp.int32, both.shape, 0)
    decay = early[DECAY_ROW : DECAY_ROW + 1] + late[DECAY_ROW : DECAY_ROW + 1]
    return jnp.where(row == TOP_ROW, joined, jnp.where(row == DECAY_ROW, decay, both))


def in_two(values):
    high = values.astype(jnp.bfloat16)
    return high, (values - high.astype(jnp.float32)).astype(jnp.bfloat16)


def as_columns(row, width):
    return jnp.broadcast_to(row, (width, row.shape[1])).T


def attend_phase(
    q_ref,
    kv_ref,
    mem_ref,
    gate_ref,
    gain_ref,
    attended_ref,
    gated_ref,
    q_all,
    kv_all,
    k_cat,
    top,
    total,
    accum,
    part_out,
    stat_out,
    part_in,
    stat_in,
    cell,
    cell_sum,
    cell_top,
    first_out,
    first_in,
    column_out,
    column_in,
    start_out,
    start_in,
    square_out,
    square_in,
    passed,
    q_send,
    q_recv,
    up_send,
    up_recv,
    down_send,
    down_recv,
    part_send,
    part_recv,
    stat_send,
    stat_recv,
    first_send,
    first_recv,
    column_send,
    column_recv,
    start_send,
    start_recv,
    square_send,
    square_recv,
    passed_send,
    passed_recv,
):
    f32, bf16 = jnp.float32, jnp.bfloat16
    z, x = lax.axis_index("z"), lax.axis_index("x")
    y, c = lax.axis_index("y"), lax.axis_index("c")
    above, below = lax.rem(z + 1, N_Z), lax.rem(z + N_Z - 1, N_Z)
    peers = [lax.rem(x + d, N_X) for d in range(1, N_X)]
    right, left = peers[0], peers[-1]
    rows_y = [lax.rem(y + d, N_Y) for d in range(1, N_Y)]
    me_tp = y * N_C + c
    half = kv_ref.shape[0] // 2
    width = PLAIN_CHANNELS

    def remote(source, target, send, recv, device):
        return pltpu.make_async_remote_copy(
            src_ref=source,
            dst_ref=target,
            send_sem=send,
            recv_sem=recv,
            device_id=device,
            device_id_type=MESH_ID,
        )

    def kv_copy(up, step, h):
        shift = (N_Z - step + 1) if up else (step - 1)
        owner = lax.rem(z + shift, N_Z)
        rows = pl.ds(h * half, half)
        source = kv_ref.at[rows] if step == 1 else kv_all.at[owner, rows]
        send, recv = (up_send, up_recv) if up else (down_send, down_recv)
        return remote(
            source,
            kv_all.at[owner, rows],
            send.at[step - 1, h],
            recv.at[step - 1, h],
            {"z": above if up else below},
        )

    q_half = ROWS // 2

    def q_copy(number):
        shift, part, to_right = (
            (0, 0, True),
            (0, 1, True),
            (0, 0, False),
            (0, 1, False),
            (N_X - 1, 0, True),
            (1, 1, False),
        )[number]
        owner = lax.rem(x + shift, N_X)
        rows = pl.ds(part * q_half, q_half)
        source = q_ref.at[rows] if shift == 0 else q_all.at[owner, rows]
        return remote(
            source,
            q_all.at[owner, rows],
            q_send.at[number],
            q_recv.at[number],
            {"x": right if to_right else left},
        )

    def part_copy(d):
        return remote(
            part_out.at[d], part_in.at[d], part_send.at[d], part_recv.at[d], {"x": peers[d]}
        )

    def far_copy(h, hop):
        rows = pl.ds(h * q_half, q_half)
        return remote(
            part_out.at[1, rows] if hop == 0 else passed.at[h],
            passed.at[h] if hop == 0 else part_in.at[1, rows],
            passed_send.at[hop, h],
            passed_recv.at[hop, h],
            {"x": right if h == 0 else left},
        )

    def stat_copy(d):
        return remote(
            stat_out.at[d], stat_in.at[d], stat_send.at[d], stat_recv.at[d], {"x": peers[d]}
        )

    def first_copy(d):
        return remote(
            first_out.at[peers[d]],
            first_in.at[x],
            first_send.at[d],
            first_recv.at[d],
            {"x": peers[d]},
        )

    def column_copy(target):
        return remote(
            column_out,
            column_in.at[z],
            column_send.at[target],
            column_recv.at[z],
            {"z": target},
        )

    def column_arrival(source):
        return remote(
            column_out,
            column_in.at[source],
            column_send.at[source],
            column_recv.at[source],
            {"z": source},
        )

    def start_copy(d):
        return remote(
            start_out.at[peers[d]],
            start_in.at[x],
            start_send.at[d],
            start_recv.at[d],
            {"x": peers[d]},
        )

    def square_copy(number):
        device = {"c": 1 - c} if number == 0 else {"y": rows_y[number - 1]}
        return remote(
            square_out.at[min(number, 1)],
            square_in.at[number],
            square_send.at[number],
            square_recv.at[number],
            device,
        )

    started = []

    def start(copy):
        copy.start()
        started.append(copy)

    relative, cumulative = gate_ref[0:1], gate_ref[1:2]
    key_scale = M_QK ** (-0.5)
    tall = 256
    for t in range(ROWS // tall):
        rows, seen = slice(t * tall, (t + 1) * tall), (t + 1) * tall
        row = lax.broadcasted_iota(jnp.int32, (tall, seen), 0) + t * tall
        col = lax.broadcasted_iota(jnp.int32, (tall, seen), 1)
        logs = jnp.where(col <= row, relative[:, :seen], -jnp.inf)
        highest = jnp.max(logs, axis=1, keepdims=True)
        affinity = lax.dot_general(
            mem_ref[rows, :M_QK],
            mem_ref[:seen, M_QK : 2 * M_QK],
            CONTRACT_LAST,
            preferred_element_type=f32,
        )
        affinity = affinity * (jnp.exp(logs - highest) * key_scale)
        values = mem_ref[:seen, 2 * M_QK : 2 * M_QK + M_V]
        cell[rows] = sum(
            jnp.dot(piece, values, preferred_element_type=f32) for piece in in_two(affinity)
        )
        cell_sum[rows] = jnp.broadcast_to(
            jnp.sum(affinity, axis=1, keepdims=True), (tall, width)
        )
        cell_top[rows] = jnp.broadcast_to(highest, (tall, width))
    ends_at = jnp.max(relative, axis=1, keepdims=True)
    weights = jnp.exp(relative - ends_at) * key_scale
    wide_key = mem_ref[:, M_QK : 2 * M_QK].astype(f32)
    normal = jnp.sum(as_columns(weights, width) * wide_key, axis=0, keepdims=True)
    values = mem_ref[:, 2 * M_QK : 2 * M_QK + M_V]
    matrix = sum(
        jnp.dot(piece, values, preferred_element_type=f32)
        for piece in in_two(wide_key.T * weights)
    )
    decay = cumulative[:, ROWS - 1 : ROWS]
    row = lax.broadcasted_iota(jnp.int32, (8, M_V), 0)
    lines = jnp.concatenate([normal, jnp.zeros_like(normal)], axis=1)
    notes = jnp.where(
        row == 0, lines, jnp.where(row == 1, ends_at + decay, jnp.where(row == 2, decay, 0.0))
    )
    for k in range(N_X):
        first_out[k, :CHUNK] = matrix[k * CHUNK : (k + 1) * CHUNK]
        first_out[k, CHUNK:] = notes
    for d in range(N_X - 1):
        start(first_copy(d))
    first_in[x] = first_out[x]

    yield

    for d in range(N_X - 1):
        first_copy(d).wait_recv()
    column = first_in[0]
    for k in range(1, N_X):
        column = merge_states(column, first_in[k])
    column_out[...] = column
    for target in range(1, N_Z):

        @pl.when(target > z)
        def _(target=target):
            column_copy(target).start()

    yield

    for h in range(2):
        for up in (True, False):
            start(kv_copy(up, 1, h))
    yield

    top[...] = jnp.full(top.shape, FAR_BELOW, f32)
    total[...] = jnp.zeros(total.shape, f32)
    for number in (0, 3, 1, 2):
        start(q_copy(number))
    accum[...] = jnp.zeros(accum.shape, f32)
    q_all[x] = q_ref[...]

    lane = lax.broadcasted_iota(jnp.int32, (ROWS // 2, width), 1)
    low = (lane < ROTARY_CHANNELS).astype(bf16)
    high = (lane >= ROTARY_CHANNELS).astype(bf16)
    scale = LOG2E * (PLAIN_CHANNELS + ROTARY_CHANNELS) ** (-0.5)

    def keys_from(ref):
        k_cat[:, :width] = ref[:ROWS]
        packed = ref[2 * ROWS :]
        k_cat[: ROWS // 2, width:] = packed * low
        k_cat[ROWS // 2 :, width:] = packed * high

    def attend_tile(t, keys, values, masked):
        shard = t // (ROWS // TALL)
        rows = pl.ds(pl.multiple_of(t * TALL, TALL), TALL)
        inner = pl.ds(pl.multiple_of((t % (ROWS // TALL)) * TALL, TALL), TALL)
        scores = lax.dot_general(
            q_all[shard, inner], keys, CONTRACT_LAST, preferred_element_type=f32
        )
        scores = scores * scale
        if masked:
            row = lax.broadcasted_iota(jnp.int32, scores.shape, 0) + t * TALL
            col = lax.broadcasted_iota(jnp.int32, scores.shape, 1) + x * ROWS
            scores = jnp.where(col <= row, scores, -jnp.inf)
        old = top[rows]
        new = jnp.maximum(old, jnp.max(scores, axis=1, keepdims=True))
        probs = jnp.exp2(scores - jnp.concatenate([new] * (ROWS // width), axis=1))
        shrink = jnp.exp2(old - new)
        added = sum(probs[:, k : k + width] for k in range(0, ROWS, width))
        total[rows] = total[rows] * shrink + added
        accum[rows] = accum[rows] * shrink + jnp.dot(
            probs.astype(bf16), values, preferred_element_type=f32
        )
        top[rows] = new

    def attend_rows(first, last, values, masked):
        def one(g, carry):
            for u in range(GROUP):
                attend_tile(g * GROUP + u, k_cat[...], values(), masked)
            return carry

        lax.fori_loop(first, last, one, 0)

    last = N_Z // 2
    steps = ROWS // (TALL * GROUP)

    def arrived(owner, useful):
        @pl.when(useful)
        def _():
            keys_from(kv_all.at[owner])
            attend_rows(0, N_X * steps, lambda: kv_all[owner, ROWS : 2 * ROWS], False)

    def take(step, h):
        for up in (True, False):
            if step == last and up != (h == 0):
                continue
            kv_copy(up, step, h).wait_recv()
            if step < last - 1 or (step == last - 1 and up == (h == 0)):
                start(kv_copy(up, step + 1, h))

    def use_up(step):
        arrived(lax.rem(z + N_Z - step, N_Z), z >= step)

    def use_down(step):
        arrived(lax.rem(z + step, N_Z), z + step >= N_Z)

    keys_from(kv_ref)
    own_values = lambda: kv_ref[ROWS : 2 * ROWS]
    attend_rows(x * steps, (x + 1) * steps, own_values, True)

    take(1, 0)
    q_copy(0).wait_recv()
    start(q_copy(4))
    q_copy(3).wait_recv()
    start(q_copy(5))

    def gather_column(k, state):
        column_arrival(k).wait_recv()
        return merge_states(state, column_in[k])

    state = lax.fori_loop(0, z, gather_column, jnp.zeros((STATE_ROWS, M_V), f32))
    for k in range(N_X):
        start_out[k] = state
        if k < N_X - 1:
            state = merge_states(state, first_in[k])
    for d in range(N_X - 1):
        start(start_copy(d))
    start_in[x] = start_out[x]
    take(1, 1)
    for number in (1, 2, 4, 5):
        q_copy(number).wait_recv()
    attend_rows((x + 1) * steps, N_X * steps, own_values, False)
    take(2, 0)
    use_up(1)
    take(2, 1)
    use_down(1)

    for d in range(N_X - 1):
        start_copy(d).wait_recv()
    carried = jnp.concatenate([start_in[k, :CHUNK] for k in range(N_X)], axis=0)
    carried_normal = start_in[0, NORMAL_ROW : NORMAL_ROW + 1, :M_QK]
    carried_top = start_in[0, TOP_ROW : TOP_ROW + 1, :width]
    queries = mem_ref[:, :M_QK]
    from_start = sum(
        jnp.dot(queries, piece, preferred_element_type=f32) for piece in in_two(carried)
    )
    highest = jnp.maximum(carried_top, cell_top[...])
    across, within = jnp.exp(carried_top - highest), jnp.exp(cell_top[...] - highest)
    twice = lambda one: jnp.concatenate([one, one], axis=1)
    numerator = cell[...] * twice(within) + from_start * twice(across)
    denominator = cell_sum[...] * within + across * jnp.sum(
        queries.astype(f32) * carried_normal, axis=1, keepdims=True
    )
    floor = jnp.exp(-(as_columns(cumulative, width) + highest))
    made = numerator / twice(jnp.maximum(jnp.abs(denominator), floor))
    cell[...] = made
    squares = jnp.sum(made * made, axis=1, keepdims=True)
    square_out[0] = jnp.broadcast_to(squares, (ROWS, width)).T[:8]
    start(square_copy(0))

    take(3, 0)
    use_up(2)
    square_copy(0).wait_recv()
    square_out[1] = square_out[0] + square_in[0]
    for number in range(1, N_Y):
        start(square_copy(number))
    take(3, 1)
    use_down(2)
    use_up(3)
    use_down(3)

    squares = square_out[1]
    for number in range(1, N_Y):
        square_copy(number).wait_recv()
        squares = squares + square_in[number]
    inverse = lax.rsqrt(squares[:1] / (MEMORY_HEADS * M_V) + SMALL_CONSTANT)
    gated = cell[...] * twice(as_columns(inverse, width)) * gain_ref[pl.ds(pl.multiple_of(me_tp * M_V, M_V), M_V)].astype(f32).reshape(1, M_V)
    gated = gated * jax.nn.sigmoid(mem_ref[:, 2 * M_QK + M_V :].astype(f32))
    gated_ref[...] = gated.astype(bf16)
    yield

    take(4, 0)
    take(4, 1)

    opposite = lax.rem(z + last, N_Z)

    @pl.when(z >= last)
    def _():
        keys_from(kv_all.at[opposite])

    def finish(shard):
        @pl.when(z >= last)
        def _():
            attend_rows(
                shard * steps,
                (shard + 1) * steps,
                lambda: kv_all[opposite, ROWS : 2 * ROWS],
                False,
            )

        rows = pl.ds(pl.multiple_of(shard * ROWS, ROWS), ROWS)
        summed = jnp.sum(total[rows], axis=1, keepdims=True)
        seen = summed > 0.0
        summed = jnp.maximum(summed, 1.0)
        log_total = jnp.where(seen, top[rows] + jnp.log2(summed), FAR_BELOW)
        return accum[rows] / summed, log_total

    for d in (1, 0, 2):
        part, log_total = finish(peers[d])
        part_out[d] = part.astype(bf16)
        stat_out[d] = log_total.T[:8]
        if d == 1:
            start(far_copy(0, 0))
            start(far_copy(1, 0))
        else:
            start(part_copy(d))
        start(stat_copy(d))
    own, own_log = finish(x)

    for h in range(2):
        far_copy(h, 0).wait_recv()
        start(far_copy(h, 1))

    logs = []
    for d in range(N_X - 1):
        stat_copy(d).wait_recv()
        logs.append(as_columns(stat_in[d, 0:1, :], width))
    highest = own_log
    for one in logs:
        highest = jnp.maximum(highest, one)
    weight = jnp.exp2(own_log - highest)
    numerator = own * weight
    denominator = weight
    for d in (0, 2, 1):
        if d == 1:
            far_copy(0, 1).wait_recv()
            far_copy(1, 1).wait_recv()
        else:
            part_copy(d).wait_recv()
        weight = jnp.exp2(logs[d] - highest)
        numerator = numerator + part_in[d].astype(f32) * weight
        denominator = denominator + weight
    attended_ref[...] = (numerator / denominator).astype(bf16)
    def finish_columns():
        for target in range(1, N_Z):

            @pl.when(target > z)
            def _(target=target):
                column_copy(target).wait_send()

    yield started, finish_columns


class TpGather:
    def __init__(self, full, sends, recvs):
        self.full, self.sends, self.recvs = full, sends, recvs
        self.y, self.c = lax.axis_index("y"), lax.axis_index("c")
        self.half = full.shape[1] // 2
        self.started = []

    def _copy(self, number, shift, part, target):
        slot = lax.rem(self.y + shift, N_Y) * N_C + self.c
        if part is None:
            ref = self.full.at[slot]
        else:
            ref = self.full.at[slot, pl.ds(part * self.half, self.half)]
        if target == "core":
            device = {"c": 1 - self.c}
        else:
            device = {"y": lax.rem(self.y + (1 if target == "up" else N_Y - 1), N_Y)}
        return pltpu.make_async_remote_copy(
            src_ref=ref,
            dst_ref=ref,
            send_sem=self.sends.at[number],
            recv_sem=self.recvs.at[number],
            device_id=device,
            device_id_type=MESH_ID,
        )

    def _start(self, *what):
        copy = self._copy(*what)
        copy.start()
        self.started.append(copy)

    def start(self):
        self._start(0, 0, 0, "up")
        self._start(3, 0, 1, "down")
        self._start(1, 0, 1, "up")
        self._start(2, 0, 0, "down")
        self._start(6, 0, None, "core")

    def relay(self):
        self._copy(0, 0, 0, "up").wait_recv()
        self._start(4, N_Y - 1, 0, "up")
        self._copy(3, 0, 1, "down").wait_recv()
        self._start(5, 1, 1, "down")
        self._copy(1, 0, 1, "up").wait_recv()
        self._start(7, N_Y - 1, None, "core")
        self._copy(2, 0, 0, "down").wait_recv()
        self._start(8, 1, None, "core")

    def near(self):
        for number, shift in ((6, 0), (7, N_Y - 1), (8, 1)):
            self._copy(number, shift, None, "core").wait_recv()

    def far(self):
        self._copy(4, 0, 0, "up").wait_recv()
        self._start(9, 2, 0, "core")
        self._copy(5, 0, 1, "down").wait_recv()
        self._start(10, 2, 1, "core")
        for part in range(2):
            self._copy(9 + part, 2, part, "core").wait_recv()

    def finish(self):
        for copy in self.started:
            copy.wait_send()


def project_phase(
    greeted,
    after_gates,
    after_exchange,
    after_keys,
    tokens_hbm,
    gain,
    query_gain,
    latent_gain,
    cosine_row,
    sine_row,
    shift_hbm,
    narrow_query,
    narrow_latent,
    narrow_rotary,
    narrow_ingate,
    narrow_forget,
    query_hbm,
    key_hbm,
    value_hbm,
    outgate_hbm,
    query_up_hbm,
    key_up_hbm,
    value_up_hbm,
    mem_ref,
    gate_ref,
    q_ref,
    kv_ref,
    rows_all,
    query_latents,
    latents,
    small,
    ingate,
    forget,
    big,
    query_up,
    key_up,
    value_up,
    tokens,
    shift_row,
    pre_gates,
    up_query,
    up_latent,
    wide_query,
    wide_latent,
    load_sem,
    row_send,
    row_recv,
    lat_send,
    lat_recv,
    query_send,
    query_recv,
):
    f32, bf16 = jnp.float32, jnp.bfloat16
    y, c = lax.axis_index("y"), lax.axis_index("c")
    mine = y * N_C + c
    width = 128
    sources = (
        (narrow_query, small.at[pl.ds(0, QUERY_PART)]),
        (narrow_latent, small.at[pl.ds(width, LATENT_PART)]),
        (narrow_rotary, small.at[pl.ds(width + LATENT_PART, ROTARY_CHANNELS)]),
        (narrow_ingate, ingate),
        (narrow_forget, forget),
        (query_up_hbm, query_up),
        (key_up_hbm, key_up),
        (value_up_hbm, value_up),
        (shift_hbm, shift_row),
    )
    loads = [
        pltpu.make_async_copy(source, target, load_sem.at[k])
        for k, (source, target) in enumerate(sources)
    ]
    at = 0
    for k, ref in enumerate((query_hbm, key_hbm, value_hbm, outgate_hbm)):
        columns = ref.shape[1]
        loads.append(
            pltpu.make_async_copy(ref, big.at[:, pl.ds(at, columns)], load_sem.at[9 + k])
        )
        at += columns
    arrival = pltpu.make_async_copy(tokens_hbm, tokens, load_sem.at[13])
    arrival.start()
    for load in loads:
        load.start()
    arrival.wait()
    wide = tokens[...].astype(f32)
    inverse = lax.rsqrt(jnp.mean(wide * wide, axis=1, keepdims=True) + SMALL_CONSTANT)
    rows_all[mine] = (wide * inverse * gain[...].astype(f32).reshape(1, -1)).astype(bf16)
    small[QUERY_PART:width] = jnp.zeros((width - QUERY_PART, small.shape[1]), bf16)

    greeted()
    gather = TpGather(rows_all, row_send, row_recv)
    gather.start()

    for load in loads:
        load.wait()
    small[QUERY_PART : QUERY_PART + 8] = ingate[...]
    small[QUERY_PART + 16 : QUERY_PART + 24] = forget[...]
    up_query[...] = jnp.zeros(up_query.shape, bf16)
    query_rows = query_up[...].astype(f32).T.astype(bf16)
    for s in range(N_Y * N_C):
        up_query[s * width : s * width + QUERY_PART] = query_rows[
            s * QUERY_PART : (s + 1) * QUERY_PART
        ]
        part = slice(s * LATENT_PART, (s + 1) * LATENT_PART)
        for h in range(2):
            at = s * width + h * LATENT_PART
            up_latent[at : at + LATENT_PART, :width] = key_up[part]
            up_latent[at : at + LATENT_PART, width:] = value_up[part]

    lane = lax.broadcasted_iota(jnp.int32, (1, width), 1)
    cosine, sine_part = (
        jnp.concatenate([ref[...]] * 4, axis=0).T for ref in (cosine_row, sine_row)
    )
    row_id = lax.broadcasted_iota(jnp.int32, (width, width), 0)
    col_id = lax.broadcasted_iota(jnp.int32, (width, width), 1)
    channels = lax.rem(col_id, ROTARY_CHANNELS)
    halfway = ROTARY_CHANNELS // 2
    twin = (row_id == channels).astype(bf16)
    partner = lax.rem(channels + halfway, ROTARY_CHANNELS)
    sign = jnp.where(channels < halfway, -1.0, 1.0)

    def duplicated(values, offset):
        return jnp.dot(
            values, (row_id == channels + offset).astype(bf16), preferred_element_type=f32
        )

    def rotated(values, offset):
        swap = jnp.where(row_id == partner + offset, sign, 0.0).astype(bf16)
        turned = jnp.dot(values, swap, preferred_element_type=f32)
        return duplicated(values, offset) * cosine + turned * sine_part

    def chip_rows(chip):
        slots = [rows_all[chip * N_C + k] for k in range(N_C)]
        return jnp.concatenate(slots, axis=0)

    span = N_C * SHARE
    tile = 256

    def project_small(chip):
        rows = pl.ds(pl.multiple_of(chip * span, span), span)
        here = chip_rows(chip)
        made = lax.dot_general(here, small[...], CONTRACT_LAST, preferred_element_type=f32)
        turned = made[:, :width].T
        for k in range(2):
            at = QUERY_PART + 16 * k
            pre_gates[k, :, rows] = turned[at : at + 8]
        rounded = made.astype(bf16)
        query_latents[mine, rows] = rounded[:, :width]
        wide_latent[rows, :width] = rounded[:, width:]

    def project_big():
        def one(t, carry):
            columns = pl.ds(pl.multiple_of(t * tile, tile), tile)
            rows = rows_all[...].reshape(ROWS, rows_all.shape[2])
            made = jnp.dot(rows, big[:, columns], preferred_element_type=f32)
            mem_ref[:, columns] = made.astype(bf16)
            return carry

        lax.fori_loop(0, big.shape[1] // tile, one, 0)

    gather.relay()
    gather.near()
    near = [y, lax.rem(y + N_Y - 1, N_Y), lax.rem(y + 1, N_Y)]
    for chip in near:
        project_small(chip)
    opposite = lax.rem(y + 2, N_Y)
    gather.far()
    project_small(opposite)

    second = wide_latent[:, :width]
    both = duplicated(second, 0)
    half = ROWS // 2
    packed = jnp.where(lane < LATENT_PART, both[:half], both[half:])
    latents[mine] = packed.astype(bf16)
    exchange = TpGather(latents, lat_send, lat_recv)
    query_exchange = TpGather(query_latents, query_send, query_recv)
    exchange.start()
    query_exchange.start()
    project_big()
    heads = lax.broadcasted_iota(jnp.int32, (8, ROWS), 0) == mine
    in_pre, forget_pre = (
        jnp.sum(jnp.where(heads, pre_gates[k], 0.0), axis=0, keepdims=True) for k in range(2)
    )
    in_gate = SOFTCAP * jnp.tanh(in_pre / SOFTCAP)
    capped = SOFTCAP * jnp.tanh((forget_pre + shift_row[...]) / SOFTCAP)
    small_part = jnp.exp(-jnp.abs(capped))
    above_one = 1.0 + small_part
    grown = jnp.where(
        above_one == 1.0, small_part, jnp.log(above_one) * small_part / (above_one - 1.0)
    )
    log_forget = jnp.minimum(capped, 0.0) - grown
    earlier = lax.broadcasted_iota(jnp.int32, (ROWS, ROWS), 0) <= lax.broadcasted_iota(
        jnp.int32, (ROWS, ROWS), 1
    )
    cumulative = jnp.dot(
        jnp.broadcast_to(log_forget, (8, ROWS)),
        earlier.astype(f32),
        precision=PRECISE,
        preferred_element_type=f32,
    )
    top_rows = lax.broadcasted_iota(jnp.int32, (8, ROWS), 0) == 0
    gate_ref[...] = jnp.where(top_rows, in_gate - cumulative, cumulative)
    after_gates()
    exchange.relay()
    query_exchange.relay()
    key_turned = rotated(second, LATENT_PART)
    kv_ref[2 * ROWS :] = jnp.where(
        lane < ROTARY_CHANNELS, key_turned[:half], key_turned[half:]
    ).astype(bf16)
    exchange.near()
    after_exchange()
    exchange.far()

    squares = jnp.zeros((half, width), f32)
    for s in range(N_Y * N_C):
        part = latents[s].astype(f32)
        squares = squares + part * part
    low = lane < LATENT_PART
    low_scale, high_scale = (
        lax.rsqrt(
            jnp.sum(jnp.where(low == first, squares, 0.0), axis=1, keepdims=True) / LATENT_WIDTH
            + SMALL_CONSTANT
        )
        for first in (True, False)
    )
    latent_scale = jnp.where(low, low_scale, high_scale)
    query_gains = jnp.broadcast_to(query_gain[...].reshape(1, -1), (8, QUERY_LATENT))
    latent_gains = jnp.broadcast_to(latent_gain[...].reshape(1, -1), (8, LATENT_WIDTH))

    def latent_gain_of(s):
        pair = slice((s // 2) * width, (s // 2 + 1) * width)
        shift = LATENT_WIDTH - LATENT_PART if s % 2 else LATENT_PART
        here = latent_gains[:1, pair]
        other = pltpu.roll(latent_gains, shift, 1)[:1, pair]
        return jnp.where(low, other, here) if s % 2 else jnp.where(low, here, other)

    def query_gain_of(s):
        turned = query_gains
        if s:
            turned = pltpu.roll(query_gains, QUERY_LATENT - s * QUERY_PART, 1)
        return turned[:1, :width]

    for s in range(N_Y * N_C):
        columns = slice(s * width, (s + 1) * width)
        part = latents[s].astype(f32)
        made = (part * latent_scale * latent_gain_of(s)).astype(bf16)
        wide_latent[:half, columns] = jnp.where(low, made, jnp.zeros_like(made))
        wide_latent[half:, columns] = jnp.where(low, jnp.zeros_like(made), made)
    made = jnp.dot(wide_latent[...], up_latent[...], preferred_element_type=f32).astype(bf16)
    kv_ref[:ROWS] = made[:, :width]
    kv_ref[ROWS : 2 * ROWS] = made[:, width:]
    after_keys()

    query_exchange.near()
    query_exchange.far()
    query_mask = (lane < QUERY_PART).astype(f32)
    squares = jnp.zeros((ROWS, width), f32)
    for s in range(N_Y * N_C):
        part = query_latents[s].astype(f32) * query_mask
        squares = squares + part * part
    query_scale = lax.rsqrt(
        jnp.sum(squares, axis=1, keepdims=True) / QUERY_LATENT + SMALL_CONSTANT
    )
    for s in range(N_Y * N_C):
        columns = slice(s * width, (s + 1) * width)
        part = query_latents[s].astype(f32) * query_mask
        wide_query[:, columns] = (part * query_scale * query_gain_of(s)).astype(bf16)
    made = jnp.dot(wide_query[...], up_query[...], preferred_element_type=f32).astype(bf16)
    q_ref[:, :width] = made[:, :width]
    turning = jnp.concatenate([made[:, width:], jnp.zeros((ROWS, ROTARY_CHANNELS), bf16)], axis=1)
    q_ref[:, width:] = rotated(turning, 0).astype(bf16)
    return gather.started + exchange.started + query_exchange.started


def output_phase(
    gated,
    attended,
    out_memory,
    out_attend,
    o_ref,
    kept,
    to_core,
    from_core,
    sums,
    passing,
    from_below,
    from_above,
    relay_in,
    core_send,
    core_recv,
    relay_send,
    relay_recv,
    up_send,
    up_recv,
    down_send,
    down_recv,
):
    f32, bf16 = jnp.float32, jnp.bfloat16
    y, c = lax.axis_index("y"), lax.axis_index("c")
    above, below = lax.rem(y + 1, N_Y), lax.rem(y + N_Y - 1, N_Y)
    opposite = lax.rem(y + 2, N_Y)
    half = out_memory.shape[1] // 2
    tile = 512

    def remote(source, target, send, recv, device):
        return pltpu.make_async_remote_copy(
            src_ref=source,
            dst_ref=target,
            send_sem=send,
            recv_sem=recv,
            device_id=device,
            device_id_type=MESH_ID,
        )

    def rows_of(ref, core):
        picked = [ref[pl.ds(pl.multiple_of((k * N_C + core) * SHARE, SHARE), SHARE)] for k in range(N_Y)]
        return jnp.concatenate(picked, axis=0)

    def columns_of(h, t):
        return slice(h * half + t * tile, h * half + (t + 1) * tile)

    for k, core in enumerate((1 - c, c)):
        memory_rows = rows_of(gated, core)
        for h in range(2):
            for t in range(half // tile):
                kept[k, h, :, t * tile : (t + 1) * tile] = jnp.dot(
                    memory_rows, out_memory[:, columns_of(h, t)], preferred_element_type=f32
                )
    yield

    def partial(k, h, store):
        attend_rows = rows_of(attended, c if k else 1 - c)
        for t in range(half // tile):
            made = jnp.dot(
                attend_rows, out_attend[:, columns_of(h, t)], preferred_element_type=f32
            )
            made = kept[k, h, :, t * tile : (t + 1) * tile] + made
            store(t * tile, made.astype(bf16).reshape(N_Y, SHARE, tile))

    def core_copy(h):
        return remote(
            to_core.at[h], from_core.at[h], core_send.at[h], core_recv.at[h], {"c": 1 - c}
        )

    def relay_copy(h):
        return remote(
            passing.at[h],
            relay_in.at[h],
            relay_send.at[h],
            relay_recv.at[h],
            {"y": above if h == 0 else below},
        )

    def up_copy(h):
        return remote(
            passing.at[2 + h], from_below.at[h], up_send.at[h], up_recv.at[h], {"y": above}
        )

    def down_copy(h):
        return remote(
            passing.at[4 + h], from_above.at[h], down_send.at[h], down_recv.at[h], {"y": below}
        )

    started = []

    def start(copy):
        copy.start()
        started.append(copy)

    for h in range(2):

        def keep(at, block, h=h):
            to_core[h, :, :, at : at + tile] = block

        partial(0, h, keep)
        start(core_copy(h))
    for h in range(2):

        def keep(at, block, h=h):
            sums[h, :, :, at : at + tile] = block.astype(f32)

        partial(1, h, keep)
    for h in range(2):
        core_copy(h).wait_recv()
        sums[h] = sums[h] + from_core[h].astype(f32)
        passing[h] = sums[h, opposite].astype(bf16)
        start(relay_copy(h))
        if h == 0:
            passing[4] = sums[0, below].astype(bf16)
            start(down_copy(0))
        else:
            passing[3] = sums[1, above].astype(bf16)
            start(up_copy(1))
    relay_copy(0).wait_recv()
    passing[2] = (sums[0, above] + relay_in[0].astype(f32)).astype(bf16)
    start(up_copy(0))
    relay_copy(1).wait_recv()
    passing[5] = (sums[1, below] + relay_in[1].astype(f32)).astype(bf16)
    start(down_copy(1))
    for h in (1, 0):
        up_copy(h).wait_recv()
        down_copy(h).wait_recv()
        made = sums[h, y] + from_below[h].astype(f32) + from_above[h].astype(f32)
        o_ref[:, h * half : (h + 1) * half] = made
    yield started


def scratch(depth, mem_width):
    f32, bf16 = jnp.float32, jnp.bfloat16
    dma = pltpu.SemaphoreType.DMA
    between = (
        pltpu.VMEM((ROWS, VALUE_CHANNELS), bf16),
        pltpu.VMEM((ROWS, M_V), bf16),
        pltpu.VMEM((ROWS, mem_width), bf16),
        pltpu.VMEM((8, ROWS), f32),
        pltpu.VMEM((ROWS, 256), bf16),
        pltpu.VMEM((ROWS * 5 // 2, 128), bf16),
        pltpu.VMEM((M_V, depth), bf16),
        pltpu.VMEM((VALUE_CHANNELS, depth), bf16),
        dma((2,)),
    )
    for_project = (
        pltpu.VMEM((N_Y * N_C, SHARE, depth), bf16),
        pltpu.VMEM((N_Y * N_C, ROWS, 128), bf16),
        pltpu.VMEM((N_Y * N_C, ROWS // 2, 128), bf16),
        pltpu.VMEM((256, depth), bf16),
        pltpu.VMEM((8, depth), bf16),
        pltpu.VMEM((8, depth), bf16),
        pltpu.VMEM((depth, mem_width), bf16),
        pltpu.VMEM((PLAIN_CHANNELS + ROTARY_CHANNELS, QUERY_LATENT), bf16),
        pltpu.VMEM((LATENT_WIDTH, PLAIN_CHANNELS), bf16),
        pltpu.VMEM((LATENT_WIDTH, VALUE_CHANNELS), bf16),
        pltpu.VMEM((SHARE, depth), bf16),
        pltpu.VMEM((1, ROWS), f32),
        pltpu.VMEM((2, 8, ROWS), f32),
        pltpu.VMEM((1024, PLAIN_CHANNELS + ROTARY_CHANNELS), bf16),
        pltpu.VMEM((1024, 256), bf16),
        pltpu.VMEM((ROWS, 1024), bf16),
        pltpu.VMEM((ROWS, 1024), bf16),
        dma((16,)),
        dma((11,)),
        dma((11,)),
        dma((11,)),
        dma((11,)),
        dma((11,)),
        dma((11,)),
    )
    for_attend = (
        pltpu.VMEM((N_X, ROWS, 256), bf16),
        pltpu.VMEM((N_Z, ROWS * 5 // 2, 128), bf16),
        pltpu.VMEM((ROWS, 256), bf16),
        pltpu.VMEM((N_X * ROWS, 128), f32),
        pltpu.VMEM((N_X * ROWS, 128), f32),
        pltpu.VMEM((N_X * ROWS, VALUE_CHANNELS), f32),
        pltpu.VMEM((N_X - 1, ROWS, VALUE_CHANNELS), bf16),
        pltpu.VMEM((N_X - 1, 8, ROWS), f32),
        pltpu.VMEM((N_X - 1, ROWS, VALUE_CHANNELS), bf16),
        pltpu.VMEM((N_X - 1, 8, ROWS), f32),
        pltpu.VMEM((ROWS, M_V), f32),
        pltpu.VMEM((ROWS, 128), f32),
        pltpu.VMEM((ROWS, 128), f32),
        pltpu.VMEM((N_X, STATE_ROWS, M_V), f32),
        pltpu.VMEM((N_X, STATE_ROWS, M_V), f32),
        pltpu.VMEM((STATE_ROWS, M_V), f32),
        pltpu.VMEM((N_Z, STATE_ROWS, M_V), f32),
        pltpu.VMEM((N_X, STATE_ROWS, M_V), f32),
        pltpu.VMEM((N_X, STATE_ROWS, M_V), f32),
        pltpu.VMEM((2, 8, ROWS), f32),
        pltpu.VMEM((N_Y, 8, ROWS), f32),
        pltpu.VMEM((2, ROWS // 2, VALUE_CHANNELS), bf16),
        dma((6,)),
        dma((6,)),
        dma((N_Z // 2, 2)),
        dma((N_Z // 2, 2)),
        dma((N_Z // 2, 2)),
        dma((N_Z // 2, 2)),
        dma((N_X - 1,)),
        dma((N_X - 1,)),
        dma((N_X - 1,)),
        dma((N_X - 1,)),
        dma((N_X - 1,)),
        dma((N_X - 1,)),
        dma((N_Z,)),
        dma((N_Z,)),
        dma((N_X - 1,)),
        dma((N_X - 1,)),
        dma((N_Y,)),
        dma((N_Y,)),
        dma((2, 2)),
        dma((2, 2)),
    )
    for_output = (
        pltpu.VMEM((2, 2, N_Y * SHARE, depth // 2), f32),
        pltpu.VMEM((2, N_Y, SHARE, depth // 2), bf16),
        pltpu.VMEM((2, N_Y, SHARE, depth // 2), bf16),
        pltpu.VMEM((2, N_Y, SHARE, depth // 2), f32),
        pltpu.VMEM((6, SHARE, depth // 2), bf16),
        pltpu.VMEM((2, SHARE, depth // 2), bf16),
        pltpu.VMEM((2, SHARE, depth // 2), bf16),
        pltpu.VMEM((2, SHARE, depth // 2), bf16),
        dma((2,)),
        dma((2,)),
        dma((2,)),
        dma((2,)),
        dma((2,)),
        dma((2,)),
        dma((2,)),
        dma((2,)),
    )
    return between, for_project, for_attend, for_output


N_INPUTS = 22
N_PROJECT_INPUTS = 19
IN_VMEM = (1, 2, 3, 4, 5, 19)


def layer_kernel(counts, *refs):
    y, c = lax.axis_index("y"), lax.axis_index("c")
    z, x = lax.axis_index("z"), lax.axis_index("x")
    project_inputs = refs[:N_PROJECT_INPUTS]
    mem_gain, out_memory_hbm, out_attend_hbm, out_ref = refs[N_PROJECT_INPUTS : N_INPUTS + 1]
    groups, at = [], N_INPUTS + 1
    for count in counts:
        groups.append(refs[at : at + count])
        at += count
    between, for_project, for_attend, for_output = groups
    attended, gated, mem, gates, queries, keys_values, out_memory, out_attend, out_sem = between

    barrier = pltpu.get_barrier_semaphore()
    devices = [{"c": 1 - c}]
    devices += [{"y": lax.rem(y + d, N_Y)} for d in range(1, N_Y)]
    devices += [{"x": lax.rem(x + d, N_X)} for d in range(1, N_X)]
    devices += [{"z": lax.rem(z + d, N_Z)} for d in range(1, N_Z)]
    for device in devices:
        pl.semaphore_signal(barrier, inc=1, device_id=device, device_id_type=MESH_ID)
    loads = [
        pltpu.make_async_copy(out_memory_hbm, out_memory, out_sem.at[0]),
        pltpu.make_async_copy(out_attend_hbm, out_attend, out_sem.at[1]),
    ]
    attending = attend_phase(
        queries, keys_values, mem, gates, mem_gain, attended, gated, *for_attend
    )
    started = project_phase(
        lambda: pl.semaphore_wait(barrier, len(devices)),
        *[lambda: next(attending)] * 3,
        *project_inputs,
        mem,
        gates,
        queries,
        keys_values,
        *for_project,
    )
    for load in loads:
        load.start()
    outputting = output_phase(gated, attended, out_memory, out_attend, out_ref, *for_output)
    next(attending)
    for load in loads:
        load.wait()
    next(outputting)
    more, finish_columns = next(attending)
    started += more
    started += next(outputting)
    for copy in started:
        copy.wait_send()
    finish_columns()


def layer(*inputs):
    depth = inputs[0].shape[1]
    mem_width = 2 * M_QK + 2 * M_V
    groups = scratch(depth, mem_width)
    vmem = pl.BlockSpec(memory_space=pltpu.VMEM)
    hbm = pl.BlockSpec(memory_space=pltpu.HBM)
    return pl.pallas_call(
        functools.partial(layer_kernel, tuple(len(group) for group in groups)),
        out_shape=jax.ShapeDtypeStruct((SHARE, depth), jnp.float32),
        in_specs=[vmem if k in IN_VMEM else hbm for k in range(N_INPUTS)],
        out_specs=vmem,
        scratch_shapes=[one for group in groups for one in group],
        compiler_params=pltpu.CompilerParams(
            collective_id=1, has_side_effects=True, vmem_limit_bytes=67_000_000
        ),
        cost_estimate=pl.CostEstimate(
            flops=8 * 10**9, bytes_accessed=2 * 10**7, transcendentals=4 * 10**6
        ),
        name="layer",
    )(*inputs)


def per_device(
    tokens,
    input_gain,
    weight_query,
    weight_key,
    weight_value,
    weight_outgate,
    weight_ingate,
    weight_forget,
    forget_shift,
    mem_gain,
    query_down_weight,
    latent_down_weight,
    down_rotary,
    query_gain,
    latent_gain,
    query_up_weight,
    key_up_weight,
    value_up_weight,
    out_memory,
    out_attend,
):
    length = forget_shift.shape[0]
    positions = lax.axis_index(SP) * length + jnp.arange(length, dtype=jnp.int32)
    halfway = ROTARY_CHANNELS // 2
    inverse = jnp.power(ROTARY_BASE, -jnp.arange(halfway, dtype=jnp.float32) / halfway)
    angles = positions.astype(jnp.float32)[None, :] * inverse[:, None]
    mixed = layer(
        tokens,
        input_gain,
        query_gain,
        latent_gain,
        jnp.cos(angles),
        jnp.sin(angles),
        forget_shift.T,
        query_down_weight.T,
        latent_down_weight.T,
        down_rotary.T,
        weight_ingate.T,
        weight_forget.T,
        weight_query,
        weight_key,
        weight_value,
        weight_outgate,
        query_up_weight.T,
        key_up_weight,
        value_up_weight,
        mem_gain,
        out_memory,
        out_attend,
    )
    return mixed.astype(jnp.bfloat16)


def solution(mesh):
    torus = Mesh(mesh.devices.reshape(N_Z, N_X, 4, 2), SP_TP)
    in_specs = (
        P(SP_TP, None),
        P(),
        P(None, TP),
        P(None, TP),
        P(None, TP),
        P(None, TP),
        P(),
        P(),
        P(SP, TP),
        P(),
        P(None, TP),
        P(None, TP),
        P(),
        P(),
        P(),
        P(None, TP),
        P(None, TP),
        P(None, TP),
        P(TP, None),
        P(TP, None),
    )
    out_specs = P(SP_TP, None)
    return jax.shard_map(
        per_device, mesh=torus, in_specs=in_specs, out_specs=out_specs, check_vma=False
    )
```

```python
import functools

import jax
import jax.numpy as jnp
from jax import lax
from jax.experimental import pallas as pl
from jax.experimental.pallas import tpu as pltpu
from jax.sharding import Mesh
from jax.sharding import PartitionSpec as P

MEMORY_HEADS = 8
M_QK = 128
M_V = 256
PLAIN_CHANNELS = 128
ROTARY_CHANNELS = 64
VALUE_CHANNELS = 128
SP = ("z", "x")
TP = ("y", "c")
SP_TP = ("z", "x", "y", "c")


SMALL_CONSTANT = 1e-06
SOFTCAP = 15.0
ROTARY_BASE = 10000.0
PRECISE = lax.Precision.HIGHEST
FAR_BELOW = -1e30

N_Y = 4
N_C = 2
SHARE = 64
QUERY_LATENT = 768
LATENT_WIDTH = 512
QUERY_PART = QUERY_LATENT // (N_Y * N_C)
LATENT_PART = LATENT_WIDTH // (N_Y * N_C)
LOG2E = 1.4426950408889634
N_Z = 8
N_X = 4
ROWS = 512
MESH_ID = pl.DeviceIdType.MESH
CONTRACT_LAST = (((1,), (1,)), ((), ()))
CHUNK = M_QK // N_X
TALL = 512
GROUP = 1
STATE_ROWS = CHUNK + 8
NORMAL_ROW, TOP_ROW, DECAY_ROW = CHUNK, CHUNK + 1, CHUNK + 2


def merge_states(early, late):
    moved = early[TOP_ROW : TOP_ROW + 1] + late[DECAY_ROW : DECAY_ROW + 1]
    late_top = late[TOP_ROW : TOP_ROW + 1]
    joined = jnp.maximum(moved, late_top)
    both = early * jnp.exp(moved - joined) + late * jnp.exp(late_top - joined)
    row = lax.broadcasted_iota(jnp.int32, both.shape, 0)
    decay = early[DECAY_ROW : DECAY_ROW + 1] + late[DECAY_ROW : DECAY_ROW + 1]
    return jnp.where(row == TOP_ROW, joined, jnp.where(row == DECAY_ROW, decay, both))


def in_two(values):
    high = values.astype(jnp.bfloat16)
    return high, (values - high.astype(jnp.float32)).astype(jnp.bfloat16)


def as_columns(row, width):
    return jnp.broadcast_to(row, (width, row.shape[1])).T


def attend_phase(
    q_ref,
    kv_ref,
    mem_ref,
    gate_ref,
    gain_ref,
    attended_ref,
    gated_ref,
    q_all,
    kv_all,
    k_cat,
    top,
    total,
    accum,
    part_out,
    stat_out,
    part_in,
    stat_in,
    cell,
    cell_sum,
    cell_top,
    first_out,
    first_in,
    column_out,
    column_in,
    start_out,
    start_in,
    square_out,
    square_in,
    passed,
    q_send,
    q_recv,
    up_send,
    up_recv,
    down_send,
    down_recv,
    part_send,
    part_recv,
    stat_send,
    stat_recv,
    first_send,
    first_recv,
    column_send,
    column_recv,
    start_send,
    start_recv,
    square_send,
    square_recv,
    passed_send,
    passed_recv,
):
    f32, bf16 = jnp.float32, jnp.bfloat16
    z, x = lax.axis_index("z"), lax.axis_index("x")
    y, c = lax.axis_index("y"), lax.axis_index("c")
    above, below = lax.rem(z + 1, N_Z), lax.rem(z + N_Z - 1, N_Z)
    peers = [lax.rem(x + d, N_X) for d in range(1, N_X)]
    right, left = peers[0], peers[-1]
    rows_y = [lax.rem(y + d, N_Y) for d in range(1, N_Y)]
    me_tp = y * N_C + c
    half = kv_ref.shape[0] // 2
    width = PLAIN_CHANNELS

    def remote(source, target, send, recv, device):
        return pltpu.make_async_remote_copy(
            src_ref=source,
            dst_ref=target,
            send_sem=send,
            recv_sem=recv,
            device_id=device,
            device_id_type=MESH_ID,
        )

    def kv_copy(up, step, h):
        shift = (N_Z - step + 1) if up else (step - 1)
        owner = lax.rem(z + shift, N_Z)
        rows = pl.ds(h * half, half)
        source = kv_ref.at[rows] if step == 1 else kv_all.at[owner, rows]
        send, recv = (up_send, up_recv) if up else (down_send, down_recv)
        return remote(
            source,
            kv_all.at[owner, rows],
            send.at[step - 1, h],
            recv.at[step - 1, h],
            {"z": above if up else below},
        )

    q_half = ROWS // 2

    def q_copy(number):
        shift, part, to_right = (
            (0, 0, True),
            (0, 1, True),
            (0, 0, False),
            (0, 1, False),
            (N_X - 1, 0, True),
            (1, 1, False),
        )[number]
        owner = lax.rem(x + shift, N_X)
        rows = pl.ds(part * q_half, q_half)
        source = q_ref.at[rows] if shift == 0 else q_all.at[owner, rows]
        return remote(
            source,
            q_all.at[owner, rows],
            q_send.at[number],
            q_recv.at[number],
            {"x": right if to_right else left},
        )

    def part_copy(d):
        return remote(
            part_out.at[d], part_in.at[d], part_send.at[d], part_recv.at[d], {"x": peers[d]}
        )

    def far_copy(h, hop):
        rows = pl.ds(h * q_half, q_half)
        return remote(
            part_out.at[1, rows] if hop == 0 else passed.at[h],
            passed.at[h] if hop == 0 else part_in.at[1, rows],
            passed_send.at[hop, h],
            passed_recv.at[hop, h],
            {"x": right if h == 0 else left},
        )

    def stat_copy(d):
        return remote(
            stat_out.at[d], stat_in.at[d], stat_send.at[d], stat_recv.at[d], {"x": peers[d]}
        )

    def first_copy(d):
        return remote(
            first_out.at[peers[d]],
            first_in.at[x],
            first_send.at[d],
            first_recv.at[d],
            {"x": peers[d]},
        )

    def column_copy(target):
        return remote(
            column_out,
            column_in.at[z],
            column_send.at[target],
            column_recv.at[z],
            {"z": target},
        )

    def column_arrival(source):
        return remote(
            column_out,
            column_in.at[source],
            column_send.at[source],
            column_recv.at[source],
            {"z": source},
        )

    def start_copy(d):
        return remote(
            start_out.at[peers[d]],
            start_in.at[x],
            start_send.at[d],
            start_recv.at[d],
            {"x": peers[d]},
        )

    def square_copy(number):
        device = {"c": 1 - c} if number == 0 else {"y": rows_y[number - 1]}
        return remote(
            square_out.at[min(number, 1)],
            square_in.at[number],
            square_send.at[number],
            square_recv.at[number],
            device,
        )

    started = []

    def start(copy):
        copy.start()
        started.append(copy)

    relative, cumulative = gate_ref[0:1], gate_ref[1:2]
    key_scale = M_QK ** (-0.5)
    tall = 256
    for t in range(ROWS // tall):
        rows, seen = slice(t * tall, (t + 1) * tall), (t + 1) * tall
        row = lax.broadcasted_iota(jnp.int32, (tall, seen), 0) + t * tall
        col = lax.broadcasted_iota(jnp.int32, (tall, seen), 1)
        logs = jnp.where(col <= row, relative[:, :seen], -jnp.inf)
        highest = jnp.max(logs, axis=1, keepdims=True)
        affinity = lax.dot_general(
            mem_ref[rows, :M_QK],
            mem_ref[:seen, M_QK : 2 * M_QK],
            CONTRACT_LAST,
            preferred_element_type=f32,
        )
        affinity = affinity * (jnp.exp(logs - highest) * key_scale)
        values = mem_ref[:seen, 2 * M_QK : 2 * M_QK + M_V]
        cell[rows] = sum(
            jnp.dot(piece, values, preferred_element_type=f32) for piece in in_two(affinity)
        )
        cell_sum[rows] = jnp.broadcast_to(
            jnp.sum(affinity, axis=1, keepdims=True), (tall, width)
        )
        cell_top[rows] = jnp.broadcast_to(highest, (tall, width))
    ends_at = jnp.max(relative, axis=1, keepdims=True)
    weights = jnp.exp(relative - ends_at) * key_scale
    wide_key = mem_ref[:, M_QK : 2 * M_QK].astype(f32)
    normal = jnp.sum(as_columns(weights, width) * wide_key, axis=0, keepdims=True)
    values = mem_ref[:, 2 * M_QK : 2 * M_QK + M_V]
    matrix = sum(
        jnp.dot(piece, values, preferred_element_type=f32)
        for piece in in_two(wide_key.T * weights)
    )
    decay = cumulative[:, ROWS - 1 : ROWS]
    row = lax.broadcasted_iota(jnp.int32, (8, M_V), 0)
    lines = jnp.concatenate([normal, jnp.zeros_like(normal)], axis=1)
    notes = jnp.where(
        row == 0, lines, jnp.where(row == 1, ends_at + decay, jnp.where(row == 2, decay, 0.0))
    )
    for k in range(N_X):
        first_out[k, :CHUNK] = matrix[k * CHUNK : (k + 1) * CHUNK]
        first_out[k, CHUNK:] = notes
    for d in range(N_X - 1):
        start(first_copy(d))
    first_in[x] = first_out[x]

    yield

    for d in range(N_X - 1):
        first_copy(d).wait_recv()
    column = first_in[0]
    for k in range(1, N_X):
        column = merge_states(column, first_in[k])
    column_out[...] = column
    for target in range(1, N_Z):

        @pl.when(target > z)
        def _(target=target):
            column_copy(target).start()

    yield

    for h in range(2):
        for up in (True, False):
            start(kv_copy(up, 1, h))
    yield

    top[...] = jnp.full(top.shape, FAR_BELOW, f32)
    total[...] = jnp.zeros(total.shape, f32)
    for number in (0, 3, 1, 2):
        start(q_copy(number))
    accum[...] = jnp.zeros(accum.shape, f32)
    q_all[x] = q_ref[...]

    lane = lax.broadcasted_iota(jnp.int32, (ROWS // 2, width), 1)
    low = (lane < ROTARY_CHANNELS).astype(bf16)
    high = (lane >= ROTARY_CHANNELS).astype(bf16)
    scale = LOG2E * (PLAIN_CHANNELS + ROTARY_CHANNELS) ** (-0.5)

    def keys_from(ref):
        k_cat[:, :width] = ref[:ROWS]
        packed = ref[2 * ROWS :]
        k_cat[: ROWS // 2, width:] = packed * low
        k_cat[ROWS // 2 :, width:] = packed * high

    def attend_tile(t, keys, values, masked):
        shard = t // (ROWS // TALL)
        rows = pl.ds(pl.multiple_of(t * TALL, TALL), TALL)
        inner = pl.ds(pl.multiple_of((t % (ROWS // TALL)) * TALL, TALL), TALL)
        scores = lax.dot_general(
            q_all[shard, inner], keys, CONTRACT_LAST, preferred_element_type=f32
        )
        scores = scores * scale
        if masked:
            row = lax.broadcasted_iota(jnp.int32, scores.shape, 0) + t * TALL
            col = lax.broadcasted_iota(jnp.int32, scores.shape, 1) + x * ROWS
            scores = jnp.where(col <= row, scores, -jnp.inf)
        old = top[rows]
        new = jnp.maximum(old, jnp.max(scores, axis=1, keepdims=True))
        probs = jnp.exp2(scores - jnp.concatenate([new] * (ROWS // width), axis=1))
        shrink = jnp.exp2(old - new)
        added = sum(probs[:, k : k + width] for k in range(0, ROWS, width))
        total[rows] = total[rows] * shrink + added
        accum[rows] = accum[rows] * shrink + jnp.dot(
            probs.astype(bf16), values, preferred_element_type=f32
        )
        top[rows] = new

    def attend_rows(first, last, values, masked):
        def one(g, carry):
            for u in range(GROUP):
                attend_tile(g * GROUP + u, k_cat[...], values(), masked)
            return carry

        lax.fori_loop(first, last, one, 0)

    last = N_Z // 2
    steps = ROWS // (TALL * GROUP)

    def arrived(owner, useful):
        @pl.when(useful)
        def _():
            keys_from(kv_all.at[owner])
            attend_rows(0, N_X * steps, lambda: kv_all[owner, ROWS : 2 * ROWS], False)

    def take(step, h):
        for up in (True, False):
            if step == last and up != (h == 0):
                continue
            kv_copy(up, step, h).wait_recv()
            if step < last - 1 or (step == last - 1 and up == (h == 0)):
                start(kv_copy(up, step + 1, h))

    def use_up(step):
        arrived(lax.rem(z + N_Z - step, N_Z), z >= step)

    def use_down(step):
        arrived(lax.rem(z + step, N_Z), z + step >= N_Z)

    keys_from(kv_ref)
    own_values = lambda: kv_ref[ROWS : 2 * ROWS]
    attend_rows(x * steps, (x + 1) * steps, own_values, True)

    take(1, 0)
    q_copy(0).wait_recv()
    start(q_copy(4))
    q_copy(3).wait_recv()
    start(q_copy(5))

    def gather_column(k, state):
        column_arrival(k).wait_recv()
        return merge_states(state, column_in[k])

    state = lax.fori_loop(0, z, gather_column, jnp.zeros((STATE_ROWS, M_V), f32))
    for k in range(N_X):
        start_out[k] = state
        if k < N_X - 1:
            state = merge_states(state, first_in[k])
    for d in range(N_X - 1):
        start(start_copy(d))
    start_in[x] = start_out[x]
    take(1, 1)
    for number in (1, 2, 4, 5):
        q_copy(number).wait_recv()
    attend_rows((x + 1) * steps, N_X * steps, own_values, False)
    use_up(1)
    take(2, 0)
    use_down(1)
    take(2, 1)
    use_up(2)

    for d in range(N_X - 1):
        start_copy(d).wait_recv()
    carried = jnp.concatenate([start_in[k, :CHUNK] for k in range(N_X)], axis=0)
    carried_normal = start_in[0, NORMAL_ROW : NORMAL_ROW + 1, :M_QK]
    carried_top = start_in[0, TOP_ROW : TOP_ROW + 1, :width]
    queries = mem_ref[:, :M_QK]
    from_start = sum(
        jnp.dot(queries, piece, preferred_element_type=f32) for piece in in_two(carried)
    )
    highest = jnp.maximum(carried_top, cell_top[...])
    across, within = jnp.exp(carried_top - highest), jnp.exp(cell_top[...] - highest)
    twice = lambda one: jnp.concatenate([one, one], axis=1)
    numerator = cell[...] * twice(within) + from_start * twice(across)
    denominator = cell_sum[...] * within + across * jnp.sum(
        queries.astype(f32) * carried_normal, axis=1, keepdims=True
    )
    floor = jnp.exp(-(as_columns(cumulative, width) + highest))
    made = numerator / twice(jnp.maximum(jnp.abs(denominator), floor))
    cell[...] = made
    squares = jnp.sum(made * made, axis=1, keepdims=True)
    square_out[0] = jnp.broadcast_to(squares, (ROWS, width)).T[:8]
    start(square_copy(0))

    take(3, 0)
    use_down(2)
    square_copy(0).wait_recv()
    square_out[1] = square_out[0] + square_in[0]
    for number in range(1, N_Y):
        start(square_copy(number))
    take(3, 1)
    use_up(3)
    use_down(3)

    take(4, 0)
    take(4, 1)

    opposite = lax.rem(z + last, N_Z)

    @pl.when(z >= last)
    def _():
        keys_from(kv_all.at[opposite])

    def finish(shard):
        @pl.when(z >= last)
        def _():
            attend_rows(
                shard * steps,
                (shard + 1) * steps,
                lambda: kv_all[opposite, ROWS : 2 * ROWS],
                False,
            )

        rows = pl.ds(pl.multiple_of(shard * ROWS, ROWS), ROWS)
        summed = jnp.sum(total[rows], axis=1, keepdims=True)
        seen = summed > 0.0
        summed = jnp.maximum(summed, 1.0)
        log_total = jnp.where(seen, top[rows] + jnp.log2(summed), FAR_BELOW)
        return accum[rows] / summed, log_total

    for d in (1, 0, 2):
        part, log_total = finish(peers[d])
        part_out[d] = part.astype(bf16)
        stat_out[d] = log_total.T[:8]
        if d == 1:
            start(far_copy(0, 0))
            start(far_copy(1, 0))
        else:
            start(part_copy(d))
        start(stat_copy(d))
    own, own_log = finish(x)

    squares = square_out[1]
    for number in range(1, N_Y):
        square_copy(number).wait_recv()
        squares = squares + square_in[number]
    inverse = lax.rsqrt(squares[:1] / (MEMORY_HEADS * M_V) + SMALL_CONSTANT)
    gated = cell[...] * twice(as_columns(inverse, width)) * gain_ref[pl.ds(pl.multiple_of(me_tp * M_V, M_V), M_V)].astype(f32).reshape(1, M_V)
    gated = gated * jax.nn.sigmoid(mem_ref[:, 2 * M_QK + M_V :].astype(f32))
    gated_ref[...] = gated.astype(bf16)
    for h in range(2):
        far_copy(h, 0).wait_recv()
        start(far_copy(h, 1))
    yield


    logs = []
    for d in range(N_X - 1):
        stat_copy(d).wait_recv()
        logs.append(as_columns(stat_in[d, 0:1, :], width))
    highest = own_log
    for one in logs:
        highest = jnp.maximum(highest, one)
    weight = jnp.exp2(own_log - highest)
    numerator = own * weight
    denominator = weight
    for d in (0, 2, 1):
        if d == 1:
            far_copy(0, 1).wait_recv()
            far_copy(1, 1).wait_recv()
        else:
            part_copy(d).wait_recv()
        weight = jnp.exp2(logs[d] - highest)
        numerator = numerator + part_in[d].astype(f32) * weight
        denominator = denominator + weight
    attended_ref[...] = (numerator / denominator).astype(bf16)
    def finish_columns():
        for target in range(1, N_Z):

            @pl.when(target > z)
            def _(target=target):
                column_copy(target).wait_send()

    yield started, finish_columns


class TpGather:
    def __init__(self, full, sends, recvs):
        self.full, self.sends, self.recvs = full, sends, recvs
        self.y, self.c = lax.axis_index("y"), lax.axis_index("c")
        self.half = full.shape[1] // 2
        self.started = []

    def _copy(self, number, shift, part, target):
        slot = lax.rem(self.y + shift, N_Y) * N_C + self.c
        if part is None:
            ref = self.full.at[slot]
        else:
            ref = self.full.at[slot, pl.ds(part * self.half, self.half)]
        if target == "core":
            device = {"c": 1 - self.c}
        else:
            device = {"y": lax.rem(self.y + (1 if target == "up" else N_Y - 1), N_Y)}
        return pltpu.make_async_remote_copy(
            src_ref=ref,
            dst_ref=ref,
            send_sem=self.sends.at[number],
            recv_sem=self.recvs.at[number],
            device_id=device,
            device_id_type=MESH_ID,
        )

    def _start(self, *what):
        copy = self._copy(*what)
        copy.start()
        self.started.append(copy)

    def start(self):
        self._start(0, 0, 0, "up")
        self._start(3, 0, 1, "down")
        self._start(1, 0, 1, "up")
        self._start(2, 0, 0, "down")
        self._start(6, 0, None, "core")

    def relay(self):
        self._copy(0, 0, 0, "up").wait_recv()
        self._start(4, N_Y - 1, 0, "up")
        self._copy(3, 0, 1, "down").wait_recv()
        self._start(5, 1, 1, "down")
        self._copy(1, 0, 1, "up").wait_recv()
        self._start(7, N_Y - 1, None, "core")
        self._copy(2, 0, 0, "down").wait_recv()
        self._start(8, 1, None, "core")

    def near(self):
        for number, shift in ((6, 0), (7, N_Y - 1), (8, 1)):
            self._copy(number, shift, None, "core").wait_recv()

    def far(self):
        self._copy(4, 0, 0, "up").wait_recv()
        self._start(9, 2, 0, "core")
        self._copy(5, 0, 1, "down").wait_recv()
        self._start(10, 2, 1, "core")
        for part in range(2):
            self._copy(9 + part, 2, part, "core").wait_recv()

    def finish(self):
        for copy in self.started:
            copy.wait_send()


def project_phase(
    greeted,
    after_gates,
    after_exchange,
    after_keys,
    tokens_hbm,
    gain,
    query_gain,
    latent_gain,
    cosine_row,
    sine_row,
    shift_hbm,
    narrow_query,
    narrow_latent,
    narrow_rotary,
    narrow_ingate,
    narrow_forget,
    query_hbm,
    key_hbm,
    value_hbm,
    outgate_hbm,
    query_up_hbm,
    key_up_hbm,
    value_up_hbm,
    mem_ref,
    gate_ref,
    q_ref,
    kv_ref,
    rows_all,
    query_latents,
    latents,
    small,
    ingate,
    forget,
    big,
    query_up,
    key_up,
    value_up,
    tokens,
    shift_row,
    pre_gates,
    up_query,
    up_latent,
    wide_query,
    wide_latent,
    load_sem,
    row_send,
    row_recv,
    lat_send,
    lat_recv,
    query_send,
    query_recv,
):
    f32, bf16 = jnp.float32, jnp.bfloat16
    y, c = lax.axis_index("y"), lax.axis_index("c")
    mine = y * N_C + c
    width = 128
    sources = (
        (narrow_query, small.at[pl.ds(0, QUERY_PART)]),
        (narrow_latent, small.at[pl.ds(width, LATENT_PART)]),
        (narrow_rotary, small.at[pl.ds(width + LATENT_PART, ROTARY_CHANNELS)]),
        (narrow_ingate, ingate),
        (narrow_forget, forget),
        (query_up_hbm, query_up),
        (key_up_hbm, key_up),
        (value_up_hbm, value_up),
        (shift_hbm, shift_row),
    )
    loads = [
        pltpu.make_async_copy(source, target, load_sem.at[k])
        for k, (source, target) in enumerate(sources)
    ]
    at = 0
    for k, ref in enumerate((query_hbm, key_hbm, value_hbm, outgate_hbm)):
        columns = ref.shape[1]
        loads.append(
            pltpu.make_async_copy(ref, big.at[:, pl.ds(at, columns)], load_sem.at[9 + k])
        )
        at += columns
    arrival = pltpu.make_async_copy(tokens_hbm, tokens, load_sem.at[13])
    arrival.start()
    for load in loads:
        load.start()
    arrival.wait()
    wide = tokens[...].astype(f32)
    inverse = lax.rsqrt(jnp.mean(wide * wide, axis=1, keepdims=True) + SMALL_CONSTANT)
    rows_all[mine] = (wide * inverse * gain[...].astype(f32).reshape(1, -1)).astype(bf16)
    small[QUERY_PART:width] = jnp.zeros((width - QUERY_PART, small.shape[1]), bf16)

    greeted()
    gather = TpGather(rows_all, row_send, row_recv)
    gather.start()

    for load in loads:
        load.wait()
    small[QUERY_PART : QUERY_PART + 8] = ingate[...]
    small[QUERY_PART + 16 : QUERY_PART + 24] = forget[...]
    up_query[...] = jnp.zeros(up_query.shape, bf16)
    query_rows = query_up[...].astype(f32).T.astype(bf16)
    for s in range(N_Y * N_C):
        up_query[s * width : s * width + QUERY_PART] = query_rows[
            s * QUERY_PART : (s + 1) * QUERY_PART
        ]
        part = slice(s * LATENT_PART, (s + 1) * LATENT_PART)
        for h in range(2):
            at = s * width + h * LATENT_PART
            up_latent[at : at + LATENT_PART, :width] = key_up[part]
            up_latent[at : at + LATENT_PART, width:] = value_up[part]

    lane = lax.broadcasted_iota(jnp.int32, (1, width), 1)
    cosine, sine_part = (
        jnp.concatenate([ref[...]] * 4, axis=0).T for ref in (cosine_row, sine_row)
    )
    row_id = lax.broadcasted_iota(jnp.int32, (width, width), 0)
    col_id = lax.broadcasted_iota(jnp.int32, (width, width), 1)
    channels = lax.rem(col_id, ROTARY_CHANNELS)
    halfway = ROTARY_CHANNELS // 2
    twin = (row_id == channels).astype(bf16)
    partner = lax.rem(channels + halfway, ROTARY_CHANNELS)
    sign = jnp.where(channels < halfway, -1.0, 1.0)

    def duplicated(values, offset):
        return jnp.dot(
            values, (row_id == channels + offset).astype(bf16), preferred_element_type=f32
        )

    def rotated(values, offset):
        swap = jnp.where(row_id == partner + offset, sign, 0.0).astype(bf16)
        turned = jnp.dot(values, swap, preferred_element_type=f32)
        return duplicated(values, offset) * cosine + turned * sine_part

    def chip_rows(chip):
        slots = [rows_all[chip * N_C + k] for k in range(N_C)]
        return jnp.concatenate(slots, axis=0)

    span = N_C * SHARE
    tile = 256

    def project_small(chip):
        rows = pl.ds(pl.multiple_of(chip * span, span), span)
        here = chip_rows(chip)
        made = lax.dot_general(here, small[...], CONTRACT_LAST, preferred_element_type=f32)
        turned = made[:, :width].T
        for k in range(2):
            at = QUERY_PART + 16 * k
            pre_gates[k, :, rows] = turned[at : at + 8]
        rounded = made.astype(bf16)
        query_latents[mine, rows] = rounded[:, :width]
        wide_latent[rows, :width] = rounded[:, width:]

    def project_big():
        def one(t, carry):
            columns = pl.ds(pl.multiple_of(t * tile, tile), tile)
            rows = rows_all[...].reshape(ROWS, rows_all.shape[2])
            made = jnp.dot(rows, big[:, columns], preferred_element_type=f32)
            mem_ref[:, columns] = made.astype(bf16)
            return carry

        lax.fori_loop(0, big.shape[1] // tile, one, 0)

    gather.relay()
    gather.near()
    near = [y, lax.rem(y + N_Y - 1, N_Y), lax.rem(y + 1, N_Y)]
    for chip in near:
        project_small(chip)
    opposite = lax.rem(y + 2, N_Y)
    gather.far()
    project_small(opposite)

    second = wide_latent[:, :width]
    both = duplicated(second, 0)
    half = ROWS // 2
    packed = jnp.where(lane < LATENT_PART, both[:half], both[half:])
    latents[mine] = packed.astype(bf16)
    exchange = TpGather(latents, lat_send, lat_recv)
    query_exchange = TpGather(query_latents, query_send, query_recv)
    exchange.start()
    query_exchange.start()
    project_big()
    heads = lax.broadcasted_iota(jnp.int32, (8, ROWS), 0) == mine
    in_pre, forget_pre = (
        jnp.sum(jnp.where(heads, pre_gates[k], 0.0), axis=0, keepdims=True) for k in range(2)
    )
    in_gate = SOFTCAP * jnp.tanh(in_pre / SOFTCAP)
    capped = SOFTCAP * jnp.tanh((forget_pre + shift_row[...]) / SOFTCAP)
    small_part = jnp.exp(-jnp.abs(capped))
    above_one = 1.0 + small_part
    grown = jnp.where(
        above_one == 1.0, small_part, jnp.log(above_one) * small_part / (above_one - 1.0)
    )
    log_forget = jnp.minimum(capped, 0.0) - grown
    earlier = lax.broadcasted_iota(jnp.int32, (ROWS, ROWS), 0) <= lax.broadcasted_iota(
        jnp.int32, (ROWS, ROWS), 1
    )
    cumulative = jnp.dot(
        jnp.broadcast_to(log_forget, (8, ROWS)),
        earlier.astype(f32),
        precision=PRECISE,
        preferred_element_type=f32,
    )
    top_rows = lax.broadcasted_iota(jnp.int32, (8, ROWS), 0) == 0
    gate_ref[...] = jnp.where(top_rows, in_gate - cumulative, cumulative)
    after_gates()
    exchange.relay()
    query_exchange.relay()
    key_turned = rotated(second, LATENT_PART)
    kv_ref[2 * ROWS :] = jnp.where(
        lane < ROTARY_CHANNELS, key_turned[:half], key_turned[half:]
    ).astype(bf16)
    exchange.near()
    after_exchange()
    exchange.far()

    squares = jnp.zeros((half, width), f32)
    for s in range(N_Y * N_C):
        part = latents[s].astype(f32)
        squares = squares + part * part
    low = lane < LATENT_PART
    low_scale, high_scale = (
        lax.rsqrt(
            jnp.sum(jnp.where(low == first, squares, 0.0), axis=1, keepdims=True) / LATENT_WIDTH
            + SMALL_CONSTANT
        )
        for first in (True, False)
    )
    latent_scale = jnp.where(low, low_scale, high_scale)
    query_gains = jnp.broadcast_to(query_gain[...].reshape(1, -1), (8, QUERY_LATENT))
    latent_gains = jnp.broadcast_to(latent_gain[...].reshape(1, -1), (8, LATENT_WIDTH))

    def latent_gain_of(s):
        pair = slice((s // 2) * width, (s // 2 + 1) * width)
        shift = LATENT_WIDTH - LATENT_PART if s % 2 else LATENT_PART
        here = latent_gains[:1, pair]
        other = pltpu.roll(latent_gains, shift, 1)[:1, pair]
        return jnp.where(low, other, here) if s % 2 else jnp.where(low, here, other)

    def query_gain_of(s):
        turned = query_gains
        if s:
            turned = pltpu.roll(query_gains, QUERY_LATENT - s * QUERY_PART, 1)
        return turned[:1, :width]

    for s in range(N_Y * N_C):
        columns = slice(s * width, (s + 1) * width)
        part = latents[s].astype(f32)
        made = (part * latent_scale * latent_gain_of(s)).astype(bf16)
        wide_latent[:half, columns] = jnp.where(low, made, jnp.zeros_like(made))
        wide_latent[half:, columns] = jnp.where(low, jnp.zeros_like(made), made)
    made = jnp.dot(wide_latent[...], up_latent[...], preferred_element_type=f32).astype(bf16)
    kv_ref[:ROWS] = made[:, :width]
    kv_ref[ROWS : 2 * ROWS] = made[:, width:]
    after_keys()

    query_exchange.near()
    query_exchange.far()
    query_mask = (lane < QUERY_PART).astype(f32)
    squares = jnp.zeros((ROWS, width), f32)
    for s in range(N_Y * N_C):
        part = query_latents[s].astype(f32) * query_mask
        squares = squares + part * part
    query_scale = lax.rsqrt(
        jnp.sum(squares, axis=1, keepdims=True) / QUERY_LATENT + SMALL_CONSTANT
    )
    for s in range(N_Y * N_C):
        columns = slice(s * width, (s + 1) * width)
        part = query_latents[s].astype(f32) * query_mask
        wide_query[:, columns] = (part * query_scale * query_gain_of(s)).astype(bf16)
    made = jnp.dot(wide_query[...], up_query[...], preferred_element_type=f32).astype(bf16)
    q_ref[:, :width] = made[:, :width]
    turning = jnp.concatenate([made[:, width:], jnp.zeros((ROWS, ROTARY_CHANNELS), bf16)], axis=1)
    q_ref[:, width:] = rotated(turning, 0).astype(bf16)
    return gather.started + exchange.started + query_exchange.started


def output_phase(
    gated,
    attended,
    out_memory,
    out_attend,
    o_ref,
    kept,
    to_core,
    from_core,
    sums,
    passing,
    from_below,
    from_above,
    relay_in,
    core_send,
    core_recv,
    relay_send,
    relay_recv,
    up_send,
    up_recv,
    down_send,
    down_recv,
):
    f32, bf16 = jnp.float32, jnp.bfloat16
    y, c = lax.axis_index("y"), lax.axis_index("c")
    above, below = lax.rem(y + 1, N_Y), lax.rem(y + N_Y - 1, N_Y)
    opposite = lax.rem(y + 2, N_Y)
    half = out_memory.shape[1] // 2
    tile = 512

    def remote(source, target, send, recv, device):
        return pltpu.make_async_remote_copy(
            src_ref=source,
            dst_ref=target,
            send_sem=send,
            recv_sem=recv,
            device_id=device,
            device_id_type=MESH_ID,
        )

    def rows_of(ref, core):
        picked = [ref[pl.ds(pl.multiple_of((k * N_C + core) * SHARE, SHARE), SHARE)] for k in range(N_Y)]
        return jnp.concatenate(picked, axis=0)

    def columns_of(h, t):
        return slice(h * half + t * tile, h * half + (t + 1) * tile)

    for k, core in enumerate((1 - c, c)):
        memory_rows = rows_of(gated, core)
        for h in range(2):
            for t in range(half // tile):
                kept[k, h, :, t * tile : (t + 1) * tile] = jnp.dot(
                    memory_rows, out_memory[:, columns_of(h, t)], preferred_element_type=f32
                )
    yield

    def partial(k, h, store):
        attend_rows = rows_of(attended, c if k else 1 - c)
        for t in range(half // tile):
            made = jnp.dot(
                attend_rows, out_attend[:, columns_of(h, t)], preferred_element_type=f32
            )
            made = kept[k, h, :, t * tile : (t + 1) * tile] + made
            store(t * tile, made.astype(bf16).reshape(N_Y, SHARE, tile))

    def core_copy(h):
        return remote(
            to_core.at[h], from_core.at[h], core_send.at[h], core_recv.at[h], {"c": 1 - c}
        )

    def relay_copy(h):
        return remote(
            passing.at[h],
            relay_in.at[h],
            relay_send.at[h],
            relay_recv.at[h],
            {"y": above if h == 0 else below},
        )

    def up_copy(h):
        return remote(
            passing.at[2 + h], from_below.at[h], up_send.at[h], up_recv.at[h], {"y": above}
        )

    def down_copy(h):
        return remote(
            passing.at[4 + h], from_above.at[h], down_send.at[h], down_recv.at[h], {"y": below}
        )

    started = []

    def start(copy):
        copy.start()
        started.append(copy)

    for h in range(2):

        def keep(at, block, h=h):
            to_core[h, :, :, at : at + tile] = block

        partial(0, h, keep)
        start(core_copy(h))
    for h in range(2):

        def keep(at, block, h=h):
            sums[h, :, :, at : at + tile] = block.astype(f32)

        partial(1, h, keep)
    for h in range(2):
        core_copy(h).wait_recv()
        sums[h] = sums[h] + from_core[h].astype(f32)
        passing[h] = sums[h, opposite].astype(bf16)
        start(relay_copy(h))
        if h == 0:
            passing[4] = sums[0, below].astype(bf16)
            start(down_copy(0))
        else:
            passing[3] = sums[1, above].astype(bf16)
            start(up_copy(1))
    relay_copy(0).wait_recv()
    passing[2] = (sums[0, above] + relay_in[0].astype(f32)).astype(bf16)
    start(up_copy(0))
    relay_copy(1).wait_recv()
    passing[5] = (sums[1, below] + relay_in[1].astype(f32)).astype(bf16)
    start(down_copy(1))
    for h in (1, 0):
        up_copy(h).wait_recv()
        down_copy(h).wait_recv()
        made = sums[h, y] + from_below[h].astype(f32) + from_above[h].astype(f32)
        o_ref[:, h * half : (h + 1) * half] = made.astype(bf16)
    yield started


def scratch(depth, mem_width):
    f32, bf16 = jnp.float32, jnp.bfloat16
    dma = pltpu.SemaphoreType.DMA
    between = (
        pltpu.VMEM((ROWS, VALUE_CHANNELS), bf16),
        pltpu.VMEM((ROWS, M_V), bf16),
        pltpu.VMEM((ROWS, mem_width), bf16),
        pltpu.VMEM((8, ROWS), f32),
        pltpu.VMEM((ROWS, 256), bf16),
        pltpu.VMEM((ROWS * 5 // 2, 128), bf16),
        pltpu.VMEM((M_V, depth), bf16),
        pltpu.VMEM((VALUE_CHANNELS, depth), bf16),
        dma((2,)),
    )
    for_project = (
        pltpu.VMEM((N_Y * N_C, SHARE, depth), bf16),
        pltpu.VMEM((N_Y * N_C, ROWS, 128), bf16),
        pltpu.VMEM((N_Y * N_C, ROWS // 2, 128), bf16),
        pltpu.VMEM((256, depth), bf16),
        pltpu.VMEM((8, depth), bf16),
        pltpu.VMEM((8, depth), bf16),
        pltpu.VMEM((depth, mem_width), bf16),
        pltpu.VMEM((PLAIN_CHANNELS + ROTARY_CHANNELS, QUERY_LATENT), bf16),
        pltpu.VMEM((LATENT_WIDTH, PLAIN_CHANNELS), bf16),
        pltpu.VMEM((LATENT_WIDTH, VALUE_CHANNELS), bf16),
        pltpu.VMEM((SHARE, depth), bf16),
        pltpu.VMEM((1, ROWS), f32),
        pltpu.VMEM((2, 8, ROWS), f32),
        pltpu.VMEM((1024, PLAIN_CHANNELS + ROTARY_CHANNELS), bf16),
        pltpu.VMEM((1024, 256), bf16),
        pltpu.VMEM((ROWS, 1024), bf16),
        pltpu.VMEM((ROWS, 1024), bf16),
        dma((16,)),
        dma((11,)),
        dma((11,)),
        dma((11,)),
        dma((11,)),
        dma((11,)),
        dma((11,)),
    )
    for_attend = (
        pltpu.VMEM((N_X, ROWS, 256), bf16),
        pltpu.VMEM((N_Z, ROWS * 5 // 2, 128), bf16),
        pltpu.VMEM((ROWS, 256), bf16),
        pltpu.VMEM((N_X * ROWS, 128), f32),
        pltpu.VMEM((N_X * ROWS, 128), f32),
        pltpu.VMEM((N_X * ROWS, VALUE_CHANNELS), f32),
        pltpu.VMEM((N_X - 1, ROWS, VALUE_CHANNELS), bf16),
        pltpu.VMEM((N_X - 1, 8, ROWS), f32),
        pltpu.VMEM((N_X - 1, ROWS, VALUE_CHANNELS), bf16),
        pltpu.VMEM((N_X - 1, 8, ROWS), f32),
        pltpu.VMEM((ROWS, M_V), f32),
        pltpu.VMEM((ROWS, 128), f32),
        pltpu.VMEM((ROWS, 128), f32),
        pltpu.VMEM((N_X, STATE_ROWS, M_V), f32),
        pltpu.VMEM((N_X, STATE_ROWS, M_V), f32),
        pltpu.VMEM((STATE_ROWS, M_V), f32),
        pltpu.VMEM((N_Z, STATE_ROWS, M_V), f32),
        pltpu.VMEM((N_X, STATE_ROWS, M_V), f32),
        pltpu.VMEM((N_X, STATE_ROWS, M_V), f32),
        pltpu.VMEM((2, 8, ROWS), f32),
        pltpu.VMEM((N_Y, 8, ROWS), f32),
        pltpu.VMEM((2, ROWS // 2, VALUE_CHANNELS), bf16),
        dma((6,)),
        dma((6,)),
        dma((N_Z // 2, 2)),
        dma((N_Z // 2, 2)),
        dma((N_Z // 2, 2)),
        dma((N_Z // 2, 2)),
        dma((N_X - 1,)),
        dma((N_X - 1,)),
        dma((N_X - 1,)),
        dma((N_X - 1,)),
        dma((N_X - 1,)),
        dma((N_X - 1,)),
        dma((N_Z,)),
        dma((N_Z,)),
        dma((N_X - 1,)),
        dma((N_X - 1,)),
        dma((N_Y,)),
        dma((N_Y,)),
        dma((2, 2)),
        dma((2, 2)),
    )
    for_output = (
        pltpu.VMEM((2, 2, N_Y * SHARE, depth // 2), f32),
        pltpu.VMEM((2, N_Y, SHARE, depth // 2), bf16),
        pltpu.VMEM((2, N_Y, SHARE, depth // 2), bf16),
        pltpu.VMEM((2, N_Y, SHARE, depth // 2), f32),
        pltpu.VMEM((6, SHARE, depth // 2), bf16),
        pltpu.VMEM((2, SHARE, depth // 2), bf16),
        pltpu.VMEM((2, SHARE, depth // 2), bf16),
        pltpu.VMEM((2, SHARE, depth // 2), bf16),
        dma((2,)),
        dma((2,)),
        dma((2,)),
        dma((2,)),
        dma((2,)),
        dma((2,)),
        dma((2,)),
        dma((2,)),
    )
    return between, for_project, for_attend, for_output


N_INPUTS = 22
N_PROJECT_INPUTS = 19
IN_VMEM = (1, 2, 3, 4, 5, 19)


def layer_kernel(counts, *refs):
    y, c = lax.axis_index("y"), lax.axis_index("c")
    z, x = lax.axis_index("z"), lax.axis_index("x")
    project_inputs = refs[:N_PROJECT_INPUTS]
    mem_gain, out_memory_hbm, out_attend_hbm, out_ref = refs[N_PROJECT_INPUTS : N_INPUTS + 1]
    groups, at = [], N_INPUTS + 1
    for count in counts:
        groups.append(refs[at : at + count])
        at += count
    between, for_project, for_attend, for_output = groups
    attended, gated, mem, gates, queries, keys_values, out_memory, out_attend, out_sem = between

    barrier = pltpu.get_barrier_semaphore()
    devices = [{"c": 1 - c}]
    devices += [{"y": lax.rem(y + d, N_Y)} for d in range(1, N_Y)]
    devices += [{"x": lax.rem(x + d, N_X)} for d in range(1, N_X)]
    devices += [{"z": lax.rem(z + d, N_Z)} for d in range(1, N_Z)]
    for device in devices:
        pl.semaphore_signal(barrier, inc=1, device_id=device, device_id_type=MESH_ID)
    loads = [
        pltpu.make_async_copy(out_memory_hbm, out_memory, out_sem.at[0]),
        pltpu.make_async_copy(out_attend_hbm, out_attend, out_sem.at[1]),
    ]
    attending = attend_phase(
        queries, keys_values, mem, gates, mem_gain, attended, gated, *for_attend
    )
    started = project_phase(
        lambda: pl.semaphore_wait(barrier, len(devices)),
        *[lambda: next(attending)] * 3,
        *project_inputs,
        mem,
        gates,
        queries,
        keys_values,
        *for_project,
    )
    for load in loads:
        load.start()
    outputting = output_phase(gated, attended, out_memory, out_attend, out_ref, *for_output)
    next(attending)
    for load in loads:
        load.wait()
    next(outputting)
    more, finish_columns = next(attending)
    started += more
    started += next(outputting)
    for copy in started:
        copy.wait_send()
    finish_columns()


def layer(*inputs):
    depth = inputs[0].shape[1]
    mem_width = 2 * M_QK + 2 * M_V
    groups = scratch(depth, mem_width)
    vmem = pl.BlockSpec(memory_space=pltpu.VMEM)
    hbm = pl.BlockSpec(memory_space=pltpu.HBM)
    return pl.pallas_call(
        functools.partial(layer_kernel, tuple(len(group) for group in groups)),
        out_shape=jax.ShapeDtypeStruct((SHARE, depth), jnp.bfloat16),
        in_specs=[vmem if k in IN_VMEM else hbm for k in range(N_INPUTS)],
        out_specs=vmem,
        scratch_shapes=[one for group in groups for one in group],
        compiler_params=pltpu.CompilerParams(
            collective_id=1, has_side_effects=True, vmem_limit_bytes=67_000_000
        ),
        cost_estimate=pl.CostEstimate(
            flops=8 * 10**9, bytes_accessed=2 * 10**7, transcendentals=4 * 10**6
        ),
        name="layer",
    )(*inputs)


def per_device(
    tokens,
    input_gain,
    weight_query,
    weight_key,
    weight_value,
    weight_outgate,
    weight_ingate,
    weight_forget,
    forget_shift,
    mem_gain,
    query_down_weight,
    latent_down_weight,
    down_rotary,
    query_gain,
    latent_gain,
    query_up_weight,
    key_up_weight,
    value_up_weight,
    out_memory,
    out_attend,
):
    length = forget_shift.shape[0]
    positions = lax.axis_index(SP) * length + jnp.arange(length, dtype=jnp.int32)
    halfway = ROTARY_CHANNELS // 2
    inverse = jnp.power(ROTARY_BASE, -jnp.arange(halfway, dtype=jnp.float32) / halfway)
    angles = positions.astype(jnp.float32)[None, :] * inverse[:, None]
    return layer(
        tokens,
        input_gain,
        query_gain,
        latent_gain,
        jnp.cos(angles),
        jnp.sin(angles),
        forget_shift.T,
        query_down_weight.T,
        latent_down_weight.T,
        down_rotary.T,
        weight_ingate.T,
        weight_forget.T,
        weight_query,
        weight_key,
        weight_value,
        weight_outgate,
        query_up_weight.T,
        key_up_weight,
        value_up_weight,
        mem_gain,
        out_memory,
        out_attend,
    )


def solution(mesh):
    torus = Mesh(mesh.devices.reshape(N_Z, N_X, 4, 2), SP_TP)
    in_specs = (
        P(SP_TP, None),
        P(),
        P(None, TP),
        P(None, TP),
        P(None, TP),
        P(None, TP),
        P(),
        P(),
        P(SP, TP),
        P(),
        P(None, TP),
        P(None, TP),
        P(),
        P(),
        P(),
        P(None, TP),
        P(None, TP),
        P(None, TP),
        P(TP, None),
        P(TP, None),
    )
    out_specs = P(SP_TP, None)
    return jax.shard_map(
        per_device, mesh=torus, in_specs=in_specs, out_specs=out_specs, check_vma=False
    )
```

```python
import functools

import jax
import jax.numpy as jnp
from jax import lax
from jax.experimental import pallas as pl
from jax.experimental.pallas import tpu as pltpu
from jax.sharding import Mesh
from jax.sharding import PartitionSpec as P

MEMORY_HEADS = 8
M_QK = 128
M_V = 256
PLAIN_CHANNELS = 128
ROTARY_CHANNELS = 64
VALUE_CHANNELS = 128
SP = ("z", "x")
TP = ("y", "c")
SP_TP = ("z", "x", "y", "c")


SMALL_CONSTANT = 1e-06
SOFTCAP = 15.0
ROTARY_BASE = 10000.0
PRECISE = lax.Precision.HIGHEST
FAR_BELOW = -1e30

N_Y = 4
N_C = 2
SHARE = 64
QUERY_LATENT = 768
LATENT_WIDTH = 512
QUERY_PART = QUERY_LATENT // (N_Y * N_C)
LATENT_PART = LATENT_WIDTH // (N_Y * N_C)
LOG2E = 1.4426950408889634
N_Z = 8
N_X = 4
ROWS = 512
MESH_ID = pl.DeviceIdType.MESH
CONTRACT_LAST = (((1,), (1,)), ((), ()))
CHUNK = M_QK // N_X
TALL = 512
GROUP = 1
TURNED = 128
KEYS_AT, VALUES_AT = TURNED, TURNED + ROWS
TURNED_AT = TURNED + 2 * ROWS
STATE_ROWS = CHUNK + 8
NORMAL_ROW, TOP_ROW, DECAY_ROW = CHUNK, CHUNK + 1, CHUNK + 2


def merge_states(early, late):
    moved = early[TOP_ROW : TOP_ROW + 1] + late[DECAY_ROW : DECAY_ROW + 1]
    late_top = late[TOP_ROW : TOP_ROW + 1]
    joined = jnp.maximum(moved, late_top)
    both = early * jnp.exp(moved - joined) + late * jnp.exp(late_top - joined)
    row = lax.broadcasted_iota(jnp.int32, both.shape, 0)
    decay = early[DECAY_ROW : DECAY_ROW + 1] + late[DECAY_ROW : DECAY_ROW + 1]
    return jnp.where(row == TOP_ROW, joined, jnp.where(row == DECAY_ROW, decay, both))


def in_two(values):
    high = values.astype(jnp.bfloat16)
    return high, (values - high.astype(jnp.float32)).astype(jnp.bfloat16)


def as_columns(row, width):
    return jnp.broadcast_to(row, (width, row.shape[1])).T


def attend_phase(
    q_ref,
    kv_ref,
    mem_ref,
    gate_ref,
    gain_ref,
    attended_ref,
    gated_ref,
    q_all,
    kv_all,
    k_cat,
    top,
    total,
    accum,
    part_out,
    stat_out,
    part_in,
    stat_in,
    cell,
    cell_sum,
    cell_top,
    first_out,
    first_in,
    column_out,
    column_in,
    start_out,
    start_in,
    square_out,
    square_in,
    passed,
    q_send,
    q_recv,
    up_send,
    up_recv,
    down_send,
    down_recv,
    part_send,
    part_recv,
    stat_send,
    stat_recv,
    first_send,
    first_recv,
    column_send,
    column_recv,
    start_send,
    start_recv,
    square_send,
    square_recv,
    passed_send,
    passed_recv,
    turned_send,
    turned_recv,
):
    f32, bf16 = jnp.float32, jnp.bfloat16
    z, x = lax.axis_index("z"), lax.axis_index("x")
    y, c = lax.axis_index("y"), lax.axis_index("c")
    above, below = lax.rem(z + 1, N_Z), lax.rem(z + N_Z - 1, N_Z)
    peers = [lax.rem(x + d, N_X) for d in range(1, N_X)]
    right, left = peers[0], peers[-1]
    rows_y = [lax.rem(y + d, N_Y) for d in range(1, N_Y)]
    me_tp = y * N_C + c
    half = (TURNED + 2 * ROWS) // 2
    width = PLAIN_CHANNELS

    def remote(source, target, send, recv, device):
        return pltpu.make_async_remote_copy(
            src_ref=source,
            dst_ref=target,
            send_sem=send,
            recv_sem=recv,
            device_id=device,
            device_id_type=MESH_ID,
        )

    def kv_copy(up, step, h):
        shift = (N_Z - step + 1) if up else (step - 1)
        owner = lax.rem(z + shift, N_Z)
        rows = pl.ds(pl.multiple_of(c * TURNED + h * half, 64), half)
        source = kv_ref.at[rows] if step == 1 else kv_all.at[owner, rows]
        send, recv = (up_send, up_recv) if up else (down_send, down_recv)
        return remote(
            source,
            kv_all.at[owner, rows],
            send.at[step - 1, h],
            recv.at[step - 1, h],
            {"z": above if up else below},
        )

    def turned_copy(step, up):
        owner = lax.rem(z + (N_Z - step if up else step), N_Z)
        rows = pl.ds(pl.multiple_of(c * TURNED_AT, TURNED), TURNED)
        return remote(
            kv_all.at[owner, rows],
            kv_all.at[owner, rows],
            turned_send.at[step - 1, int(up)],
            turned_recv.at[step - 1, int(up)],
            {"c": 1 - c},
        )

    q_half = ROWS // 2

    def q_copy(number):
        shift, part, to_right = (
            (0, 0, True),
            (0, 1, True),
            (0, 0, False),
            (0, 1, False),
            (N_X - 1, 0, True),
            (1, 1, False),
        )[number]
        owner = lax.rem(x + shift, N_X)
        rows = pl.ds(part * q_half, q_half)
        source = q_ref.at[rows] if shift == 0 else q_all.at[owner, rows]
        return remote(
            source,
            q_all.at[owner, rows],
            q_send.at[number],
            q_recv.at[number],
            {"x": right if to_right else left},
        )

    def part_copy(d):
        return remote(
            part_out.at[d], part_in.at[d], part_send.at[d], part_recv.at[d], {"x": peers[d]}
        )

    def far_copy(h, hop):
        rows = pl.ds(h * q_half, q_half)
        return remote(
            part_out.at[1, rows] if hop == 0 else passed.at[h],
            passed.at[h] if hop == 0 else part_in.at[1, rows],
            passed_send.at[hop, h],
            passed_recv.at[hop, h],
            {"x": right if h == 0 else left},
        )

    def stat_copy(d):
        return remote(
            stat_out.at[d], stat_in.at[d], stat_send.at[d], stat_recv.at[d], {"x": peers[d]}
        )

    def first_copy(d):
        return remote(
            first_out.at[peers[d]],
            first_in.at[x],
            first_send.at[d],
            first_recv.at[d],
            {"x": peers[d]},
        )

    def column_copy(target):
        return remote(
            column_out,
            column_in.at[z],
            column_send.at[target],
            column_recv.at[z],
            {"z": target},
        )

    def column_arrival(source):
        return remote(
            column_out,
            column_in.at[source],
            column_send.at[source],
            column_recv.at[source],
            {"z": source},
        )

    def start_copy(d):
        return remote(
            start_out.at[peers[d]],
            start_in.at[x],
            start_send.at[d],
            start_recv.at[d],
            {"x": peers[d]},
        )

    def square_copy(number):
        device = {"c": 1 - c} if number == 0 else {"y": rows_y[number - 1]}
        return remote(
            square_out.at[min(number, 1)],
            square_in.at[number],
            square_send.at[number],
            square_recv.at[number],
            device,
        )

    started = []

    def start(copy):
        copy.start()
        started.append(copy)

    relative, cumulative = gate_ref[0:1], gate_ref[1:2]
    key_scale = M_QK ** (-0.5)
    tall = 256
    for t in range(ROWS // tall):
        rows, seen = slice(t * tall, (t + 1) * tall), (t + 1) * tall
        row = lax.broadcasted_iota(jnp.int32, (tall, seen), 0) + t * tall
        col = lax.broadcasted_iota(jnp.int32, (tall, seen), 1)
        logs = jnp.where(col <= row, relative[:, :seen], -jnp.inf)
        highest = jnp.max(logs, axis=1, keepdims=True)
        affinity = lax.dot_general(
            mem_ref[rows, :M_QK],
            mem_ref[:seen, M_QK : 2 * M_QK],
            CONTRACT_LAST,
            preferred_element_type=f32,
        )
        affinity = affinity * (jnp.exp(logs - highest) * key_scale)
        values = mem_ref[:seen, 2 * M_QK : 2 * M_QK + M_V]
        cell[rows] = sum(
            jnp.dot(piece, values, preferred_element_type=f32) for piece in in_two(affinity)
        )
        cell_sum[rows] = jnp.broadcast_to(
            jnp.sum(affinity, axis=1, keepdims=True), (tall, width)
        )
        cell_top[rows] = jnp.broadcast_to(highest, (tall, width))
    ends_at = jnp.max(relative, axis=1, keepdims=True)
    weights = jnp.exp(relative - ends_at) * key_scale
    wide_key = mem_ref[:, M_QK : 2 * M_QK].astype(f32)
    normal = jnp.sum(as_columns(weights, width) * wide_key, axis=0, keepdims=True)
    values = mem_ref[:, 2 * M_QK : 2 * M_QK + M_V]
    matrix = sum(
        jnp.dot(piece, values, preferred_element_type=f32)
        for piece in in_two(wide_key.T * weights)
    )
    decay = cumulative[:, ROWS - 1 : ROWS]
    row = lax.broadcasted_iota(jnp.int32, (8, M_V), 0)
    lines = jnp.concatenate([normal, jnp.zeros_like(normal)], axis=1)
    notes = jnp.where(
        row == 0, lines, jnp.where(row == 1, ends_at + decay, jnp.where(row == 2, decay, 0.0))
    )
    for k in range(N_X):
        first_out[k, :CHUNK] = matrix[k * CHUNK : (k + 1) * CHUNK]
        first_out[k, CHUNK:] = notes
    for d in range(N_X - 1):
        start(first_copy(d))
    first_in[x] = first_out[x]

    yield

    for d in range(N_X - 1):
        first_copy(d).wait_recv()
    column = first_in[0]
    for k in range(1, N_X):
        column = merge_states(column, first_in[k])
    column_out[...] = column
    for target in range(1, N_Z):

        @pl.when(target > z)
        def _(target=target):
            column_copy(target).start()

    yield

    for h in range(2):
        for up in (True, False):
            start(kv_copy(up, 1, h))
    yield

    top[...] = jnp.full(top.shape, FAR_BELOW, f32)
    total[...] = jnp.zeros(total.shape, f32)
    for number in (0, 3, 1, 2):
        start(q_copy(number))
    accum[...] = jnp.zeros(accum.shape, f32)
    q_all[x] = q_ref[...]

    lane = lax.broadcasted_iota(jnp.int32, (TURNED, width), 1)
    low = (lane < ROTARY_CHANNELS).astype(bf16)
    high = (lane >= ROTARY_CHANNELS).astype(bf16)
    scale = LOG2E * (PLAIN_CHANNELS + ROTARY_CHANNELS) ** (-0.5)

    def keys_from(ref):
        k_cat[:, :width] = ref[KEYS_AT : KEYS_AT + ROWS]
        for k, mask in enumerate((low, low, high, high)):
            at = TURNED_AT if k % 2 else 0
            k_cat[k * TURNED : (k + 1) * TURNED, width:] = ref[at : at + TURNED] * mask

    def attend_tile(t, keys, values, masked):
        shard = t // (ROWS // TALL)
        rows = pl.ds(pl.multiple_of(t * TALL, TALL), TALL)
        inner = pl.ds(pl.multiple_of((t % (ROWS // TALL)) * TALL, TALL), TALL)
        scores = lax.dot_general(
            q_all[shard, inner], keys, CONTRACT_LAST, preferred_element_type=f32
        )
        scores = scores * scale
        if masked:
            row = lax.broadcasted_iota(jnp.int32, scores.shape, 0) + t * TALL
            col = lax.broadcasted_iota(jnp.int32, scores.shape, 1) + x * ROWS
            scores = jnp.where(col <= row, scores, -jnp.inf)
        old = top[rows]
        new = jnp.maximum(old, jnp.max(scores, axis=1, keepdims=True))
        probs = jnp.exp2(scores - jnp.concatenate([new] * (ROWS // width), axis=1))
        shrink = jnp.exp2(old - new)
        added = sum(probs[:, k : k + width] for k in range(0, ROWS, width))
        total[rows] = total[rows] * shrink + added
        accum[rows] = accum[rows] * shrink + jnp.dot(
            probs.astype(bf16), values, preferred_element_type=f32
        )
        top[rows] = new

    def attend_rows(first, last, values, masked):
        def one(g, carry):
            for u in range(GROUP):
                attend_tile(g * GROUP + u, k_cat[...], values(), masked)
            return carry

        lax.fori_loop(first, last, one, 0)

    last = N_Z // 2
    steps = ROWS // (TALL * GROUP)

    def arrived(owner, useful):
        @pl.when(useful)
        def _():
            keys_from(kv_all.at[owner])
            attend_rows(0, N_X * steps, lambda: kv_all[owner, VALUES_AT : VALUES_AT + ROWS], False)

    def take(step, h):
        for up in (True, False):
            if step == last and up != (h == 0):
                continue
            kv_copy(up, step, h).wait_recv()
            if step < last - 1 or (step == last - 1 and up == (h == 0)):
                start(kv_copy(up, step + 1, h))
        if h == 1:
            for up in (True, False):
                if step < last or up:
                    start(turned_copy(step, up))

    def use_up(step):
        turned_copy(step, True).wait_recv()
        arrived(lax.rem(z + N_Z - step, N_Z), z >= step)

    def use_down(step):
        turned_copy(step, False).wait_recv()
        arrived(lax.rem(z + step, N_Z), z + step >= N_Z)

    keys_from(kv_ref)
    own_values = lambda: kv_ref[VALUES_AT : VALUES_AT + ROWS]
    attend_rows(x * steps, (x + 1) * steps, own_values, True)

    take(1, 0)
    q_copy(0).wait_recv()
    start(q_copy(4))
    q_copy(3).wait_recv()
    start(q_copy(5))

    def gather_column(k, state):
        column_arrival(k).wait_recv()
        return merge_states(state, column_in[k])

    state = lax.fori_loop(0, z, gather_column, jnp.zeros((STATE_ROWS, M_V), f32))
    for k in range(N_X):
        start_out[k] = state
        if k < N_X - 1:
            state = merge_states(state, first_in[k])
    for d in range(N_X - 1):
        start(start_copy(d))
    start_in[x] = start_out[x]
    take(1, 1)
    for number in (1, 2, 4, 5):
        q_copy(number).wait_recv()
    attend_rows((x + 1) * steps, N_X * steps, own_values, False)
    use_up(1)
    take(2, 0)
    use_down(1)
    take(2, 1)
    use_up(2)

    for d in range(N_X - 1):
        start_copy(d).wait_recv()
    carried = jnp.concatenate([start_in[k, :CHUNK] for k in range(N_X)], axis=0)
    carried_normal = start_in[0, NORMAL_ROW : NORMAL_ROW + 1, :M_QK]
    carried_top = start_in[0, TOP_ROW : TOP_ROW + 1, :width]
    queries = mem_ref[:, :M_QK]
    from_start = sum(
        jnp.dot(queries, piece, preferred_element_type=f32) for piece in in_two(carried)
    )
    highest = jnp.maximum(carried_top, cell_top[...])
    across, within = jnp.exp(carried_top - highest), jnp.exp(cell_top[...] - highest)
    twice = lambda one: jnp.concatenate([one, one], axis=1)
    numerator = cell[...] * twice(within) + from_start * twice(across)
    denominator = cell_sum[...] * within + across * jnp.sum(
        queries.astype(f32) * carried_normal, axis=1, keepdims=True
    )
    floor = jnp.exp(-(as_columns(cumulative, width) + highest))
    made = numerator / twice(jnp.maximum(jnp.abs(denominator), floor))
    cell[...] = made
    squares = jnp.sum(made * made, axis=1, keepdims=True)
    square_out[0] = jnp.broadcast_to(squares, (ROWS, width)).T[:8]
    start(square_copy(0))

    take(3, 0)
    use_down(2)
    square_copy(0).wait_recv()
    square_out[1] = square_out[0] + square_in[0]
    for number in range(1, N_Y):
        start(square_copy(number))
    take(3, 1)
    use_up(3)
    use_down(3)

    take(4, 0)
    take(4, 1)
    turned_copy(last, True).wait_recv()

    opposite = lax.rem(z + last, N_Z)

    @pl.when(z >= last)
    def _():
        keys_from(kv_all.at[opposite])

    def finish(shard):
        @pl.when(z >= last)
        def _():
            attend_rows(
                shard * steps,
                (shard + 1) * steps,
                lambda: kv_all[opposite, VALUES_AT : VALUES_AT + ROWS],
                False,
            )

        rows = pl.ds(pl.multiple_of(shard * ROWS, ROWS), ROWS)
        summed = jnp.sum(total[rows], axis=1, keepdims=True)
        seen = summed > 0.0
        summed = jnp.maximum(summed, 1.0)
        log_total = jnp.where(seen, top[rows] + jnp.log2(summed), FAR_BELOW)
        return accum[rows] / summed, log_total

    for d in (1, 0, 2):
        part, log_total = finish(peers[d])
        part_out[d] = part.astype(bf16)
        stat_out[d] = log_total.T[:8]
        if d == 1:
            start(far_copy(0, 0))
            start(far_copy(1, 0))
        else:
            start(part_copy(d))
        start(stat_copy(d))
    own, own_log = finish(x)

    squares = square_out[1]
    for number in range(1, N_Y):
        square_copy(number).wait_recv()
        squares = squares + square_in[number]
    inverse = lax.rsqrt(squares[:1] / (MEMORY_HEADS * M_V) + SMALL_CONSTANT)
    gated = cell[...] * twice(as_columns(inverse, width)) * gain_ref[pl.ds(pl.multiple_of(me_tp * M_V, M_V), M_V)].astype(f32).reshape(1, M_V)
    gated = gated * jax.nn.sigmoid(mem_ref[:, 2 * M_QK + M_V :].astype(f32))
    gated_ref[...] = gated.astype(bf16)
    for h in range(2):
        far_copy(h, 0).wait_recv()
        start(far_copy(h, 1))
    yield


    logs = []
    for d in range(N_X - 1):
        stat_copy(d).wait_recv()
        logs.append(as_columns(stat_in[d, 0:1, :], width))
    highest = own_log
    for one in logs:
        highest = jnp.maximum(highest, one)
    weight = jnp.exp2(own_log - highest)
    numerator = own * weight
    denominator = weight
    for d in (0, 2, 1):
        if d == 1:
            far_copy(0, 1).wait_recv()
            far_copy(1, 1).wait_recv()
        else:
            part_copy(d).wait_recv()
        weight = jnp.exp2(logs[d] - highest)
        numerator = numerator + part_in[d].astype(f32) * weight
        denominator = denominator + weight
    attended_ref[...] = (numerator / denominator).astype(bf16)
    def finish_columns():
        for target in range(1, N_Z):

            @pl.when(target > z)
            def _(target=target):
                column_copy(target).wait_send()

    yield started, finish_columns


class TpGather:
    def __init__(self, full, sends, recvs):
        self.full, self.sends, self.recvs = full, sends, recvs
        self.y, self.c = lax.axis_index("y"), lax.axis_index("c")
        self.half = full.shape[1] // 2
        self.started = []

    def _copy(self, number, shift, part, target):
        slot = lax.rem(self.y + shift, N_Y) * N_C + self.c
        if part is None:
            ref = self.full.at[slot]
        else:
            ref = self.full.at[slot, pl.ds(part * self.half, self.half)]
        if target == "core":
            device = {"c": 1 - self.c}
        else:
            device = {"y": lax.rem(self.y + (1 if target == "up" else N_Y - 1), N_Y)}
        return pltpu.make_async_remote_copy(
            src_ref=ref,
            dst_ref=ref,
            send_sem=self.sends.at[number],
            recv_sem=self.recvs.at[number],
            device_id=device,
            device_id_type=MESH_ID,
        )

    def _start(self, *what):
        copy = self._copy(*what)
        copy.start()
        self.started.append(copy)

    def start(self):
        self._start(0, 0, 0, "up")
        self._start(3, 0, 1, "down")
        self._start(1, 0, 1, "up")
        self._start(2, 0, 0, "down")
        self._start(6, 0, None, "core")

    def relay(self):
        self._copy(0, 0, 0, "up").wait_recv()
        self._start(4, N_Y - 1, 0, "up")
        self._copy(3, 0, 1, "down").wait_recv()
        self._start(5, 1, 1, "down")
        self._copy(1, 0, 1, "up").wait_recv()
        self._start(7, N_Y - 1, None, "core")
        self._copy(2, 0, 0, "down").wait_recv()
        self._start(8, 1, None, "core")

    def near(self):
        for number, shift in ((6, 0), (7, N_Y - 1), (8, 1)):
            self._copy(number, shift, None, "core").wait_recv()

    def far(self):
        self._copy(4, 0, 0, "up").wait_recv()
        self._start(9, 2, 0, "core")
        self._copy(5, 0, 1, "down").wait_recv()
        self._start(10, 2, 1, "core")
        for part in range(2):
            self._copy(9 + part, 2, part, "core").wait_recv()

    def finish(self):
        for copy in self.started:
            copy.wait_send()


def project_phase(
    greeted,
    after_gates,
    after_exchange,
    after_keys,
    tokens_hbm,
    gain,
    query_gain,
    latent_gain,
    cosine_row,
    sine_row,
    shift_hbm,
    narrow_query,
    narrow_latent,
    narrow_rotary,
    narrow_ingate,
    narrow_forget,
    query_hbm,
    key_hbm,
    value_hbm,
    outgate_hbm,
    query_up_hbm,
    key_up_hbm,
    value_up_hbm,
    mem_ref,
    gate_ref,
    q_ref,
    kv_ref,
    rows_all,
    query_latents,
    latents,
    small,
    ingate,
    forget,
    big,
    query_up,
    key_up,
    value_up,
    tokens,
    shift_row,
    pre_gates,
    up_query,
    up_latent,
    wide_query,
    wide_latent,
    load_sem,
    row_send,
    row_recv,
    lat_send,
    lat_recv,
    query_send,
    query_recv,
):
    f32, bf16 = jnp.float32, jnp.bfloat16
    y, c = lax.axis_index("y"), lax.axis_index("c")
    mine = y * N_C + c
    width = 128
    sources = (
        (narrow_query, small.at[pl.ds(0, QUERY_PART)]),
        (narrow_latent, small.at[pl.ds(width, LATENT_PART)]),
        (narrow_rotary, small.at[pl.ds(width + LATENT_PART, ROTARY_CHANNELS)]),
        (narrow_ingate, ingate),
        (narrow_forget, forget),
        (query_up_hbm, query_up),
        (key_up_hbm, key_up),
        (value_up_hbm, value_up),
        (shift_hbm, shift_row),
    )
    loads = [
        pltpu.make_async_copy(source, target, load_sem.at[k])
        for k, (source, target) in enumerate(sources)
    ]
    at = 0
    for k, ref in enumerate((query_hbm, key_hbm, value_hbm, outgate_hbm)):
        columns = ref.shape[1]
        loads.append(
            pltpu.make_async_copy(ref, big.at[:, pl.ds(at, columns)], load_sem.at[9 + k])
        )
        at += columns
    arrival = pltpu.make_async_copy(tokens_hbm, tokens, load_sem.at[13])
    arrival.start()
    for load in loads:
        load.start()
    arrival.wait()
    wide = tokens[...].astype(f32)
    inverse = lax.rsqrt(jnp.mean(wide * wide, axis=1, keepdims=True) + SMALL_CONSTANT)
    rows_all[mine] = (wide * inverse * gain[...].astype(f32).reshape(1, -1)).astype(bf16)
    small[QUERY_PART:width] = jnp.zeros((width - QUERY_PART, small.shape[1]), bf16)

    greeted()
    gather = TpGather(rows_all, row_send, row_recv)
    gather.start()

    for load in loads:
        load.wait()
    small[QUERY_PART : QUERY_PART + 8] = ingate[...]
    small[QUERY_PART + 16 : QUERY_PART + 24] = forget[...]
    up_query[...] = jnp.zeros(up_query.shape, bf16)
    query_rows = query_up[...].astype(f32).T.astype(bf16)
    for s in range(N_Y * N_C):
        up_query[s * width : s * width + QUERY_PART] = query_rows[
            s * QUERY_PART : (s + 1) * QUERY_PART
        ]
        part = slice(s * LATENT_PART, (s + 1) * LATENT_PART)
        for h in range(2):
            at = s * width + h * LATENT_PART
            up_latent[at : at + LATENT_PART, :width] = key_up[part]
            up_latent[at : at + LATENT_PART, width:] = value_up[part]

    lane = lax.broadcasted_iota(jnp.int32, (1, width), 1)
    cosine, sine_part = (
        jnp.concatenate([ref[...]] * 4, axis=0).T for ref in (cosine_row, sine_row)
    )
    row_id = lax.broadcasted_iota(jnp.int32, (width, width), 0)
    col_id = lax.broadcasted_iota(jnp.int32, (width, width), 1)
    channels = lax.rem(col_id, ROTARY_CHANNELS)
    halfway = ROTARY_CHANNELS // 2
    twin = (row_id == channels).astype(bf16)
    partner = lax.rem(channels + halfway, ROTARY_CHANNELS)
    sign = jnp.where(channels < halfway, -1.0, 1.0)

    def duplicated(values, offset):
        return jnp.dot(
            values, (row_id == channels + offset).astype(bf16), preferred_element_type=f32
        )

    def rotated(values, offset):
        swap = jnp.where(row_id == partner + offset, sign, 0.0).astype(bf16)
        turned = jnp.dot(values, swap, preferred_element_type=f32)
        return duplicated(values, offset) * cosine + turned * sine_part

    def chip_rows(chip):
        slots = [rows_all[chip * N_C + k] for k in range(N_C)]
        return jnp.concatenate(slots, axis=0)

    span = N_C * SHARE
    tile = 256

    def project_small(chip):
        rows = pl.ds(pl.multiple_of(chip * span, span), span)
        here = chip_rows(chip)
        made = lax.dot_general(here, small[...], CONTRACT_LAST, preferred_element_type=f32)
        turned = made[:, :width].T
        for k in range(2):
            at = QUERY_PART + 16 * k
            pre_gates[k, :, rows] = turned[at : at + 8]
        rounded = made.astype(bf16)
        query_latents[mine, rows] = rounded[:, :width]
        wide_latent[rows, :width] = rounded[:, width:]

    def project_big():
        def one(t, carry):
            columns = pl.ds(pl.multiple_of(t * tile, tile), tile)
            rows = rows_all[...].reshape(ROWS, rows_all.shape[2])
            made = jnp.dot(rows, big[:, columns], preferred_element_type=f32)
            mem_ref[:, columns] = made.astype(bf16)
            return carry

        lax.fori_loop(0, big.shape[1] // tile, one, 0)

    gather.relay()
    gather.near()
    near = [y, lax.rem(y + N_Y - 1, N_Y), lax.rem(y + 1, N_Y)]
    for chip in near:
        project_small(chip)
    opposite = lax.rem(y + 2, N_Y)
    gather.far()
    project_small(opposite)

    second = wide_latent[:, :width]
    both = duplicated(second, 0)
    half = ROWS // 2
    packed = jnp.where(lane < LATENT_PART, both[:half], both[half:])
    latents[mine] = packed.astype(bf16)
    exchange = TpGather(latents, lat_send, lat_recv)
    query_exchange = TpGather(query_latents, query_send, query_recv)
    exchange.start()
    query_exchange.start()
    project_big()
    heads = lax.broadcasted_iota(jnp.int32, (8, ROWS), 0) == mine
    in_pre, forget_pre = (
        jnp.sum(jnp.where(heads, pre_gates[k], 0.0), axis=0, keepdims=True) for k in range(2)
    )
    in_gate = SOFTCAP * jnp.tanh(in_pre / SOFTCAP)
    capped = SOFTCAP * jnp.tanh((forget_pre + shift_row[...]) / SOFTCAP)
    small_part = jnp.exp(-jnp.abs(capped))
    above_one = 1.0 + small_part
    grown = jnp.where(
        above_one == 1.0, small_part, jnp.log(above_one) * small_part / (above_one - 1.0)
    )
    log_forget = jnp.minimum(capped, 0.0) - grown
    earlier = lax.broadcasted_iota(jnp.int32, (ROWS, ROWS), 0) <= lax.broadcasted_iota(
        jnp.int32, (ROWS, ROWS), 1
    )
    cumulative = jnp.dot(
        jnp.broadcast_to(log_forget, (8, ROWS)),
        earlier.astype(f32),
        precision=PRECISE,
        preferred_element_type=f32,
    )
    top_rows = lax.broadcasted_iota(jnp.int32, (8, ROWS), 0) == 0
    gate_ref[...] = jnp.where(top_rows, in_gate - cumulative, cumulative)
    after_gates()
    exchange.relay()
    query_exchange.relay()
    key_turned = rotated(second, LATENT_PART)
    key_turned = jnp.where(
        lane < ROTARY_CHANNELS, key_turned[:half], key_turned[half:]
    ).astype(bf16)
    kv_ref[:TURNED] = key_turned[:TURNED]
    kv_ref[TURNED_AT:] = key_turned[TURNED:]
    exchange.near()
    after_exchange()
    exchange.far()

    squares = jnp.zeros((half, width), f32)
    for s in range(N_Y * N_C):
        part = latents[s].astype(f32)
        squares = squares + part * part
    low = lane < LATENT_PART
    low_scale, high_scale = (
        lax.rsqrt(
            jnp.sum(jnp.where(low == first, squares, 0.0), axis=1, keepdims=True) / LATENT_WIDTH
            + SMALL_CONSTANT
        )
        for first in (True, False)
    )
    latent_scale = jnp.where(low, low_scale, high_scale)
    query_gains = jnp.broadcast_to(query_gain[...].reshape(1, -1), (8, QUERY_LATENT))
    latent_gains = jnp.broadcast_to(latent_gain[...].reshape(1, -1), (8, LATENT_WIDTH))

    def latent_gain_of(s):
        pair = slice((s // 2) * width, (s // 2 + 1) * width)
        shift = LATENT_WIDTH - LATENT_PART if s % 2 else LATENT_PART
        here = latent_gains[:1, pair]
        other = pltpu.roll(latent_gains, shift, 1)[:1, pair]
        return jnp.where(low, other, here) if s % 2 else jnp.where(low, here, other)

    def query_gain_of(s):
        turned = query_gains
        if s:
            turned = pltpu.roll(query_gains, QUERY_LATENT - s * QUERY_PART, 1)
        return turned[:1, :width]

    for s in range(N_Y * N_C):
        columns = slice(s * width, (s + 1) * width)
        part = latents[s].astype(f32)
        made = (part * latent_scale * latent_gain_of(s)).astype(bf16)
        wide_latent[:half, columns] = jnp.where(low, made, jnp.zeros_like(made))
        wide_latent[half:, columns] = jnp.where(low, jnp.zeros_like(made), made)
    made = jnp.dot(wide_latent[...], up_latent[...], preferred_element_type=f32).astype(bf16)
    kv_ref[KEYS_AT : KEYS_AT + ROWS] = made[:, :width]
    kv_ref[VALUES_AT : VALUES_AT + ROWS] = made[:, width:]
    after_keys()

    query_exchange.near()
    query_exchange.far()
    query_mask = (lane < QUERY_PART).astype(f32)
    squares = jnp.zeros((ROWS, width), f32)
    for s in range(N_Y * N_C):
        part = query_latents[s].astype(f32) * query_mask
        squares = squares + part * part
    query_scale = lax.rsqrt(
        jnp.sum(squares, axis=1, keepdims=True) / QUERY_LATENT + SMALL_CONSTANT
    )
    for s in range(N_Y * N_C):
        columns = slice(s * width, (s + 1) * width)
        part = query_latents[s].astype(f32) * query_mask
        wide_query[:, columns] = (part * query_scale * query_gain_of(s)).astype(bf16)
    made = jnp.dot(wide_query[...], up_query[...], preferred_element_type=f32).astype(bf16)
    q_ref[:, :width] = made[:, :width]
    turning = jnp.concatenate([made[:, width:], jnp.zeros((ROWS, ROTARY_CHANNELS), bf16)], axis=1)
    q_ref[:, width:] = rotated(turning, 0).astype(bf16)
    return gather.started + exchange.started + query_exchange.started


def output_phase(
    gated,
    attended,
    out_memory,
    out_attend,
    o_ref,
    kept,
    to_core,
    from_core,
    sums,
    passing,
    from_below,
    from_above,
    relay_in,
    core_send,
    core_recv,
    relay_send,
    relay_recv,
    up_send,
    up_recv,
    down_send,
    down_recv,
):
    f32, bf16 = jnp.float32, jnp.bfloat16
    y, c = lax.axis_index("y"), lax.axis_index("c")
    above, below = lax.rem(y + 1, N_Y), lax.rem(y + N_Y - 1, N_Y)
    opposite = lax.rem(y + 2, N_Y)
    half = out_memory.shape[1] // 2
    tile = 512

    def remote(source, target, send, recv, device):
        return pltpu.make_async_remote_copy(
            src_ref=source,
            dst_ref=target,
            send_sem=send,
            recv_sem=recv,
            device_id=device,
            device_id_type=MESH_ID,
        )

    def rows_of(ref, core):
        picked = [ref[pl.ds(pl.multiple_of((k * N_C + core) * SHARE, SHARE), SHARE)] for k in range(N_Y)]
        return jnp.concatenate(picked, axis=0)

    def columns_of(h, t):
        return slice(h * half + t * tile, h * half + (t + 1) * tile)

    for k, core in enumerate((1 - c, c)):
        memory_rows = rows_of(gated, core)
        for h in range(2):
            for t in range(half // tile):
                kept[k, h, :, t * tile : (t + 1) * tile] = jnp.dot(
                    memory_rows, out_memory[:, columns_of(h, t)], preferred_element_type=f32
                )
    yield

    def partial(k, h, store):
        attend_rows = rows_of(attended, c if k else 1 - c)
        for t in range(half // tile):
            made = jnp.dot(
                attend_rows, out_attend[:, columns_of(h, t)], preferred_element_type=f32
            )
            made = kept[k, h, :, t * tile : (t + 1) * tile] + made
            store(t * tile, made.astype(bf16).reshape(N_Y, SHARE, tile))

    def core_copy(h):
        return remote(
            to_core.at[h], from_core.at[h], core_send.at[h], core_recv.at[h], {"c": 1 - c}
        )

    def relay_copy(h):
        return remote(
            passing.at[h],
            relay_in.at[h],
            relay_send.at[h],
            relay_recv.at[h],
            {"y": above if h == 0 else below},
        )

    def up_copy(h):
        return remote(
            passing.at[2 + h], from_below.at[h], up_send.at[h], up_recv.at[h], {"y": above}
        )

    def down_copy(h):
        return remote(
            passing.at[4 + h], from_above.at[h], down_send.at[h], down_recv.at[h], {"y": below}
        )

    started = []

    def start(copy):
        copy.start()
        started.append(copy)

    for h in range(2):

        def keep(at, block, h=h):
            to_core[h, :, :, at : at + tile] = block

        partial(0, h, keep)
        start(core_copy(h))
    for h in range(2):

        def keep(at, block, h=h):
            sums[h, :, :, at : at + tile] = block.astype(f32)

        partial(1, h, keep)
    for h in range(2):
        core_copy(h).wait_recv()
        sums[h] = sums[h] + from_core[h].astype(f32)
        passing[h] = sums[h, opposite].astype(bf16)
        start(relay_copy(h))
        if h == 0:
            passing[4] = sums[0, below].astype(bf16)
            start(down_copy(0))
        else:
            passing[3] = sums[1, above].astype(bf16)
            start(up_copy(1))
    relay_copy(0).wait_recv()
    passing[2] = (sums[0, above] + relay_in[0].astype(f32)).astype(bf16)
    start(up_copy(0))
    relay_copy(1).wait_recv()
    passing[5] = (sums[1, below] + relay_in[1].astype(f32)).astype(bf16)
    start(down_copy(1))
    for h in (1, 0):
        up_copy(h).wait_recv()
        down_copy(h).wait_recv()
        made = sums[h, y] + from_below[h].astype(f32) + from_above[h].astype(f32)
        o_ref[:, h * half : (h + 1) * half] = made.astype(bf16)
    yield started


def scratch(depth, mem_width):
    f32, bf16 = jnp.float32, jnp.bfloat16
    dma = pltpu.SemaphoreType.DMA
    between = (
        pltpu.VMEM((ROWS, VALUE_CHANNELS), bf16),
        pltpu.VMEM((ROWS, M_V), bf16),
        pltpu.VMEM((ROWS, mem_width), bf16),
        pltpu.VMEM((8, ROWS), f32),
        pltpu.VMEM((ROWS, 256), bf16),
        pltpu.VMEM((ROWS * 5 // 2, 128), bf16),
        pltpu.VMEM((M_V, depth), bf16),
        pltpu.VMEM((VALUE_CHANNELS, depth), bf16),
        dma((2,)),
    )
    for_project = (
        pltpu.VMEM((N_Y * N_C, SHARE, depth), bf16),
        pltpu.VMEM((N_Y * N_C, ROWS, 128), bf16),
        pltpu.VMEM((N_Y * N_C, ROWS // 2, 128), bf16),
        pltpu.VMEM((256, depth), bf16),
        pltpu.VMEM((8, depth), bf16),
        pltpu.VMEM((8, depth), bf16),
        pltpu.VMEM((depth, mem_width), bf16),
        pltpu.VMEM((PLAIN_CHANNELS + ROTARY_CHANNELS, QUERY_LATENT), bf16),
        pltpu.VMEM((LATENT_WIDTH, PLAIN_CHANNELS), bf16),
        pltpu.VMEM((LATENT_WIDTH, VALUE_CHANNELS), bf16),
        pltpu.VMEM((SHARE, depth), bf16),
        pltpu.VMEM((1, ROWS), f32),
        pltpu.VMEM((2, 8, ROWS), f32),
        pltpu.VMEM((1024, PLAIN_CHANNELS + ROTARY_CHANNELS), bf16),
        pltpu.VMEM((1024, 256), bf16),
        pltpu.VMEM((ROWS, 1024), bf16),
        pltpu.VMEM((ROWS, 1024), bf16),
        dma((16,)),
        dma((11,)),
        dma((11,)),
        dma((11,)),
        dma((11,)),
        dma((11,)),
        dma((11,)),
    )
    for_attend = (
        pltpu.VMEM((N_X, ROWS, 256), bf16),
        pltpu.VMEM((N_Z, ROWS * 5 // 2, 128), bf16),
        pltpu.VMEM((ROWS, 256), bf16),
        pltpu.VMEM((N_X * ROWS, 128), f32),
        pltpu.VMEM((N_X * ROWS, 128), f32),
        pltpu.VMEM((N_X * ROWS, VALUE_CHANNELS), f32),
        pltpu.VMEM((N_X - 1, ROWS, VALUE_CHANNELS), bf16),
        pltpu.VMEM((N_X - 1, 8, ROWS), f32),
        pltpu.VMEM((N_X - 1, ROWS, VALUE_CHANNELS), bf16),
        pltpu.VMEM((N_X - 1, 8, ROWS), f32),
        pltpu.VMEM((ROWS, M_V), f32),
        pltpu.VMEM((ROWS, 128), f32),
        pltpu.VMEM((ROWS, 128), f32),
        pltpu.VMEM((N_X, STATE_ROWS, M_V), f32),
        pltpu.VMEM((N_X, STATE_ROWS, M_V), f32),
        pltpu.VMEM((STATE_ROWS, M_V), f32),
        pltpu.VMEM((N_Z, STATE_ROWS, M_V), f32),
        pltpu.VMEM((N_X, STATE_ROWS, M_V), f32),
        pltpu.VMEM((N_X, STATE_ROWS, M_V), f32),
        pltpu.VMEM((2, 8, ROWS), f32),
        pltpu.VMEM((N_Y, 8, ROWS), f32),
        pltpu.VMEM((2, ROWS // 2, VALUE_CHANNELS), bf16),
        dma((6,)),
        dma((6,)),
        dma((N_Z // 2, 2)),
        dma((N_Z // 2, 2)),
        dma((N_Z // 2, 2)),
        dma((N_Z // 2, 2)),
        dma((N_X - 1,)),
        dma((N_X - 1,)),
        dma((N_X - 1,)),
        dma((N_X - 1,)),
        dma((N_X - 1,)),
        dma((N_X - 1,)),
        dma((N_Z,)),
        dma((N_Z,)),
        dma((N_X - 1,)),
        dma((N_X - 1,)),
        dma((N_Y,)),
        dma((N_Y,)),
        dma((2, 2)),
        dma((2, 2)),
        dma((N_Z // 2, 2)),
        dma((N_Z // 2, 2)),
    )
    for_output = (
        pltpu.VMEM((2, 2, N_Y * SHARE, depth // 2), f32),
        pltpu.VMEM((2, N_Y, SHARE, depth // 2), bf16),
        pltpu.VMEM((2, N_Y, SHARE, depth // 2), bf16),
        pltpu.VMEM((2, N_Y, SHARE, depth // 2), f32),
        pltpu.VMEM((6, SHARE, depth // 2), bf16),
        pltpu.VMEM((2, SHARE, depth // 2), bf16),
        pltpu.VMEM((2, SHARE, depth // 2), bf16),
        pltpu.VMEM((2, SHARE, depth // 2), bf16),
        dma((2,)),
        dma((2,)),
        dma((2,)),
        dma((2,)),
        dma((2,)),
        dma((2,)),
        dma((2,)),
        dma((2,)),
    )
    return between, for_project, for_attend, for_output


N_INPUTS = 22
N_PROJECT_INPUTS = 19
IN_VMEM = (1, 2, 3, 4, 5, 19)


def layer_kernel(counts, *refs):
    y, c = lax.axis_index("y"), lax.axis_index("c")
    z, x = lax.axis_index("z"), lax.axis_index("x")
    project_inputs = refs[:N_PROJECT_INPUTS]
    mem_gain, out_memory_hbm, out_attend_hbm, out_ref = refs[N_PROJECT_INPUTS : N_INPUTS + 1]
    groups, at = [], N_INPUTS + 1
    for count in counts:
        groups.append(refs[at : at + count])
        at += count
    between, for_project, for_attend, for_output = groups
    attended, gated, mem, gates, queries, keys_values, out_memory, out_attend, out_sem = between

    barrier = pltpu.get_barrier_semaphore()
    devices = [{"c": 1 - c}]
    devices += [{"y": lax.rem(y + d, N_Y)} for d in range(1, N_Y)]
    devices += [{"x": lax.rem(x + d, N_X)} for d in range(1, N_X)]
    devices += [{"z": lax.rem(z + d, N_Z)} for d in range(1, N_Z)]
    for device in devices:
        pl.semaphore_signal(barrier, inc=1, device_id=device, device_id_type=MESH_ID)
    loads = [
        pltpu.make_async_copy(out_memory_hbm, out_memory, out_sem.at[0]),
        pltpu.make_async_copy(out_attend_hbm, out_attend, out_sem.at[1]),
    ]
    attending = attend_phase(
        queries, keys_values, mem, gates, mem_gain, attended, gated, *for_attend
    )
    started = project_phase(
        lambda: pl.semaphore_wait(barrier, len(devices)),
        *[lambda: next(attending)] * 3,
        *project_inputs,
        mem,
        gates,
        queries,
        keys_values,
        *for_project,
    )
    for load in loads:
        load.start()
    outputting = output_phase(gated, attended, out_memory, out_attend, out_ref, *for_output)
    next(attending)
    for load in loads:
        load.wait()
    next(outputting)
    more, finish_columns = next(attending)
    started += more
    started += next(outputting)
    for copy in started:
        copy.wait_send()
    finish_columns()


def layer(*inputs):
    depth = inputs[0].shape[1]
    mem_width = 2 * M_QK + 2 * M_V
    groups = scratch(depth, mem_width)
    vmem = pl.BlockSpec(memory_space=pltpu.VMEM)
    hbm = pl.BlockSpec(memory_space=pltpu.HBM)
    return pl.pallas_call(
        functools.partial(layer_kernel, tuple(len(group) for group in groups)),
        out_shape=jax.ShapeDtypeStruct((SHARE, depth), jnp.bfloat16),
        in_specs=[vmem if k in IN_VMEM else hbm for k in range(N_INPUTS)],
        out_specs=vmem,
        scratch_shapes=[one for group in groups for one in group],
        compiler_params=pltpu.CompilerParams(
            collective_id=1, has_side_effects=True, vmem_limit_bytes=67_000_000
        ),
        cost_estimate=pl.CostEstimate(
            flops=8 * 10**9, bytes_accessed=2 * 10**7, transcendentals=4 * 10**6
        ),
        name="layer",
    )(*inputs)


def per_device(
    tokens,
    input_gain,
    weight_query,
    weight_key,
    weight_value,
    weight_outgate,
    weight_ingate,
    weight_forget,
    forget_shift,
    mem_gain,
    query_down_weight,
    latent_down_weight,
    down_rotary,
    query_gain,
    latent_gain,
    query_up_weight,
    key_up_weight,
    value_up_weight,
    out_memory,
    out_attend,
):
    length = forget_shift.shape[0]
    positions = lax.axis_index(SP) * length + jnp.arange(length, dtype=jnp.int32)
    halfway = ROTARY_CHANNELS // 2
    inverse = jnp.power(ROTARY_BASE, -jnp.arange(halfway, dtype=jnp.float32) / halfway)
    angles = positions.astype(jnp.float32)[None, :] * inverse[:, None]
    return layer(
        tokens,
        input_gain,
        query_gain,
        latent_gain,
        jnp.cos(angles),
        jnp.sin(angles),
        forget_shift.T,
        query_down_weight.T,
        latent_down_weight.T,
        down_rotary.T,
        weight_ingate.T,
        weight_forget.T,
        weight_query,
        weight_key,
        weight_value,
        weight_outgate,
        query_up_weight.T,
        key_up_weight,
        value_up_weight,
        mem_gain,
        out_memory,
        out_attend,
    )


def solution(mesh):
    torus = Mesh(mesh.devices.reshape(N_Z, N_X, 4, 2), SP_TP)
    in_specs = (
        P(SP_TP, None),
        P(),
        P(None, TP),
        P(None, TP),
        P(None, TP),
        P(None, TP),
        P(),
        P(),
        P(SP, TP),
        P(),
        P(None, TP),
        P(None, TP),
        P(),
        P(),
        P(),
        P(None, TP),
        P(None, TP),
        P(None, TP),
        P(TP, None),
        P(TP, None),
    )
    out_specs = P(SP_TP, None)
    return jax.shard_map(
        per_device, mesh=torus, in_specs=in_specs, out_specs=out_specs, check_vma=False
    )
```

```python
import functools

import jax
import jax.numpy as jnp
from jax import lax
from jax.experimental import pallas as pl
from jax.experimental.pallas import tpu as pltpu
from jax.sharding import Mesh
from jax.sharding import PartitionSpec as P

MEMORY_HEADS = 8
M_QK = 128
M_V = 256
PLAIN_CHANNELS = 128
ROTARY_CHANNELS = 64
VALUE_CHANNELS = 128
SP = ("z", "x")
TP = ("y", "c")
SP_TP = ("z", "x", "y", "c")


SMALL_CONSTANT = 1e-06
SOFTCAP = 15.0
ROTARY_BASE = 10000.0
PRECISE = lax.Precision.HIGHEST
FAR_BELOW = -1e30

N_Y = 4
N_C = 2
SHARE = 64
QUERY_LATENT = 768
LATENT_WIDTH = 512
QUERY_PART = QUERY_LATENT // (N_Y * N_C)
LATENT_PART = LATENT_WIDTH // (N_Y * N_C)
LOG2E = 1.4426950408889634
N_Z = 8
N_X = 4
ROWS = 512
MESH_ID = pl.DeviceIdType.MESH
CONTRACT_LAST = (((1,), (1,)), ((), ()))
CHUNK = M_QK // N_X
TALL = 512
GROUP = 1
STATE_ROWS = CHUNK + 8
NORMAL_ROW, TOP_ROW, DECAY_ROW = CHUNK, CHUNK + 1, CHUNK + 2


def merge_states(early, late):
    moved = early[TOP_ROW : TOP_ROW + 1] + late[DECAY_ROW : DECAY_ROW + 1]
    late_top = late[TOP_ROW : TOP_ROW + 1]
    joined = jnp.maximum(moved, late_top)
    both = early * jnp.exp(moved - joined) + late * jnp.exp(late_top - joined)
    row = lax.broadcasted_iota(jnp.int32, both.shape, 0)
    decay = early[DECAY_ROW : DECAY_ROW + 1] + late[DECAY_ROW : DECAY_ROW + 1]
    return jnp.where(row == TOP_ROW, joined, jnp.where(row == DECAY_ROW, decay, both))


def in_two(values):
    high = values.astype(jnp.bfloat16)
    return high, (values - high.astype(jnp.float32)).astype(jnp.bfloat16)


def as_columns(row, width):
    return jnp.broadcast_to(row, (width, row.shape[1])).T


def attend_phase(
    q_ref,
    kv_ref,
    mem_ref,
    gate_ref,
    gain_ref,
    attended_ref,
    gated_ref,
    q_all,
    kv_all,
    k_cat,
    top,
    total,
    accum,
    part_out,
    stat_out,
    part_in,
    stat_in,
    cell,
    cell_sum,
    cell_top,
    first_out,
    first_in,
    column_out,
    column_in,
    start_out,
    start_in,
    square_out,
    square_in,
    passed,
    q_send,
    q_recv,
    up_send,
    up_recv,
    down_send,
    down_recv,
    part_send,
    part_recv,
    stat_send,
    stat_recv,
    first_send,
    first_recv,
    column_send,
    column_recv,
    start_send,
    start_recv,
    square_send,
    square_recv,
    passed_send,
    passed_recv,
):
    f32, bf16 = jnp.float32, jnp.bfloat16
    z, x = lax.axis_index("z"), lax.axis_index("x")
    y, c = lax.axis_index("y"), lax.axis_index("c")
    above, below = lax.rem(z + 1, N_Z), lax.rem(z + N_Z - 1, N_Z)
    peers = [lax.rem(x + d, N_X) for d in range(1, N_X)]
    right, left = peers[0], peers[-1]
    rows_y = [lax.rem(y + d, N_Y) for d in range(1, N_Y)]
    me_tp = y * N_C + c
    half = kv_ref.shape[0] // 2
    width = PLAIN_CHANNELS

    def remote(source, target, send, recv, device):
        return pltpu.make_async_remote_copy(
            src_ref=source,
            dst_ref=target,
            send_sem=send,
            recv_sem=recv,
            device_id=device,
            device_id_type=MESH_ID,
        )

    def kv_copy(up, step, h):
        shift = (N_Z - step + 1) if up else (step - 1)
        owner = lax.rem(z + shift, N_Z)
        rows = pl.ds(h * half, half)
        source = kv_ref.at[rows] if step == 1 else kv_all.at[owner, rows]
        send, recv = (up_send, up_recv) if up else (down_send, down_recv)
        return remote(
            source,
            kv_all.at[owner, rows],
            send.at[step - 1, h],
            recv.at[step - 1, h],
            {"z": above if up else below},
        )

    q_half = ROWS // 2

    def q_copy(number):
        shift, part, to_right = (
            (0, 0, True),
            (0, 1, True),
            (0, 0, False),
            (0, 1, False),
            (N_X - 1, 0, True),
            (1, 1, False),
        )[number]
        owner = lax.rem(x + shift, N_X)
        rows = pl.ds(part * q_half, q_half)
        source = q_ref.at[rows] if shift == 0 else q_all.at[owner, rows]
        return remote(
            source,
            q_all.at[owner, rows],
            q_send.at[number],
            q_recv.at[number],
            {"x": right if to_right else left},
        )

    def part_copy(d):
        return remote(
            part_out.at[d], part_in.at[d], part_send.at[d], part_recv.at[d], {"x": peers[d]}
        )

    def far_copy(h, hop):
        rows = pl.ds(h * q_half, q_half)
        return remote(
            part_out.at[1, rows] if hop == 0 else passed.at[h],
            passed.at[h] if hop == 0 else part_in.at[1, rows],
            passed_send.at[hop, h],
            passed_recv.at[hop, h],
            {"x": right if h == 0 else left},
        )

    def stat_copy(d):
        return remote(
            stat_out.at[d], stat_in.at[d], stat_send.at[d], stat_recv.at[d], {"x": peers[d]}
        )

    def first_copy(d):
        return remote(
            first_out.at[peers[d]],
            first_in.at[x],
            first_send.at[d],
            first_recv.at[d],
            {"x": peers[d]},
        )

    def column_copy(target):
        return remote(
            column_out,
            column_in.at[z],
            column_send.at[target],
            column_recv.at[z],
            {"z": target},
        )

    def column_arrival(source):
        return remote(
            column_out,
            column_in.at[source],
            column_send.at[source],
            column_recv.at[source],
            {"z": source},
        )

    def start_copy(d):
        return remote(
            start_out.at[peers[d]],
            start_in.at[x],
            start_send.at[d],
            start_recv.at[d],
            {"x": peers[d]},
        )

    def square_copy(number):
        device = {"c": 1 - c} if number == 0 else {"y": rows_y[number - 1]}
        return remote(
            square_out.at[min(number, 1)],
            square_in.at[number],
            square_send.at[number],
            square_recv.at[number],
            device,
        )

    started = []

    def start(copy):
        copy.start()
        started.append(copy)

    relative, cumulative = gate_ref[0:1], gate_ref[1:2]
    key_scale = M_QK ** (-0.5)
    tall = 256
    for t in range(ROWS // tall):
        rows, seen = slice(t * tall, (t + 1) * tall), (t + 1) * tall
        row = lax.broadcasted_iota(jnp.int32, (tall, seen), 0) + t * tall
        col = lax.broadcasted_iota(jnp.int32, (tall, seen), 1)
        logs = jnp.where(col <= row, relative[:, :seen], -jnp.inf)
        highest = jnp.max(logs, axis=1, keepdims=True)
        affinity = lax.dot_general(
            mem_ref[rows, :M_QK],
            mem_ref[:seen, M_QK : 2 * M_QK],
            CONTRACT_LAST,
            preferred_element_type=f32,
        )
        affinity = affinity * (jnp.exp(logs - highest) * key_scale)
        values = mem_ref[:seen, 2 * M_QK : 2 * M_QK + M_V]
        cell[rows] = sum(
            jnp.dot(piece, values, preferred_element_type=f32) for piece in in_two(affinity)
        )
        cell_sum[rows] = jnp.broadcast_to(
            jnp.sum(affinity, axis=1, keepdims=True), (tall, width)
        )
        cell_top[rows] = jnp.broadcast_to(highest, (tall, width))
    ends_at = jnp.max(relative, axis=1, keepdims=True)
    weights = jnp.exp(relative - ends_at) * key_scale
    wide_key = mem_ref[:, M_QK : 2 * M_QK].astype(f32)
    normal = jnp.sum(as_columns(weights, width) * wide_key, axis=0, keepdims=True)
    values = mem_ref[:, 2 * M_QK : 2 * M_QK + M_V]
    matrix = sum(
        jnp.dot(piece, values, preferred_element_type=f32)
        for piece in in_two(wide_key.T * weights)
    )
    decay = cumulative[:, ROWS - 1 : ROWS]
    row = lax.broadcasted_iota(jnp.int32, (8, M_V), 0)
    lines = jnp.concatenate([normal, jnp.zeros_like(normal)], axis=1)
    notes = jnp.where(
        row == 0, lines, jnp.where(row == 1, ends_at + decay, jnp.where(row == 2, decay, 0.0))
    )
    for k in range(N_X):
        first_out[k, :CHUNK] = matrix[k * CHUNK : (k + 1) * CHUNK]
        first_out[k, CHUNK:] = notes
    for d in range(N_X - 1):
        start(first_copy(d))
    first_in[x] = first_out[x]

    yield

    for d in range(N_X - 1):
        first_copy(d).wait_recv()
    column = first_in[0]
    for k in range(1, N_X):
        column = merge_states(column, first_in[k])
    column_out[...] = column
    for target in range(1, N_Z):

        @pl.when(target > z)
        def _(target=target):
            column_copy(target).start()

    yield

    for h in range(2):
        for up in (True, False):
            start(kv_copy(up, 1, h))
    yield

    top[...] = jnp.full(top.shape, FAR_BELOW, f32)
    total[...] = jnp.zeros(total.shape, f32)
    for number in (0, 3, 1, 2):
        start(q_copy(number))
    accum[...] = jnp.zeros(accum.shape, f32)
    q_all[x] = q_ref[...]

    lane = lax.broadcasted_iota(jnp.int32, (ROWS // 2, width), 1)
    low = (lane < ROTARY_CHANNELS).astype(bf16)
    high = (lane >= ROTARY_CHANNELS).astype(bf16)
    scale = LOG2E * (PLAIN_CHANNELS + ROTARY_CHANNELS) ** (-0.5)

    def keys_from(ref):
        k_cat[:, :width] = ref[:ROWS]
        packed = ref[2 * ROWS :]
        k_cat[: ROWS // 2, width:] = packed * low
        k_cat[ROWS // 2 :, width:] = packed * high

    def attend_tile(t, keys, values, masked):
        shard = t // (ROWS // TALL)
        rows = pl.ds(pl.multiple_of(t * TALL, TALL), TALL)
        inner = pl.ds(pl.multiple_of((t % (ROWS // TALL)) * TALL, TALL), TALL)
        scores = lax.dot_general(
            q_all[shard, inner], keys, CONTRACT_LAST, preferred_element_type=f32
        )
        scores = scores * scale
        if masked:
            row = lax.broadcasted_iota(jnp.int32, scores.shape, 0) + t * TALL
            col = lax.broadcasted_iota(jnp.int32, scores.shape, 1) + x * ROWS
            scores = jnp.where(col <= row, scores, -jnp.inf)
        old = top[rows]
        new = jnp.maximum(old, jnp.max(scores, axis=1, keepdims=True))
        probs = jnp.exp2(scores - jnp.concatenate([new] * (ROWS // width), axis=1))
        shrink = jnp.exp2(old - new)
        added = sum(probs[:, k : k + width] for k in range(0, ROWS, width))
        total[rows] = total[rows] * shrink + added
        accum[rows] = accum[rows] * shrink + jnp.dot(
            probs.astype(bf16), values, preferred_element_type=f32
        )
        top[rows] = new

    def attend_rows(first, last, values, masked):
        def one(g, carry):
            for u in range(GROUP):
                attend_tile(g * GROUP + u, k_cat[...], values(), masked)
            return carry

        lax.fori_loop(first, last, one, 0)

    last = N_Z // 2
    steps = ROWS // (TALL * GROUP)

    def arrived(owner, useful):
        @pl.when(useful)
        def _():
            keys_from(kv_all.at[owner])
            attend_rows(0, N_X * steps, lambda: kv_all[owner, ROWS : 2 * ROWS], False)

    def take(step, h):
        for up in (True, False):
            if step == last and up != (h == 0):
                continue
            kv_copy(up, step, h).wait_recv()
            if step < last - 1 or (step == last - 1 and up == (h == 0)):
                start(kv_copy(up, step + 1, h))

    def use_up(step):
        arrived(lax.rem(z + N_Z - step, N_Z), z >= step)

    def use_down(step):
        arrived(lax.rem(z + step, N_Z), z + step >= N_Z)

    keys_from(kv_ref)
    own_values = lambda: kv_ref[ROWS : 2 * ROWS]
    attend_rows(x * steps, (x + 1) * steps, own_values, True)

    take(1, 0)
    q_copy(0).wait_recv()
    start(q_copy(4))
    q_copy(3).wait_recv()
    start(q_copy(5))

    def gather_column(k, state):
        column_arrival(k).wait_recv()
        return merge_states(state, column_in[k])

    state = lax.fori_loop(0, z, gather_column, jnp.zeros((STATE_ROWS, M_V), f32))
    for k in range(N_X):
        start_out[k] = state
        if k < N_X - 1:
            state = merge_states(state, first_in[k])
    for d in range(N_X - 1):
        start(start_copy(d))
    start_in[x] = start_out[x]
    take(1, 1)
    for number in (1, 2, 4, 5):
        q_copy(number).wait_recv()
    attend_rows((x + 1) * steps, N_X * steps, own_values, False)
    use_up(1)
    take(2, 0)
    use_down(1)
    take(2, 1)
    use_up(2)

    for d in range(N_X - 1):
        start_copy(d).wait_recv()
    carried = jnp.concatenate([start_in[k, :CHUNK] for k in range(N_X)], axis=0)
    carried_normal = start_in[0, NORMAL_ROW : NORMAL_ROW + 1, :M_QK]
    carried_top = start_in[0, TOP_ROW : TOP_ROW + 1, :width]
    queries = mem_ref[:, :M_QK]
    from_start = sum(
        jnp.dot(queries, piece, preferred_element_type=f32) for piece in in_two(carried)
    )
    highest = jnp.maximum(carried_top, cell_top[...])
    across, within = jnp.exp(carried_top - highest), jnp.exp(cell_top[...] - highest)
    twice = lambda one: jnp.concatenate([one, one], axis=1)
    numerator = cell[...] * twice(within) + from_start * twice(across)
    denominator = cell_sum[...] * within + across * jnp.sum(
        queries.astype(f32) * carried_normal, axis=1, keepdims=True
    )
    floor = jnp.exp(-(as_columns(cumulative, width) + highest))
    made = numerator / twice(jnp.maximum(jnp.abs(denominator), floor))
    cell[...] = made
    squares = jnp.sum(made * made, axis=1, keepdims=True)
    square_out[0] = jnp.broadcast_to(squares, (ROWS, width)).T[:8]
    start(square_copy(0))

    take(3, 0)
    use_down(2)
    square_copy(0).wait_recv()
    square_out[1] = square_out[0] + square_in[0]
    for number in range(1, N_Y):
        start(square_copy(number))
    take(3, 1)
    use_up(3)
    use_down(3)

    take(4, 0)
    take(4, 1)

    opposite = lax.rem(z + last, N_Z)

    @pl.when(z >= last)
    def _():
        keys_from(kv_all.at[opposite])

    def finish(shard):
        @pl.when(z >= last)
        def _():
            attend_rows(
                shard * steps,
                (shard + 1) * steps,
                lambda: kv_all[opposite, ROWS : 2 * ROWS],
                False,
            )

        rows = pl.ds(pl.multiple_of(shard * ROWS, ROWS), ROWS)
        summed = jnp.sum(total[rows], axis=1, keepdims=True)
        seen = summed > 0.0
        summed = jnp.maximum(summed, 1.0)
        log_total = jnp.where(seen, top[rows] + jnp.log2(summed), FAR_BELOW)
        return accum[rows] / summed, log_total

    for d in (1, 0, 2):
        part, log_total = finish(peers[d])
        part_out[d] = part.astype(bf16)
        stat_out[d] = log_total.T[:8]
        if d == 1:
            start(far_copy(0, 0))
            start(far_copy(1, 0))
        else:
            start(part_copy(d))
        start(stat_copy(d))
    own, own_log = finish(x)

    squares = square_out[1]
    for number in range(1, N_Y):
        square_copy(number).wait_recv()
        squares = squares + square_in[number]
    inverse = lax.rsqrt(squares[:1] / (MEMORY_HEADS * M_V) + SMALL_CONSTANT)
    gated = cell[...] * twice(as_columns(inverse, width)) * gain_ref[pl.ds(pl.multiple_of(me_tp * M_V, M_V), M_V)].astype(f32).reshape(1, M_V)
    gated = gated * jax.nn.sigmoid(mem_ref[:, 2 * M_QK + M_V :].astype(f32))
    gated_ref[...] = gated.astype(bf16)
    for h in range(2):
        far_copy(h, 0).wait_recv()
        start(far_copy(h, 1))
    yield


    logs = []
    for d in range(N_X - 1):
        stat_copy(d).wait_recv()
        logs.append(as_columns(stat_in[d, 0:1, :], width))
    highest = own_log
    for one in logs:
        highest = jnp.maximum(highest, one)
    weight = jnp.exp2(own_log - highest)
    numerator = own * weight
    denominator = weight
    for d in (0, 2, 1):
        if d == 1:
            far_copy(0, 1).wait_recv()
            far_copy(1, 1).wait_recv()
        else:
            part_copy(d).wait_recv()
        weight = jnp.exp2(logs[d] - highest)
        numerator = numerator + part_in[d].astype(f32) * weight
        denominator = denominator + weight
    attended_ref[...] = (numerator / denominator).astype(bf16)
    def finish_columns():
        for target in range(1, N_Z):

            @pl.when(target > z)
            def _(target=target):
                column_copy(target).wait_send()

    yield started, finish_columns


class TpGather:
    def __init__(self, full, sends, recvs):
        self.full, self.sends, self.recvs = full, sends, recvs
        self.y, self.c = lax.axis_index("y"), lax.axis_index("c")
        self.half = full.shape[1] // 2
        self.started = []

    def _copy(self, number, shift, part, target):
        slot = lax.rem(self.y + shift, N_Y) * N_C + self.c
        if part is None:
            ref = self.full.at[slot]
        else:
            ref = self.full.at[slot, pl.ds(part * self.half, self.half)]
        if target == "core":
            device = {"c": 1 - self.c}
        else:
            device = {"y": lax.rem(self.y + (1 if target == "up" else N_Y - 1), N_Y)}
        return pltpu.make_async_remote_copy(
            src_ref=ref,
            dst_ref=ref,
            send_sem=self.sends.at[number],
            recv_sem=self.recvs.at[number],
            device_id=device,
            device_id_type=MESH_ID,
        )

    def _start(self, *what):
        copy = self._copy(*what)
        copy.start()
        self.started.append(copy)

    def start(self):
        self._start(0, 0, 0, "up")
        self._start(3, 0, 1, "down")
        self._start(1, 0, 1, "up")
        self._start(2, 0, 0, "down")
        self._start(6, 0, None, "core")

    def relay(self):
        self._copy(0, 0, 0, "up").wait_recv()
        self._start(4, N_Y - 1, 0, "up")
        self._copy(3, 0, 1, "down").wait_recv()
        self._start(5, 1, 1, "down")
        self._copy(1, 0, 1, "up").wait_recv()
        self._start(7, N_Y - 1, None, "core")
        self._copy(2, 0, 0, "down").wait_recv()
        self._start(8, 1, None, "core")

    def near(self):
        for number, shift in ((6, 0), (7, N_Y - 1), (8, 1)):
            self._copy(number, shift, None, "core").wait_recv()

    def far(self):
        self._copy(4, 0, 0, "up").wait_recv()
        self._start(9, 2, 0, "core")
        self._copy(5, 0, 1, "down").wait_recv()
        self._start(10, 2, 1, "core")
        for part in range(2):
            self._copy(9 + part, 2, part, "core").wait_recv()

    def finish(self):
        for copy in self.started:
            copy.wait_send()


def project_phase(
    greeted,
    after_gates,
    after_exchange,
    after_keys,
    tokens_hbm,
    gain,
    query_gain,
    latent_gain,
    cosine_row,
    sine_row,
    shift_hbm,
    narrow_query,
    narrow_latent,
    narrow_rotary,
    narrow_ingate,
    narrow_forget,
    query_hbm,
    key_hbm,
    value_hbm,
    outgate_hbm,
    query_up_hbm,
    key_up_hbm,
    value_up_hbm,
    mem_ref,
    gate_ref,
    q_ref,
    kv_ref,
    rows_all,
    query_latents,
    latents,
    small,
    ingate,
    forget,
    big,
    query_up,
    key_up,
    value_up,
    tokens,
    shift_row,
    pre_gates,
    up_query,
    up_latent,
    wide_query,
    wide_latent,
    load_sem,
    row_send,
    row_recv,
    lat_send,
    lat_recv,
    query_send,
    query_recv,
):
    f32, bf16 = jnp.float32, jnp.bfloat16
    y, c = lax.axis_index("y"), lax.axis_index("c")
    mine = y * N_C + c
    width = 128
    sources = (
        (narrow_query, small.at[pl.ds(0, QUERY_PART)]),
        (narrow_latent, small.at[pl.ds(width, LATENT_PART)]),
        (narrow_rotary, small.at[pl.ds(width + LATENT_PART, ROTARY_CHANNELS)]),
        (narrow_ingate, ingate),
        (narrow_forget, forget),
        (query_up_hbm, query_up),
        (key_up_hbm, key_up),
        (value_up_hbm, value_up),
        (shift_hbm, shift_row),
    )
    loads = [
        pltpu.make_async_copy(source, target, load_sem.at[k])
        for k, (source, target) in enumerate(sources)
    ]
    at = 0
    for k, ref in enumerate((query_hbm, key_hbm, value_hbm, outgate_hbm)):
        columns = ref.shape[1]
        loads.append(
            pltpu.make_async_copy(ref, big.at[:, pl.ds(at, columns)], load_sem.at[9 + k])
        )
        at += columns
    arrival = pltpu.make_async_copy(tokens_hbm, tokens, load_sem.at[13])
    arrival.start()
    for load in loads:
        load.start()
    arrival.wait()
    wide = tokens[...].astype(f32)
    inverse = lax.rsqrt(jnp.mean(wide * wide, axis=1, keepdims=True) + SMALL_CONSTANT)
    rows_all[mine] = (wide * inverse * gain[...].astype(f32).reshape(1, -1)).astype(bf16)
    small[QUERY_PART:width] = jnp.zeros((width - QUERY_PART, small.shape[1]), bf16)

    greeted()
    gather = TpGather(rows_all, row_send, row_recv)
    gather.start()

    for load in loads:
        load.wait()
    small[QUERY_PART : QUERY_PART + 8] = ingate[...]
    small[QUERY_PART + 16 : QUERY_PART + 24] = forget[...]
    up_query[...] = jnp.zeros(up_query.shape, bf16)
    query_rows = query_up[...].astype(f32).T.astype(bf16)
    for s in range(N_Y * N_C):
        up_query[s * width : s * width + QUERY_PART] = query_rows[
            s * QUERY_PART : (s + 1) * QUERY_PART
        ]
        part = slice(s * LATENT_PART, (s + 1) * LATENT_PART)
        for h in range(2):
            at = s * width + h * LATENT_PART
            up_latent[at : at + LATENT_PART, :width] = key_up[part]
            up_latent[at : at + LATENT_PART, width:] = value_up[part]

    lane = lax.broadcasted_iota(jnp.int32, (1, width), 1)
    cosine, sine_part = (
        jnp.concatenate([ref[...]] * 4, axis=0).T for ref in (cosine_row, sine_row)
    )
    row_id = lax.broadcasted_iota(jnp.int32, (width, width), 0)
    col_id = lax.broadcasted_iota(jnp.int32, (width, width), 1)
    channels = lax.rem(col_id, ROTARY_CHANNELS)
    halfway = ROTARY_CHANNELS // 2
    twin = (row_id == channels).astype(bf16)
    partner = lax.rem(channels + halfway, ROTARY_CHANNELS)
    sign = jnp.where(channels < halfway, -1.0, 1.0)

    def duplicated(values, offset):
        return jnp.dot(
            values, (row_id == channels + offset).astype(bf16), preferred_element_type=f32
        )

    def rotated(values, offset):
        swap = jnp.where(row_id == partner + offset, sign, 0.0).astype(bf16)
        turned = jnp.dot(values, swap, preferred_element_type=f32)
        return duplicated(values, offset) * cosine + turned * sine_part

    def chip_rows(chip):
        slots = [rows_all[chip * N_C + k] for k in range(N_C)]
        return jnp.concatenate(slots, axis=0)

    span = N_C * SHARE
    tile = 256

    def project_small(chip):
        rows = pl.ds(pl.multiple_of(chip * span, span), span)
        here = chip_rows(chip)
        made = lax.dot_general(here, small[...], CONTRACT_LAST, preferred_element_type=f32)
        turned = made[:, :width].T
        for k in range(2):
            at = QUERY_PART + 16 * k
            pre_gates[k, :, rows] = turned[at : at + 8]
        rounded = made.astype(bf16)
        query_latents[mine, rows] = rounded[:, :width]
        wide_latent[rows, :width] = rounded[:, width:]

    def project_big():
        def one(t, carry):
            columns = pl.ds(pl.multiple_of(t * tile, tile), tile)
            rows = rows_all[...].reshape(ROWS, rows_all.shape[2])
            made = jnp.dot(rows, big[:, columns], preferred_element_type=f32)
            mem_ref[:, columns] = made.astype(bf16)
            return carry

        lax.fori_loop(0, big.shape[1] // tile, one, 0)

    gather.relay()
    gather.near()
    near = [y, lax.rem(y + N_Y - 1, N_Y), lax.rem(y + 1, N_Y)]
    for chip in near:
        project_small(chip)
    opposite = lax.rem(y + 2, N_Y)
    gather.far()
    project_small(opposite)

    second = wide_latent[:, :width]
    both = duplicated(second, 0)
    half = ROWS // 2
    packed = jnp.where(lane < LATENT_PART, both[:half], both[half:])
    latents[mine] = packed.astype(bf16)
    exchange = TpGather(latents, lat_send, lat_recv)
    query_exchange = TpGather(query_latents, query_send, query_recv)
    exchange.start()
    query_exchange.start()
    project_big()
    heads = lax.broadcasted_iota(jnp.int32, (8, ROWS), 0) == mine
    in_pre, forget_pre = (
        jnp.sum(jnp.where(heads, pre_gates[k], 0.0), axis=0, keepdims=True) for k in range(2)
    )
    in_gate = SOFTCAP * jnp.tanh(in_pre / SOFTCAP)
    capped = SOFTCAP * jnp.tanh((forget_pre + shift_row[...]) / SOFTCAP)
    small_part = jnp.exp(-jnp.abs(capped))
    above_one = 1.0 + small_part
    grown = jnp.where(
        above_one == 1.0, small_part, jnp.log(above_one) * small_part / (above_one - 1.0)
    )
    log_forget = jnp.minimum(capped, 0.0) - grown
    earlier = lax.broadcasted_iota(jnp.int32, (ROWS, ROWS), 0) <= lax.broadcasted_iota(
        jnp.int32, (ROWS, ROWS), 1
    )
    cumulative = jnp.dot(
        jnp.broadcast_to(log_forget, (8, ROWS)),
        earlier.astype(f32),
        precision=PRECISE,
        preferred_element_type=f32,
    )
    top_rows = lax.broadcasted_iota(jnp.int32, (8, ROWS), 0) == 0
    gate_ref[...] = jnp.where(top_rows, in_gate - cumulative, cumulative)
    exchange.relay()
    after_gates()
    query_exchange.relay()
    key_turned = rotated(second, LATENT_PART)
    kv_ref[2 * ROWS :] = jnp.where(
        lane < ROTARY_CHANNELS, key_turned[:half], key_turned[half:]
    ).astype(bf16)
    exchange.near()
    after_exchange()
    exchange.far()

    squares = jnp.zeros((half, width), f32)
    for s in range(N_Y * N_C):
        part = latents[s].astype(f32)
        squares = squares + part * part
    low = lane < LATENT_PART
    low_scale, high_scale = (
        lax.rsqrt(
            jnp.sum(jnp.where(low == first, squares, 0.0), axis=1, keepdims=True) / LATENT_WIDTH
            + SMALL_CONSTANT
        )
        for first in (True, False)
    )
    latent_scale = jnp.where(low, low_scale, high_scale)
    query_gains = jnp.broadcast_to(query_gain[...].reshape(1, -1), (8, QUERY_LATENT))
    latent_gains = jnp.broadcast_to(latent_gain[...].reshape(1, -1), (8, LATENT_WIDTH))

    def latent_gain_of(s):
        pair = slice((s // 2) * width, (s // 2 + 1) * width)
        shift = LATENT_WIDTH - LATENT_PART if s % 2 else LATENT_PART
        here = latent_gains[:1, pair]
        other = pltpu.roll(latent_gains, shift, 1)[:1, pair]
        return jnp.where(low, other, here) if s % 2 else jnp.where(low, here, other)

    def query_gain_of(s):
        turned = query_gains
        if s:
            turned = pltpu.roll(query_gains, QUERY_LATENT - s * QUERY_PART, 1)
        return turned[:1, :width]

    for s in range(N_Y * N_C):
        columns = slice(s * width, (s + 1) * width)
        part = latents[s].astype(f32)
        made = (part * latent_scale * latent_gain_of(s)).astype(bf16)
        wide_latent[:half, columns] = jnp.where(low, made, jnp.zeros_like(made))
        wide_latent[half:, columns] = jnp.where(low, jnp.zeros_like(made), made)
    made = jnp.dot(wide_latent[...], up_latent[...], preferred_element_type=f32).astype(bf16)
    kv_ref[:ROWS] = made[:, :width]
    kv_ref[ROWS : 2 * ROWS] = made[:, width:]
    after_keys()

    query_exchange.near()
    query_exchange.far()
    query_mask = (lane < QUERY_PART).astype(f32)
    squares = jnp.zeros((ROWS, width), f32)
    for s in range(N_Y * N_C):
        part = query_latents[s].astype(f32) * query_mask
        squares = squares + part * part
    query_scale = lax.rsqrt(
        jnp.sum(squares, axis=1, keepdims=True) / QUERY_LATENT + SMALL_CONSTANT
    )
    for s in range(N_Y * N_C):
        columns = slice(s * width, (s + 1) * width)
        part = query_latents[s].astype(f32) * query_mask
        wide_query[:, columns] = (part * query_scale * query_gain_of(s)).astype(bf16)
    made = jnp.dot(wide_query[...], up_query[...], preferred_element_type=f32).astype(bf16)
    q_ref[:, :width] = made[:, :width]
    turning = jnp.concatenate([made[:, width:], jnp.zeros((ROWS, ROTARY_CHANNELS), bf16)], axis=1)
    q_ref[:, width:] = rotated(turning, 0).astype(bf16)
    return gather.started + exchange.started + query_exchange.started


def output_phase(
    gated,
    attended,
    out_memory,
    out_attend,
    o_ref,
    kept,
    to_core,
    from_core,
    sums,
    passing,
    from_below,
    from_above,
    relay_in,
    core_send,
    core_recv,
    relay_send,
    relay_recv,
    up_send,
    up_recv,
    down_send,
    down_recv,
):
    f32, bf16 = jnp.float32, jnp.bfloat16
    y, c = lax.axis_index("y"), lax.axis_index("c")
    above, below = lax.rem(y + 1, N_Y), lax.rem(y + N_Y - 1, N_Y)
    opposite = lax.rem(y + 2, N_Y)
    half = out_memory.shape[1] // 2
    tile = 512

    def remote(source, target, send, recv, device):
        return pltpu.make_async_remote_copy(
            src_ref=source,
            dst_ref=target,
            send_sem=send,
            recv_sem=recv,
            device_id=device,
            device_id_type=MESH_ID,
        )

    def rows_of(ref, core):
        picked = [ref[pl.ds(pl.multiple_of((k * N_C + core) * SHARE, SHARE), SHARE)] for k in range(N_Y)]
        return jnp.concatenate(picked, axis=0)

    def columns_of(h, t):
        return slice(h * half + t * tile, h * half + (t + 1) * tile)

    for k, core in enumerate((1 - c, c)):
        memory_rows = rows_of(gated, core)
        for h in range(2):
            for t in range(half // tile):
                kept[k, h, :, t * tile : (t + 1) * tile] = jnp.dot(
                    memory_rows, out_memory[:, columns_of(h, t)], preferred_element_type=f32
                )
    yield

    def partial(k, h, store):
        attend_rows = rows_of(attended, c if k else 1 - c)
        for t in range(half // tile):
            made = jnp.dot(
                attend_rows, out_attend[:, columns_of(h, t)], preferred_element_type=f32
            )
            made = kept[k, h, :, t * tile : (t + 1) * tile] + made
            store(t * tile, made.astype(bf16).reshape(N_Y, SHARE, tile))

    def core_copy(h):
        return remote(
            to_core.at[h], from_core.at[h], core_send.at[h], core_recv.at[h], {"c": 1 - c}
        )

    def relay_copy(h):
        return remote(
            passing.at[h],
            relay_in.at[h],
            relay_send.at[h],
            relay_recv.at[h],
            {"y": above if h == 0 else below},
        )

    def up_copy(h):
        return remote(
            passing.at[2 + h], from_below.at[h], up_send.at[h], up_recv.at[h], {"y": above}
        )

    def down_copy(h):
        return remote(
            passing.at[4 + h], from_above.at[h], down_send.at[h], down_recv.at[h], {"y": below}
        )

    started = []

    def start(copy):
        copy.start()
        started.append(copy)

    for h in range(2):

        def keep(at, block, h=h):
            to_core[h, :, :, at : at + tile] = block

        partial(0, h, keep)
        start(core_copy(h))
    for h in range(2):

        def keep(at, block, h=h):
            sums[h, :, :, at : at + tile] = block.astype(f32)

        partial(1, h, keep)
    for h in range(2):
        core_copy(h).wait_recv()
        sums[h] = sums[h] + from_core[h].astype(f32)
        passing[h] = sums[h, opposite].astype(bf16)
        start(relay_copy(h))
        if h == 0:
            passing[4] = sums[0, below].astype(bf16)
            start(down_copy(0))
        else:
            passing[3] = sums[1, above].astype(bf16)
            start(up_copy(1))
    relay_copy(0).wait_recv()
    passing[2] = (sums[0, above] + relay_in[0].astype(f32)).astype(bf16)
    start(up_copy(0))
    relay_copy(1).wait_recv()
    passing[5] = (sums[1, below] + relay_in[1].astype(f32)).astype(bf16)
    start(down_copy(1))
    for h in (1, 0):
        up_copy(h).wait_recv()
        down_copy(h).wait_recv()
        made = sums[h, y] + from_below[h].astype(f32) + from_above[h].astype(f32)
        o_ref[:, h * half : (h + 1) * half] = made.astype(bf16)
    yield started


def scratch(depth, mem_width):
    f32, bf16 = jnp.float32, jnp.bfloat16
    dma = pltpu.SemaphoreType.DMA
    between = (
        pltpu.VMEM((ROWS, VALUE_CHANNELS), bf16),
        pltpu.VMEM((ROWS, M_V), bf16),
        pltpu.VMEM((ROWS, mem_width), bf16),
        pltpu.VMEM((8, ROWS), f32),
        pltpu.VMEM((ROWS, 256), bf16),
        pltpu.VMEM((ROWS * 5 // 2, 128), bf16),
        pltpu.VMEM((M_V, depth), bf16),
        pltpu.VMEM((VALUE_CHANNELS, depth), bf16),
        dma((2,)),
    )
    for_project = (
        pltpu.VMEM((N_Y * N_C, SHARE, depth), bf16),
        pltpu.VMEM((N_Y * N_C, ROWS, 128), bf16),
        pltpu.VMEM((N_Y * N_C, ROWS // 2, 128), bf16),
        pltpu.VMEM((256, depth), bf16),
        pltpu.VMEM((8, depth), bf16),
        pltpu.VMEM((8, depth), bf16),
        pltpu.VMEM((depth, mem_width), bf16),
        pltpu.VMEM((PLAIN_CHANNELS + ROTARY_CHANNELS, QUERY_LATENT), bf16),
        pltpu.VMEM((LATENT_WIDTH, PLAIN_CHANNELS), bf16),
        pltpu.VMEM((LATENT_WIDTH, VALUE_CHANNELS), bf16),
        pltpu.VMEM((SHARE, depth), bf16),
        pltpu.VMEM((1, ROWS), f32),
        pltpu.VMEM((2, 8, ROWS), f32),
        pltpu.VMEM((1024, PLAIN_CHANNELS + ROTARY_CHANNELS), bf16),
        pltpu.VMEM((1024, 256), bf16),
        pltpu.VMEM((ROWS, 1024), bf16),
        pltpu.VMEM((ROWS, 1024), bf16),
        dma((16,)),
        dma((11,)),
        dma((11,)),
        dma((11,)),
        dma((11,)),
        dma((11,)),
        dma((11,)),
    )
    for_attend = (
        pltpu.VMEM((N_X, ROWS, 256), bf16),
        pltpu.VMEM((N_Z, ROWS * 5 // 2, 128), bf16),
        pltpu.VMEM((ROWS, 256), bf16),
        pltpu.VMEM((N_X * ROWS, 128), f32),
        pltpu.VMEM((N_X * ROWS, 128), f32),
        pltpu.VMEM((N_X * ROWS, VALUE_CHANNELS), f32),
        pltpu.VMEM((N_X - 1, ROWS, VALUE_CHANNELS), bf16),
        pltpu.VMEM((N_X - 1, 8, ROWS), f32),
        pltpu.VMEM((N_X - 1, ROWS, VALUE_CHANNELS), bf16),
        pltpu.VMEM((N_X - 1, 8, ROWS), f32),
        pltpu.VMEM((ROWS, M_V), f32),
        pltpu.VMEM((ROWS, 128), f32),
        pltpu.VMEM((ROWS, 128), f32),
        pltpu.VMEM((N_X, STATE_ROWS, M_V), f32),
        pltpu.VMEM((N_X, STATE_ROWS, M_V), f32),
        pltpu.VMEM((STATE_ROWS, M_V), f32),
        pltpu.VMEM((N_Z, STATE_ROWS, M_V), f32),
        pltpu.VMEM((N_X, STATE_ROWS, M_V), f32),
        pltpu.VMEM((N_X, STATE_ROWS, M_V), f32),
        pltpu.VMEM((2, 8, ROWS), f32),
        pltpu.VMEM((N_Y, 8, ROWS), f32),
        pltpu.VMEM((2, ROWS // 2, VALUE_CHANNELS), bf16),
        dma((6,)),
        dma((6,)),
        dma((N_Z // 2, 2)),
        dma((N_Z // 2, 2)),
        dma((N_Z // 2, 2)),
        dma((N_Z // 2, 2)),
        dma((N_X - 1,)),
        dma((N_X - 1,)),
        dma((N_X - 1,)),
        dma((N_X - 1,)),
        dma((N_X - 1,)),
        dma((N_X - 1,)),
        dma((N_Z,)),
        dma((N_Z,)),
        dma((N_X - 1,)),
        dma((N_X - 1,)),
        dma((N_Y,)),
        dma((N_Y,)),
        dma((2, 2)),
        dma((2, 2)),
    )
    for_output = (
        pltpu.VMEM((2, 2, N_Y * SHARE, depth // 2), f32),
        pltpu.VMEM((2, N_Y, SHARE, depth // 2), bf16),
        pltpu.VMEM((2, N_Y, SHARE, depth // 2), bf16),
        pltpu.VMEM((2, N_Y, SHARE, depth // 2), f32),
        pltpu.VMEM((6, SHARE, depth // 2), bf16),
        pltpu.VMEM((2, SHARE, depth // 2), bf16),
        pltpu.VMEM((2, SHARE, depth // 2), bf16),
        pltpu.VMEM((2, SHARE, depth // 2), bf16),
        dma((2,)),
        dma((2,)),
        dma((2,)),
        dma((2,)),
        dma((2,)),
        dma((2,)),
        dma((2,)),
        dma((2,)),
    )
    return between, for_project, for_attend, for_output


N_INPUTS = 22
N_PROJECT_INPUTS = 19
IN_VMEM = (1, 2, 3, 4, 5, 19)


def layer_kernel(counts, *refs):
    y, c = lax.axis_index("y"), lax.axis_index("c")
    z, x = lax.axis_index("z"), lax.axis_index("x")
    project_inputs = refs[:N_PROJECT_INPUTS]
    mem_gain, out_memory_hbm, out_attend_hbm, out_ref = refs[N_PROJECT_INPUTS : N_INPUTS + 1]
    groups, at = [], N_INPUTS + 1
    for count in counts:
        groups.append(refs[at : at + count])
        at += count
    between, for_project, for_attend, for_output = groups
    attended, gated, mem, gates, queries, keys_values, out_memory, out_attend, out_sem = between

    barrier = pltpu.get_barrier_semaphore()
    devices = [{"c": 1 - c}]
    devices += [{"y": lax.rem(y + d, N_Y)} for d in range(1, N_Y)]
    devices += [{"x": lax.rem(x + d, N_X)} for d in range(1, N_X)]
    devices += [{"z": lax.rem(z + d, N_Z)} for d in range(1, N_Z)]
    for device in devices:
        pl.semaphore_signal(barrier, inc=1, device_id=device, device_id_type=MESH_ID)
    loads = [
        pltpu.make_async_copy(out_memory_hbm, out_memory, out_sem.at[0]),
        pltpu.make_async_copy(out_attend_hbm, out_attend, out_sem.at[1]),
    ]
    attending = attend_phase(
        queries, keys_values, mem, gates, mem_gain, attended, gated, *for_attend
    )
    started = project_phase(
        lambda: pl.semaphore_wait(barrier, len(devices)),
        *[lambda: next(attending)] * 3,
        *project_inputs,
        mem,
        gates,
        queries,
        keys_values,
        *for_project,
    )
    for load in loads:
        load.start()
    outputting = output_phase(gated, attended, out_memory, out_attend, out_ref, *for_output)
    next(attending)
    for load in loads:
        load.wait()
    next(outputting)
    more, finish_columns = next(attending)
    started += more
    started += next(outputting)
    for copy in started:
        copy.wait_send()
    finish_columns()


def layer(*inputs):
    depth = inputs[0].shape[1]
    mem_width = 2 * M_QK + 2 * M_V
    groups = scratch(depth, mem_width)
    vmem = pl.BlockSpec(memory_space=pltpu.VMEM)
    hbm = pl.BlockSpec(memory_space=pltpu.HBM)
    return pl.pallas_call(
        functools.partial(layer_kernel, tuple(len(group) for group in groups)),
        out_shape=jax.ShapeDtypeStruct((SHARE, depth), jnp.bfloat16),
        in_specs=[vmem if k in IN_VMEM else hbm for k in range(N_INPUTS)],
        out_specs=vmem,
        scratch_shapes=[one for group in groups for one in group],
        compiler_params=pltpu.CompilerParams(
            collective_id=1, has_side_effects=True, vmem_limit_bytes=67_000_000
        ),
        cost_estimate=pl.CostEstimate(
            flops=8 * 10**9, bytes_accessed=2 * 10**7, transcendentals=4 * 10**6
        ),
        name="layer",
    )(*inputs)


def per_device(
    tokens,
    input_gain,
    weight_query,
    weight_key,
    weight_value,
    weight_outgate,
    weight_ingate,
    weight_forget,
    forget_shift,
    mem_gain,
    query_down_weight,
    latent_down_weight,
    down_rotary,
    query_gain,
    latent_gain,
    query_up_weight,
    key_up_weight,
    value_up_weight,
    out_memory,
    out_attend,
):
    length = forget_shift.shape[0]
    positions = lax.axis_index(SP) * length + jnp.arange(length, dtype=jnp.int32)
    halfway = ROTARY_CHANNELS // 2
    inverse = jnp.power(ROTARY_BASE, -jnp.arange(halfway, dtype=jnp.float32) / halfway)
    angles = positions.astype(jnp.float32)[None, :] * inverse[:, None]
    return layer(
        tokens,
        input_gain,
        query_gain,
        latent_gain,
        jnp.cos(angles),
        jnp.sin(angles),
        forget_shift.T,
        query_down_weight.T,
        latent_down_weight.T,
        down_rotary.T,
        weight_ingate.T,
        weight_forget.T,
        weight_query,
        weight_key,
        weight_value,
        weight_outgate,
        query_up_weight.T,
        key_up_weight,
        value_up_weight,
        mem_gain,
        out_memory,
        out_attend,
    )


def solution(mesh):
    torus = Mesh(mesh.devices.reshape(N_Z, N_X, 4, 2), SP_TP)
    in_specs = (
        P(SP_TP, None),
        P(),
        P(None, TP),
        P(None, TP),
        P(None, TP),
        P(None, TP),
        P(),
        P(),
        P(SP, TP),
        P(),
        P(None, TP),
        P(None, TP),
        P(),
        P(),
        P(),
        P(None, TP),
        P(None, TP),
        P(None, TP),
        P(TP, None),
        P(TP, None),
    )
    out_specs = P(SP_TP, None)
    return jax.shard_map(
        per_device, mesh=torus, in_specs=in_specs, out_specs=out_specs, check_vma=False
    )
```
